32 devices in a mesh: sp: 4 (over z), fs: 4 (over y, x), tp: 2 (over core).
Axes of the slice: x: 2, y: 2, z: 4, core: 2. Of those that a mesh axis runs over, the one named last changes fastest.
Arguments:
- hidden_in: bfloat16 [4, 1024, 2048], P('fs', 'sp', 'tp'), may hold values from -6 to 6
- sb_query_w: bfloat16 [2048, 1024], P('fs', 'tp'), may hold values from -0.21875 to 0.21875
- sb_key_w: bfloat16 [2048, 1024], P('fs', 'tp'), may hold values from -0.21875 to 0.21875
- sb_value_w: bfloat16 [2048, 1024], P('fs', 'tp'), may hold values from -0.125 to 0.125
- sb_offset: float32 [16], P('tp'), may hold values from -16 to -6
- delta_query_w: bfloat16 [2048, 1024], P('fs', 'tp'), may hold values from -0.125 to 0.125
- delta_key_w: bfloat16 [2048, 1024], P('fs', 'tp'), may hold values from -0.125 to 0.125
- delta_value_w: bfloat16 [2048, 1024], P('fs', 'tp'), may hold values from -0.125 to 0.125
- decay_w: bfloat16 [2048, 8], P(None, 'tp'), may hold values from -0.125 to 0.125
- write_w: bfloat16 [2048, 8], P(None, 'tp'), may hold values from -0.125 to 0.125
- write_bias: float32 [8], P('tp'), may hold values from -7 to 1.5
- decay_log_scale: float32 [8], P('tp'), may hold values from -14 to -3
- decay_shift: float32 [4, 8, 1024], P('fs', 'tp', 'sp'), may hold values from -3 to 0
- head_gain: float32 [128], replicated, may hold values from 0.1 to 1.9
- sb_out_w: bfloat16 [1024, 2048], P('tp'), may hold values from -0.125 to 0.125
- delta_out_w: bfloat16 [1024, 2048], P('tp'), may hold values from -0.125 to 0.125
Outputs:
- mixed_out: bfloat16 [4, 1024, 2048], P('fs', ('sp', 'tp'))
The draws below stay inside these ranges and needn't reach their ends.
All inputs are finite; a program needn't handle non-finite values.
Results may differ from the reference program's by a relative error of at most 0.015.
Values may be sent and summed in bfloat16 or wider, within the bound.
A program may use at most 128 MiB of HBM per device.

```python
import jax
import jax.numpy as jnp
from jax import lax

D = 2048
SB_HEADS = 16
SB_DIM = 64
GDN_HEADS = 8
GDN_DIM = 128
BLOCK = 64
TOK_DEV = 256
LEN = 1024
SEQS = 4
N_TP = 2


def head_kinds(key, fast_share):
    return jax.random.uniform(jax.random.fold_in(key, 71), (GDN_HEADS,), jnp.float32) < fast_share


def draw_sb_offset(key, part):
    reach_term = jax.random.uniform(key, (SB_HEADS,), jnp.float32, -1.0, 2.5)
    return reach_term - jnp.log(jnp.float32(LEN)) - 4.5


def draw_write_bias(key, part):
    fast_share = 0.5
    chosen = head_kinds(key, fast_share)
    strong_term = jax.random.uniform(jax.random.fold_in(key, 5), (GDN_HEADS,), jnp.float32, -1.0, 1.5)
    faint_summand = jax.random.uniform(jax.random.fold_in(key, 6), (GDN_HEADS,), jnp.float32, -7.0, -5.5)
    return jnp.where(chosen, strong_term, faint_summand)


def draw_decay_log_scale(key, part):
    split_keys = jax.random.split(key, 3)
    fast_share = 0.5
    chosen = head_kinds(key, fast_share)
    fast_rate = jax.random.uniform(split_keys[1], (GDN_HEADS,), jnp.float32, 0.015, 0.04)
    slow_rate = jax.random.uniform(split_keys[2], (GDN_HEADS,), jnp.float32, 2e-06, 8e-06)
    return jnp.log(jnp.where(chosen, fast_rate, slow_rate))


def draw_decay_shift(key, part):
    split_keys = jax.random.split(key, 3)
    blocks_count = LEN // TOK_DEV
    minimal_level = 0.15
    highest = 1.2
    rates = jnp.exp(jax.random.uniform(split_keys[0], (SEQS, GDN_HEADS, blocks_count), jnp.float32, jnp.log(minimal_level), jnp.log(highest)))
    unweighted_result = jnp.repeat(rates, TOK_DEV, axis=2) * (-1.0 / LEN)
    destination_indices = jax.random.randint(split_keys[1], (SEQS, GDN_HEADS, 3), 0, LEN)
    forgetting_amounts = jnp.log(jax.random.uniform(split_keys[2], (SEQS, GDN_HEADS, 3), jnp.float32, 0.5, 0.8))
    cell_locations = jnp.arange(LEN, dtype=jnp.int32)
    storing_pulses = jnp.sum(jnp.where(cell_locations[None, None, None, :] == destination_indices[..., None], forgetting_amounts[..., None], 0.0), axis=2)
    return unweighted_result + storing_pulses


def shard_levels(own_key, dims, pieces, smallest, top_value):
    gain, own = 1.0, jax.random.fold_in(own_key, 6)
    for axis_at, blocks in pieces:
        heights = jnp.exp(jax.random.uniform(jax.random.fold_in(own, axis_at), (blocks,), jnp.float32, smallest / len(pieces), top_value / len(pieces)))
        gain = gain * jnp.repeat(heights, dims[axis_at] // blocks).reshape([-1 if axis == axis_at else 1 for axis in range(len(dims))])
    return gain


def gaussian(own_key, dims, scale, reach, shards=(), kind=jnp.bfloat16):
    drawn = jax.random.normal(own_key, dims, jnp.float32) * scale
    if len(shards) > 0:
        drawn = shard_levels(own_key, dims, shards, -0.22, 0.18) * drawn
    return jnp.clip(drawn, min=-reach, max=reach).astype(kind)


def setup_inputs(seed: int = 0) -> dict:
    streams_of = jax.random.split(jax.random.key(seed), 17)
    hidden_in = gaussian(streams_of[0], (SEQS, LEN, D), 1.0, 6.0, ((0, 4), (1, 4), (2, 2)))
    sb_query_w = gaussian(streams_of[1], (D, SB_HEADS * SB_DIM), (D // 3) ** -0.5, 0.21875, ((0, 4), (1, 2)))
    sb_key_w = gaussian(streams_of[2], (D, SB_HEADS * SB_DIM), (D // 3) ** -0.5, 0.21875, ((0, 4), (1, 2)))
    sb_value_w = gaussian(streams_of[3], (D, SB_HEADS * SB_DIM), D ** -0.5, 0.125, ((0, 4), (1, 2)))
    sb_offset = draw_sb_offset(jax.random.fold_in(streams_of[16], 71), 0)
    delta_query_w = gaussian(streams_of[5], (D, GDN_HEADS * GDN_DIM), D ** -0.5, 0.125, ((0, 4), (1, 2)))
    delta_key_w = gaussian(streams_of[6], (D, GDN_HEADS * GDN_DIM), D ** -0.5, 0.125, ((0, 4), (1, 2)))
    delta_value_w = gaussian(streams_of[7], (D, GDN_HEADS * GDN_DIM), D ** -0.5, 0.125, ((0, 4), (1, 2)))
    decay_w = gaussian(streams_of[8], (D, GDN_HEADS), D ** -0.5, 0.125, ((1, 2),))
    write_w = gaussian(streams_of[9], (D, GDN_HEADS), D ** -0.5, 0.125, ((1, 2),))
    write_bias = draw_write_bias(jax.random.fold_in(streams_of[16], 71), 0)
    decay_log_scale = draw_decay_log_scale(jax.random.fold_in(streams_of[16], 71), 0)
    decay_shift = draw_decay_shift(jax.random.fold_in(streams_of[16], 71), 0)
    head_gain = jnp.clip(1.0 + 0.18 * jax.random.normal(streams_of[13], (GDN_DIM,), jnp.float32), 0.1, 1.9)
    sb_out_w = gaussian(streams_of[14], (SB_HEADS * SB_DIM, D), (SB_HEADS * SB_DIM + GDN_HEADS * GDN_DIM) ** -0.5, 0.125, ((0, 2),))
    delta_out_w = gaussian(streams_of[15], (GDN_HEADS * GDN_DIM, D), (SB_HEADS * SB_DIM + GDN_HEADS * GDN_DIM) ** -0.5, 0.125, ((0, 2),))
    return dict(hidden_in=hidden_in, sb_query_w=sb_query_w, sb_key_w=sb_key_w, sb_value_w=sb_value_w, sb_offset=sb_offset, delta_query_w=delta_query_w, delta_key_w=delta_key_w, delta_value_w=delta_value_w, decay_w=decay_w, write_w=write_w, write_bias=write_bias, decay_log_scale=decay_log_scale, decay_shift=decay_shift, head_gain=head_gain, sb_out_w=sb_out_w, delta_out_w=delta_out_w)


EXACT_MATMUL = lax.Precision.HIGHEST
NORM_EPS = 1e-06

def unit_lower_inverse(strict_part):
    order_size = strict_part.shape[-1]
    powered = strict_part
    inverse = jnp.eye(order_size, dtype=strict_part.dtype) - strict_part
    for repeat_number in range(max(1, (order_size - 1).bit_length()) - 1):
        powered = jnp.einsum('...ij,...jk->...ik', powered, powered, precision=EXACT_MATMUL)
        inverse = inverse + jnp.einsum('...ij,...jk->...ik', inverse, powered, precision=EXACT_MATMUL)
    return inverse

def to_blocks(row_data, block_span):
    blocks_count = row_data.shape[0] // block_span
    shaped = row_data.reshape((blocks_count, block_span) + row_data.shape[1:])
    return jnp.swapaxes(shaped, 1, 2)

def from_blocks(blocked):
    swapped = jnp.swapaxes(blocked, 1, 2)
    return swapped.reshape((-1,) + swapped.shape[2:])

def unit_rows(vectors):
    return vectors * lax.rsqrt(lax.optimization_barrier(jnp.sum(vectors * vectors, axis=-1, keepdims=True)) + NORM_EPS)

def delta_inputs(query_proj, key_proj, value_proj, decay_pre, write_pre, write_bias, decay_log_scale, shift_rows, head_count, head_size):
    query_act = jax.nn.silu(query_proj.astype(jnp.float32)).reshape(-1, head_count, head_size)
    key_act = jax.nn.silu(key_proj.astype(jnp.float32)).reshape(-1, head_count, head_size)
    value_rows = jax.nn.silu(value_proj.astype(jnp.float32)).reshape(-1, head_count, head_size)
    queries = unit_rows(query_act) * head_size ** (-0.5)
    key_rows = unit_rows(key_act)
    log_decay = -jnp.exp(decay_log_scale) * jax.nn.softplus(decay_pre) + shift_rows
    strength = jax.nn.sigmoid(write_pre + write_bias)
    return (queries, key_rows, value_rows, log_decay, strength)

def delta_prepare(queries, key_rows, value_rows, log_decay, strength):
    block_span = queries.shape[2]
    cumulative = jnp.cumsum(log_decay, axis=-1)
    row_place = lax.broadcasted_iota(jnp.int32, (block_span, block_span), 0)
    col_place = lax.broadcasted_iota(jnp.int32, (block_span, block_span), 1)
    inclusive = col_place <= row_place
    strictly = col_place < row_place
    spread = cumulative[..., :, None] - cumulative[..., None, :]
    decay_table = jnp.where(inclusive, jnp.exp(jnp.where(inclusive, spread, 0.0)), 0.0)
    keys_beta = key_rows * strength[..., None]
    lower_part = jnp.where(strictly, jnp.einsum('nhik,nhjk->nhij', keys_beta, key_rows, precision=EXACT_MATMUL) * decay_table, 0.0)
    inverse = unit_lower_inverse(lower_part)
    growth = jnp.exp(cumulative)
    state_updates = jnp.einsum('nhij,nhjv->nhiv', inverse, value_rows * strength[..., None], precision=EXACT_MATMUL)
    erase_term = jnp.einsum('nhij,nhjk->nhik', inverse, keys_beta * growth[..., None], precision=EXACT_MATMUL)
    inside_block = jnp.einsum('nhik,nhjk->nhij', queries, key_rows, precision=EXACT_MATMUL) * decay_table
    boosted_query = queries * growth[..., None]
    damped_keys = key_rows * jnp.exp(cumulative[..., -1:] - cumulative)[..., None]
    decay_per_block = jnp.exp(cumulative[..., -1])
    return (state_updates, erase_term, inside_block, boosted_query, damped_keys, decay_per_block)

def delta_step(memory_state, inputs):
    state_updates, erase_term, inside_block, boosted_query, damped_keys, decay_per_block = inputs
    fixed_values = state_updates - jnp.einsum('mzq,mqc->mzc', erase_term, memory_state, precision=EXACT_MATMUL)
    produced_rows = jnp.einsum('mzq,mqc->mzc', boosted_query, memory_state, precision=EXACT_MATMUL) + jnp.einsum('efq,eqn->efn', inside_block, fixed_values, precision=EXACT_MATMUL)
    memory_state = memory_state * decay_per_block[:, None, None] + jnp.einsum('wam,waz->wmz', damped_keys, fixed_values, precision=EXACT_MATMUL)
    return (memory_state, produced_rows)

def stick_block(queries, key_rows, value_rows, query_place, key_place, offsets):
    scale_factor = queries.shape[-1] ** (-0.5)
    scores = jnp.einsum('qhd,khd->hqk', queries.astype(jnp.float32), key_rows.astype(jnp.float32)) * scale_factor + offsets[:, None, None]
    visible = key_place[None, :] < query_place[:, None]
    skipped = jnp.where(visible, jax.nn.log_sigmoid(-scores), 0.0)
    beyond = lax.cumsum(skipped, axis=2, reverse=True) - skipped
    weights = jnp.where(visible, jnp.exp(jax.nn.log_sigmoid(scores) + beyond), 0.0).astype(jnp.bfloat16)
    weights = lax.optimization_barrier(weights).astype(jnp.float32)
    partial_value = jnp.einsum('hqk,khd->qhd', weights, value_rows.astype(jnp.float32))
    return (partial_value, lax.optimization_barrier(jnp.sum(skipped, axis=2)).T)

def stick_combine(partials, totals):
    beyond = jnp.cumsum(totals[::-1], axis=0)[::-1] - totals
    return lax.optimization_barrier(jnp.sum(partials * jnp.exp(beyond)[..., None], axis=0))

def stick_sequence(queries, key_rows, value_rows, offsets):
    blocks_count = LEN // TOK_DEV
    query_blocks = queries.reshape((blocks_count, TOK_DEV) + queries.shape[1:])
    key_blocks = key_rows.reshape((blocks_count, TOK_DEV) + key_rows.shape[1:])
    value_blocks = value_rows.reshape((blocks_count, TOK_DEV) + value_rows.shape[1:])
    cell_locations = jnp.arange(LEN, dtype=jnp.int32).reshape(blocks_count, TOK_DEV)
    head_count = queries.shape[1]
    head_size = value_rows.shape[2]

    def per_query(query_index):

        def per_key(key_index):

            def active(unused_arg):
                return stick_block(query_blocks[query_index], key_blocks[key_index], value_blocks[key_index], cell_locations[query_index], cell_locations[key_index], offsets)

            def inactive(unused_arg):
                return (jnp.zeros((TOK_DEV, head_count, head_size), jnp.float32), jnp.zeros((TOK_DEV, head_count), jnp.float32))
            return lax.cond(key_index <= query_index, active, inactive, 0)
        partials, totals = lax.map(per_key, jnp.arange(blocks_count, dtype=jnp.int32))
        return stick_combine(partials, totals)
    gathered = lax.map(per_query, jnp.arange(blocks_count, dtype=jnp.int32))
    return gathered.reshape(LEN, head_count, head_size)

def reference(hidden_in, sb_query_w, sb_key_w, sb_value_w, sb_offset, delta_query_w, delta_key_w, delta_value_w, decay_w, write_w, write_bias, decay_log_scale, decay_shift, head_gain, sb_out_w, delta_out_w):

    def one_sequence(inputs):
        sequence_rows, shift_rows = inputs

        def project(weight):
            return jnp.dot(sequence_rows, weight, preferred_element_type=jnp.float32).astype(jnp.bfloat16)
        sb_query = project(sb_query_w).reshape(LEN, SB_HEADS, SB_DIM)
        sb_keys = project(sb_key_w).reshape(LEN, SB_HEADS, SB_DIM)
        sb_values = project(sb_value_w).reshape(LEN, SB_HEADS, SB_DIM)
        sb_mixed = stick_sequence(sb_query, sb_keys, sb_values, sb_offset).astype(jnp.bfloat16).reshape(LEN, SB_HEADS * SB_DIM)
        decay_pre = jnp.dot(sequence_rows, decay_w, preferred_element_type=jnp.float32)
        write_pre = jnp.dot(sequence_rows, write_w, preferred_element_type=jnp.float32)
        queries, key_rows, value_rows, log_decay, strength = delta_inputs(project(delta_query_w), project(delta_key_w), project(delta_value_w), decay_pre, write_pre, write_bias, decay_log_scale, shift_rows.T, GDN_HEADS, GDN_DIM)
        prepared = delta_prepare(to_blocks(queries, BLOCK), to_blocks(key_rows, BLOCK), to_blocks(value_rows, BLOCK), to_blocks(log_decay, BLOCK), to_blocks(strength, BLOCK))
        initial = jnp.zeros((GDN_HEADS, GDN_DIM, GDN_DIM), jnp.float32)
        unused_memory, produced_rows = lax.scan(delta_step, initial, prepared)
        produced_rows = from_blocks(produced_rows)
        normed = produced_rows * lax.rsqrt(lax.optimization_barrier(jnp.mean(produced_rows * produced_rows, axis=-1, keepdims=True)) + NORM_EPS) * head_gain
        delta_mixed = normed.astype(jnp.bfloat16).reshape(LEN, GDN_HEADS * GDN_DIM)
        sb_group = SB_HEADS * SB_DIM // N_TP
        delta_group = GDN_HEADS * GDN_DIM // N_TP
        accumulated = jnp.zeros((LEN, D), jnp.float32)
        for group_number in range(N_TP):
            sb_cols = slice(group_number * sb_group, (group_number + 1) * sb_group)
            delta_cols = slice(group_number * delta_group, (group_number + 1) * delta_group)
            term = jnp.dot(sb_mixed[:, sb_cols], sb_out_w[sb_cols], preferred_element_type=jnp.float32) + jnp.dot(delta_mixed[:, delta_cols], delta_out_w[delta_cols], preferred_element_type=jnp.float32)
            rounded = lax.optimization_barrier(term.astype(jnp.bfloat16))
            accumulated = accumulated + rounded.astype(jnp.float32)
        return accumulated.astype(jnp.bfloat16)
    return lax.map(one_sequence, (hidden_in, decay_shift))
```

```python
import jax
import jax.numpy as jnp
from jax import lax
from jax.experimental import pallas as pl
from jax.experimental.pallas import tpu as pltpu
from jax.sharding import PartitionSpec as P

MESH = pl.DeviceIdType.MESH
ALL_VMEM = 67043328

SB_DIM = 64
GDN_DIM = 128
BLOCK = 64


EXACT_MATMUL = lax.Precision.HIGHEST
NORM_EPS = 1e-06


def carried_in(value, axis, combine, identity):
    devices, index = (lax.axis_size(axis), lax.axis_index(axis))
    everything = jax.tree.map(
        lambda part, kind: lax.all_gather(part.astype(kind), axis),
        value,
        (jnp.bfloat16, jnp.bfloat16),
    )
    start = jax.tree.map(
        lambda part, zero: jnp.broadcast_to(jnp.asarray(zero, part.dtype), part.shape),
        value,
        identity,
    )

    def lap(k, before):
        reached = k < index
        new = combine(
            before, jax.tree.map(lambda part, own: part[k].astype(own.dtype), everything, value)
        )
        return jax.tree.map(lambda a, b: jnp.where(reached, a, b), new, before)

    return lax.fori_loop(0, devices, lap, start)


def unit_lower_inverse(strict_part):
    order_size = strict_part.shape[-1]
    powered = strict_part
    inverse = jnp.eye(order_size, dtype=strict_part.dtype) - strict_part
    for repeat_number in range(max(1, (order_size - 1).bit_length()) - 1):
        powered = jnp.einsum("...ij,...jk->...ik", powered, powered, precision=EXACT_MATMUL)
        inverse = inverse + jnp.einsum(
            "...ij,...jk->...ik", inverse, powered, precision=EXACT_MATMUL
        )
    return inverse


def to_blocks(row_data, block_span):
    blocks_count = row_data.shape[0] // block_span
    shaped = row_data.reshape((blocks_count, block_span) + row_data.shape[1:])
    return jnp.swapaxes(shaped, 1, 2)


def from_blocks(blocked):
    swapped = jnp.swapaxes(blocked, 1, 2)
    return swapped.reshape((-1,) + swapped.shape[2:])


def unit_rows(vectors):
    return vectors * lax.rsqrt(jnp.sum(vectors * vectors, axis=-1, keepdims=True) + NORM_EPS)


def delta_inputs(
    query_proj,
    key_proj,
    value_proj,
    decay_pre,
    write_pre,
    write_bias,
    decay_log_scale,
    shift_rows,
    head_count,
    head_size,
):
    query_act = jax.nn.silu(query_proj.astype(jnp.float32)).reshape(-1, head_count, head_size)
    key_act = jax.nn.silu(key_proj.astype(jnp.float32)).reshape(-1, head_count, head_size)
    value_rows = jax.nn.silu(value_proj.astype(jnp.float32)).reshape(-1, head_count, head_size)
    queries = unit_rows(query_act) * head_size ** (-0.5)
    key_rows = unit_rows(key_act)
    log_decay = -jnp.exp(decay_log_scale) * jax.nn.softplus(decay_pre) + shift_rows
    strength = jax.nn.sigmoid(write_pre + write_bias)
    return (queries, key_rows, value_rows, log_decay, strength)


def delta_prepare(queries, key_rows, value_rows, log_decay, strength):
    block_span = queries.shape[2]
    cumulative = jnp.cumsum(log_decay, axis=-1)
    row_place = lax.broadcasted_iota(jnp.int32, (block_span, block_span), 0)
    col_place = lax.broadcasted_iota(jnp.int32, (block_span, block_span), 1)
    inclusive = col_place <= row_place
    strictly = col_place < row_place
    spread = cumulative[..., :, None] - cumulative[..., None, :]
    decay_table = jnp.where(inclusive, jnp.exp(jnp.where(inclusive, spread, 0.0)), 0.0)
    keys_beta = key_rows * strength[..., None]
    lower_part = jnp.where(
        strictly,
        jnp.einsum("nhik,nhjk->nhij", keys_beta, key_rows, precision=EXACT_MATMUL) * decay_table,
        0.0,
    )
    inverse = unit_lower_inverse(lower_part)
    growth = jnp.exp(cumulative)
    state_updates = jnp.einsum(
        "nhij,nhjv->nhiv", inverse, value_rows * strength[..., None], precision=EXACT_MATMUL
    )
    erase_term = jnp.einsum(
        "nhij,nhjk->nhik", inverse, keys_beta * growth[..., None], precision=EXACT_MATMUL
    )
    inside_block = (
        jnp.einsum("nhik,nhjk->nhij", queries, key_rows, precision=EXACT_MATMUL) * decay_table
    )
    boosted_query = queries * growth[..., None]
    damped_keys = key_rows * jnp.exp(cumulative[..., -1:] - cumulative)[..., None]
    decay_per_block = jnp.exp(cumulative[..., -1])
    return (state_updates, erase_term, inside_block, boosted_query, damped_keys, decay_per_block)


def delta_step(memory_state, inputs):
    state_updates, erase_term, inside_block, boosted_query, damped_keys, decay_per_block = inputs
    fixed_values = state_updates - jnp.einsum(
        "mzq,mqc->mzc", erase_term, memory_state, precision=EXACT_MATMUL
    )
    produced_rows = jnp.einsum(
        "mzq,mqc->mzc", boosted_query, memory_state, precision=EXACT_MATMUL
    ) + jnp.einsum("efq,eqn->efn", inside_block, fixed_values, precision=EXACT_MATMUL)
    memory_state = memory_state * decay_per_block[:, None, None] + jnp.einsum(
        "wam,waz->wmz", damped_keys, fixed_values, precision=EXACT_MATMUL
    )
    return (memory_state, produced_rows)


def transition_step(carried, inputs):
    memory_state, transfer = carried
    state_updates, erase_term, inside_block, boosted_query, damped_keys, decay_per_block = inputs
    fixed_values = state_updates - jnp.einsum(
        "mzq,mqc->mzc", erase_term, memory_state, precision=EXACT_MATMUL
    )
    coupling = jnp.einsum("hik,hil->hkl", damped_keys, erase_term, precision=EXACT_MATMUL)
    memory_state = memory_state * decay_per_block[:, None, None] + jnp.einsum(
        "wam,waz->wmz", damped_keys, fixed_values, precision=EXACT_MATMUL
    )
    transfer = transfer * decay_per_block[:, None, None] - jnp.einsum(
        "hkl,hlm->hkm", coupling, transfer, precision=EXACT_MATMUL
    )
    return ((memory_state, transfer), None)


def compose(prior_blocks, following_blocks):
    joined_map = jnp.einsum(
        "hkl,hlm->hkm", following_blocks[0], prior_blocks[0], precision=EXACT_MATMUL
    )
    joined_state = (
        jnp.einsum("djo,dog->djg", following_blocks[0], prior_blocks[1], precision=EXACT_MATMUL)
        + following_blocks[1]
    )
    return (joined_map, joined_state)


def stick_block(queries, key_rows, value_rows, query_place, key_place, offsets):
    scale_factor = queries.shape[-1] ** (-0.5)
    scores = (
        jnp.einsum("qhd,khd->hqk", queries, key_rows, preferred_element_type=jnp.float32)
        * scale_factor
        + offsets[:, None, None]
    )
    visible = key_place[None, :] < query_place[:, None]
    skipped = jnp.where(visible, jax.nn.log_sigmoid(-scores), 0.0)
    beyond = lax.cumsum(skipped, axis=2, reverse=True) - skipped
    weights = jnp.where(visible, jnp.exp(jax.nn.log_sigmoid(scores) + beyond), 0.0).astype(
        jnp.bfloat16
    )
    partial_value = jnp.einsum(
        "hqk,khd->qhd", weights, value_rows, preferred_element_type=jnp.float32
    )
    return (partial_value, jnp.sum(skipped, axis=2).T)


def stick_combine(partials, totals):
    beyond = jnp.cumsum(totals[::-1], axis=0)[::-1] - totals
    return jnp.sum(partials * jnp.exp(beyond)[..., None], axis=0)


def on_device_split(
    hidden_in,
    sb_query_w,
    sb_key_w,
    sb_value_w,
    sb_offset,
    delta_query_w,
    delta_key_w,
    delta_value_w,
    decay_w,
    write_w,
    write_bias,
    decay_log_scale,
    decay_shift,
    head_gain,
    sb_out_w,
    delta_out_w,
):
    token_rows = hidden_in.shape[1]
    local_in = hidden_in.reshape(token_rows, hidden_in.shape[2])
    gathered = (
        lax.all_gather(sb_query_w, "fs", axis=0, tiled=True),
        lax.all_gather(sb_key_w, "fs", axis=0, tiled=True),
        lax.all_gather(sb_value_w, "fs", axis=0, tiled=True),
        lax.all_gather(delta_query_w, "fs", axis=0, tiled=True),
        lax.all_gather(delta_key_w, "fs", axis=0, tiled=True),
        lax.all_gather(delta_value_w, "fs", axis=0, tiled=True),
    )
    in_weights = tuple(gathered) + (decay_w, write_w)
    portion = lax.all_gather(local_in, "tp", axis=1, tiled=True)
    projected = tuple(
        (jnp.dot(portion, weight, preferred_element_type=jnp.float32) for weight in in_weights)
    )
    sb_heads = sb_offset.shape[0]
    delta_heads = decay_log_scale.shape[0]
    sb_query = projected[0].astype(jnp.bfloat16).reshape(token_rows, sb_heads, SB_DIM)
    sb_keys = projected[1].astype(jnp.bfloat16)
    sb_values = projected[2].astype(jnp.bfloat16)
    shift_rows = decay_shift.reshape(delta_heads, token_rows).T
    queries, key_rows, value_rows, log_decay, strength = delta_inputs(
        projected[3].astype(jnp.bfloat16),
        projected[4].astype(jnp.bfloat16),
        projected[5].astype(jnp.bfloat16),
        projected[6],
        projected[7],
        write_bias,
        decay_log_scale,
        shift_rows,
        delta_heads,
        GDN_DIM,
    )
    prepared = delta_prepare(
        to_blocks(queries, BLOCK),
        to_blocks(key_rows, BLOCK),
        to_blocks(value_rows, BLOCK),
        to_blocks(log_decay, BLOCK),
        to_blocks(strength, BLOCK),
    )
    identity_map = jnp.broadcast_to(
        jnp.eye(GDN_DIM, dtype=jnp.float32), (delta_heads, GDN_DIM, GDN_DIM)
    )
    empty_state = jnp.zeros((delta_heads, GDN_DIM, GDN_DIM), jnp.float32)
    (local_end, local_map), unused_out = lax.scan(
        transition_step, (empty_state, identity_map), prepared
    )
    own_first = lax.axis_index("sp") * token_rows
    query_place = own_first + lax.iota(jnp.int32, token_rows)
    sp_count = lax.axis_size("sp")
    slot_out = jnp.zeros((sp_count, token_rows, sb_heads, SB_DIM), jnp.float32)
    slot_total = jnp.zeros((sp_count, token_rows, sb_heads), jnp.float32)

    def absorb(slot_arrays, address_portion, value_part, shard_first):

        def active(current):
            partial_value, totals = stick_block(
                sb_query,
                address_portion.reshape(token_rows, sb_heads, SB_DIM),
                value_part.reshape(token_rows, sb_heads, SB_DIM),
                query_place,
                shard_first + lax.iota(jnp.int32, token_rows),
                sb_offset,
            )
            slot_index = shard_first // token_rows
            return (
                lax.dynamic_update_index_in_dim(current[0], partial_value, slot_index, 0),
                lax.dynamic_update_index_in_dim(current[1], totals, slot_index, 0),
            )

        def inactive(current):
            return current

        usable = jnp.logical_and(shard_first >= 0, shard_first <= own_first)
        return lax.cond(usable, active, inactive, slot_arrays)

    key_block = lax.all_gather(sb_keys, "sp", axis=0, tiled=True)
    value_block = lax.all_gather(sb_values, "sp", axis=0, tiled=True)

    def per_shard(shard_number, current):
        row_begin = shard_number * token_rows
        return absorb(
            current,
            lax.dynamic_slice_in_dim(key_block, row_begin, token_rows, 0),
            lax.dynamic_slice_in_dim(value_block, row_begin, token_rows, 0),
            row_begin,
        )

    slot_arrays = lax.fori_loop(
        0, key_block.shape[0] // token_rows, per_shard, (slot_out, slot_total)
    )
    unused_map, incoming = carried_in(
        (local_map, local_end), "sp", compose, (identity_map, empty_state)
    )
    sb_mixed = (
        stick_combine(slot_arrays[0], slot_arrays[1])
        .astype(jnp.bfloat16)
        .reshape(token_rows, sb_heads * SB_DIM)
    )
    unused_end, produced_rows = lax.scan(delta_step, incoming, prepared)
    produced_rows = from_blocks(produced_rows)
    normed = (
        produced_rows
        * lax.rsqrt(jnp.mean(produced_rows * produced_rows, axis=-1, keepdims=True) + NORM_EPS)
        * head_gain
    )
    delta_mixed = normed.astype(jnp.bfloat16).reshape(token_rows, delta_heads * GDN_DIM)
    result = lax.psum_scatter(
        (
            jnp.dot(sb_mixed, sb_out_w, preferred_element_type=jnp.float32)
            + jnp.dot(delta_mixed, delta_out_w, preferred_element_type=jnp.float32)
        ).astype(jnp.bfloat16),
        "tp",
        scatter_dimension=0,
        tiled=True,
    ).astype(jnp.float32)
    return result.astype(jnp.bfloat16).reshape(1, result.shape[0], result.shape[1])


def remote(src, dst, send, recv, axis, index):
    return pltpu.make_async_remote_copy(
        src_ref=src, dst_ref=dst, send_sem=send, recv_sem=recv,
        device_id={axis: index}, device_id_type=MESH,
    )


def greet(axes):
    barrier = pltpu.get_barrier_semaphore()
    count = 0
    for axis in axes:
        size, me = lax.axis_size(axis), lax.axis_index(axis)
        for k in range(1, size):
            pl.semaphore_signal(
                barrier, inc=1, device_id={axis: lax.rem(me + k, size)}, device_id_type=MESH
            )
            count += 1
    pl.semaphore_wait(barrier, count)


def halves(a):
    high = a.astype(jnp.bfloat16)
    return high, (a - high.astype(jnp.float32)).astype(jnp.bfloat16)


def dot_f32(a, b, dims=((1,), (0,))):
    return lax.dot_general(a, b, (dims, ((), ())), preferred_element_type=jnp.float32)


def wide_rhs(high, low, axis):
    top = jnp.concatenate([high, low], axis=axis)
    bottom = jnp.concatenate([high, jnp.zeros_like(low)], axis=axis)
    return jnp.concatenate([top, bottom], axis=1 - axis)


def folded(a):
    half = a.shape[1] // 2
    return a[:, :half] + a[:, half:]


def layer_kernel(
    offset_ref, decay_scale_ref, write_bias_ref,
    x_ref, w0, w1, w2, w3, w4, w5, decay_w_ref, write_w_ref, shift_ref, gain_ref, sw_hbm, dw_hbm,
    out_ref,
    xs, ws, gate_w, gates, shifts_ref,
    proj, acc, later, maps, adds, stick_out, delta_out,
    sticks, deltas, sw_ref, dw_ref, partial, outgoing, incoming, own,
    x_send, x_recv, f_send, f_recv, w_send, w_recv, s_send, s_recv, l_sem, lw_sem,
    a_send, a_recv, c_send, c_recv,
):
    weights = (w0, w1, w2, w3, w4, w5)
    sp, tp = lax.axis_size("sp"), lax.axis_size("tp")
    z, f, t = lax.axis_index("sp"), lax.axis_index("fs"), lax.axis_index("tp")
    rows, half = x_ref.shape
    depth = w0.shape[0]
    cols = ws.shape[1] // len(weights)
    parts = x_send.shape[2]
    heads = decay_w_ref.shape[0]
    slot = pl.ds(pl.multiple_of(t * half, half), half)
    local = [
        pltpu.make_async_copy(x_ref, xs.at[z, :, slot], l_sem.at[0]),
        pltpu.make_async_copy(shift_ref, shifts_ref.at[z], l_sem.at[1]),
        pltpu.make_async_copy(decay_w_ref, gate_w.at[0], l_sem.at[2]),
        pltpu.make_async_copy(write_w_ref, gate_w.at[1], l_sem.at[3]),
    ]
    late = [
        pltpu.make_async_copy(sw_hbm, sw_ref, l_sem.at[4]),
        pltpu.make_async_copy(dw_hbm, dw_ref, l_sem.at[5]),
    ]

    def w_src(i):
        return weights[i].at[:, pl.ds(pl.multiple_of(z * cols, cols), cols)]

    def w_at(i, who):
        return ws.at[pl.ds(pl.multiple_of(who * depth, depth), depth), pl.ds(i * cols, cols)]

    local += [
        pltpu.make_async_copy(w_src(i), w_at(i, f), lw_sem.at[i]) for i in range(len(weights))
    ]
    for c in local:
        c.start()
    greet(("sp", "fs", "tp"))

    near = (f + 1 - 2 * (f % 2), f + 2 - 4 * (f // 2))
    count = len(weights)
    orders = (tuple(range(count)), tuple(range(count // 2, count)) + tuple(range(count // 2)))

    def x_copy(way, step, part):
        block = z - (step - 1) if way == 0 else z + (step - 1)
        piece = pl.ds(part * (rows // parts), rows // parts)
        there = xs.at[block, piece, slot]
        return remote(
            x_ref.at[piece, :] if step == 1 else there, there,
            x_send.at[way, step, part], x_recv.at[way, step, part],
            "sp", z + 1 if way == 0 else z - 1,
        )

    def onward(way):
        return z + 1 < sp if way == 0 else z > 0

    def comes(way, step):
        return z >= step if way == 0 else z + step < sp

    def sends(way, step):
        return jnp.logical_and(onward(way), comes(way, step - 1))

    def forward(way, step, part):
        block = z - step if way == 0 else z + step
        piece = pl.ds(part * (rows // parts), rows // parts)
        there = xs.at[block, piece, slot]
        return remote(
            x_ref.at[piece, :] if step == 0 else there, there,
            f_send.at[way, step, part], f_recv.at[way, step, part], "tp", lax.rem(t + 1, tp),
        )

    for part in range(parts):
        for way in range(2):
            @pl.when(onward(way))
            def _():
                x_copy(way, 1, part).start()

    w_copies = {}
    for order_at in range(count):
        for side in range(2):
            i = orders[side][order_at]
            c = remote(
                w_src(i), w_at(i, f), w_send.at[side, i], w_recv.at[side, i], "fs", near[side]
            )
            c.start()
            w_copies[side, i] = c
    s_copies = []
    for k in range(1, sp):
        c = remote(
            shift_ref, shifts_ref.at[z], s_send.at[k], s_recv.at[k], "sp", lax.rem(z + k, sp)
        )
        c.start()
        s_copies.append(c)
    for part in range(parts):
        forward(0, 0, part).start()
    for c in late:
        c.start()

    relays = []

    def relay(position):
        for side in range(2):
            i = orders[side][position]
            w_copies[side, i].wait_recv()
            there = w_at(i, near[side])
            c = remote(
                there, there, w_send.at[2 + side, i], w_recv.at[2 + side, i],
                "fs", near[1 - side],
            )
            c.start()
            relays.append(c)

    def arrive(step, part):
        for way in range(2):
            @pl.when(comes(way, step))
            def _():
                x_copy(way, step, part).wait_recv()
                forward(way, step, part).start()
                if step + 1 < sp:
                    @pl.when(onward(way))
                    def _():
                        x_copy(way, step + 1, part).start()

    early = [(step, part) for step in range(1, sp - 1) for part in range(parts)]
    relay(0)
    arrive(*early[0])
    for position in range(1, count // 2):
        relay(position)
    for step, part in early[1:]:
        arrive(step, part)
    for c in local:
        c.wait()
    for side in range(2):
        for position in range(count // 2, count):
            w_copies[side, orders[side][position]].wait_recv()
    for c in relays:
        c.wait_recv()
    for c in s_copies:
        c.wait_recv()
    for part in range(parts):
        forward(0, 0, part).wait_recv()

    size = offset_ref.shape[0] // sp
    sb_size = cols // size
    scale = sb_size ** (-0.5)
    tile = rows // 2
    below = lax.broadcasted_iota(jnp.int32, (rows, rows), 0)
    across = lax.broadcasted_iota(jnp.int32, (rows, rows), 1)
    after = jnp.where(below > across, 1.0, 0.0).astype(jnp.bfloat16)

    def at_block(b, start=0, extent=rows):
        return pl.ds(pl.multiple_of(b * rows + start, extent), extent)

    def pair(i, j, masked):
        for part in range(rows // tile):
            span = (part + 1) * tile if masked else rows
            mine = at_block(i, part * tile, tile)
            q = proj[0, mine, :]
            keys, values = proj[1, at_block(j), :], proj[2, at_block(j), :]
            keys, values = keys[:span], values[:span]
            lane = lax.broadcasted_iota(jnp.int32, (tile, cols), 1)
            if masked:
                seen = across[:tile, :span] < below[:tile, :span] + part * tile
            mixed = total = None
            for h in range(size):
                query = jnp.where(lane // sb_size == h, q, jnp.zeros_like(q))
                score = dot_f32(query, keys, ((1,), (1,))) * scale + offset_ref[z * size + h]
                skip = jnp.maximum(
                    score, jnp.log(1.0 + jnp.exp(jnp.minimum(score, 80.0)))
                )
                weight = score - skip
                if masked:
                    skip = jnp.where(seen, skip, 0.0)
                beyond = dot_f32(skip.astype(jnp.bfloat16), after[:span, :span])
                weight = jnp.exp(weight - beyond)
                if masked:
                    weight = jnp.where(seen, weight, 0.0)
                part_out = dot_f32(weight.astype(jnp.bfloat16), values)
                whole = jnp.broadcast_to(beyond[:, :1] + skip[:, :1], (tile, cols))
                mixed = part_out if h == 0 else jnp.where(lane // sb_size == h, part_out, mixed)
                total = whole if h == 0 else jnp.where(lane // sb_size == h, whole, total)
            if masked:
                acc[mine, :] = mixed
                later[mine, :] = total
            else:
                passed = later[mine, :]
                acc[mine, :] = acc[mine, :] + mixed * jnp.exp(-passed)
                later[mine, :] = passed + total

    span = BLOCK
    duo = 2 * span
    blocks = rows // span
    width = GDN_DIM
    seg_row = lax.broadcasted_iota(jnp.int32, (rows, rows), 0)
    seg_col = lax.broadcasted_iota(jnp.int32, (rows, rows), 1)
    together = seg_row // span == seg_col // span
    upto = jnp.where(jnp.logical_and(together, seg_row <= seg_col), 1.0, 0.0).astype(jnp.bfloat16)
    beyond_it = jnp.where(jnp.logical_and(together, seg_row > seg_col), 1.0, 0.0).astype(
        jnp.bfloat16
    )
    prow = lax.broadcasted_iota(jnp.int32, (span, duo), 0)
    plane = lax.broadcasted_iota(jnp.int32, (span, duo), 1)
    first = plane < span
    pcol = jnp.where(first, plane, plane - span)
    inclusive, strictly = pcol <= prow, pcol < prow
    unit = jnp.where(pcol == prow, 1.0, 0.0)
    diagonal = lax.broadcasted_iota(jnp.int32, (width, width), 0) == lax.broadcasted_iota(
        jnp.int32, (width, width), 1
    )
    eighth = lax.broadcasted_iota(jnp.int32, (8, rows), 0)

    def silu(a):
        return a * (1.0 / (1.0 + jnp.exp(-a)))

    def unit_of(a):
        return a * lax.rsqrt(jnp.sum(a * a, axis=-1, keepdims=True) + NORM_EPS)

    def apart(a):
        lanes = lax.broadcasted_iota(jnp.int32, a.shape, 1) < span
        zero = jnp.zeros_like(a)
        return jnp.concatenate([jnp.where(lanes, a, zero), jnp.where(lanes, zero, a)], axis=0)

    def squared(left, power):
        high, low = halves(power)
        lhigh, llow = halves(left)
        return folded(
            dot_f32(
                jnp.concatenate([lhigh, llow], axis=1), wide_rhs(apart(high), apart(low), 1)
            )
        )

    def prepare(b, dq, dk, dv):
        for side in range(2):
            gates[side * heads : (side + 1) * heads, :] = dot_f32(
                gate_w[side], xs[b], ((1,), (1,))
            )
        pre = gates[pl.ds(z, 1), :]
        write = gates[pl.ds(heads + z, 1), :] + write_bias_ref[z]
        rate = jnp.exp(jnp.full((1, rows), decay_scale_ref[z], jnp.float32))
        soft = jnp.maximum(pre, 0.0) + jnp.log(1.0 + jnp.exp(-jnp.abs(pre)))
        decay = shifts_ref[b, pl.ds(z, 1), :] - rate * soft
        strength = 1.0 / (1.0 + jnp.exp(-write))
        d1 = decay.astype(jnp.bfloat16).astype(jnp.float32)
        d2 = (decay - d1).astype(jnp.bfloat16).astype(jnp.float32)
        d3 = decay - d1 - d2
        three = jnp.where(
            eighth == 0, d1, jnp.where(eighth == 1, d2, jnp.where(eighth == 2, d3, 0.0))
        ).astype(jnp.bfloat16)
        cum_row = jnp.sum(dot_f32(three, upto), axis=0, keepdims=True)
        rest_row = jnp.sum(dot_f32(three, beyond_it), axis=0, keepdims=True)
        stack = jnp.where(
            eighth == 0, strength,
            jnp.where(
                eighth == 1, jnp.exp(cum_row),
                jnp.where(eighth == 2, jnp.exp(rest_row), cum_row),
            ),
        )
        columns = stack.T
        s_col, grow, damp, cum = (columns[:, n : n + 1] for n in range(4))
        q = unit_of(silu(dq)) * width ** (-0.5)
        k = unit_of(silu(dk))
        v = silu(dv)
        boosted = q * grow
        damped = k * damp
        right = jnp.concatenate([v * s_col, k * (s_col * grow)], axis=1)
        kh, kl = halves(k)
        qh, ql = halves(q)
        work = []
        for duo_at in range(rows // duo):
            lo = duo_at * duo
            here = slice(lo, lo + duo)
            left = jnp.concatenate(
                [
                    jnp.concatenate([kh[here], kl[here]], axis=1),
                    jnp.concatenate([qh[here], ql[here]], axis=1),
                ],
                axis=0,
            )
            gram = folded(
                dot_f32(left, wide_rhs(kh[here], kl[here], 0), ((1,), (1,)))
            )
            spread = (
                jnp.where(first, cum[lo : lo + span], cum[lo + span : lo + duo])
                - cum_row[:, here]
            )
            table = jnp.where(inclusive, jnp.exp(jnp.where(inclusive, spread, 0.0)), 0.0)
            scale_col = jnp.where(first, s_col[lo : lo + span], s_col[lo + span : lo + duo])
            near_k = jnp.where(first, gram[:span], gram[span:duo])
            near_q = jnp.where(first, gram[duo : duo + span], gram[duo + span :])
            strict = jnp.where(strictly, near_k * table * scale_col, 0.0)
            work.append([unit - strict, strict, near_q * table])
        for w in work:
            w[1] = squared(w[1], w[1])
        levels = max(1, (span - 1).bit_length()) - 1
        for level in range(levels):
            for w in work:
                if level + 1 < levels:
                    both = squared(jnp.concatenate([w[1], w[0]], axis=0), w[1])
                    w[1], w[0] = both[:span], w[0] + both[span:]
                else:
                    w[0] = w[0] + squared(w[0], w[1])
        for duo_at, (inverse, _, inside) in enumerate(work):
            lo = duo_at * duo
            here = slice(lo, lo + duo)
            ih, il = (apart(a) for a in halves(inverse))
            rh, rl = halves(right[here])
            solved = dot_f32(
                jnp.concatenate([ih, il], axis=1), jnp.concatenate([rh, rh], axis=0)
            ) + dot_f32(ih, rl)
            lh, ll = (
                apart(a) for a in halves(jnp.concatenate([damped[here].T, inside], axis=0))
            )
            sh, sl = halves(solved)
            made = dot_f32(
                jnp.concatenate([lh, ll], axis=1), jnp.concatenate([sh, sh], axis=0)
            ) + dot_f32(lh, sl)
            for side in range(2):
                at = lo + side * span
                mine = made[side * (width + span) : (side + 1) * (width + span)]
                n = b * blocks + 2 * duo_at + side
                keep = grow[at + span - 1 : at + span]
                step_map = jnp.where(diagonal, keep, 0.0) - mine[:width, width:]
                query = boosted[at : at + span] - mine[width:, width:]
                high, low = halves(jnp.concatenate([step_map, query], axis=0))
                maps[n, :, :width] = high
                maps[n, :, width:] = low
                adds[n] = mine[:, :width]

    def wait_x(way, step):
        for part in range(parts):
            if step == sp - 1:
                x_copy(way, step, part).wait_recv()
                forward(way, step, part).start()
        for part in range(parts):
            forward(way, step, part).wait_recv()

    shorter = jnp.minimum(z, sp - 1 - z)
    down_last = z > sp - 1 - z

    def event(n, reach):
        lowest, highest = reach
        both = n <= 2 * shorter
        way_n = jnp.where(both, lax.rem(n + 1, 2), jnp.where(down_last, 0, 1))
        step_n = jnp.where(n == 0, 0, jnp.where(both, (n + 1) // 2, n - shorter))
        for step in range(1, sp):
            for way in range(2):
                @pl.when(jnp.logical_and(step_n == step, way_n == way))
                def _():
                    wait_x(way, step)
        down = jnp.logical_and(way_n == 0, n > 0)
        b = jnp.where(down, z - step_n, z + step_n)
        for i in range(0, 3 * cols, 3 * cols // 3):
            proj[i // cols, at_block(b), :] = dot_f32(
                xs[b], ws[:, i : i + cols]
            ).astype(jnp.bfloat16)
        drows = dot_f32(xs[b], ws[:, 3 * cols :]).astype(jnp.bfloat16).astype(jnp.float32)
        prepare(b, drows[:, :cols], drows[:, cols : 2 * cols], drows[:, 2 * cols :])
        pair(b, b, True)

        def off(m, c):
            i = jnp.where(down, b + 1 + m, b)
            j = jnp.where(down, b, b - 1 - m)
            pair(i, j, False)
            return c

        lowest = jnp.minimum(lowest, b)
        highest = jnp.maximum(highest, b)
        lax.fori_loop(0, highest - lowest, off, 0)
        return lowest, highest

    lax.fori_loop(0, sp, event, (z, z))

    out_copies = []

    def give(kind, out, target):
        which = 0 if kind == "stick" else 1
        here = target.at[:, pl.ds(pl.multiple_of(z * cols, cols), cols)]

        def send(g, k):
            return remote(
                out.at[g * rows : (g + 1) * rows, :], here,
                a_send.at[k, which], a_recv.at[k, which], "sp", g,
            )

        def started(g):
            for k in range(1, sp):
                @pl.when(lax.rem(z + k, sp) == g)
                def _():
                    send(g, k).start()

        def finished():
            for g in range(sp):
                for k in range(1, sp):
                    @pl.when(lax.rem(z + k, sp) == g)
                    def _():
                        send(g, k).wait_send()

        def came():
            for k in range(1, sp):
                send(0, k).wait_recv()

        return started, finished, came

    stick_started, stick_finished, stick_came = give("stick", stick_out, sticks)
    delta_started, delta_finished, delta_came = give("delta", delta_out, deltas)

    for g in range(sp):
        at = slice(g * rows, (g + 1) * rows)
        stick_out[at, :] = acc[at, :].astype(jnp.bfloat16)
        if g > 0:
            stick_started(g - 1)

    def walk(n, memory):
        high, low = halves(memory)
        new = folded(dot_f32(maps[n], wide_rhs(high, low, 1))) + adds[n]
        made = new[width:]
        made = made * lax.rsqrt(jnp.mean(made * made, axis=-1, keepdims=True) + NORM_EPS)
        at = pl.ds(pl.multiple_of(n * span, span), span)
        delta_out[at, :] = (made * gain_ref[...]).astype(delta_out.dtype)
        return new[:width]

    memory = jnp.zeros((width, width), jnp.float32)
    for g in range(sp):
        memory = lax.fori_loop(g * blocks, (g + 1) * blocks, walk, memory)
        if g == 0:
            stick_started(sp - 1)
        else:
            delta_started(g - 1)

    mine_z = pl.ds(pl.multiple_of(z * rows, rows), rows)
    lanes = pl.ds(pl.multiple_of(z * cols, cols), cols)
    sticks[:, lanes] = stick_out[mine_z, :]
    deltas[:, lanes] = delta_out[mine_z, :]
    for c in late:
        c.wait()
    delta_started(sp - 1)
    stick_came()
    chunks, wide = outgoing.shape[0], outgoing.shape[2]
    share = rows // tp
    for c in range(chunks):
        columns = slice(c * wide, (c + 1) * wide)
        partial[:, columns] = dot_f32(sticks[...], sw_ref[:, columns])
    delta_came()
    mine = pl.ds(pl.multiple_of(t * share, share), share)
    partner = lax.rem(t + 1, tp)
    theirs = pl.ds(pl.multiple_of(partner * share, share), share)

    def finish(which, c):
        columns = slice(c * wide, (c + 1) * wide)
        return (
            partial[which, columns] + dot_f32(deltas[which, :], dw_ref[:, columns])
        ).astype(jnp.bfloat16)

    swaps = [
        remote(outgoing.at[c], incoming.at[c], c_send.at[c], c_recv.at[c], "tp", partner)
        for c in range(chunks)
    ]
    for c in range(chunks):
        outgoing[c] = finish(theirs, c)
        if c > 0:
            swaps[c - 1].start()
    for c in range(chunks):
        own[c] = finish(mine, c)
        if c == 0:
            swaps[chunks - 1].start()
    for c in range(chunks):
        swaps[c].wait_recv()
        out_ref[:, c * wide : (c + 1) * wide] = (
            own[c].astype(jnp.float32) + incoming[c].astype(jnp.float32)
        ).astype(out_ref.dtype)

    for c in list(w_copies.values()) + relays + s_copies + swaps:
        c.wait_send()
    for part in range(parts):
        forward(0, 0, part).wait_send()
        for step in range(1, sp):
            for way in range(2):
                @pl.when(sends(way, step))
                def _():
                    x_copy(way, step, part).wait_send()

                @pl.when(comes(way, step))
                def _():
                    forward(way, step, part).wait_send()
    stick_finished()
    delta_finished()


ANYWHERE = pl.BlockSpec(memory_space=pltpu.HBM)
ON_CORE = pl.BlockSpec(memory_space=pltpu.VMEM)
SCALARS = pl.BlockSpec(memory_space=pltpu.SMEM)


def on_device_heads(
    hidden_in, sb_query_w, sb_key_w, sb_value_w, sb_offset,
    delta_query_w, delta_key_w, delta_value_w, decay_w, write_w, write_bias,
    decay_log_scale, decay_shift, head_gain, sb_out_w, delta_out_w,
):
    sp, fs, tp = lax.axis_size("sp"), lax.axis_size("fs"), lax.axis_size("tp")
    rows, half = hidden_in.shape[1:]
    width = half * tp
    length = rows * sp
    heads = decay_log_scale.shape[0]
    cols = sb_query_w.shape[1] // sp
    parts, chunks = 2, 4
    share = rows // tp
    blocks = length // BLOCK
    dma = pltpu.SemaphoreType.DMA
    bf16, f32 = jnp.bfloat16, jnp.float32
    result = pl.pallas_call(
        layer_kernel,
        name="layer",
        out_shape=jax.ShapeDtypeStruct((share, width), bf16),
        in_specs=[SCALARS] * 3 + [ANYWHERE] * 10 + [ON_CORE] + [ANYWHERE] * 2,
        out_specs=ON_CORE,
        scratch_shapes=[
            pltpu.VMEM((sp, rows, width), bf16),
            pltpu.VMEM((width, 6 * cols), bf16),
            pltpu.VMEM((2, heads, width), bf16),
            pltpu.VMEM((2 * heads, rows), f32),
            pltpu.VMEM((sp, heads, rows), f32),
            pltpu.VMEM((3, length, cols), bf16),
            pltpu.VMEM((length, cols), f32),
            pltpu.VMEM((length, cols), f32),
            pltpu.VMEM((blocks, cols + BLOCK, 2 * cols), bf16),
            pltpu.VMEM((blocks, cols + BLOCK, cols), f32),
            pltpu.VMEM((length, cols), bf16),
            pltpu.VMEM((length, cols), bf16),
            pltpu.VMEM((rows, cols * sp), bf16),
            pltpu.VMEM((rows, cols * sp), bf16),
            pltpu.VMEM(sb_out_w.shape, bf16),
            pltpu.VMEM(delta_out_w.shape, bf16),
            pltpu.VMEM((rows, width), f32),
            pltpu.VMEM((chunks, share, width // chunks), bf16),
            pltpu.VMEM((chunks, share, width // chunks), bf16),
            pltpu.VMEM((chunks, share, width // chunks), bf16),
            dma((2, sp, parts)), dma((2, sp, parts)), dma((2, sp, parts)), dma((2, sp, parts)),
            dma((fs, 6)), dma((fs, 6)), dma((sp,)), dma((sp,)), dma((6,)), dma((6,)),
            dma((sp, 2)), dma((sp, 2)), dma((chunks,)), dma((chunks,)),
        ],
        compiler_params=pltpu.CompilerParams(
            collective_id=0, has_side_effects=True, vmem_limit_bytes=ALL_VMEM
        ),
    )(
        sb_offset, decay_log_scale, write_bias,
        hidden_in.reshape(rows, half), sb_query_w, sb_key_w, sb_value_w,
        delta_query_w, delta_key_w, delta_value_w, decay_w.T, write_w.T,
        decay_shift.reshape(heads, rows), head_gain.reshape(1, -1), sb_out_w, delta_out_w,
    )
    return result.reshape(1, share, width)


def on_device(*inputs):
    delta_heads = inputs[11].shape[0]
    square = lax.axis_size("fs") == 4 and lax.axis_size("tp") == 2
    if square and delta_heads == lax.axis_size("sp") and inputs[4].shape[0] % delta_heads == 0:
        return on_device_heads(*inputs)
    return on_device_split(*inputs)


def solution(mesh):
    return jax.shard_map(
        on_device,
        mesh=mesh,
        in_specs=(
            P("fs", "sp", "tp"),
            P("fs", "tp"),
            P("fs", "tp"),
            P("fs", "tp"),
            P("tp"),
            P("fs", "tp"),
            P("fs", "tp"),
            P("fs", "tp"),
            P(None, "tp"),
            P(None, "tp"),
            P("tp"),
            P("tp"),
            P("fs", "tp", "sp"),
            P(),
            P("tp", None),
            P("tp", None),
        ),
        out_specs=P("fs", ("sp", "tp"), None),
        check_vma=False,
    )
```

```python
import jax
import jax.numpy as jnp
from jax import lax
from jax.experimental import pallas as pl
from jax.experimental.pallas import tpu as pltpu
from jax.sharding import PartitionSpec as P

MESH = pl.DeviceIdType.MESH
ALL_VMEM = 67043328

SB_DIM = 64
GDN_DIM = 128
BLOCK = 64


EXACT_MATMUL = lax.Precision.HIGHEST
NORM_EPS = 1e-06


def carried_in(value, axis, combine, identity):
    devices, index = (lax.axis_size(axis), lax.axis_index(axis))
    everything = jax.tree.map(
        lambda part, kind: lax.all_gather(part.astype(kind), axis),
        value,
        (jnp.bfloat16, jnp.bfloat16),
    )
    start = jax.tree.map(
        lambda part, zero: jnp.broadcast_to(jnp.asarray(zero, part.dtype), part.shape),
        value,
        identity,
    )

    def lap(k, before):
        reached = k < index
        new = combine(
            before, jax.tree.map(lambda part, own: part[k].astype(own.dtype), everything, value)
        )
        return jax.tree.map(lambda a, b: jnp.where(reached, a, b), new, before)

    return lax.fori_loop(0, devices, lap, start)


def unit_lower_inverse(strict_part):
    order_size = strict_part.shape[-1]
    powered = strict_part
    inverse = jnp.eye(order_size, dtype=strict_part.dtype) - strict_part
    for repeat_number in range(max(1, (order_size - 1).bit_length()) - 1):
        powered = jnp.einsum("...ij,...jk->...ik", powered, powered, precision=EXACT_MATMUL)
        inverse = inverse + jnp.einsum(
            "...ij,...jk->...ik", inverse, powered, precision=EXACT_MATMUL
        )
    return inverse


def to_blocks(row_data, block_span):
    blocks_count = row_data.shape[0] // block_span
    shaped = row_data.reshape((blocks_count, block_span) + row_data.shape[1:])
    return jnp.swapaxes(shaped, 1, 2)


def from_blocks(blocked):
    swapped = jnp.swapaxes(blocked, 1, 2)
    return swapped.reshape((-1,) + swapped.shape[2:])


def unit_rows(vectors):
    return vectors * lax.rsqrt(jnp.sum(vectors * vectors, axis=-1, keepdims=True) + NORM_EPS)


def delta_inputs(
    query_proj,
    key_proj,
    value_proj,
    decay_pre,
    write_pre,
    write_bias,
    decay_log_scale,
    shift_rows,
    head_count,
    head_size,
):
    query_act = jax.nn.silu(query_proj.astype(jnp.float32)).reshape(-1, head_count, head_size)
    key_act = jax.nn.silu(key_proj.astype(jnp.float32)).reshape(-1, head_count, head_size)
    value_rows = jax.nn.silu(value_proj.astype(jnp.float32)).reshape(-1, head_count, head_size)
    queries = unit_rows(query_act) * head_size ** (-0.5)
    key_rows = unit_rows(key_act)
    log_decay = -jnp.exp(decay_log_scale) * jax.nn.softplus(decay_pre) + shift_rows
    strength = jax.nn.sigmoid(write_pre + write_bias)
    return (queries, key_rows, value_rows, log_decay, strength)


def delta_prepare(queries, key_rows, value_rows, log_decay, strength):
    block_span = queries.shape[2]
    cumulative = jnp.cumsum(log_decay, axis=-1)
    row_place = lax.broadcasted_iota(jnp.int32, (block_span, block_span), 0)
    col_place = lax.broadcasted_iota(jnp.int32, (block_span, block_span), 1)
    inclusive = col_place <= row_place
    strictly = col_place < row_place
    spread = cumulative[..., :, None] - cumulative[..., None, :]
    decay_table = jnp.where(inclusive, jnp.exp(jnp.where(inclusive, spread, 0.0)), 0.0)
    keys_beta = key_rows * strength[..., None]
    lower_part = jnp.where(
        strictly,
        jnp.einsum("nhik,nhjk->nhij", keys_beta, key_rows, precision=EXACT_MATMUL) * decay_table,
        0.0,
    )
    inverse = unit_lower_inverse(lower_part)
    growth = jnp.exp(cumulative)
    state_updates = jnp.einsum(
        "nhij,nhjv->nhiv", inverse, value_rows * strength[..., None], precision=EXACT_MATMUL
    )
    erase_term = jnp.einsum(
        "nhij,nhjk->nhik", inverse, keys_beta * growth[..., None], precision=EXACT_MATMUL
    )
    inside_block = (
        jnp.einsum("nhik,nhjk->nhij", queries, key_rows, precision=EXACT_MATMUL) * decay_table
    )
    boosted_query = queries * growth[..., None]
    damped_keys = key_rows * jnp.exp(cumulative[..., -1:] - cumulative)[..., None]
    decay_per_block = jnp.exp(cumulative[..., -1])
    return (state_updates, erase_term, inside_block, boosted_query, damped_keys, decay_per_block)


def delta_step(memory_state, inputs):
    state_updates, erase_term, inside_block, boosted_query, damped_keys, decay_per_block = inputs
    fixed_values = state_updates - jnp.einsum(
        "mzq,mqc->mzc", erase_term, memory_state, precision=EXACT_MATMUL
    )
    produced_rows = jnp.einsum(
        "mzq,mqc->mzc", boosted_query, memory_state, precision=EXACT_MATMUL
    ) + jnp.einsum("efq,eqn->efn", inside_block, fixed_values, precision=EXACT_MATMUL)
    memory_state = memory_state * decay_per_block[:, None, None] + jnp.einsum(
        "wam,waz->wmz", damped_keys, fixed_values, precision=EXACT_MATMUL
    )
    return (memory_state, produced_rows)


def transition_step(carried, inputs):
    memory_state, transfer = carried
    state_updates, erase_term, inside_block, boosted_query, damped_keys, decay_per_block = inputs
    fixed_values = state_updates - jnp.einsum(
        "mzq,mqc->mzc", erase_term, memory_state, precision=EXACT_MATMUL
    )
    coupling = jnp.einsum("hik,hil->hkl", damped_keys, erase_term, precision=EXACT_MATMUL)
    memory_state = memory_state * decay_per_block[:, None, None] + jnp.einsum(
        "wam,waz->wmz", damped_keys, fixed_values, precision=EXACT_MATMUL
    )
    transfer = transfer * decay_per_block[:, None, None] - jnp.einsum(
        "hkl,hlm->hkm", coupling, transfer, precision=EXACT_MATMUL
    )
    return ((memory_state, transfer), None)


def compose(prior_blocks, following_blocks):
    joined_map = jnp.einsum(
        "hkl,hlm->hkm", following_blocks[0], prior_blocks[0], precision=EXACT_MATMUL
    )
    joined_state = (
        jnp.einsum("djo,dog->djg", following_blocks[0], prior_blocks[1], precision=EXACT_MATMUL)
        + following_blocks[1]
    )
    return (joined_map, joined_state)


def stick_block(queries, key_rows, value_rows, query_place, key_place, offsets):
    scale_factor = queries.shape[-1] ** (-0.5)
    scores = (
        jnp.einsum("qhd,khd->hqk", queries, key_rows, preferred_element_type=jnp.float32)
        * scale_factor
        + offsets[:, None, None]
    )
    visible = key_place[None, :] < query_place[:, None]
    skipped = jnp.where(visible, jax.nn.log_sigmoid(-scores), 0.0)
    beyond = lax.cumsum(skipped, axis=2, reverse=True) - skipped
    weights = jnp.where(visible, jnp.exp(jax.nn.log_sigmoid(scores) + beyond), 0.0).astype(
        jnp.bfloat16
    )
    partial_value = jnp.einsum(
        "hqk,khd->qhd", weights, value_rows, preferred_element_type=jnp.float32
    )
    return (partial_value, jnp.sum(skipped, axis=2).T)


def stick_combine(partials, totals):
    beyond = jnp.cumsum(totals[::-1], axis=0)[::-1] - totals
    return jnp.sum(partials * jnp.exp(beyond)[..., None], axis=0)


def on_device_split(
    hidden_in,
    sb_query_w,
    sb_key_w,
    sb_value_w,
    sb_offset,
    delta_query_w,
    delta_key_w,
    delta_value_w,
    decay_w,
    write_w,
    write_bias,
    decay_log_scale,
    decay_shift,
    head_gain,
    sb_out_w,
    delta_out_w,
):
    token_rows = hidden_in.shape[1]
    local_in = hidden_in.reshape(token_rows, hidden_in.shape[2])
    gathered = (
        lax.all_gather(sb_query_w, "fs", axis=0, tiled=True),
        lax.all_gather(sb_key_w, "fs", axis=0, tiled=True),
        lax.all_gather(sb_value_w, "fs", axis=0, tiled=True),
        lax.all_gather(delta_query_w, "fs", axis=0, tiled=True),
        lax.all_gather(delta_key_w, "fs", axis=0, tiled=True),
        lax.all_gather(delta_value_w, "fs", axis=0, tiled=True),
    )
    in_weights = tuple(gathered) + (decay_w, write_w)
    portion = lax.all_gather(local_in, "tp", axis=1, tiled=True)
    projected = tuple(
        (jnp.dot(portion, weight, preferred_element_type=jnp.float32) for weight in in_weights)
    )
    sb_heads = sb_offset.shape[0]
    delta_heads = decay_log_scale.shape[0]
    sb_query = projected[0].astype(jnp.bfloat16).reshape(token_rows, sb_heads, SB_DIM)
    sb_keys = projected[1].astype(jnp.bfloat16)
    sb_values = projected[2].astype(jnp.bfloat16)
    shift_rows = decay_shift.reshape(delta_heads, token_rows).T
    queries, key_rows, value_rows, log_decay, strength = delta_inputs(
        projected[3].astype(jnp.bfloat16),
        projected[4].astype(jnp.bfloat16),
        projected[5].astype(jnp.bfloat16),
        projected[6],
        projected[7],
        write_bias,
        decay_log_scale,
        shift_rows,
        delta_heads,
        GDN_DIM,
    )
    prepared = delta_prepare(
        to_blocks(queries, BLOCK),
        to_blocks(key_rows, BLOCK),
        to_blocks(value_rows, BLOCK),
        to_blocks(log_decay, BLOCK),
        to_blocks(strength, BLOCK),
    )
    identity_map = jnp.broadcast_to(
        jnp.eye(GDN_DIM, dtype=jnp.float32), (delta_heads, GDN_DIM, GDN_DIM)
    )
    empty_state = jnp.zeros((delta_heads, GDN_DIM, GDN_DIM), jnp.float32)
    (local_end, local_map), unused_out = lax.scan(
        transition_step, (empty_state, identity_map), prepared
    )
    own_first = lax.axis_index("sp") * token_rows
    query_place = own_first + lax.iota(jnp.int32, token_rows)
    sp_count = lax.axis_size("sp")
    slot_out = jnp.zeros((sp_count, token_rows, sb_heads, SB_DIM), jnp.float32)
    slot_total = jnp.zeros((sp_count, token_rows, sb_heads), jnp.float32)

    def absorb(slot_arrays, address_portion, value_part, shard_first):

        def active(current):
            partial_value, totals = stick_block(
                sb_query,
                address_portion.reshape(token_rows, sb_heads, SB_DIM),
                value_part.reshape(token_rows, sb_heads, SB_DIM),
                query_place,
                shard_first + lax.iota(jnp.int32, token_rows),
                sb_offset,
            )
            slot_index = shard_first // token_rows
            return (
                lax.dynamic_update_index_in_dim(current[0], partial_value, slot_index, 0),
                lax.dynamic_update_index_in_dim(current[1], totals, slot_index, 0),
            )

        def inactive(current):
            return current

        usable = jnp.logical_and(shard_first >= 0, shard_first <= own_first)
        return lax.cond(usable, active, inactive, slot_arrays)

    key_block = lax.all_gather(sb_keys, "sp", axis=0, tiled=True)
    value_block = lax.all_gather(sb_values, "sp", axis=0, tiled=True)

    def per_shard(shard_number, current):
        row_begin = shard_number * token_rows
        return absorb(
            current,
            lax.dynamic_slice_in_dim(key_block, row_begin, token_rows, 0),
            lax.dynamic_slice_in_dim(value_block, row_begin, token_rows, 0),
            row_begin,
        )

    slot_arrays = lax.fori_loop(
        0, key_block.shape[0] // token_rows, per_shard, (slot_out, slot_total)
    )
    unused_map, incoming = carried_in(
        (local_map, local_end), "sp", compose, (identity_map, empty_state)
    )
    sb_mixed = (
        stick_combine(slot_arrays[0], slot_arrays[1])
        .astype(jnp.bfloat16)
        .reshape(token_rows, sb_heads * SB_DIM)
    )
    unused_end, produced_rows = lax.scan(delta_step, incoming, prepared)
    produced_rows = from_blocks(produced_rows)
    normed = (
        produced_rows
        * lax.rsqrt(jnp.mean(produced_rows * produced_rows, axis=-1, keepdims=True) + NORM_EPS)
        * head_gain
    )
    delta_mixed = normed.astype(jnp.bfloat16).reshape(token_rows, delta_heads * GDN_DIM)
    result = lax.psum_scatter(
        (
            jnp.dot(sb_mixed, sb_out_w, preferred_element_type=jnp.float32)
            + jnp.dot(delta_mixed, delta_out_w, preferred_element_type=jnp.float32)
        ).astype(jnp.bfloat16),
        "tp",
        scatter_dimension=0,
        tiled=True,
    ).astype(jnp.float32)
    return result.astype(jnp.bfloat16).reshape(1, result.shape[0], result.shape[1])


def remote(src, dst, send, recv, axis, index):
    return pltpu.make_async_remote_copy(
        src_ref=src, dst_ref=dst, send_sem=send, recv_sem=recv,
        device_id={axis: index}, device_id_type=MESH,
    )


def greet(axes):
    barrier = pltpu.get_barrier_semaphore()
    count = 0
    for axis in axes:
        size, me = lax.axis_size(axis), lax.axis_index(axis)
        for k in range(1, size):
            pl.semaphore_signal(
                barrier, inc=1, device_id={axis: lax.rem(me + k, size)}, device_id_type=MESH
            )
            count += 1
    pl.semaphore_wait(barrier, count)


def halves(a):
    high = a.astype(jnp.bfloat16)
    return high, (a - high.astype(jnp.float32)).astype(jnp.bfloat16)


def dot_f32(a, b, dims=((1,), (0,))):
    return lax.dot_general(a, b, (dims, ((), ())), preferred_element_type=jnp.float32)


def wide_rhs(high, low, axis):
    top = jnp.concatenate([high, low], axis=axis)
    bottom = jnp.concatenate([high, jnp.zeros_like(low)], axis=axis)
    return jnp.concatenate([top, bottom], axis=1 - axis)


def folded(a):
    half = a.shape[1] // 2
    return a[:, :half] + a[:, half:]


def layer_kernel(
    offset_hbm, decay_scale_hbm, write_bias_hbm,
    x_ref, w0, w1, w2, w3, w4, w5, decay_w_ref, write_w_ref, shift_ref, gain_hbm, sw_hbm, dw_hbm,
    out_ref,
    offset_ref, decay_scale_ref, write_bias_ref, gain_ref,
    xs, ws, gate_w, gate_all, gates, shifts_ref,
    proj, acc, later, maps, adds, stick_out, delta_out,
    sticks, deltas, sw_ref, dw_ref, partial, outgoing, incoming, own,
    x_send, x_recv, f_send, f_recv, w_send, w_recv, s_send, s_recv, l_sem, lw_sem,
    a_send, a_recv, c_send, c_recv,
):
    weights = (w0, w1, w2, w3, w4, w5)
    sp, tp = lax.axis_size("sp"), lax.axis_size("tp")
    z, f, t = lax.axis_index("sp"), lax.axis_index("fs"), lax.axis_index("tp")
    rows, half = x_ref.shape
    depth = w0.shape[0]
    cols = ws.shape[1] // len(weights)
    parts = x_send.shape[2]
    heads = decay_w_ref.shape[0]
    slot = pl.ds(pl.multiple_of(t * half, half), half)
    local = [
        pltpu.make_async_copy(x_ref, xs.at[z, :, slot], l_sem.at[0]),
        pltpu.make_async_copy(shift_ref, shifts_ref.at[z], l_sem.at[1]),
        pltpu.make_async_copy(decay_w_ref, gate_w.at[0], l_sem.at[2]),
        pltpu.make_async_copy(write_w_ref, gate_w.at[1], l_sem.at[3]),
        pltpu.make_async_copy(offset_hbm, offset_ref, l_sem.at[6]),
        pltpu.make_async_copy(decay_scale_hbm, decay_scale_ref, l_sem.at[7]),
        pltpu.make_async_copy(write_bias_hbm, write_bias_ref, l_sem.at[8]),
        pltpu.make_async_copy(gain_hbm, gain_ref, l_sem.at[9]),
    ]
    late = [
        pltpu.make_async_copy(sw_hbm, sw_ref, l_sem.at[4]),
        pltpu.make_async_copy(dw_hbm, dw_ref, l_sem.at[5]),
    ]

    def w_src(i):
        return weights[i].at[:, pl.ds(pl.multiple_of(z * cols, cols), cols)]

    def w_at(i, who):
        return ws.at[pl.ds(pl.multiple_of(who * depth, depth), depth), pl.ds(i * cols, cols)]

    local += [
        pltpu.make_async_copy(w_src(i), w_at(i, f), lw_sem.at[i]) for i in range(len(weights))
    ]
    near = (f + 1 - 2 * (f % 2), f + 2 - 4 * (f // 2))
    count = len(weights)
    delta_kinds, stick_kinds = (3, 4, 5), (0, 1, 2)

    def onward(way):
        return z + 1 < sp if way == 0 else z > 0

    def ahead(way):
        return z + 1 if way == 0 else z - 1

    barrier = pltpu.get_barrier_semaphore()
    for way in range(2):
        @pl.when(onward(way))
        def _():
            pl.semaphore_signal(
                barrier, inc=1, device_id={"sp": ahead(way)}, device_id_type=MESH
            )
    for side in range(2):
        pl.semaphore_signal(barrier, inc=1, device_id={"fs": near[side]}, device_id_type=MESH)
    pl.semaphore_signal(
        barrier, inc=1, device_id={"tp": lax.rem(t + 1, tp)}, device_id_type=MESH
    )
    for c in local:
        c.start()
    peers = onward(0).astype(jnp.int32) + onward(1).astype(jnp.int32) + 3
    pl.semaphore_wait(barrier, peers)

    def x_copy(way, step, part):
        block = z - (step - 1) if way == 0 else z + (step - 1)
        piece = pl.ds(part * (rows // parts), rows // parts)
        there = xs.at[block, piece, slot]
        return remote(
            x_ref.at[piece, :] if step == 1 else there, there,
            x_send.at[way, step, part], x_recv.at[way, step, part], "sp", ahead(way),
        )

    def shift_copy(way, step):
        block = z - (step - 1) if way == 0 else z + (step - 1)
        there = shifts_ref.at[block]
        return remote(
            shift_ref if step == 1 else there, there,
            s_send.at[way, step], s_recv.at[way, step], "sp", ahead(way),
        )

    def comes(way, step):
        return z >= step if way == 0 else z + step < sp

    def sends(way, step):
        return jnp.logical_and(onward(way), comes(way, step - 1))

    def forward(way, step, part):
        block = z - step if way == 0 else z + step
        piece = pl.ds(part * (rows // parts), rows // parts)
        there = xs.at[block, piece, slot]
        return remote(
            x_ref.at[piece, :] if step == 0 else there, there,
            f_send.at[way, step, part], f_recv.at[way, step, part], "tp", lax.rem(t + 1, tp),
        )

    def w_copy(side, i):
        return remote(
            w_src(i), w_at(i, f), w_send.at[side, i], w_recv.at[side, i], "fs", near[side]
        )

    def w_relay(side, i):
        part = depth // 2
        start = pl.multiple_of(near[side] * depth + side * part, part)
        there = ws.at[pl.ds(start, part), pl.ds(i * cols, cols)]
        return remote(
            there, there, w_send.at[2 + side, i], w_recv.at[2 + side, i], "fs", near[1 - side]
        )

    for part in range(parts):
        for way in range(2):
            @pl.when(onward(way))
            def _():
                x_copy(way, 1, part).start()
                if part == 0:
                    shift_copy(way, 1).start()
    for i in delta_kinds:
        for side in range(2):
            w_copy(side, i).start()
    for part in range(parts):
        forward(0, 0, part).start()

    def relay(i):
        for side in range(2):
            w_copy(side, i).wait_recv()
            w_relay(side, i).start()

    def arrive(step, part):
        for way in range(2):
            @pl.when(comes(way, step))
            def _():
                x_copy(way, step, part).wait_recv()
                forward(way, step, part).start()
                if step + 1 < sp:
                    @pl.when(onward(way))
                    def _():
                        x_copy(way, step + 1, part).start()
                if part == 0:
                    shift_copy(way, step).wait_recv()
                    if step + 1 < sp:
                        @pl.when(onward(way))
                        def _():
                            shift_copy(way, step + 1).start()

    early = [(step, part) for step in range(1, sp - 1) for part in range(parts)]
    relay(delta_kinds[0])
    arrive(*early[0])
    for i in delta_kinds[1:]:
        relay(i)
    for i in stick_kinds:
        for side in range(2):
            w_copy(side, i).start()
    for c in late:
        c.start()
    for step, part in early[1:parts]:
        arrive(step, part)
    for c in local:
        c.wait()
    gate_all[...] = jnp.concatenate(
        [gate_w[0].astype(jnp.float32), gate_w[1].astype(jnp.float32)], axis=0
    ).astype(jnp.bfloat16)
    for part in range(parts):
        forward(0, 0, part).wait_recv()

    def relayed(kinds):
        for i in kinds:
            for side in range(2):
                w_relay(side, i).wait_recv()

    relayed(delta_kinds)

    size = offset_ref.shape[0] // sp
    sb_size = cols // size
    scale = sb_size ** (-0.5)
    tile = rows // 2
    below = lax.broadcasted_iota(jnp.int32, (rows, rows), 0)
    across = lax.broadcasted_iota(jnp.int32, (rows, rows), 1)
    after = jnp.where(below > across, 1.0, 0.0).astype(jnp.bfloat16)

    def at_block(b, start=0, extent=rows):
        return pl.ds(pl.multiple_of(b * rows + start, extent), extent)

    def pair(i, j, masked):
        for part in range(rows // tile):
            span = (part + 1) * tile if masked else rows
            mine = at_block(i, part * tile, tile)
            q = proj[0, mine, :]
            keys, values = proj[1, at_block(j), :], proj[2, at_block(j), :]
            keys, values = keys[:span], values[:span]
            lane = lax.broadcasted_iota(jnp.int32, (tile, cols), 1)
            if masked:
                seen = across[:tile, :span] < below[:tile, :span] + part * tile
            mixed = total = None
            for h in range(size):
                query = jnp.where(lane // sb_size == h, q, jnp.zeros_like(q))
                score = dot_f32(query, keys, ((1,), (1,))) * scale + offset_ref[z * size + h]
                skip = jnp.maximum(
                    score, jnp.log(1.0 + jnp.exp(jnp.minimum(score, 80.0)))
                )
                weight = score - skip
                if masked:
                    skip = jnp.where(seen, skip, 0.0)
                beyond = dot_f32(skip.astype(jnp.bfloat16), after[:span, :span])
                weight = jnp.exp(weight - beyond)
                if masked:
                    weight = jnp.where(seen, weight, 0.0)
                part_out = dot_f32(weight.astype(jnp.bfloat16), values)
                whole = jnp.broadcast_to(beyond[:, :1] + skip[:, :1], (tile, cols))
                mixed = part_out if h == 0 else jnp.where(lane // sb_size == h, part_out, mixed)
                total = whole if h == 0 else jnp.where(lane // sb_size == h, whole, total)
            if masked:
                acc[mine, :] = mixed
                later[mine, :] = total
            else:
                passed = later[mine, :]
                acc[mine, :] = acc[mine, :] + mixed * jnp.exp(-passed)
                later[mine, :] = passed + total

    span = BLOCK
    duo = 2 * span
    blocks = rows // span
    width = GDN_DIM
    seg_row = lax.broadcasted_iota(jnp.int32, (rows, rows), 0)
    seg_col = lax.broadcasted_iota(jnp.int32, (rows, rows), 1)
    together = seg_row // span == seg_col // span
    upto = jnp.where(jnp.logical_and(together, seg_row <= seg_col), 1.0, 0.0).astype(jnp.bfloat16)
    beyond_it = jnp.where(jnp.logical_and(together, seg_row > seg_col), 1.0, 0.0).astype(
        jnp.bfloat16
    )
    prow = lax.broadcasted_iota(jnp.int32, (span, duo), 0)
    plane = lax.broadcasted_iota(jnp.int32, (span, duo), 1)
    first = plane < span
    pcol = jnp.where(first, plane, plane - span)
    inclusive, strictly = pcol <= prow, pcol < prow
    unit = jnp.where(pcol == prow, 1.0, 0.0)
    diagonal = lax.broadcasted_iota(jnp.int32, (width, width), 0) == lax.broadcasted_iota(
        jnp.int32, (width, width), 1
    )
    eighth = lax.broadcasted_iota(jnp.int32, (8, rows), 0)

    def silu(a):
        return a * (1.0 / (1.0 + jnp.exp(-a)))

    def unit_of(a):
        return a * lax.rsqrt(jnp.sum(a * a, axis=-1, keepdims=True) + NORM_EPS)

    def apart(a):
        lanes = lax.broadcasted_iota(jnp.int32, a.shape, 1) < span
        zero = jnp.zeros_like(a)
        return jnp.concatenate([jnp.where(lanes, a, zero), jnp.where(lanes, zero, a)], axis=0)

    def squared(left, power):
        high, low = halves(power)
        lhigh, llow = halves(left)
        return folded(
            dot_f32(
                jnp.concatenate([lhigh, llow], axis=1), wide_rhs(apart(high), apart(low), 1)
            )
        )

    def prepare(b, dq, dk, dv):
        gates[...] = dot_f32(gate_all[...], xs[b], ((1,), (1,)))
        pre = gates[pl.ds(z, 1), :]
        write = gates[pl.ds(heads + z, 1), :] + write_bias_ref[z]
        rate = jnp.exp(jnp.full((1, rows), decay_scale_ref[z], jnp.float32))
        soft = jnp.maximum(pre, 0.0) + jnp.log(1.0 + jnp.exp(-jnp.abs(pre)))
        decay = shifts_ref[b, pl.ds(z, 1), :] - rate * soft
        strength = 1.0 / (1.0 + jnp.exp(-write))
        d1 = decay.astype(jnp.bfloat16).astype(jnp.float32)
        d2 = (decay - d1).astype(jnp.bfloat16).astype(jnp.float32)
        d3 = decay - d1 - d2
        three = jnp.where(
            eighth == 0, d1, jnp.where(eighth == 1, d2, jnp.where(eighth == 2, d3, 0.0))
        ).astype(jnp.bfloat16)
        cum_row = jnp.sum(dot_f32(three, upto), axis=0, keepdims=True)
        rest_row = jnp.sum(dot_f32(three, beyond_it), axis=0, keepdims=True)
        stack = jnp.where(
            eighth == 0, strength,
            jnp.where(
                eighth == 1, jnp.exp(cum_row),
                jnp.where(eighth == 2, jnp.exp(rest_row), cum_row),
            ),
        )
        columns = stack.T
        s_col, grow, damp, cum = (columns[:, n : n + 1] for n in range(4))
        q = unit_of(silu(dq)) * width ** (-0.5)
        k = unit_of(silu(dk))
        v = silu(dv)
        boosted = q * grow
        damped = k * damp
        right = jnp.concatenate([v * s_col, k * (s_col * grow)], axis=1)
        kh, kl = halves(k)
        qh, ql = halves(q)
        work = []
        for duo_at in range(rows // duo):
            lo = duo_at * duo
            here = slice(lo, lo + duo)
            left = jnp.concatenate(
                [
                    jnp.concatenate([kh[here], kl[here]], axis=1),
                    jnp.concatenate([qh[here], ql[here]], axis=1),
                ],
                axis=0,
            )
            gram = folded(
                dot_f32(left, wide_rhs(kh[here], kl[here], 0), ((1,), (1,)))
            )
            spread = (
                jnp.where(first, cum[lo : lo + span], cum[lo + span : lo + duo])
                - cum_row[:, here]
            )
            table = jnp.where(inclusive, jnp.exp(jnp.where(inclusive, spread, 0.0)), 0.0)
            scale_col = jnp.where(first, s_col[lo : lo + span], s_col[lo + span : lo + duo])
            near_k = jnp.where(first, gram[:span], gram[span:duo])
            near_q = jnp.where(first, gram[duo : duo + span], gram[duo + span :])
            strict = jnp.where(strictly, near_k * table * scale_col, 0.0)
            work.append([unit - strict, strict, near_q * table])
        for w in work:
            w[1] = squared(w[1], w[1])
        levels = max(1, (span - 1).bit_length()) - 1
        for level in range(levels):
            for w in work:
                if level + 1 < levels:
                    both = squared(jnp.concatenate([w[1], w[0]], axis=0), w[1])
                    w[1], w[0] = both[:span], w[0] + both[span:]
                else:
                    w[0] = w[0] + squared(w[0], w[1])
        for duo_at, (inverse, _, inside) in enumerate(work):
            lo = duo_at * duo
            here = slice(lo, lo + duo)
            ih, il = (apart(a) for a in halves(inverse))
            rh, rl = halves(right[here])
            solved = dot_f32(
                jnp.concatenate([ih, il], axis=1), jnp.concatenate([rh, rh], axis=0)
            ) + dot_f32(ih, rl)
            lh, ll = (
                apart(a) for a in halves(jnp.concatenate([damped[here].T, inside], axis=0))
            )
            sh, sl = halves(solved)
            made = dot_f32(
                jnp.concatenate([lh, ll], axis=1), jnp.concatenate([sh, sh], axis=0)
            ) + dot_f32(lh, sl)
            for side in range(2):
                at = lo + side * span
                mine = made[side * (width + span) : (side + 1) * (width + span)]
                n = b * blocks + 2 * duo_at + side
                keep = grow[at + span - 1 : at + span]
                step_map = jnp.where(diagonal, keep, 0.0) - mine[:width, width:]
                query = boosted[at : at + span] - mine[width:, width:]
                high, low = halves(jnp.concatenate([step_map, query], axis=0))
                maps[n, :, :width] = high
                maps[n, :, width:] = low
                adds[n] = mine[:, :width]

    def wait_x(way, step):
        for part in range(parts):
            if step == sp - 1:
                x_copy(way, step, part).wait_recv()
                forward(way, step, part).start()
                if part == 0:
                    shift_copy(way, step).wait_recv()
        for part in range(parts):
            forward(way, step, part).wait_recv()

    def give(which, out, target):
        here = target.at[:, pl.ds(pl.multiple_of(z * cols, cols), cols)]

        def send(g, k):
            return remote(
                out.at[at_block(g), :], here,
                a_send.at[k, which], a_recv.at[k, which], "sp", g,
            )

        def started(g):
            for k in range(1, sp):
                @pl.when(lax.rem(z + k, sp) == g)
                def _():
                    send(lax.rem(z + k, sp), k).start()

        def finished():
            for k in range(1, sp):
                send(lax.rem(z + k, sp), k).wait_send()

        def came():
            for k in range(1, sp):
                send(lax.rem(z + k, sp), k).wait_recv()

        return started, finished, came

    stick_started, stick_finished, stick_came = give(0, stick_out, sticks)
    delta_started, delta_finished, delta_came = give(1, delta_out, deltas)

    shorter = jnp.minimum(z, sp - 1 - z)
    down_last = z > sp - 1 - z

    def place(n):
        both = n <= 2 * shorter
        way_n = jnp.where(both, lax.rem(n + 1, 2), jnp.where(down_last, 0, 1))
        step_n = jnp.where(n == 0, 0, jnp.where(both, (n + 1) // 2, n - shorter))
        down = jnp.logical_and(way_n == 0, n > 0)
        return way_n, step_n, down, jnp.where(down, z - step_n, z + step_n)

    def delta_event(n):
        way_n, step_n, down, b = place(n)
        for step in range(1, sp):
            for way in range(2):
                @pl.when(jnp.logical_and(step_n == step, way_n == way))
                def _():
                    wait_x(way, step)
        drows = dot_f32(xs[b], ws[:, 3 * cols :]).astype(jnp.bfloat16).astype(jnp.float32)
        prepare(b, drows[:, :cols], drows[:, cols : 2 * cols], drows[:, 2 * cols :])

    def stick_event(n, reach):
        lowest, highest = reach
        way_n, step_n, down, b = place(n)
        lowest = jnp.minimum(lowest, b)
        highest = jnp.maximum(highest, b)
        out = dot_f32(xs[b], ws[:, : 3 * cols]).astype(jnp.bfloat16)
        for i in range(3):
            proj[i, at_block(b), :] = out[:, i * cols : (i + 1) * cols]
        pair(b, b, True)

        def settle(i):
            stick_out[at_block(i), :] = acc[at_block(i), :].astype(jnp.bfloat16)

        first_key = b == 0

        @pl.when(first_key)
        def _():
            settle(b)

        def off(m, c):
            i = jnp.where(down, b + 1 + m, b)
            j = jnp.where(down, b, b - 1 - m)
            pair(i, j, False)

            @pl.when(first_key)
            def _():
                stick_started(i - 1)
                settle(i)
            return c

        lax.fori_loop(0, highest - lowest, off, 0)

        @pl.when(jnp.logical_and(lowest == 0, b > 0))
        def _():
            settle(b)

        @pl.when(lowest == 0)
        def _():
            stick_started(jnp.where(first_key, highest, b))
        return lowest, highest

    def early_delta(n, carry):
        @pl.when(n == 1)
        def _():
            relay(stick_kinds[0])

        @pl.when(n == sp - 2)
        def _():
            for c in early[parts:-1]:
                arrive(*c)
            for i in stick_kinds[1:]:
                relay(i)
            arrive(*early[-1])
        delta_event(n)
        return carry

    lax.fori_loop(0, sp - 1, early_delta, 0)
    relayed(stick_kinds)

    def walk(n, memory):
        high, low = halves(memory)
        new = folded(dot_f32(maps[n], wide_rhs(high, low, 1))) + adds[n]
        made = new[width:]
        made = made * lax.rsqrt(jnp.mean(made * made, axis=-1, keepdims=True) + NORM_EPS)
        at = pl.ds(pl.multiple_of(n * span, span), span)
        delta_out[at, :] = (made * gain_ref[...]).astype(delta_out.dtype)
        return new[:width]

    def stick_loop(n, reach):
        @pl.when(n == sp - 1)
        def _():
            delta_event(n)
            memory = jnp.zeros((width, width), jnp.float32)
            for g in range(sp):
                memory = lax.fori_loop(g * blocks, (g + 1) * blocks, walk, memory)
                if g > 0:
                    delta_started(g - 1)
            delta_started(sp - 1)
        return stick_event(n, reach)

    lax.fori_loop(0, sp, stick_loop, (z, z))

    mine_z = pl.ds(pl.multiple_of(z * rows, rows), rows)
    lanes = pl.ds(pl.multiple_of(z * cols, cols), cols)
    sticks[:, lanes] = stick_out[mine_z, :]
    deltas[:, lanes] = delta_out[mine_z, :]
    for c in late:
        c.wait()
    stick_came()
    chunks, wide = outgoing.shape[0], outgoing.shape[2]
    share = rows // tp
    for c in range(chunks):
        columns = slice(c * wide, (c + 1) * wide)
        partial[:, columns] = dot_f32(sticks[...], sw_ref[:, columns])
    delta_came()
    mine = pl.ds(pl.multiple_of(t * share, share), share)
    partner = lax.rem(t + 1, tp)
    theirs = pl.ds(pl.multiple_of(partner * share, share), share)

    def finish(which, c):
        columns = slice(c * wide, (c + 1) * wide)
        return (
            partial[which, columns] + dot_f32(deltas[which, :], dw_ref[:, columns])
        ).astype(jnp.bfloat16)

    swaps = [
        remote(outgoing.at[c], incoming.at[c], c_send.at[c], c_recv.at[c], "tp", partner)
        for c in range(chunks)
    ]
    for c in range(chunks):
        outgoing[c] = finish(theirs, c)
        if c > 0:
            swaps[c - 1].start()
    for c in range(chunks):
        own[c] = finish(mine, c)
        if c == 0:
            swaps[chunks - 1].start()
    for c in range(chunks):
        swaps[c].wait_recv()
        out_ref[:, c * wide : (c + 1) * wide] = (
            own[c].astype(jnp.float32) + incoming[c].astype(jnp.float32)
        ).astype(out_ref.dtype)

    for c in swaps:
        c.wait_send()
    for i in range(count):
        for side in range(2):
            w_copy(side, i).wait_send()
            w_relay(side, i).wait_send()
    for part in range(parts):
        forward(0, 0, part).wait_send()
        for step in range(1, sp):
            for way in range(2):
                @pl.when(sends(way, step))
                def _():
                    x_copy(way, step, part).wait_send()
                    if part == 0:
                        shift_copy(way, step).wait_send()

                @pl.when(comes(way, step))
                def _():
                    forward(way, step, part).wait_send()
    stick_finished()
    delta_finished()


ANYWHERE = pl.BlockSpec(memory_space=pltpu.HBM)
ON_CORE = pl.BlockSpec(memory_space=pltpu.VMEM)


def on_device_heads(
    hidden_in, sb_query_w, sb_key_w, sb_value_w, sb_offset,
    delta_query_w, delta_key_w, delta_value_w, decay_w, write_w, write_bias,
    decay_log_scale, decay_shift, head_gain, sb_out_w, delta_out_w,
):
    sp, fs, tp = lax.axis_size("sp"), lax.axis_size("fs"), lax.axis_size("tp")
    rows, half = hidden_in.shape[1:]
    width = half * tp
    length = rows * sp
    heads = decay_log_scale.shape[0]
    cols = sb_query_w.shape[1] // sp
    parts, chunks = 2, 4
    share = rows // tp
    blocks = length // BLOCK
    dma = pltpu.SemaphoreType.DMA
    bf16, f32 = jnp.bfloat16, jnp.float32
    result = pl.pallas_call(
        layer_kernel,
        name="layer",
        out_shape=jax.ShapeDtypeStruct((share, width), bf16),
        in_specs=[ANYWHERE] * 16,
        out_specs=ON_CORE,
        scratch_shapes=[
            pltpu.SMEM(sb_offset.shape, f32),
            pltpu.SMEM(decay_log_scale.shape, f32),
            pltpu.SMEM(write_bias.shape, f32),
            pltpu.VMEM((1, head_gain.shape[0]), f32),
            pltpu.VMEM((sp, rows, width), bf16),
            pltpu.VMEM((width, 6 * cols), bf16),
            pltpu.VMEM((2, heads, width), bf16),
            pltpu.VMEM((2 * heads, width), bf16),
            pltpu.VMEM((2 * heads, rows), f32),
            pltpu.VMEM((sp, heads, rows), f32),
            pltpu.VMEM((3, length, cols), bf16),
            pltpu.VMEM((length, cols), f32),
            pltpu.VMEM((length, cols), f32),
            pltpu.VMEM((blocks, cols + BLOCK, 2 * cols), bf16),
            pltpu.VMEM((blocks, cols + BLOCK, cols), f32),
            pltpu.VMEM((length, cols), bf16),
            pltpu.VMEM((length, cols), bf16),
            pltpu.VMEM((rows, cols * sp), bf16),
            pltpu.VMEM((rows, cols * sp), bf16),
            pltpu.VMEM(sb_out_w.shape, bf16),
            pltpu.VMEM(delta_out_w.shape, bf16),
            pltpu.VMEM((rows, width), f32),
            pltpu.VMEM((chunks, share, width // chunks), bf16),
            pltpu.VMEM((chunks, share, width // chunks), bf16),
            pltpu.VMEM((chunks, share, width // chunks), bf16),
            dma((2, sp, parts)), dma((2, sp, parts)), dma((2, sp, parts)), dma((2, sp, parts)),
            dma((fs, 6)), dma((fs, 6)), dma((2, sp)), dma((2, sp)), dma((10,)), dma((6,)),
            dma((sp, 2)), dma((sp, 2)), dma((chunks,)), dma((chunks,)),
        ],
        compiler_params=pltpu.CompilerParams(
            collective_id=0, has_side_effects=True, vmem_limit_bytes=ALL_VMEM
        ),
    )(
        sb_offset, decay_log_scale, write_bias,
        hidden_in.reshape(rows, half), sb_query_w, sb_key_w, sb_value_w,
        delta_query_w, delta_key_w, delta_value_w, decay_w.T, write_w.T,
        decay_shift.reshape(heads, rows), head_gain.reshape(1, -1), sb_out_w, delta_out_w,
    )
    return result.reshape(1, share, width)


def on_device(*inputs):
    delta_heads = inputs[11].shape[0]
    square = lax.axis_size("fs") == 4 and lax.axis_size("tp") == 2
    if square and delta_heads == lax.axis_size("sp") and inputs[4].shape[0] % delta_heads == 0:
        return on_device_heads(*inputs)
    return on_device_split(*inputs)


def solution(mesh):
    return jax.shard_map(
        on_device,
        mesh=mesh,
        in_specs=(
            P("fs", "sp", "tp"),
            P("fs", "tp"),
            P("fs", "tp"),
            P("fs", "tp"),
            P("tp"),
            P("fs", "tp"),
            P("fs", "tp"),
            P("fs", "tp"),
            P(None, "tp"),
            P(None, "tp"),
            P("tp"),
            P("tp"),
            P("fs", "tp", "sp"),
            P(),
            P("tp", None),
            P("tp", None),
        ),
        out_specs=P("fs", ("sp", "tp"), None),
        check_vma=False,
    )
```

```python
import jax
import jax.numpy as jnp
from jax import lax
from jax.experimental import pallas as pl
from jax.experimental.pallas import tpu as pltpu
from jax.sharding import PartitionSpec as P

MESH = pl.DeviceIdType.MESH
ALL_VMEM = 67043328

SB_DIM = 64
GDN_DIM = 128
BLOCK = 64


EXACT_MATMUL = lax.Precision.HIGHEST
NORM_EPS = 1e-06


def carried_in(value, axis, combine, identity):
    devices, index = (lax.axis_size(axis), lax.axis_index(axis))
    everything = jax.tree.map(
        lambda part, kind: lax.all_gather(part.astype(kind), axis),
        value,
        (jnp.bfloat16, jnp.bfloat16),
    )
    start = jax.tree.map(
        lambda part, zero: jnp.broadcast_to(jnp.asarray(zero, part.dtype), part.shape),
        value,
        identity,
    )

    def lap(k, before):
        reached = k < index
        new = combine(
            before, jax.tree.map(lambda part, own: part[k].astype(own.dtype), everything, value)
        )
        return jax.tree.map(lambda a, b: jnp.where(reached, a, b), new, before)

    return lax.fori_loop(0, devices, lap, start)


def unit_lower_inverse(strict_part):
    order_size = strict_part.shape[-1]
    powered = strict_part
    inverse = jnp.eye(order_size, dtype=strict_part.dtype) - strict_part
    for repeat_number in range(max(1, (order_size - 1).bit_length()) - 1):
        powered = jnp.einsum("...ij,...jk->...ik", powered, powered, precision=EXACT_MATMUL)
        inverse = inverse + jnp.einsum(
            "...ij,...jk->...ik", inverse, powered, precision=EXACT_MATMUL
        )
    return inverse


def to_blocks(row_data, block_span):
    blocks_count = row_data.shape[0] // block_span
    shaped = row_data.reshape((blocks_count, block_span) + row_data.shape[1:])
    return jnp.swapaxes(shaped, 1, 2)


def from_blocks(blocked):
    swapped = jnp.swapaxes(blocked, 1, 2)
    return swapped.reshape((-1,) + swapped.shape[2:])


def unit_rows(vectors):
    return vectors * lax.rsqrt(jnp.sum(vectors * vectors, axis=-1, keepdims=True) + NORM_EPS)


def delta_inputs(
    query_proj,
    key_proj,
    value_proj,
    decay_pre,
    write_pre,
    write_bias,
    decay_log_scale,
    shift_rows,
    head_count,
    head_size,
):
    query_act = jax.nn.silu(query_proj.astype(jnp.float32)).reshape(-1, head_count, head_size)
    key_act = jax.nn.silu(key_proj.astype(jnp.float32)).reshape(-1, head_count, head_size)
    value_rows = jax.nn.silu(value_proj.astype(jnp.float32)).reshape(-1, head_count, head_size)
    queries = unit_rows(query_act) * head_size ** (-0.5)
    key_rows = unit_rows(key_act)
    log_decay = -jnp.exp(decay_log_scale) * jax.nn.softplus(decay_pre) + shift_rows
    strength = jax.nn.sigmoid(write_pre + write_bias)
    return (queries, key_rows, value_rows, log_decay, strength)


def delta_prepare(queries, key_rows, value_rows, log_decay, strength):
    block_span = queries.shape[2]
    cumulative = jnp.cumsum(log_decay, axis=-1)
    row_place = lax.broadcasted_iota(jnp.int32, (block_span, block_span), 0)
    col_place = lax.broadcasted_iota(jnp.int32, (block_span, block_span), 1)
    inclusive = col_place <= row_place
    strictly = col_place < row_place
    spread = cumulative[..., :, None] - cumulative[..., None, :]
    decay_table = jnp.where(inclusive, jnp.exp(jnp.where(inclusive, spread, 0.0)), 0.0)
    keys_beta = key_rows * strength[..., None]
    lower_part = jnp.where(
        strictly,
        jnp.einsum("nhik,nhjk->nhij", keys_beta, key_rows, precision=EXACT_MATMUL) * decay_table,
        0.0,
    )
    inverse = unit_lower_inverse(lower_part)
    growth = jnp.exp(cumulative)
    state_updates = jnp.einsum(
        "nhij,nhjv->nhiv", inverse, value_rows * strength[..., None], precision=EXACT_MATMUL
    )
    erase_term = jnp.einsum(
        "nhij,nhjk->nhik", inverse, keys_beta * growth[..., None], precision=EXACT_MATMUL
    )
    inside_block = (
        jnp.einsum("nhik,nhjk->nhij", queries, key_rows, precision=EXACT_MATMUL) * decay_table
    )
    boosted_query = queries * growth[..., None]
    damped_keys = key_rows * jnp.exp(cumulative[..., -1:] - cumulative)[..., None]
    decay_per_block = jnp.exp(cumulative[..., -1])
    return (state_updates, erase_term, inside_block, boosted_query, damped_keys, decay_per_block)


def delta_step(memory_state, inputs):
    state_updates, erase_term, inside_block, boosted_query, damped_keys, decay_per_block = inputs
    fixed_values = state_updates - jnp.einsum(
        "mzq,mqc->mzc", erase_term, memory_state, precision=EXACT_MATMUL
    )
    produced_rows = jnp.einsum(
        "mzq,mqc->mzc", boosted_query, memory_state, precision=EXACT_MATMUL
    ) + jnp.einsum("efq,eqn->efn", inside_block, fixed_values, precision=EXACT_MATMUL)
    memory_state = memory_state * decay_per_block[:, None, None] + jnp.einsum(
        "wam,waz->wmz", damped_keys, fixed_values, precision=EXACT_MATMUL
    )
    return (memory_state, produced_rows)


def transition_step(carried, inputs):
    memory_state, transfer = carried
    state_updates, erase_term, inside_block, boosted_query, damped_keys, decay_per_block = inputs
    fixed_values = state_updates - jnp.einsum(
        "mzq,mqc->mzc", erase_term, memory_state, precision=EXACT_MATMUL
    )
    coupling = jnp.einsum("hik,hil->hkl", damped_keys, erase_term, precision=EXACT_MATMUL)
    memory_state = memory_state * decay_per_block[:, None, None] + jnp.einsum(
        "wam,waz->wmz", damped_keys, fixed_values, precision=EXACT_MATMUL
    )
    transfer = transfer * decay_per_block[:, None, None] - jnp.einsum(
        "hkl,hlm->hkm", coupling, transfer, precision=EXACT_MATMUL
    )
    return ((memory_state, transfer), None)


def compose(prior_blocks, following_blocks):
    joined_map = jnp.einsum(
        "hkl,hlm->hkm", following_blocks[0], prior_blocks[0], precision=EXACT_MATMUL
    )
    joined_state = (
        jnp.einsum("djo,dog->djg", following_blocks[0], prior_blocks[1], precision=EXACT_MATMUL)
        + following_blocks[1]
    )
    return (joined_map, joined_state)


def stick_block(queries, key_rows, value_rows, query_place, key_place, offsets):
    scale_factor = queries.shape[-1] ** (-0.5)
    scores = (
        jnp.einsum("qhd,khd->hqk", queries, key_rows, preferred_element_type=jnp.float32)
        * scale_factor
        + offsets[:, None, None]
    )
    visible = key_place[None, :] < query_place[:, None]
    skipped = jnp.where(visible, jax.nn.log_sigmoid(-scores), 0.0)
    beyond = lax.cumsum(skipped, axis=2, reverse=True) - skipped
    weights = jnp.where(visible, jnp.exp(jax.nn.log_sigmoid(scores) + beyond), 0.0).astype(
        jnp.bfloat16
    )
    partial_value = jnp.einsum(
        "hqk,khd->qhd", weights, value_rows, preferred_element_type=jnp.float32
    )
    return (partial_value, jnp.sum(skipped, axis=2).T)


def stick_combine(partials, totals):
    beyond = jnp.cumsum(totals[::-1], axis=0)[::-1] - totals
    return jnp.sum(partials * jnp.exp(beyond)[..., None], axis=0)


def on_device_split(
    hidden_in,
    sb_query_w,
    sb_key_w,
    sb_value_w,
    sb_offset,
    delta_query_w,
    delta_key_w,
    delta_value_w,
    decay_w,
    write_w,
    write_bias,
    decay_log_scale,
    decay_shift,
    head_gain,
    sb_out_w,
    delta_out_w,
):
    token_rows = hidden_in.shape[1]
    local_in = hidden_in.reshape(token_rows, hidden_in.shape[2])
    gathered = (
        lax.all_gather(sb_query_w, "fs", axis=0, tiled=True),
        lax.all_gather(sb_key_w, "fs", axis=0, tiled=True),
        lax.all_gather(sb_value_w, "fs", axis=0, tiled=True),
        lax.all_gather(delta_query_w, "fs", axis=0, tiled=True),
        lax.all_gather(delta_key_w, "fs", axis=0, tiled=True),
        lax.all_gather(delta_value_w, "fs", axis=0, tiled=True),
    )
    in_weights = tuple(gathered) + (decay_w, write_w)
    portion = lax.all_gather(local_in, "tp", axis=1, tiled=True)
    projected = tuple(
        (jnp.dot(portion, weight, preferred_element_type=jnp.float32) for weight in in_weights)
    )
    sb_heads = sb_offset.shape[0]
    delta_heads = decay_log_scale.shape[0]
    sb_query = projected[0].astype(jnp.bfloat16).reshape(token_rows, sb_heads, SB_DIM)
    sb_keys = projected[1].astype(jnp.bfloat16)
    sb_values = projected[2].astype(jnp.bfloat16)
    shift_rows = decay_shift.reshape(delta_heads, token_rows).T
    queries, key_rows, value_rows, log_decay, strength = delta_inputs(
        projected[3].astype(jnp.bfloat16),
        projected[4].astype(jnp.bfloat16),
        projected[5].astype(jnp.bfloat16),
        projected[6],
        projected[7],
        write_bias,
        decay_log_scale,
        shift_rows,
        delta_heads,
        GDN_DIM,
    )
    prepared = delta_prepare(
        to_blocks(queries, BLOCK),
        to_blocks(key_rows, BLOCK),
        to_blocks(value_rows, BLOCK),
        to_blocks(log_decay, BLOCK),
        to_blocks(strength, BLOCK),
    )
    identity_map = jnp.broadcast_to(
        jnp.eye(GDN_DIM, dtype=jnp.float32), (delta_heads, GDN_DIM, GDN_DIM)
    )
    empty_state = jnp.zeros((delta_heads, GDN_DIM, GDN_DIM), jnp.float32)
    (local_end, local_map), unused_out = lax.scan(
        transition_step, (empty_state, identity_map), prepared
    )
    own_first = lax.axis_index("sp") * token_rows
    query_place = own_first + lax.iota(jnp.int32, token_rows)
    sp_count = lax.axis_size("sp")
    slot_out = jnp.zeros((sp_count, token_rows, sb_heads, SB_DIM), jnp.float32)
    slot_total = jnp.zeros((sp_count, token_rows, sb_heads), jnp.float32)

    def absorb(slot_arrays, address_portion, value_part, shard_first):

        def active(current):
            partial_value, totals = stick_block(
                sb_query,
                address_portion.reshape(token_rows, sb_heads, SB_DIM),
                value_part.reshape(token_rows, sb_heads, SB_DIM),
                query_place,
                shard_first + lax.iota(jnp.int32, token_rows),
                sb_offset,
            )
            slot_index = shard_first // token_rows
            return (
                lax.dynamic_update_index_in_dim(current[0], partial_value, slot_index, 0),
                lax.dynamic_update_index_in_dim(current[1], totals, slot_index, 0),
            )

        def inactive(current):
            return current

        usable = jnp.logical_and(shard_first >= 0, shard_first <= own_first)
        return lax.cond(usable, active, inactive, slot_arrays)

    key_block = lax.all_gather(sb_keys, "sp", axis=0, tiled=True)
    value_block = lax.all_gather(sb_values, "sp", axis=0, tiled=True)

    def per_shard(shard_number, current):
        row_begin = shard_number * token_rows
        return absorb(
            current,
            lax.dynamic_slice_in_dim(key_block, row_begin, token_rows, 0),
            lax.dynamic_slice_in_dim(value_block, row_begin, token_rows, 0),
            row_begin,
        )

    slot_arrays = lax.fori_loop(
        0, key_block.shape[0] // token_rows, per_shard, (slot_out, slot_total)
    )
    unused_map, incoming = carried_in(
        (local_map, local_end), "sp", compose, (identity_map, empty_state)
    )
    sb_mixed = (
        stick_combine(slot_arrays[0], slot_arrays[1])
        .astype(jnp.bfloat16)
        .reshape(token_rows, sb_heads * SB_DIM)
    )
    unused_end, produced_rows = lax.scan(delta_step, incoming, prepared)
    produced_rows = from_blocks(produced_rows)
    normed = (
        produced_rows
        * lax.rsqrt(jnp.mean(produced_rows * produced_rows, axis=-1, keepdims=True) + NORM_EPS)
        * head_gain
    )
    delta_mixed = normed.astype(jnp.bfloat16).reshape(token_rows, delta_heads * GDN_DIM)
    result = lax.psum_scatter(
        (
            jnp.dot(sb_mixed, sb_out_w, preferred_element_type=jnp.float32)
            + jnp.dot(delta_mixed, delta_out_w, preferred_element_type=jnp.float32)
        ).astype(jnp.bfloat16),
        "tp",
        scatter_dimension=0,
        tiled=True,
    ).astype(jnp.float32)
    return result.astype(jnp.bfloat16).reshape(1, result.shape[0], result.shape[1])


def remote(src, dst, send, recv, axis, index):
    return pltpu.make_async_remote_copy(
        src_ref=src, dst_ref=dst, send_sem=send, recv_sem=recv,
        device_id={axis: index}, device_id_type=MESH,
    )


def greet(axes):
    barrier = pltpu.get_barrier_semaphore()
    count = 0
    for axis in axes:
        size, me = lax.axis_size(axis), lax.axis_index(axis)
        for k in range(1, size):
            pl.semaphore_signal(
                barrier, inc=1, device_id={axis: lax.rem(me + k, size)}, device_id_type=MESH
            )
            count += 1
    pl.semaphore_wait(barrier, count)


def halves(a):
    high = a.astype(jnp.bfloat16)
    return high, (a - high.astype(jnp.float32)).astype(jnp.bfloat16)


def dot_f32(a, b, dims=((1,), (0,))):
    return lax.dot_general(a, b, (dims, ((), ())), preferred_element_type=jnp.float32)


def wide_rhs(high, low, axis):
    top = jnp.concatenate([high, low], axis=axis)
    bottom = jnp.concatenate([high, jnp.zeros_like(low)], axis=axis)
    return jnp.concatenate([top, bottom], axis=1 - axis)


def folded(a):
    half = a.shape[1] // 2
    return a[:, :half] + a[:, half:]


def layer_kernel(
    offset_hbm, decay_scale_hbm, write_bias_hbm,
    x_ref, w0, w1, w2, w3, w4, w5, decay_w_ref, write_w_ref, shift_ref, gain_hbm, sw_hbm, dw_hbm,
    own, incoming,
    offset_ref, decay_scale_ref, write_bias_ref, gain_ref,
    xs, ws, gate_w, gate_all, gates, shifts_ref,
    proj, acc, later, maps, adds, stick_out, delta_out,
    sticks, deltas, sw_ref, dw_ref, partial, outgoing,
    x_send, x_recv, f_send, f_recv, w_send, w_recv, s_send, s_recv, l_sem, lw_sem,
    a_send, a_recv, c_send, c_recv,
):
    weights = (w0, w1, w2, w3, w4, w5)
    sp, tp = lax.axis_size("sp"), lax.axis_size("tp")
    z, f, t = lax.axis_index("sp"), lax.axis_index("fs"), lax.axis_index("tp")
    rows, half = x_ref.shape
    depth = w0.shape[0]
    cols = ws.shape[1] // len(weights)
    parts = x_send.shape[2]
    heads = decay_w_ref.shape[0]
    slot = pl.ds(pl.multiple_of(t * half, half), half)
    local = [
        pltpu.make_async_copy(x_ref, xs.at[z, :, slot], l_sem.at[0]),
        pltpu.make_async_copy(shift_ref, shifts_ref.at[z], l_sem.at[1]),
        pltpu.make_async_copy(decay_w_ref, gate_w.at[0], l_sem.at[2]),
        pltpu.make_async_copy(write_w_ref, gate_w.at[1], l_sem.at[3]),
        pltpu.make_async_copy(offset_hbm, offset_ref, l_sem.at[6]),
        pltpu.make_async_copy(decay_scale_hbm, decay_scale_ref, l_sem.at[7]),
        pltpu.make_async_copy(write_bias_hbm, write_bias_ref, l_sem.at[8]),
        pltpu.make_async_copy(gain_hbm, gain_ref, l_sem.at[9]),
    ]
    late = [
        pltpu.make_async_copy(sw_hbm, sw_ref, l_sem.at[4]),
        pltpu.make_async_copy(dw_hbm, dw_ref, l_sem.at[5]),
    ]

    def w_src(i):
        return weights[i].at[:, pl.ds(pl.multiple_of(z * cols, cols), cols)]

    def w_at(i, who):
        return ws.at[pl.ds(pl.multiple_of(who * depth, depth), depth), pl.ds(i * cols, cols)]

    local += [
        pltpu.make_async_copy(w_src(i), w_at(i, f), lw_sem.at[i]) for i in range(len(weights))
    ]
    near = (f + 1 - 2 * (f % 2), f + 2 - 4 * (f // 2))
    count = len(weights)
    delta_kinds, stick_kinds = (3, 4, 5), (0, 1, 2)

    def onward(way):
        return z + 1 < sp if way == 0 else z > 0

    def ahead(way):
        return z + 1 if way == 0 else z - 1

    barrier = pltpu.get_barrier_semaphore()
    for way in range(2):
        @pl.when(onward(way))
        def _():
            pl.semaphore_signal(
                barrier, inc=1, device_id={"sp": ahead(way)}, device_id_type=MESH
            )
    for side in range(2):
        pl.semaphore_signal(barrier, inc=1, device_id={"fs": near[side]}, device_id_type=MESH)
    pl.semaphore_signal(
        barrier, inc=1, device_id={"tp": lax.rem(t + 1, tp)}, device_id_type=MESH
    )
    for c in local:
        c.start()
    peers = onward(0).astype(jnp.int32) + onward(1).astype(jnp.int32) + 3
    pl.semaphore_wait(barrier, peers)

    def x_copy(way, step, part):
        block = z - (step - 1) if way == 0 else z + (step - 1)
        piece = pl.ds(part * (rows // parts), rows // parts)
        there = xs.at[block, piece, slot]
        return remote(
            x_ref.at[piece, :] if step == 1 else there, there,
            x_send.at[way, step, part], x_recv.at[way, step, part], "sp", ahead(way),
        )

    def shift_copy(way, step):
        block = z - (step - 1) if way == 0 else z + (step - 1)
        there = shifts_ref.at[block]
        return remote(
            shift_ref if step == 1 else there, there,
            s_send.at[way, step], s_recv.at[way, step], "sp", ahead(way),
        )

    def comes(way, step):
        return z >= step if way == 0 else z + step < sp

    def sends(way, step):
        return jnp.logical_and(onward(way), comes(way, step - 1))

    def forward(way, step, part):
        block = z - step if way == 0 else z + step
        piece = pl.ds(part * (rows // parts), rows // parts)
        there = xs.at[block, piece, slot]
        return remote(
            x_ref.at[piece, :] if step == 0 else there, there,
            f_send.at[way, step, part], f_recv.at[way, step, part], "tp", lax.rem(t + 1, tp),
        )

    def w_copy(side, i):
        return remote(
            w_src(i), w_at(i, f), w_send.at[side, i], w_recv.at[side, i], "fs", near[side]
        )

    def w_relay(side, i):
        part = depth // 2
        start = pl.multiple_of(near[side] * depth + side * part, part)
        there = ws.at[pl.ds(start, part), pl.ds(i * cols, cols)]
        return remote(
            there, there, w_send.at[2 + side, i], w_recv.at[2 + side, i], "fs", near[1 - side]
        )

    for part in range(parts):
        for way in range(2):
            @pl.when(onward(way))
            def _():
                x_copy(way, 1, part).start()
                if part == 0:
                    shift_copy(way, 1).start()
    for i in delta_kinds:
        for side in range(2):
            w_copy(side, i).start()
    for part in range(parts):
        forward(0, 0, part).start()

    def relay(i):
        for side in range(2):
            w_copy(side, i).wait_recv()
            w_relay(side, i).start()

    def arrive(step, part):
        for way in range(2):
            @pl.when(comes(way, step))
            def _():
                x_copy(way, step, part).wait_recv()
                forward(way, step, part).start()
                if step + 1 < sp:
                    @pl.when(onward(way))
                    def _():
                        x_copy(way, step + 1, part).start()
                if part == 0:
                    shift_copy(way, step).wait_recv()
                    if step + 1 < sp:
                        @pl.when(onward(way))
                        def _():
                            shift_copy(way, step + 1).start()

    early = [(step, part) for step in range(1, sp - 1) for part in range(parts)]
    relay(delta_kinds[0])
    arrive(*early[0])
    for i in delta_kinds[1:]:
        relay(i)
    for i in stick_kinds:
        for side in range(2):
            w_copy(side, i).start()
    for c in late:
        c.start()
    for step, part in early[1:parts]:
        arrive(step, part)
    for c in local:
        c.wait()
    gate_all[...] = jnp.concatenate(
        [gate_w[0].astype(jnp.float32), gate_w[1].astype(jnp.float32)], axis=0
    ).astype(jnp.bfloat16)
    for part in range(parts):
        forward(0, 0, part).wait_recv()

    def relayed(kinds):
        for i in kinds:
            for side in range(2):
                w_relay(side, i).wait_recv()

    relayed(delta_kinds)

    size = offset_ref.shape[0] // sp
    sb_size = cols // size
    scale = sb_size ** (-0.5)
    tile = rows // 2
    below = lax.broadcasted_iota(jnp.int32, (rows, rows), 0)
    across = lax.broadcasted_iota(jnp.int32, (rows, rows), 1)
    after = jnp.where(below > across, 1.0, 0.0).astype(jnp.bfloat16)

    def at_block(b, start=0, extent=rows):
        return pl.ds(pl.multiple_of(b * rows + start, extent), extent)

    def pair(i, j, masked, fresh):
        for part in range(rows // tile):
            span = (part + 1) * tile if fresh else rows
            mine = at_block(i, part * tile, tile)
            q = proj[0, mine, :]
            keys, values = proj[1, at_block(j), :], proj[2, at_block(j), :]
            keys, values = keys[:span], values[:span]
            lane = lax.broadcasted_iota(jnp.int32, (tile, cols), 1)
            if masked:
                seen = across[:tile, :span] < below[:tile, :span] + part * tile + (i - j) * rows
            mixed = total = None
            for h in range(size):
                query = jnp.where(lane // sb_size == h, q, jnp.zeros_like(q))
                score = dot_f32(query, keys, ((1,), (1,))) * scale + offset_ref[z * size + h]
                skip = jnp.maximum(
                    score, jnp.log(1.0 + jnp.exp(jnp.minimum(score, 80.0)))
                )
                weight = score - skip
                if masked:
                    skip = jnp.where(seen, skip, 0.0)
                beyond = dot_f32(skip.astype(jnp.bfloat16), after[:span, :span])
                weight = jnp.exp(weight - beyond)
                if masked:
                    weight = jnp.where(seen, weight, 0.0)
                part_out = dot_f32(weight.astype(jnp.bfloat16), values)
                whole = jnp.broadcast_to(beyond[:, :1] + skip[:, :1], (tile, cols))
                mixed = part_out if h == 0 else jnp.where(lane // sb_size == h, part_out, mixed)
                total = whole if h == 0 else jnp.where(lane // sb_size == h, whole, total)
            if fresh:
                acc[mine, :] = mixed
                later[mine, :] = total
            else:
                passed = later[mine, :]
                acc[mine, :] = acc[mine, :] + mixed * jnp.exp(-passed)
                later[mine, :] = passed + total

    span = BLOCK
    duo = 2 * span
    blocks = rows // span
    width = GDN_DIM
    seg_row = lax.broadcasted_iota(jnp.int32, (rows, rows), 0)
    seg_col = lax.broadcasted_iota(jnp.int32, (rows, rows), 1)
    together = seg_row // span == seg_col // span
    upto = jnp.where(jnp.logical_and(together, seg_row <= seg_col), 1.0, 0.0).astype(jnp.bfloat16)
    beyond_it = jnp.where(jnp.logical_and(together, seg_row > seg_col), 1.0, 0.0).astype(
        jnp.bfloat16
    )
    prow = lax.broadcasted_iota(jnp.int32, (span, duo), 0)
    plane = lax.broadcasted_iota(jnp.int32, (span, duo), 1)
    first = plane < span
    pcol = jnp.where(first, plane, plane - span)
    inclusive, strictly = pcol <= prow, pcol < prow
    unit = jnp.where(pcol == prow, 1.0, 0.0)
    diagonal = lax.broadcasted_iota(jnp.int32, (width, width), 0) == lax.broadcasted_iota(
        jnp.int32, (width, width), 1
    )
    eighth = lax.broadcasted_iota(jnp.int32, (8, rows), 0)

    def silu(a):
        return a * (1.0 / (1.0 + jnp.exp(-a)))

    def unit_of(a):
        return a * lax.rsqrt(jnp.sum(a * a, axis=-1, keepdims=True) + NORM_EPS)

    def apart(a):
        lanes = lax.broadcasted_iota(jnp.int32, a.shape, 1) < span
        zero = jnp.zeros_like(a)
        return jnp.concatenate([jnp.where(lanes, a, zero), jnp.where(lanes, zero, a)], axis=0)

    def squared(left, power):
        high, low = halves(power)
        lhigh, llow = halves(left)
        return folded(
            dot_f32(
                jnp.concatenate([lhigh, llow], axis=1), wide_rhs(apart(high), apart(low), 1)
            )
        )

    def prepare(b, dq, dk, dv):
        gates[...] = dot_f32(gate_all[...], xs[b], ((1,), (1,)))
        pre = gates[pl.ds(z, 1), :]
        write = gates[pl.ds(heads + z, 1), :] + write_bias_ref[z]
        rate = jnp.exp(jnp.full((1, rows), decay_scale_ref[z], jnp.float32))
        soft = jnp.maximum(pre, 0.0) + jnp.log(1.0 + jnp.exp(-jnp.abs(pre)))
        decay = shifts_ref[b, pl.ds(z, 1), :] - rate * soft
        strength = 1.0 / (1.0 + jnp.exp(-write))
        d1 = decay.astype(jnp.bfloat16).astype(jnp.float32)
        d2 = (decay - d1).astype(jnp.bfloat16).astype(jnp.float32)
        d3 = decay - d1 - d2
        three = jnp.where(
            eighth == 0, d1, jnp.where(eighth == 1, d2, jnp.where(eighth == 2, d3, 0.0))
        ).astype(jnp.bfloat16)
        cum_row = jnp.sum(dot_f32(three, upto), axis=0, keepdims=True)
        rest_row = jnp.sum(dot_f32(three, beyond_it), axis=0, keepdims=True)
        stack = jnp.where(
            eighth == 0, strength,
            jnp.where(
                eighth == 1, jnp.exp(cum_row),
                jnp.where(eighth == 2, jnp.exp(rest_row), cum_row),
            ),
        )
        columns = stack.T
        s_col, grow, damp, cum = (columns[:, n : n + 1] for n in range(4))
        q = unit_of(silu(dq)) * width ** (-0.5)
        k = unit_of(silu(dk))
        v = silu(dv)
        boosted = q * grow
        damped = k * damp
        right = jnp.concatenate([v * s_col, k * (s_col * grow)], axis=1)
        kh, kl = halves(k)
        qh, ql = halves(q)
        work = []
        for duo_at in range(rows // duo):
            lo = duo_at * duo
            here = slice(lo, lo + duo)
            left = jnp.concatenate(
                [
                    jnp.concatenate([kh[here], kl[here]], axis=1),
                    jnp.concatenate([qh[here], ql[here]], axis=1),
                ],
                axis=0,
            )
            gram = folded(
                dot_f32(left, wide_rhs(kh[here], kl[here], 0), ((1,), (1,)))
            )
            spread = (
                jnp.where(first, cum[lo : lo + span], cum[lo + span : lo + duo])
                - cum_row[:, here]
            )
            table = jnp.where(inclusive, jnp.exp(jnp.where(inclusive, spread, 0.0)), 0.0)
            scale_col = jnp.where(first, s_col[lo : lo + span], s_col[lo + span : lo + duo])
            near_k = jnp.where(first, gram[:span], gram[span:duo])
            near_q = jnp.where(first, gram[duo : duo + span], gram[duo + span :])
            strict = jnp.where(strictly, near_k * table * scale_col, 0.0)
            work.append([unit - strict, strict, near_q * table])
        for w in work:
            w[1] = squared(w[1], w[1])
        levels = max(1, (span - 1).bit_length()) - 1
        for level in range(levels):
            for w in work:
                if level + 1 < levels:
                    both = squared(jnp.concatenate([w[1], w[0]], axis=0), w[1])
                    w[1], w[0] = both[:span], w[0] + both[span:]
                else:
                    w[0] = w[0] + squared(w[0], w[1])
        for duo_at, (inverse, _, inside) in enumerate(work):
            lo = duo_at * duo
            here = slice(lo, lo + duo)
            ih, il = (apart(a) for a in halves(inverse))
            rh, rl = halves(right[here])
            solved = dot_f32(
                jnp.concatenate([ih, il], axis=1), jnp.concatenate([rh, rh], axis=0)
            ) + dot_f32(ih, rl)
            lh, ll = (
                apart(a) for a in halves(jnp.concatenate([damped[here].T, inside], axis=0))
            )
            sh, sl = halves(solved)
            made = dot_f32(
                jnp.concatenate([lh, ll], axis=1), jnp.concatenate([sh, sh], axis=0)
            ) + dot_f32(lh, sl)
            for side in range(2):
                at = lo + side * span
                mine = made[side * (width + span) : (side + 1) * (width + span)]
                n = b * blocks + 2 * duo_at + side
                keep = grow[at + span - 1 : at + span]
                step_map = jnp.where(diagonal, keep, 0.0) - mine[:width, width:]
                query = boosted[at : at + span] - mine[width:, width:]
                high, low = halves(jnp.concatenate([step_map, query], axis=0))
                maps[n, :, :width] = high
                maps[n, :, width:] = low
                adds[n] = mine[:, :width]

    def wait_x(way, step):
        for part in range(parts):
            if step == sp - 1:
                x_copy(way, step, part).wait_recv()
                forward(way, step, part).start()
                if part == 0:
                    shift_copy(way, step).wait_recv()
        for part in range(parts):
            forward(way, step, part).wait_recv()

    def give(which, out, target):
        here = target.at[:, pl.ds(pl.multiple_of(z * cols, cols), cols)]

        def send(g, k):
            return remote(
                out.at[at_block(g), :], here,
                a_send.at[k, which], a_recv.at[k, which], "sp", g,
            )

        def started(g):
            for k in range(1, sp):
                @pl.when(lax.rem(z + k, sp) == g)
                def _():
                    send(lax.rem(z + k, sp), k).start()

        def finished():
            for k in range(1, sp):
                send(lax.rem(z + k, sp), k).wait_send()

        def came():
            for k in range(1, sp):
                send(lax.rem(z + k, sp), k).wait_recv()

        return started, finished, came

    stick_started, stick_finished, stick_came = give(0, stick_out, sticks)
    delta_started, delta_finished, delta_came = give(1, delta_out, deltas)

    shorter = jnp.minimum(z, sp - 1 - z)
    down_last = z > sp - 1 - z

    def place(n):
        both = n <= 2 * shorter
        way_n = jnp.where(both, lax.rem(n + 1, 2), jnp.where(down_last, 0, 1))
        step_n = jnp.where(n == 0, 0, jnp.where(both, (n + 1) // 2, n - shorter))
        down = jnp.logical_and(way_n == 0, n > 0)
        return way_n, step_n, down, jnp.where(down, z - step_n, z + step_n)

    def delta_event(n):
        way_n, step_n, down, b = place(n)
        for step in range(1, sp):
            for way in range(2):
                @pl.when(jnp.logical_and(step_n == step, way_n == way))
                def _():
                    wait_x(way, step)
        drows = dot_f32(xs[b], ws[:, 3 * cols :]).astype(jnp.bfloat16).astype(jnp.float32)
        prepare(b, drows[:, :cols], drows[:, cols : 2 * cols], drows[:, 2 * cols :])

    def settle(i):
        stick_out[at_block(i), :] = acc[at_block(i), :].astype(jnp.bfloat16)

    def stick_project(b):
        out = dot_f32(xs[b], ws[:, : 3 * cols]).astype(jnp.bfloat16)
        for i in range(3):
            proj[i, at_block(b), :] = out[:, i * cols : (i + 1) * cols]

    def stick_event(n, reach):
        lowest, highest = reach
        way_n, step_n, down, b = place(n)
        lowest = jnp.minimum(lowest, b)
        highest = jnp.maximum(highest, b)
        stick_project(b)
        pair(b, b, True, True)
        first_key = b == 0

        @pl.when(first_key)
        def _():
            settle(b)

        def off(m, c):
            i = jnp.where(down, b + 1 + m, b)
            j = jnp.where(down, b, b - 1 - m)
            pair(i, j, False, False)

            @pl.when(first_key)
            def _():
                stick_started(i - 1)
                settle(i)
            return c

        lax.fori_loop(0, highest - lowest, off, 0)

        @pl.when(jnp.logical_and(lowest == 0, b > 0))
        def _():
            settle(b)

        @pl.when(lowest == 0)
        def _():
            stick_started(jnp.where(first_key, highest, b))
        return lowest, highest

    def early_delta(n, carry):
        @pl.when(n == 1)
        def _():
            relay(stick_kinds[0])

        @pl.when(n == sp - 2)
        def _():
            for c in early[parts:-1]:
                arrive(*c)
            for i in stick_kinds[1:]:
                relay(i)
            arrive(*early[-1])
        delta_event(n)
        return carry

    lax.fori_loop(0, sp - 1, early_delta, 0)
    relayed(stick_kinds)

    def walk(n, memory):
        high, low = halves(memory)
        new = folded(dot_f32(maps[n], wide_rhs(high, low, 1))) + adds[n]
        made = new[width:]
        made = made * lax.rsqrt(jnp.mean(made * made, axis=-1, keepdims=True) + NORM_EPS)
        at = pl.ds(pl.multiple_of(n * span, span), span)
        delta_out[at, :] = (made * gain_ref[...]).astype(delta_out.dtype)
        return new[:width]

    lax.fori_loop(0, sp - 1, stick_event, (z, z))

    delta_event(sp - 1)
    _, _, down, b = place(sp - 1)
    stick_project(b)
    acc[at_block(b), :] = jnp.zeros((rows, cols), jnp.float32)
    later[at_block(b), :] = jnp.zeros((rows, cols), jnp.float32)

    def last_pairs(m, memory):
        i = jnp.where(down, m, b)
        j = jnp.where(down, b, b - m)
        pair(i, j, True, False)
        for n in range(blocks):
            memory = walk(m * blocks + n, memory)
        delta_started(m - 1)

        @pl.when(down)
        def _():
            stick_started(m - 1)
            settle(i)
        return memory

    lax.fori_loop(0, sp, last_pairs, jnp.zeros((width, width), jnp.float32))
    delta_started(sp - 1)

    @pl.when(down)
    def _():
        stick_started(sp - 1)

    @pl.when(jnp.logical_not(down))
    def _():
        settle(b)
        stick_started(b)

    mine_z = pl.ds(pl.multiple_of(z * rows, rows), rows)
    lanes = pl.ds(pl.multiple_of(z * cols, cols), cols)
    sticks[:, lanes] = stick_out[mine_z, :]
    deltas[:, lanes] = delta_out[mine_z, :]
    for c in late:
        c.wait()
    stick_came()
    chunks, wide = outgoing.shape[0], outgoing.shape[2]
    share = rows // tp
    for c in range(chunks):
        columns = slice(c * wide, (c + 1) * wide)
        partial[:, columns] = dot_f32(sticks[...], sw_ref[:, columns])
    delta_came()
    mine = pl.ds(pl.multiple_of(t * share, share), share)
    partner = lax.rem(t + 1, tp)
    theirs = pl.ds(pl.multiple_of(partner * share, share), share)

    def finish(which, c):
        columns = slice(c * wide, (c + 1) * wide)
        return (
            partial[which, columns] + dot_f32(deltas[which, :], dw_ref[:, columns])
        ).astype(jnp.bfloat16)

    swaps = [
        remote(
            outgoing.at[c], incoming.at[:, c * wide : (c + 1) * wide],
            c_send.at[c], c_recv.at[c], "tp", partner,
        )
        for c in range(chunks)
    ]
    for c in range(chunks):
        outgoing[c] = finish(theirs, c)
        if c > 0:
            swaps[c - 1].start()
    for c in range(chunks):
        own[:, c * wide : (c + 1) * wide] = finish(mine, c)
        if c == 0:
            swaps[chunks - 1].start()
    for c in range(chunks):
        swaps[c].wait_recv()

    for c in swaps:
        c.wait_send()
    for i in range(count):
        for side in range(2):
            w_copy(side, i).wait_send()
            w_relay(side, i).wait_send()
    for part in range(parts):
        forward(0, 0, part).wait_send()
        for step in range(1, sp):
            for way in range(2):
                @pl.when(sends(way, step))
                def _():
                    x_copy(way, step, part).wait_send()
                    if part == 0:
                        shift_copy(way, step).wait_send()

                @pl.when(comes(way, step))
                def _():
                    forward(way, step, part).wait_send()
    stick_finished()
    delta_finished()


ANYWHERE = pl.BlockSpec(memory_space=pltpu.HBM)
ON_CORE = pl.BlockSpec(memory_space=pltpu.VMEM)


def on_device_heads(
    hidden_in, sb_query_w, sb_key_w, sb_value_w, sb_offset,
    delta_query_w, delta_key_w, delta_value_w, decay_w, write_w, write_bias,
    decay_log_scale, decay_shift, head_gain, sb_out_w, delta_out_w,
):
    sp, fs, tp = lax.axis_size("sp"), lax.axis_size("fs"), lax.axis_size("tp")
    rows, half = hidden_in.shape[1:]
    width = half * tp
    length = rows * sp
    heads = decay_log_scale.shape[0]
    cols = sb_query_w.shape[1] // sp
    parts, chunks = 2, 4
    share = rows // tp
    blocks = length // BLOCK
    dma = pltpu.SemaphoreType.DMA
    bf16, f32 = jnp.bfloat16, jnp.float32
    own, incoming = pl.pallas_call(
        layer_kernel,
        name="layer",
        out_shape=(pltpu.VMEM((share, width), bf16),) * 2,
        in_specs=[ANYWHERE] * 16,
        out_specs=(ON_CORE,) * 2,
        scratch_shapes=[
            pltpu.SMEM(sb_offset.shape, f32),
            pltpu.SMEM(decay_log_scale.shape, f32),
            pltpu.SMEM(write_bias.shape, f32),
            pltpu.VMEM((1, head_gain.shape[0]), f32),
            pltpu.VMEM((sp, rows, width), bf16),
            pltpu.VMEM((width, 6 * cols), bf16),
            pltpu.VMEM((2, heads, width), bf16),
            pltpu.VMEM((2 * heads, width), bf16),
            pltpu.VMEM((2 * heads, rows), f32),
            pltpu.VMEM((sp, heads, rows), f32),
            pltpu.VMEM((3, length, cols), bf16),
            pltpu.VMEM((length, cols), f32),
            pltpu.VMEM((length, cols), f32),
            pltpu.VMEM((blocks, cols + BLOCK, 2 * cols), bf16),
            pltpu.VMEM((blocks, cols + BLOCK, cols), f32),
            pltpu.VMEM((length, cols), bf16),
            pltpu.VMEM((length, cols), bf16),
            pltpu.VMEM((rows, cols * sp), bf16),
            pltpu.VMEM((rows, cols * sp), bf16),
            pltpu.VMEM(sb_out_w.shape, bf16),
            pltpu.VMEM(delta_out_w.shape, bf16),
            pltpu.VMEM((rows, width), f32),
            pltpu.VMEM((chunks, share, width // chunks), bf16),
            dma((2, sp, parts)), dma((2, sp, parts)), dma((2, sp, parts)), dma((2, sp, parts)),
            dma((fs, 6)), dma((fs, 6)), dma((2, sp)), dma((2, sp)), dma((10,)), dma((6,)),
            dma((sp, 2)), dma((sp, 2)), dma((chunks,)), dma((chunks,)),
        ],
        compiler_params=pltpu.CompilerParams(
            collective_id=0, has_side_effects=True,
            vmem_limit_bytes=ALL_VMEM - 5 * share * width,
        ),
    )(
        sb_offset, decay_log_scale, write_bias,
        hidden_in.reshape(rows, half), sb_query_w, sb_key_w, sb_value_w,
        delta_query_w, delta_key_w, delta_value_w, decay_w.T, write_w.T,
        decay_shift.reshape(heads, rows), head_gain.reshape(1, -1), sb_out_w, delta_out_w,
    )
    result = (own.astype(f32) + incoming.astype(f32)).astype(bf16)
    return result.reshape(1, share, width)


def on_device(*inputs):
    delta_heads = inputs[11].shape[0]
    square = lax.axis_size("fs") == 4 and lax.axis_size("tp") == 2
    if square and delta_heads == lax.axis_size("sp") and inputs[4].shape[0] % delta_heads == 0:
        return on_device_heads(*inputs)
    return on_device_split(*inputs)


def solution(mesh):
    return jax.shard_map(
        on_device,
        mesh=mesh,
        in_specs=(
            P("fs", "sp", "tp"),
            P("fs", "tp"),
            P("fs", "tp"),
            P("fs", "tp"),
            P("tp"),
            P("fs", "tp"),
            P("fs", "tp"),
            P("fs", "tp"),
            P(None, "tp"),
            P(None, "tp"),
            P("tp"),
            P("tp"),
            P("fs", "tp", "sp"),
            P(),
            P("tp", None),
            P("tp", None),
        ),
        out_specs=P("fs", ("sp", "tp"), None),
        check_vma=False,
    )
```

```python
import jax
import jax.numpy as jnp
from jax import lax
from jax.experimental import pallas as pl
from jax.experimental.pallas import tpu as pltpu
from jax.sharding import PartitionSpec as P

MESH = pl.DeviceIdType.MESH
ALL_VMEM = 67043328

SB_DIM = 64
GDN_DIM = 128
BLOCK = 64


EXACT_MATMUL = lax.Precision.HIGHEST
NORM_EPS = 1e-06


def carried_in(value, axis, combine, identity):
    devices, index = (lax.axis_size(axis), lax.axis_index(axis))
    everything = jax.tree.map(
        lambda part, kind: lax.all_gather(part.astype(kind), axis),
        value,
        (jnp.bfloat16, jnp.bfloat16),
    )
    start = jax.tree.map(
        lambda part, zero: jnp.broadcast_to(jnp.asarray(zero, part.dtype), part.shape),
        value,
        identity,
    )

    def lap(k, before):
        reached = k < index
        new = combine(
            before, jax.tree.map(lambda part, own: part[k].astype(own.dtype), everything, value)
        )
        return jax.tree.map(lambda a, b: jnp.where(reached, a, b), new, before)

    return lax.fori_loop(0, devices, lap, start)


def unit_lower_inverse(strict_part):
    order_size = strict_part.shape[-1]
    powered = strict_part
    inverse = jnp.eye(order_size, dtype=strict_part.dtype) - strict_part
    for repeat_number in range(max(1, (order_size - 1).bit_length()) - 1):
        powered = jnp.einsum("...ij,...jk->...ik", powered, powered, precision=EXACT_MATMUL)
        inverse = inverse + jnp.einsum(
            "...ij,...jk->...ik", inverse, powered, precision=EXACT_MATMUL
        )
    return inverse


def to_blocks(row_data, block_span):
    blocks_count = row_data.shape[0] // block_span
    shaped = row_data.reshape((blocks_count, block_span) + row_data.shape[1:])
    return jnp.swapaxes(shaped, 1, 2)


def from_blocks(blocked):
    swapped = jnp.swapaxes(blocked, 1, 2)
    return swapped.reshape((-1,) + swapped.shape[2:])


def unit_rows(vectors):
    return vectors * lax.rsqrt(jnp.sum(vectors * vectors, axis=-1, keepdims=True) + NORM_EPS)


def delta_inputs(
    query_proj,
    key_proj,
    value_proj,
    decay_pre,
    write_pre,
    write_bias,
    decay_log_scale,
    shift_rows,
    head_count,
    head_size,
):
    query_act = jax.nn.silu(query_proj.astype(jnp.float32)).reshape(-1, head_count, head_size)
    key_act = jax.nn.silu(key_proj.astype(jnp.float32)).reshape(-1, head_count, head_size)
    value_rows = jax.nn.silu(value_proj.astype(jnp.float32)).reshape(-1, head_count, head_size)
    queries = unit_rows(query_act) * head_size ** (-0.5)
    key_rows = unit_rows(key_act)
    log_decay = -jnp.exp(decay_log_scale) * jax.nn.softplus(decay_pre) + shift_rows
    strength = jax.nn.sigmoid(write_pre + write_bias)
    return (queries, key_rows, value_rows, log_decay, strength)


def delta_prepare(queries, key_rows, value_rows, log_decay, strength):
    block_span = queries.shape[2]
    cumulative = jnp.cumsum(log_decay, axis=-1)
    row_place = lax.broadcasted_iota(jnp.int32, (block_span, block_span), 0)
    col_place = lax.broadcasted_iota(jnp.int32, (block_span, block_span), 1)
    inclusive = col_place <= row_place
    strictly = col_place < row_place
    spread = cumulative[..., :, None] - cumulative[..., None, :]
    decay_table = jnp.where(inclusive, jnp.exp(jnp.where(inclusive, spread, 0.0)), 0.0)
    keys_beta = key_rows * strength[..., None]
    lower_part = jnp.where(
        strictly,
        jnp.einsum("nhik,nhjk->nhij", keys_beta, key_rows, precision=EXACT_MATMUL) * decay_table,
        0.0,
    )
    inverse = unit_lower_inverse(lower_part)
    growth = jnp.exp(cumulative)
    state_updates = jnp.einsum(
        "nhij,nhjv->nhiv", inverse, value_rows * strength[..., None], precision=EXACT_MATMUL
    )
    erase_term = jnp.einsum(
        "nhij,nhjk->nhik", inverse, keys_beta * growth[..., None], precision=EXACT_MATMUL
    )
    inside_block = (
        jnp.einsum("nhik,nhjk->nhij", queries, key_rows, precision=EXACT_MATMUL) * decay_table
    )
    boosted_query = queries * growth[..., None]
    damped_keys = key_rows * jnp.exp(cumulative[..., -1:] - cumulative)[..., None]
    decay_per_block = jnp.exp(cumulative[..., -1])
    return (state_updates, erase_term, inside_block, boosted_query, damped_keys, decay_per_block)


def delta_step(memory_state, inputs):
    state_updates, erase_term, inside_block, boosted_query, damped_keys, decay_per_block = inputs
    fixed_values = state_updates - jnp.einsum(
        "mzq,mqc->mzc", erase_term, memory_state, precision=EXACT_MATMUL
    )
    produced_rows = jnp.einsum(
        "mzq,mqc->mzc", boosted_query, memory_state, precision=EXACT_MATMUL
    ) + jnp.einsum("efq,eqn->efn", inside_block, fixed_values, precision=EXACT_MATMUL)
    memory_state = memory_state * decay_per_block[:, None, None] + jnp.einsum(
        "wam,waz->wmz", damped_keys, fixed_values, precision=EXACT_MATMUL
    )
    return (memory_state, produced_rows)


def transition_step(carried, inputs):
    memory_state, transfer = carried
    state_updates, erase_term, inside_block, boosted_query, damped_keys, decay_per_block = inputs
    fixed_values = state_updates - jnp.einsum(
        "mzq,mqc->mzc", erase_term, memory_state, precision=EXACT_MATMUL
    )
    coupling = jnp.einsum("hik,hil->hkl", damped_keys, erase_term, precision=EXACT_MATMUL)
    memory_state = memory_state * decay_per_block[:, None, None] + jnp.einsum(
        "wam,waz->wmz", damped_keys, fixed_values, precision=EXACT_MATMUL
    )
    transfer = transfer * decay_per_block[:, None, None] - jnp.einsum(
        "hkl,hlm->hkm", coupling, transfer, precision=EXACT_MATMUL
    )
    return ((memory_state, transfer), None)


def compose(prior_blocks, following_blocks):
    joined_map = jnp.einsum(
        "hkl,hlm->hkm", following_blocks[0], prior_blocks[0], precision=EXACT_MATMUL
    )
    joined_state = (
        jnp.einsum("djo,dog->djg", following_blocks[0], prior_blocks[1], precision=EXACT_MATMUL)
        + following_blocks[1]
    )
    return (joined_map, joined_state)


def stick_block(queries, key_rows, value_rows, query_place, key_place, offsets):
    scale_factor = queries.shape[-1] ** (-0.5)
    scores = (
        jnp.einsum("qhd,khd->hqk", queries, key_rows, preferred_element_type=jnp.float32)
        * scale_factor
        + offsets[:, None, None]
    )
    visible = key_place[None, :] < query_place[:, None]
    skipped = jnp.where(visible, jax.nn.log_sigmoid(-scores), 0.0)
    beyond = lax.cumsum(skipped, axis=2, reverse=True) - skipped
    weights = jnp.where(visible, jnp.exp(jax.nn.log_sigmoid(scores) + beyond), 0.0).astype(
        jnp.bfloat16
    )
    partial_value = jnp.einsum(
        "hqk,khd->qhd", weights, value_rows, preferred_element_type=jnp.float32
    )
    return (partial_value, jnp.sum(skipped, axis=2).T)


def stick_combine(partials, totals):
    beyond = jnp.cumsum(totals[::-1], axis=0)[::-1] - totals
    return jnp.sum(partials * jnp.exp(beyond)[..., None], axis=0)


def on_device_split(
    hidden_in,
    sb_query_w,
    sb_key_w,
    sb_value_w,
    sb_offset,
    delta_query_w,
    delta_key_w,
    delta_value_w,
    decay_w,
    write_w,
    write_bias,
    decay_log_scale,
    decay_shift,
    head_gain,
    sb_out_w,
    delta_out_w,
):
    token_rows = hidden_in.shape[1]
    local_in = hidden_in.reshape(token_rows, hidden_in.shape[2])
    gathered = (
        lax.all_gather(sb_query_w, "fs", axis=0, tiled=True),
        lax.all_gather(sb_key_w, "fs", axis=0, tiled=True),
        lax.all_gather(sb_value_w, "fs", axis=0, tiled=True),
        lax.all_gather(delta_query_w, "fs", axis=0, tiled=True),
        lax.all_gather(delta_key_w, "fs", axis=0, tiled=True),
        lax.all_gather(delta_value_w, "fs", axis=0, tiled=True),
    )
    in_weights = tuple(gathered) + (decay_w, write_w)
    portion = lax.all_gather(local_in, "tp", axis=1, tiled=True)
    projected = tuple(
        (jnp.dot(portion, weight, preferred_element_type=jnp.float32) for weight in in_weights)
    )
    sb_heads = sb_offset.shape[0]
    delta_heads = decay_log_scale.shape[0]
    sb_query = projected[0].astype(jnp.bfloat16).reshape(token_rows, sb_heads, SB_DIM)
    sb_keys = projected[1].astype(jnp.bfloat16)
    sb_values = projected[2].astype(jnp.bfloat16)
    shift_rows = decay_shift.reshape(delta_heads, token_rows).T
    queries, key_rows, value_rows, log_decay, strength = delta_inputs(
        projected[3].astype(jnp.bfloat16),
        projected[4].astype(jnp.bfloat16),
        projected[5].astype(jnp.bfloat16),
        projected[6],
        projected[7],
        write_bias,
        decay_log_scale,
        shift_rows,
        delta_heads,
        GDN_DIM,
    )
    prepared = delta_prepare(
        to_blocks(queries, BLOCK),
        to_blocks(key_rows, BLOCK),
        to_blocks(value_rows, BLOCK),
        to_blocks(log_decay, BLOCK),
        to_blocks(strength, BLOCK),
    )
    identity_map = jnp.broadcast_to(
        jnp.eye(GDN_DIM, dtype=jnp.float32), (delta_heads, GDN_DIM, GDN_DIM)
    )
    empty_state = jnp.zeros((delta_heads, GDN_DIM, GDN_DIM), jnp.float32)
    (local_end, local_map), unused_out = lax.scan(
        transition_step, (empty_state, identity_map), prepared
    )
    own_first = lax.axis_index("sp") * token_rows
    query_place = own_first + lax.iota(jnp.int32, token_rows)
    sp_count = lax.axis_size("sp")
    slot_out = jnp.zeros((sp_count, token_rows, sb_heads, SB_DIM), jnp.float32)
    slot_total = jnp.zeros((sp_count, token_rows, sb_heads), jnp.float32)

    def absorb(slot_arrays, address_portion, value_part, shard_first):

        def active(current):
            partial_value, totals = stick_block(
                sb_query,
                address_portion.reshape(token_rows, sb_heads, SB_DIM),
                value_part.reshape(token_rows, sb_heads, SB_DIM),
                query_place,
                shard_first + lax.iota(jnp.int32, token_rows),
                sb_offset,
            )
            slot_index = shard_first // token_rows
            return (
                lax.dynamic_update_index_in_dim(current[0], partial_value, slot_index, 0),
                lax.dynamic_update_index_in_dim(current[1], totals, slot_index, 0),
            )

        def inactive(current):
            return current

        usable = jnp.logical_and(shard_first >= 0, shard_first <= own_first)
        return lax.cond(usable, active, inactive, slot_arrays)

    key_block = lax.all_gather(sb_keys, "sp", axis=0, tiled=True)
    value_block = lax.all_gather(sb_values, "sp", axis=0, tiled=True)

    def per_shard(shard_number, current):
        row_begin = shard_number * token_rows
        return absorb(
            current,
            lax.dynamic_slice_in_dim(key_block, row_begin, token_rows, 0),
            lax.dynamic_slice_in_dim(value_block, row_begin, token_rows, 0),
            row_begin,
        )

    slot_arrays = lax.fori_loop(
        0, key_block.shape[0] // token_rows, per_shard, (slot_out, slot_total)
    )
    unused_map, incoming = carried_in(
        (local_map, local_end), "sp", compose, (identity_map, empty_state)
    )
    sb_mixed = (
        stick_combine(slot_arrays[0], slot_arrays[1])
        .astype(jnp.bfloat16)
        .reshape(token_rows, sb_heads * SB_DIM)
    )
    unused_end, produced_rows = lax.scan(delta_step, incoming, prepared)
    produced_rows = from_blocks(produced_rows)
    normed = (
        produced_rows
        * lax.rsqrt(jnp.mean(produced_rows * produced_rows, axis=-1, keepdims=True) + NORM_EPS)
        * head_gain
    )
    delta_mixed = normed.astype(jnp.bfloat16).reshape(token_rows, delta_heads * GDN_DIM)
    result = lax.psum_scatter(
        (
            jnp.dot(sb_mixed, sb_out_w, preferred_element_type=jnp.float32)
            + jnp.dot(delta_mixed, delta_out_w, preferred_element_type=jnp.float32)
        ).astype(jnp.bfloat16),
        "tp",
        scatter_dimension=0,
        tiled=True,
    ).astype(jnp.float32)
    return result.astype(jnp.bfloat16).reshape(1, result.shape[0], result.shape[1])


def remote(src, dst, send, recv, axis, index):
    return pltpu.make_async_remote_copy(
        src_ref=src, dst_ref=dst, send_sem=send, recv_sem=recv,
        device_id={axis: index}, device_id_type=MESH,
    )


def greet(axes):
    barrier = pltpu.get_barrier_semaphore()
    count = 0
    for axis in axes:
        size, me = lax.axis_size(axis), lax.axis_index(axis)
        for k in range(1, size):
            pl.semaphore_signal(
                barrier, inc=1, device_id={axis: lax.rem(me + k, size)}, device_id_type=MESH
            )
            count += 1
    pl.semaphore_wait(barrier, count)


def halves(a):
    high = a.astype(jnp.bfloat16)
    return high, (a - high.astype(jnp.float32)).astype(jnp.bfloat16)


def dot_f32(a, b, dims=((1,), (0,))):
    return lax.dot_general(a, b, (dims, ((), ())), preferred_element_type=jnp.float32)


def wide_rhs(high, low, axis):
    top = jnp.concatenate([high, low], axis=axis)
    bottom = jnp.concatenate([high, jnp.zeros_like(low)], axis=axis)
    return jnp.concatenate([top, bottom], axis=1 - axis)


def folded(a):
    half = a.shape[1] // 2
    return a[:, :half] + a[:, half:]


def layer_kernel(
    offset_hbm, decay_scale_hbm, write_bias_hbm,
    x_ref, w0, w1, w2, w3, w4, w5, decay_w_ref, write_w_ref, shift_ref, gain_hbm, sw_hbm, dw_hbm,
    own, incoming,
    offset_ref, decay_scale_ref, write_bias_ref, gain_ref,
    xs, ws, gate_w, gate_all, gates, shifts_ref, after,
    proj, acc, later, maps, adds, stick_out, delta_out,
    sticks, deltas, sw_ref, dw_ref, partial, outgoing,
    x_send, x_recv, f_send, f_recv, w_send, w_recv, s_send, s_recv, l_sem, lw_sem,
    a_send, a_recv, c_send, c_recv,
):
    weights = (w0, w1, w2, w3, w4, w5)
    sp, tp = lax.axis_size("sp"), lax.axis_size("tp")
    z, f, t = lax.axis_index("sp"), lax.axis_index("fs"), lax.axis_index("tp")
    rows, half = x_ref.shape
    depth = w0.shape[0]
    cols = ws.shape[1] // len(weights)
    parts = x_send.shape[2]
    heads = decay_w_ref.shape[0]
    slot = pl.ds(pl.multiple_of(t * half, half), half)
    local = [
        pltpu.make_async_copy(x_ref, xs.at[z, :, slot], l_sem.at[0]),
        pltpu.make_async_copy(shift_ref, shifts_ref.at[z], l_sem.at[1]),
        pltpu.make_async_copy(decay_w_ref, gate_w.at[0], l_sem.at[2]),
        pltpu.make_async_copy(write_w_ref, gate_w.at[1], l_sem.at[3]),
        pltpu.make_async_copy(offset_hbm, offset_ref, l_sem.at[6]),
        pltpu.make_async_copy(decay_scale_hbm, decay_scale_ref, l_sem.at[7]),
        pltpu.make_async_copy(write_bias_hbm, write_bias_ref, l_sem.at[8]),
        pltpu.make_async_copy(gain_hbm, gain_ref, l_sem.at[9]),
    ]
    late = [
        pltpu.make_async_copy(sw_hbm, sw_ref, l_sem.at[4]),
        pltpu.make_async_copy(dw_hbm, dw_ref, l_sem.at[5]),
    ]

    def w_src(i):
        return weights[i].at[:, pl.ds(pl.multiple_of(z * cols, cols), cols)]

    def w_at(i, who):
        return ws.at[pl.ds(pl.multiple_of(who * depth, depth), depth), pl.ds(i * cols, cols)]

    local += [
        pltpu.make_async_copy(w_src(i), w_at(i, f), lw_sem.at[i]) for i in range(len(weights))
    ]
    near = (f + 1 - 2 * (f % 2), f + 2 - 4 * (f // 2))
    count = len(weights)
    delta_kinds, stick_kinds = (3, 4, 5), (0, 1, 2)

    def onward(way):
        return z + 1 < sp if way == 0 else z > 0

    def ahead(way):
        return z + 1 if way == 0 else z - 1

    barrier = pltpu.get_barrier_semaphore()
    for way in range(2):
        @pl.when(onward(way))
        def _():
            pl.semaphore_signal(
                barrier, inc=1, device_id={"sp": ahead(way)}, device_id_type=MESH
            )
    for side in range(2):
        pl.semaphore_signal(barrier, inc=1, device_id={"fs": near[side]}, device_id_type=MESH)
    pl.semaphore_signal(
        barrier, inc=1, device_id={"tp": lax.rem(t + 1, tp)}, device_id_type=MESH
    )
    for c in local:
        c.start()
    peers = onward(0).astype(jnp.int32) + onward(1).astype(jnp.int32) + 3
    pl.semaphore_wait(barrier, peers)

    def x_copy(way, step, part):
        block = z - (step - 1) if way == 0 else z + (step - 1)
        piece = pl.ds(part * (rows // parts), rows // parts)
        there = xs.at[block, piece, slot]
        return remote(
            x_ref.at[piece, :] if step == 1 else there, there,
            x_send.at[way, step, part], x_recv.at[way, step, part], "sp", ahead(way),
        )

    def shift_copy(way, step):
        block = z - (step - 1) if way == 0 else z + (step - 1)
        there = shifts_ref.at[block]
        return remote(
            shift_ref if step == 1 else there, there,
            s_send.at[way, step], s_recv.at[way, step], "sp", ahead(way),
        )

    def comes(way, step):
        return z >= step if way == 0 else z + step < sp

    def sends(way, step):
        return jnp.logical_and(onward(way), comes(way, step - 1))

    def forward(way, step, part):
        block = z - step if way == 0 else z + step
        piece = pl.ds(part * (rows // parts), rows // parts)
        there = xs.at[block, piece, slot]
        return remote(
            x_ref.at[piece, :] if step == 0 else there, there,
            f_send.at[way, step, part], f_recv.at[way, step, part], "tp", lax.rem(t + 1, tp),
        )

    def w_copy(side, i):
        return remote(
            w_src(i), w_at(i, f), w_send.at[side, i], w_recv.at[side, i], "fs", near[side]
        )

    def w_relay(side, i):
        part = depth // 2
        start = pl.multiple_of(near[side] * depth + side * part, part)
        there = ws.at[pl.ds(start, part), pl.ds(i * cols, cols)]
        return remote(
            there, there, w_send.at[2 + side, i], w_recv.at[2 + side, i], "fs", near[1 - side]
        )

    for part in range(parts):
        for way in range(2):
            @pl.when(onward(way))
            def _():
                x_copy(way, 1, part).start()
                if part == 0:
                    shift_copy(way, 1).start()
    for i in delta_kinds:
        for side in range(2):
            w_copy(side, i).start()
    for part in range(parts):
        forward(0, 0, part).start()

    def relay(i):
        for side in range(2):
            w_copy(side, i).wait_recv()
            w_relay(side, i).start()

    def arrive(step, part):
        for way in range(2):
            @pl.when(comes(way, step))
            def _():
                x_copy(way, step, part).wait_recv()
                forward(way, step, part).start()
                if step + 1 < sp:
                    @pl.when(onward(way))
                    def _():
                        x_copy(way, step + 1, part).start()
                if part == 0:
                    shift_copy(way, step).wait_recv()
                    if step + 1 < sp:
                        @pl.when(onward(way))
                        def _():
                            shift_copy(way, step + 1).start()

    early = [(step, part) for step in range(1, sp - 1) for part in range(parts)]
    relay(delta_kinds[0])
    arrive(*early[0])
    for i in delta_kinds[1:]:
        relay(i)
    for i in stick_kinds:
        for side in range(2):
            w_copy(side, i).start()
    for c in late:
        c.start()
    for step, part in early[1:parts]:
        arrive(step, part)
    for c in local:
        c.wait()
    gate_all[...] = jnp.concatenate(
        [gate_w[0].astype(jnp.float32), gate_w[1].astype(jnp.float32)], axis=0
    ).astype(jnp.bfloat16)
    for part in range(parts):
        forward(0, 0, part).wait_recv()

    def relayed(kinds):
        for i in kinds:
            for side in range(2):
                w_relay(side, i).wait_recv()

    relayed(delta_kinds)

    size = offset_ref.shape[0] // sp
    sb_size = cols // size
    scale = sb_size ** (-0.5)
    tile = rows // 2
    below = lax.broadcasted_iota(jnp.int32, (rows, rows), 0)
    across = lax.broadcasted_iota(jnp.int32, (rows, rows), 1)
    after[:, :rows] = jnp.where(below > across, 1.0, 0.0).astype(jnp.bfloat16)
    after[:, rows:] = jnp.ones((rows, cols), jnp.bfloat16)

    def at_block(b, start=0, extent=rows):
        return pl.ds(pl.multiple_of(b * rows + start, extent), extent)

    def pair(i, j, masked, fresh):
        for part in range(rows // tile):
            span = (part + 1) * tile if fresh else rows
            mine = at_block(i, part * tile, tile)
            q = proj[0, mine, :]
            keys, values = proj[1, at_block(j), :], proj[2, at_block(j), :]
            keys, values = keys[:span], values[:span]
            lane = lax.broadcasted_iota(jnp.int32, (tile, cols), 1)
            query = jnp.concatenate(
                [jnp.where(lane // sb_size == h, q, jnp.zeros_like(q)) for h in range(size)], axis=0
            )
            score = dot_f32(query, keys, ((1,), (1,)))
            score = jnp.concatenate(
                [
                    score[h * tile : (h + 1) * tile] * scale + offset_ref[z * size + h]
                    for h in range(size)
                ],
                axis=0,
            )
            skip = jnp.maximum(score, jnp.log(1.0 + jnp.exp(jnp.minimum(score, 80.0))))
            weight = score - skip
            if masked:
                seen = across[:tile, :span] < below[:tile, :span] + part * tile + (i - j) * rows
                seen = jnp.concatenate([seen] * size, axis=0)
                skip = jnp.where(seen, skip, 0.0)
            suffix = after[:span, :]
            if span < rows:
                suffix = jnp.concatenate([suffix[:, :span], suffix[:, rows:]], axis=1)
            sums = dot_f32(skip.astype(jnp.bfloat16), suffix)
            weight = jnp.exp(weight - sums[:, :span])
            if masked:
                weight = jnp.where(seen, weight, 0.0)
            out = dot_f32(weight.astype(jnp.bfloat16), values)
            mixed, total = out[:tile], sums[:tile, span:]
            for h in range(1, size):
                at = slice(h * tile, (h + 1) * tile)
                mixed = jnp.where(lane // sb_size == h, out[at], mixed)
                total = jnp.where(lane // sb_size == h, sums[at, span:], total)
            if fresh:
                acc[mine, :] = mixed
                later[mine, :] = total
            else:
                passed = later[mine, :]
                acc[mine, :] = acc[mine, :] + mixed * jnp.exp(-passed)
                later[mine, :] = passed + total

    span = BLOCK
    duo = 2 * span
    blocks = rows // span
    width = GDN_DIM
    seg_row = lax.broadcasted_iota(jnp.int32, (rows, rows), 0)
    seg_col = lax.broadcasted_iota(jnp.int32, (rows, rows), 1)
    together = seg_row // span == seg_col // span
    upto = jnp.where(jnp.logical_and(together, seg_row <= seg_col), 1.0, 0.0).astype(jnp.bfloat16)
    beyond_it = jnp.where(jnp.logical_and(together, seg_row > seg_col), 1.0, 0.0).astype(
        jnp.bfloat16
    )
    prow = lax.broadcasted_iota(jnp.int32, (span, duo), 0)
    plane = lax.broadcasted_iota(jnp.int32, (span, duo), 1)
    first = plane < span
    pcol = jnp.where(first, plane, plane - span)
    inclusive, strictly = pcol <= prow, pcol < prow
    unit = jnp.where(pcol == prow, 1.0, 0.0)
    diagonal = lax.broadcasted_iota(jnp.int32, (width, width), 0) == lax.broadcasted_iota(
        jnp.int32, (width, width), 1
    )
    eighth = lax.broadcasted_iota(jnp.int32, (8, rows), 0)

    def silu(a):
        return a * (1.0 / (1.0 + jnp.exp(-a)))

    def unit_of(a):
        return a * lax.rsqrt(jnp.sum(a * a, axis=-1, keepdims=True) + NORM_EPS)

    def apart(a):
        lanes = lax.broadcasted_iota(jnp.int32, a.shape, 1) < span
        zero = jnp.zeros_like(a)
        return jnp.concatenate([jnp.where(lanes, a, zero), jnp.where(lanes, zero, a)], axis=0)

    def squared(left, power):
        high, low = halves(power)
        lhigh, llow = halves(left)
        return folded(
            dot_f32(
                jnp.concatenate([lhigh, llow], axis=1), wide_rhs(apart(high), apart(low), 1)
            )
        )

    def prepare(b, dq, dk, dv):
        gates[...] = dot_f32(gate_all[...], xs[b], ((1,), (1,)))
        pre = gates[pl.ds(z, 1), :]
        write = gates[pl.ds(heads + z, 1), :] + write_bias_ref[z]
        rate = jnp.exp(jnp.full((1, rows), decay_scale_ref[z], jnp.float32))
        soft = jnp.maximum(pre, 0.0) + jnp.log(1.0 + jnp.exp(-jnp.abs(pre)))
        decay = shifts_ref[b, pl.ds(z, 1), :] - rate * soft
        strength = 1.0 / (1.0 + jnp.exp(-write))
        d1 = decay.astype(jnp.bfloat16).astype(jnp.float32)
        d2 = (decay - d1).astype(jnp.bfloat16).astype(jnp.float32)
        d3 = decay - d1 - d2
        three = jnp.where(
            eighth == 0, d1, jnp.where(eighth == 1, d2, jnp.where(eighth == 2, d3, 0.0))
        ).astype(jnp.bfloat16)
        cum_row = jnp.sum(dot_f32(three, upto), axis=0, keepdims=True)
        rest_row = jnp.sum(dot_f32(three, beyond_it), axis=0, keepdims=True)
        stack = jnp.where(
            eighth == 0, strength,
            jnp.where(
                eighth == 1, jnp.exp(cum_row),
                jnp.where(eighth == 2, jnp.exp(rest_row), cum_row),
            ),
        )
        columns = stack.T
        s_col, grow, damp, cum = (columns[:, n : n + 1] for n in range(4))
        q = unit_of(silu(dq)) * width ** (-0.5)
        k = unit_of(silu(dk))
        v = silu(dv)
        boosted = q * grow
        damped = k * damp
        right = jnp.concatenate([v * s_col, k * (s_col * grow)], axis=1)
        kh, kl = halves(k)
        qh, ql = halves(q)
        work = []
        for duo_at in range(rows // duo):
            lo = duo_at * duo
            here = slice(lo, lo + duo)
            left = jnp.concatenate(
                [
                    jnp.concatenate([kh[here], kl[here]], axis=1),
                    jnp.concatenate([qh[here], ql[here]], axis=1),
                ],
                axis=0,
            )
            gram = folded(
                dot_f32(left, wide_rhs(kh[here], kl[here], 0), ((1,), (1,)))
            )
            spread = (
                jnp.where(first, cum[lo : lo + span], cum[lo + span : lo + duo])
                - cum_row[:, here]
            )
            table = jnp.where(inclusive, jnp.exp(jnp.where(inclusive, spread, 0.0)), 0.0)
            scale_col = jnp.where(first, s_col[lo : lo + span], s_col[lo + span : lo + duo])
            near_k = jnp.where(first, gram[:span], gram[span:duo])
            near_q = jnp.where(first, gram[duo : duo + span], gram[duo + span :])
            strict = jnp.where(strictly, near_k * table * scale_col, 0.0)
            work.append([unit - strict, strict, near_q * table])
        for w in work:
            w[1] = squared(w[1], w[1])
        levels = max(1, (span - 1).bit_length()) - 1
        for level in range(levels):
            for w in work:
                if level + 1 < levels:
                    both = squared(jnp.concatenate([w[1], w[0]], axis=0), w[1])
                    w[1], w[0] = both[:span], w[0] + both[span:]
                else:
                    w[0] = w[0] + squared(w[0], w[1])
        for duo_at, (inverse, _, inside) in enumerate(work):
            lo = duo_at * duo
            here = slice(lo, lo + duo)
            ih, il = (apart(a) for a in halves(inverse))
            rh, rl = halves(right[here])
            solved = dot_f32(
                jnp.concatenate([ih, il], axis=1), jnp.concatenate([rh, rh], axis=0)
            ) + dot_f32(ih, rl)
            lh, ll = (
                apart(a) for a in halves(jnp.concatenate([damped[here].T, inside], axis=0))
            )
            sh, sl = halves(solved)
            made = dot_f32(
                jnp.concatenate([lh, ll], axis=1), jnp.concatenate([sh, sh], axis=0)
            ) + dot_f32(lh, sl)
            for side in range(2):
                at = lo + side * span
                mine = made[side * (width + span) : (side + 1) * (width + span)]
                n = b * blocks + 2 * duo_at + side
                keep = grow[at + span - 1 : at + span]
                step_map = jnp.where(diagonal, keep, 0.0) - mine[:width, width:]
                query = boosted[at : at + span] - mine[width:, width:]
                high, low = halves(jnp.concatenate([step_map, query], axis=0))
                maps[n, :, :width] = high
                maps[n, :, width:] = low
                adds[n] = mine[:, :width]

    def wait_x(way, step):
        for part in range(parts):
            forward(way, step, part).wait_recv()

    def give(which, out, target):
        here = target.at[:, pl.ds(pl.multiple_of(z * cols, cols), cols)]

        def send(g, k):
            return remote(
                out.at[at_block(g), :], here,
                a_send.at[k, which], a_recv.at[k, which], "sp", g,
            )

        def started(g):
            for k in range(1, sp):
                @pl.when(lax.rem(z + k, sp) == g)
                def _():
                    send(lax.rem(z + k, sp), k).start()

        def finished():
            for k in range(1, sp):
                send(lax.rem(z + k, sp), k).wait_send()

        def came():
            for k in range(1, sp):
                send(lax.rem(z + k, sp), k).wait_recv()

        return started, finished, came

    stick_started, stick_finished, stick_came = give(0, stick_out, sticks)
    delta_started, delta_finished, delta_came = give(1, delta_out, deltas)

    shorter = jnp.minimum(z, sp - 1 - z)
    down_last = z > sp - 1 - z

    def place(n):
        both = n <= 2 * shorter
        way_n = jnp.where(both, lax.rem(n + 1, 2), jnp.where(down_last, 0, 1))
        step_n = jnp.where(n == 0, 0, jnp.where(both, (n + 1) // 2, n - shorter))
        down = jnp.logical_and(way_n == 0, n > 0)
        return way_n, step_n, down, jnp.where(down, z - step_n, z + step_n)

    last_way = jnp.logical_or(z == 0, z == sp - 1)

    def delta_event(n):
        way_n, step_n, down, b = place(n)
        for step in range(1, sp):
            for way in range(2):
                @pl.when(jnp.logical_and(step_n == step, way_n == way))
                def _():
                    wait_x(way, step)
        drows = dot_f32(xs[b], ws[:, 3 * cols :]).astype(jnp.bfloat16).astype(jnp.float32)
        prepare(b, drows[:, :cols], drows[:, cols : 2 * cols], drows[:, 2 * cols :])

    def settle(i):
        stick_out[at_block(i), :] = acc[at_block(i), :].astype(jnp.bfloat16)

    def stick_project(b):
        out = dot_f32(xs[b], ws[:, : 3 * cols]).astype(jnp.bfloat16)
        for i in range(3):
            proj[i, at_block(b), :] = out[:, i * cols : (i + 1) * cols]

    def stick_place(n):
        down = n > sp - 1 - z
        return down, jnp.where(down, sp - 1 - n, z + n)

    def stick_event(n, reach):
        lowest, highest = reach
        down, b = stick_place(n)
        lowest = jnp.minimum(lowest, b)
        highest = jnp.maximum(highest, b)

        @pl.when(last_way)
        def _():
            for part in range(2):
                @pl.when(n == sp - 3 + part)
                def _():
                    arrive(sp - 1, part)

        stick_project(b)
        pair(b, b, True, True)
        first_key = b == 0

        @pl.when(first_key)
        def _():
            settle(b)

        @pl.when(jnp.logical_and(last_way, n == sp - 2))
        def _():
            arrive(sp - 1, 2)

        def off(m, c):
            i = jnp.where(down, highest - m, b)
            j = jnp.where(down, b, b - 1 - m)
            pair(i, j, False, False)

            @pl.when(first_key)
            def _():
                stick_started(jnp.where(m == 0, b, i + 1))
                settle(i)
            return c

        lax.fori_loop(0, highest - lowest, off, 0)

        @pl.when(jnp.logical_and(lowest == 0, b > 0))
        def _():
            settle(b)

        @pl.when(lowest == 0)
        def _():
            stick_started(jnp.where(jnp.logical_and(first_key, highest > b), b + 1, b))
        return lowest, highest

    def early_delta(n, carry):
        @pl.when(n == 1)
        def _():
            relay(stick_kinds[0])

        @pl.when(n == sp - 2)
        def _():
            for c in early[parts:-1]:
                arrive(*c)
            for i in stick_kinds[1:]:
                relay(i)
            arrive(*early[-1])
        delta_event(n)
        return carry

    events = jnp.where(last_way, sp - 1, sp)
    lax.fori_loop(0, events, early_delta, 0)

    def walk(n, memory):
        high, low = halves(memory)
        new = folded(dot_f32(maps[n], wide_rhs(high, low, 1))) + adds[n]
        made = new[width:]
        made = made * lax.rsqrt(jnp.mean(made * made, axis=-1, keepdims=True) + NORM_EPS)
        at = pl.ds(pl.multiple_of(n * span, span), span)
        delta_out[at, :] = (made * gain_ref[...]).astype(delta_out.dtype)
        return new[:width]

    def walk_group(g, memory):
        for n in range(blocks):
            memory = walk(g * blocks + n, memory)
        delta_started(g - 1)
        return memory

    empty = jnp.zeros((width, width), jnp.float32)

    @pl.when(jnp.logical_not(last_way))
    def _():
        lax.fori_loop(0, sp, walk_group, empty)
        delta_started(sp - 1)

    relayed(stick_kinds)
    lax.fori_loop(0, events, stick_event, (z, z))

    @pl.when(last_way)
    def _():
        for part in range(3, parts):
            arrive(sp - 1, part)
        delta_event(sp - 1)
        down, b = stick_place(sp - 1)
        stick_project(b)
        acc[at_block(b), :] = jnp.zeros((rows, cols), jnp.float32)
        later[at_block(b), :] = jnp.zeros((rows, cols), jnp.float32)

        def last_pairs(m, memory):
            i = jnp.where(down, m, b)
            j = jnp.where(down, b, b - m)
            pair(i, j, True, False)
            memory = walk_group(m, memory)

            @pl.when(down)
            def _():
                stick_started(m - 1)
                settle(i)
            return memory

        lax.fori_loop(0, sp, last_pairs, empty)
        delta_started(sp - 1)

        @pl.when(down)
        def _():
            stick_started(sp - 1)

        @pl.when(jnp.logical_not(down))
        def _():
            settle(b)
            stick_started(b)

    mine_z = pl.ds(pl.multiple_of(z * rows, rows), rows)
    lanes = pl.ds(pl.multiple_of(z * cols, cols), cols)
    sticks[:, lanes] = stick_out[mine_z, :]
    deltas[:, lanes] = delta_out[mine_z, :]
    for c in late:
        c.wait()
    stick_came()
    chunks, wide = outgoing.shape[0], outgoing.shape[2]
    share = rows // tp
    for c in range(chunks):
        columns = slice(c * wide, (c + 1) * wide)
        partial[:, columns] = dot_f32(sticks[...], sw_ref[:, columns])
    delta_came()
    mine = pl.ds(pl.multiple_of(t * share, share), share)
    partner = lax.rem(t + 1, tp)
    theirs = pl.ds(pl.multiple_of(partner * share, share), share)

    def finish(which, c):
        columns = slice(c * wide, (c + 1) * wide)
        return (
            partial[which, columns] + dot_f32(deltas[which, :], dw_ref[:, columns])
        ).astype(jnp.bfloat16)

    swaps = [
        remote(
            outgoing.at[c], incoming.at[:, c * wide : (c + 1) * wide],
            c_send.at[c], c_recv.at[c], "tp", partner,
        )
        for c in range(chunks)
    ]
    for c in range(chunks):
        outgoing[c] = finish(theirs, c)
        if c > 0:
            swaps[c - 1].start()
    for c in range(chunks):
        own[:, c * wide : (c + 1) * wide] = finish(mine, c)
        if c == 0:
            swaps[chunks - 1].start()
    for c in range(chunks):
        swaps[c].wait_recv()

    for c in swaps:
        c.wait_send()
    for i in range(count):
        for side in range(2):
            w_copy(side, i).wait_send()
            w_relay(side, i).wait_send()
    for part in range(parts):
        forward(0, 0, part).wait_send()
        for step in range(1, sp):
            for way in range(2):
                @pl.when(sends(way, step))
                def _():
                    x_copy(way, step, part).wait_send()
                    if part == 0:
                        shift_copy(way, step).wait_send()

                @pl.when(comes(way, step))
                def _():
                    forward(way, step, part).wait_send()
    stick_finished()
    delta_finished()


ANYWHERE = pl.BlockSpec(memory_space=pltpu.HBM)
ON_CORE = pl.BlockSpec(memory_space=pltpu.VMEM)


def on_device_heads(
    hidden_in, sb_query_w, sb_key_w, sb_value_w, sb_offset,
    delta_query_w, delta_key_w, delta_value_w, decay_w, write_w, write_bias,
    decay_log_scale, decay_shift, head_gain, sb_out_w, delta_out_w,
):
    sp, fs, tp = lax.axis_size("sp"), lax.axis_size("fs"), lax.axis_size("tp")
    rows, half = hidden_in.shape[1:]
    width = half * tp
    length = rows * sp
    heads = decay_log_scale.shape[0]
    cols = sb_query_w.shape[1] // sp
    parts, chunks = 4, 4
    share = rows // tp
    blocks = length // BLOCK
    dma = pltpu.SemaphoreType.DMA
    bf16, f32 = jnp.bfloat16, jnp.float32
    own, incoming = pl.pallas_call(
        layer_kernel,
        name="layer",
        out_shape=(pltpu.VMEM((share, width), bf16),) * 2,
        in_specs=[ANYWHERE] * 16,
        out_specs=(ON_CORE,) * 2,
        scratch_shapes=[
            pltpu.SMEM(sb_offset.shape, f32),
            pltpu.SMEM(decay_log_scale.shape, f32),
            pltpu.SMEM(write_bias.shape, f32),
            pltpu.VMEM((1, head_gain.shape[0]), f32),
            pltpu.VMEM((sp, rows, width), bf16),
            pltpu.VMEM((width, 6 * cols), bf16),
            pltpu.VMEM((2, heads, width), bf16),
            pltpu.VMEM((2 * heads, width), bf16),
            pltpu.VMEM((2 * heads, rows), f32),
            pltpu.VMEM((sp, heads, rows), f32),
            pltpu.VMEM((rows, rows + cols), bf16),
            pltpu.VMEM((3, length, cols), bf16),
            pltpu.VMEM((length, cols), f32),
            pltpu.VMEM((length, cols), f32),
            pltpu.VMEM((blocks, cols + BLOCK, 2 * cols), bf16),
            pltpu.VMEM((blocks, cols + BLOCK, cols), f32),
            pltpu.VMEM((length, cols), bf16),
            pltpu.VMEM((length, cols), bf16),
            pltpu.VMEM((rows, cols * sp), bf16),
            pltpu.VMEM((rows, cols * sp), bf16),
            pltpu.VMEM(sb_out_w.shape, bf16),
            pltpu.VMEM(delta_out_w.shape, bf16),
            pltpu.VMEM((rows, width), f32),
            pltpu.VMEM((chunks, share, width // chunks), bf16),
            dma((2, sp, parts)), dma((2, sp, parts)), dma((2, sp, parts)), dma((2, sp, parts)),
            dma((fs, 6)), dma((fs, 6)), dma((2, sp)), dma((2, sp)), dma((10,)), dma((6,)),
            dma((sp, 2)), dma((sp, 2)), dma((chunks,)), dma((chunks,)),
        ],
        compiler_params=pltpu.CompilerParams(
            collective_id=0, has_side_effects=True,
            vmem_limit_bytes=ALL_VMEM - 5 * share * width,
        ),
    )(
        sb_offset, decay_log_scale, write_bias,
        hidden_in.reshape(rows, half), sb_query_w, sb_key_w, sb_value_w,
        delta_query_w, delta_key_w, delta_value_w, decay_w.T, write_w.T,
        decay_shift.reshape(heads, rows), head_gain.reshape(1, -1), sb_out_w, delta_out_w,
    )
    result = (own.astype(f32) + incoming.astype(f32)).astype(bf16)
    return result.reshape(1, share, width)


def on_device(*inputs):
    delta_heads = inputs[11].shape[0]
    square = lax.axis_size("fs") == 4 and lax.axis_size("tp") == 2
    if square and delta_heads == lax.axis_size("sp") and inputs[4].shape[0] % delta_heads == 0:
        return on_device_heads(*inputs)
    return on_device_split(*inputs)


def solution(mesh):
    return jax.shard_map(
        on_device,
        mesh=mesh,
        in_specs=(
            P("fs", "sp", "tp"),
            P("fs", "tp"),
            P("fs", "tp"),
            P("fs", "tp"),
            P("tp"),
            P("fs", "tp"),
            P("fs", "tp"),
            P("fs", "tp"),
            P(None, "tp"),
            P(None, "tp"),
            P("tp"),
            P("tp"),
            P("fs", "tp", "sp"),
            P(),
            P("tp", None),
            P("tp", None),
        ),
        out_specs=P("fs", ("sp", "tp"), None),
        check_vma=False,
    )
```

```python
import jax
import jax.numpy as jnp
from jax import lax
from jax.experimental import pallas as pl
from jax.experimental.pallas import tpu as pltpu
from jax.sharding import PartitionSpec as P

MESH = pl.DeviceIdType.MESH
ALL_VMEM = 67043328

SB_DIM = 64
GDN_DIM = 128
BLOCK = 64


EXACT_MATMUL = lax.Precision.HIGHEST
NORM_EPS = 1e-06


def carried_in(value, axis, combine, identity):
    devices, index = (lax.axis_size(axis), lax.axis_index(axis))
    everything = jax.tree.map(
        lambda part, kind: lax.all_gather(part.astype(kind), axis),
        value,
        (jnp.bfloat16, jnp.bfloat16),
    )
    start = jax.tree.map(
        lambda part, zero: jnp.broadcast_to(jnp.asarray(zero, part.dtype), part.shape),
        value,
        identity,
    )

    def lap(k, before):
        reached = k < index
        new = combine(
            before, jax.tree.map(lambda part, own: part[k].astype(own.dtype), everything, value)
        )
        return jax.tree.map(lambda a, b: jnp.where(reached, a, b), new, before)

    return lax.fori_loop(0, devices, lap, start)


def unit_lower_inverse(strict_part):
    order_size = strict_part.shape[-1]
    powered = strict_part
    inverse = jnp.eye(order_size, dtype=strict_part.dtype) - strict_part
    for repeat_number in range(max(1, (order_size - 1).bit_length()) - 1):
        powered = jnp.einsum("...ij,...jk->...ik", powered, powered, precision=EXACT_MATMUL)
        inverse = inverse + jnp.einsum(
            "...ij,...jk->...ik", inverse, powered, precision=EXACT_MATMUL
        )
    return inverse


def to_blocks(row_data, block_span):
    blocks_count = row_data.shape[0] // block_span
    shaped = row_data.reshape((blocks_count, block_span) + row_data.shape[1:])
    return jnp.swapaxes(shaped, 1, 2)


def from_blocks(blocked):
    swapped = jnp.swapaxes(blocked, 1, 2)
    return swapped.reshape((-1,) + swapped.shape[2:])


def unit_rows(vectors):
    return vectors * lax.rsqrt(jnp.sum(vectors * vectors, axis=-1, keepdims=True) + NORM_EPS)


def delta_inputs(
    query_proj,
    key_proj,
    value_proj,
    decay_pre,
    write_pre,
    write_bias,
    decay_log_scale,
    shift_rows,
    head_count,
    head_size,
):
    query_act = jax.nn.silu(query_proj.astype(jnp.float32)).reshape(-1, head_count, head_size)
    key_act = jax.nn.silu(key_proj.astype(jnp.float32)).reshape(-1, head_count, head_size)
    value_rows = jax.nn.silu(value_proj.astype(jnp.float32)).reshape(-1, head_count, head_size)
    queries = unit_rows(query_act) * head_size ** (-0.5)
    key_rows = unit_rows(key_act)
    log_decay = -jnp.exp(decay_log_scale) * jax.nn.softplus(decay_pre) + shift_rows
    strength = jax.nn.sigmoid(write_pre + write_bias)
    return (queries, key_rows, value_rows, log_decay, strength)


def delta_prepare(queries, key_rows, value_rows, log_decay, strength):
    block_span = queries.shape[2]
    cumulative = jnp.cumsum(log_decay, axis=-1)
    row_place = lax.broadcasted_iota(jnp.int32, (block_span, block_span), 0)
    col_place = lax.broadcasted_iota(jnp.int32, (block_span, block_span), 1)
    inclusive = col_place <= row_place
    strictly = col_place < row_place
    spread = cumulative[..., :, None] - cumulative[..., None, :]
    decay_table = jnp.where(inclusive, jnp.exp(jnp.where(inclusive, spread, 0.0)), 0.0)
    keys_beta = key_rows * strength[..., None]
    lower_part = jnp.where(
        strictly,
        jnp.einsum("nhik,nhjk->nhij", keys_beta, key_rows, precision=EXACT_MATMUL) * decay_table,
        0.0,
    )
    inverse = unit_lower_inverse(lower_part)
    growth = jnp.exp(cumulative)
    state_updates = jnp.einsum(
        "nhij,nhjv->nhiv", inverse, value_rows * strength[..., None], precision=EXACT_MATMUL
    )
    erase_term = jnp.einsum(
        "nhij,nhjk->nhik", inverse, keys_beta * growth[..., None], precision=EXACT_MATMUL
    )
    inside_block = (
        jnp.einsum("nhik,nhjk->nhij", queries, key_rows, precision=EXACT_MATMUL) * decay_table
    )
    boosted_query = queries * growth[..., None]
    damped_keys = key_rows * jnp.exp(cumulative[..., -1:] - cumulative)[..., None]
    decay_per_block = jnp.exp(cumulative[..., -1])
    return (state_updates, erase_term, inside_block, boosted_query, damped_keys, decay_per_block)


def delta_step(memory_state, inputs):
    state_updates, erase_term, inside_block, boosted_query, damped_keys, decay_per_block = inputs
    fixed_values = state_updates - jnp.einsum(
        "mzq,mqc->mzc", erase_term, memory_state, precision=EXACT_MATMUL
    )
    produced_rows = jnp.einsum(
        "mzq,mqc->mzc", boosted_query, memory_state, precision=EXACT_MATMUL
    ) + jnp.einsum("efq,eqn->efn", inside_block, fixed_values, precision=EXACT_MATMUL)
    memory_state = memory_state * decay_per_block[:, None, None] + jnp.einsum(
        "wam,waz->wmz", damped_keys, fixed_values, precision=EXACT_MATMUL
    )
    return (memory_state, produced_rows)


def transition_step(carried, inputs):
    memory_state, transfer = carried
    state_updates, erase_term, inside_block, boosted_query, damped_keys, decay_per_block = inputs
    fixed_values = state_updates - jnp.einsum(
        "mzq,mqc->mzc", erase_term, memory_state, precision=EXACT_MATMUL
    )
    coupling = jnp.einsum("hik,hil->hkl", damped_keys, erase_term, precision=EXACT_MATMUL)
    memory_state = memory_state * decay_per_block[:, None, None] + jnp.einsum(
        "wam,waz->wmz", damped_keys, fixed_values, precision=EXACT_MATMUL
    )
    transfer = transfer * decay_per_block[:, None, None] - jnp.einsum(
        "hkl,hlm->hkm", coupling, transfer, precision=EXACT_MATMUL
    )
    return ((memory_state, transfer), None)


def compose(prior_blocks, following_blocks):
    joined_map = jnp.einsum(
        "hkl,hlm->hkm", following_blocks[0], prior_blocks[0], precision=EXACT_MATMUL
    )
    joined_state = (
        jnp.einsum("djo,dog->djg", following_blocks[0], prior_blocks[1], precision=EXACT_MATMUL)
        + following_blocks[1]
    )
    return (joined_map, joined_state)


def stick_block(queries, key_rows, value_rows, query_place, key_place, offsets):
    scale_factor = queries.shape[-1] ** (-0.5)
    scores = (
        jnp.einsum("qhd,khd->hqk", queries, key_rows, preferred_element_type=jnp.float32)
        * scale_factor
        + offsets[:, None, None]
    )
    visible = key_place[None, :] < query_place[:, None]
    skipped = jnp.where(visible, jax.nn.log_sigmoid(-scores), 0.0)
    beyond = lax.cumsum(skipped, axis=2, reverse=True) - skipped
    weights = jnp.where(visible, jnp.exp(jax.nn.log_sigmoid(scores) + beyond), 0.0).astype(
        jnp.bfloat16
    )
    partial_value = jnp.einsum(
        "hqk,khd->qhd", weights, value_rows, preferred_element_type=jnp.float32
    )
    return (partial_value, jnp.sum(skipped, axis=2).T)


def stick_combine(partials, totals):
    beyond = jnp.cumsum(totals[::-1], axis=0)[::-1] - totals
    return jnp.sum(partials * jnp.exp(beyond)[..., None], axis=0)


def on_device_split(
    hidden_in,
    sb_query_w,
    sb_key_w,
    sb_value_w,
    sb_offset,
    delta_query_w,
    delta_key_w,
    delta_value_w,
    decay_w,
    write_w,
    write_bias,
    decay_log_scale,
    decay_shift,
    head_gain,
    sb_out_w,
    delta_out_w,
):
    token_rows = hidden_in.shape[1]
    local_in = hidden_in.reshape(token_rows, hidden_in.shape[2])
    gathered = (
        lax.all_gather(sb_query_w, "fs", axis=0, tiled=True),
        lax.all_gather(sb_key_w, "fs", axis=0, tiled=True),
        lax.all_gather(sb_value_w, "fs", axis=0, tiled=True),
        lax.all_gather(delta_query_w, "fs", axis=0, tiled=True),
        lax.all_gather(delta_key_w, "fs", axis=0, tiled=True),
        lax.all_gather(delta_value_w, "fs", axis=0, tiled=True),
    )
    in_weights = tuple(gathered) + (decay_w, write_w)
    portion = lax.all_gather(local_in, "tp", axis=1, tiled=True)
    projected = tuple(
        (jnp.dot(portion, weight, preferred_element_type=jnp.float32) for weight in in_weights)
    )
    sb_heads = sb_offset.shape[0]
    delta_heads = decay_log_scale.shape[0]
    sb_query = projected[0].astype(jnp.bfloat16).reshape(token_rows, sb_heads, SB_DIM)
    sb_keys = projected[1].astype(jnp.bfloat16)
    sb_values = projected[2].astype(jnp.bfloat16)
    shift_rows = decay_shift.reshape(delta_heads, token_rows).T
    queries, key_rows, value_rows, log_decay, strength = delta_inputs(
        projected[3].astype(jnp.bfloat16),
        projected[4].astype(jnp.bfloat16),
        projected[5].astype(jnp.bfloat16),
        projected[6],
        projected[7],
        write_bias,
        decay_log_scale,
        shift_rows,
        delta_heads,
        GDN_DIM,
    )
    prepared = delta_prepare(
        to_blocks(queries, BLOCK),
        to_blocks(key_rows, BLOCK),
        to_blocks(value_rows, BLOCK),
        to_blocks(log_decay, BLOCK),
        to_blocks(strength, BLOCK),
    )
    identity_map = jnp.broadcast_to(
        jnp.eye(GDN_DIM, dtype=jnp.float32), (delta_heads, GDN_DIM, GDN_DIM)
    )
    empty_state = jnp.zeros((delta_heads, GDN_DIM, GDN_DIM), jnp.float32)
    (local_end, local_map), unused_out = lax.scan(
        transition_step, (empty_state, identity_map), prepared
    )
    own_first = lax.axis_index("sp") * token_rows
    query_place = own_first + lax.iota(jnp.int32, token_rows)
    sp_count = lax.axis_size("sp")
    slot_out = jnp.zeros((sp_count, token_rows, sb_heads, SB_DIM), jnp.float32)
    slot_total = jnp.zeros((sp_count, token_rows, sb_heads), jnp.float32)

    def absorb(slot_arrays, address_portion, value_part, shard_first):

        def active(current):
            partial_value, totals = stick_block(
                sb_query,
                address_portion.reshape(token_rows, sb_heads, SB_DIM),
                value_part.reshape(token_rows, sb_heads, SB_DIM),
                query_place,
                shard_first + lax.iota(jnp.int32, token_rows),
                sb_offset,
            )
            slot_index = shard_first // token_rows
            return (
                lax.dynamic_update_index_in_dim(current[0], partial_value, slot_index, 0),
                lax.dynamic_update_index_in_dim(current[1], totals, slot_index, 0),
            )

        def inactive(current):
            return current

        usable = jnp.logical_and(shard_first >= 0, shard_first <= own_first)
        return lax.cond(usable, active, inactive, slot_arrays)

    key_block = lax.all_gather(sb_keys, "sp", axis=0, tiled=True)
    value_block = lax.all_gather(sb_values, "sp", axis=0, tiled=True)

    def per_shard(shard_number, current):
        row_begin = shard_number * token_rows
        return absorb(
            current,
            lax.dynamic_slice_in_dim(key_block, row_begin, token_rows, 0),
            lax.dynamic_slice_in_dim(value_block, row_begin, token_rows, 0),
            row_begin,
        )

    slot_arrays = lax.fori_loop(
        0, key_block.shape[0] // token_rows, per_shard, (slot_out, slot_total)
    )
    unused_map, incoming = carried_in(
        (local_map, local_end), "sp", compose, (identity_map, empty_state)
    )
    sb_mixed = (
        stick_combine(slot_arrays[0], slot_arrays[1])
        .astype(jnp.bfloat16)
        .reshape(token_rows, sb_heads * SB_DIM)
    )
    unused_end, produced_rows = lax.scan(delta_step, incoming, prepared)
    produced_rows = from_blocks(produced_rows)
    normed = (
        produced_rows
        * lax.rsqrt(jnp.mean(produced_rows * produced_rows, axis=-1, keepdims=True) + NORM_EPS)
        * head_gain
    )
    delta_mixed = normed.astype(jnp.bfloat16).reshape(token_rows, delta_heads * GDN_DIM)
    result = lax.psum_scatter(
        (
            jnp.dot(sb_mixed, sb_out_w, preferred_element_type=jnp.float32)
            + jnp.dot(delta_mixed, delta_out_w, preferred_element_type=jnp.float32)
        ).astype(jnp.bfloat16),
        "tp",
        scatter_dimension=0,
        tiled=True,
    ).astype(jnp.float32)
    return result.astype(jnp.bfloat16).reshape(1, result.shape[0], result.shape[1])


def remote(src, dst, send, recv, axis, index):
    return pltpu.make_async_remote_copy(
        src_ref=src, dst_ref=dst, send_sem=send, recv_sem=recv,
        device_id={axis: index}, device_id_type=MESH,
    )


def greet(axes):
    barrier = pltpu.get_barrier_semaphore()
    count = 0
    for axis in axes:
        size, me = lax.axis_size(axis), lax.axis_index(axis)
        for k in range(1, size):
            pl.semaphore_signal(
                barrier, inc=1, device_id={axis: lax.rem(me + k, size)}, device_id_type=MESH
            )
            count += 1
    pl.semaphore_wait(barrier, count)


def halves(a):
    high = a.astype(jnp.bfloat16)
    return high, (a - high.astype(jnp.float32)).astype(jnp.bfloat16)


def dot_f32(a, b, dims=((1,), (0,))):
    return lax.dot_general(a, b, (dims, ((), ())), preferred_element_type=jnp.float32)


def wide_rhs(high, low, axis):
    top = jnp.concatenate([high, low], axis=axis)
    bottom = jnp.concatenate([high, jnp.zeros_like(low)], axis=axis)
    return jnp.concatenate([top, bottom], axis=1 - axis)


def folded(a):
    half = a.shape[1] // 2
    return a[:, :half] + a[:, half:]


def layer_kernel(
    offset_hbm, decay_scale_hbm, write_bias_hbm,
    x_ref, w0, w1, w2, w3, w4, w5, decay_w_ref, write_w_ref, shift_ref, gain_hbm, sw_hbm, dw_hbm,
    own, incoming,
    offset_ref, decay_scale_ref, write_bias_ref, gain_ref,
    xs, ws, gate_w, gate_all, gates, shifts_ref, after,
    proj, acc, later, memory_ref, maps, adds, stick_out, delta_out,
    sticks, deltas, sw_ref, dw_ref, partial, outgoing,
    x_send, x_recv, f_send, f_recv, w_send, w_recv, r_recv, s_send, s_recv, l_sem,
    a_send, a_recv, c_sem,
):
    weights = (w0, w1, w2, w3, w4, w5)
    sp, tp = lax.axis_size("sp"), lax.axis_size("tp")
    z, f, t = lax.axis_index("sp"), lax.axis_index("fs"), lax.axis_index("tp")
    rows, half = x_ref.shape
    depth = w0.shape[0]
    cols = ws.shape[1] // len(weights)
    parts = x_recv.shape[2]
    heads = decay_w_ref.shape[0]
    slot = pl.ds(pl.multiple_of(t * half, half), half)
    local = [
        pltpu.make_async_copy(x_ref, xs.at[z, :, slot], l_sem.at[0]),
        pltpu.make_async_copy(shift_ref, shifts_ref.at[z], l_sem.at[1]),
        pltpu.make_async_copy(decay_w_ref, gate_w.at[0], l_sem.at[2]),
        pltpu.make_async_copy(write_w_ref, gate_w.at[1], l_sem.at[3]),
        pltpu.make_async_copy(offset_hbm, offset_ref, l_sem.at[6]),
        pltpu.make_async_copy(decay_scale_hbm, decay_scale_ref, l_sem.at[7]),
        pltpu.make_async_copy(write_bias_hbm, write_bias_ref, l_sem.at[8]),
        pltpu.make_async_copy(gain_hbm, gain_ref, l_sem.at[9]),
    ]
    late = [
        pltpu.make_async_copy(sw_hbm, sw_ref, l_sem.at[4]),
        pltpu.make_async_copy(dw_hbm, dw_ref, l_sem.at[5]),
    ]

    def w_src(i):
        return weights[i].at[:, pl.ds(pl.multiple_of(z * cols, cols), cols)]

    def w_at(i, who):
        return ws.at[pl.ds(pl.multiple_of(who * depth, depth), depth), pl.ds(i * cols, cols)]

    local_w = [
        pltpu.make_async_copy(w_src(i), w_at(i, f), l_sem.at[10]) for i in range(len(weights))
    ]
    near = (f + 1 - 2 * (f % 2), f + 2 - 4 * (f // 2))
    count = len(weights)
    delta_kinds, stick_kinds = (3, 4, 5), (0, 1, 2)

    def onward(way):
        return z + 1 < sp if way == 0 else z > 0

    def ahead(way):
        return z + 1 if way == 0 else z - 1

    barrier = pltpu.get_barrier_semaphore()
    for way in range(2):
        @pl.when(onward(way))
        def _():
            pl.semaphore_signal(
                barrier, inc=1, device_id={"sp": ahead(way)}, device_id_type=MESH
            )
    for side in range(2):
        pl.semaphore_signal(barrier, inc=1, device_id={"fs": near[side]}, device_id_type=MESH)
    pl.semaphore_signal(
        barrier, inc=1, device_id={"tp": lax.rem(t + 1, tp)}, device_id_type=MESH
    )
    for c in local + local_w:
        c.start()
    peers = onward(0).astype(jnp.int32) + onward(1).astype(jnp.int32) + 3
    pl.semaphore_wait(barrier, peers)

    def x_copy(way, step, part):
        block = z - (step - 1) if way == 0 else z + (step - 1)
        piece = pl.ds(part * (rows // parts), rows // parts)
        there = xs.at[block, piece, slot]
        return remote(
            x_ref.at[piece, :] if step == 1 else there, there,
            x_send.at[way], x_recv.at[way, step - 1, part], "sp", ahead(way),
        )

    def shift_copy(way, step):
        block = z - (step - 1) if way == 0 else z + (step - 1)
        there = shifts_ref.at[block]
        return remote(
            shift_ref if step == 1 else there, there,
            s_send.at[way], s_recv.at[way, step - 1], "sp", ahead(way),
        )

    def comes(way, step):
        return z >= step if way == 0 else z + step < sp

    def sends(way, step):
        return jnp.logical_and(onward(way), comes(way, step - 1))

    def forward(way, step, part):
        block = z - step if way == 0 else z + step
        piece = pl.ds(part * (rows // parts), rows // parts)
        there = xs.at[block, piece, slot]
        return remote(
            x_ref.at[piece, :] if step == 0 else there, there,
            f_send.at[0], f_recv.at[way * (sp - 1) + step], "tp", lax.rem(t + 1, tp),
        )

    def w_copy(side, i):
        return remote(
            w_src(i), w_at(i, f), w_send.at[0], w_recv.at[side, i], "fs", near[side]
        )

    def w_relay(side, i):
        part = depth // 2
        start = pl.multiple_of(near[side] * depth + side * part, part)
        there = ws.at[pl.ds(start, part), pl.ds(i * cols, cols)]
        return remote(
            there, there, w_send.at[0], r_recv.at[i // 3], "fs", near[1 - side]
        )

    for part in range(parts):
        for way in range(2):
            @pl.when(onward(way))
            def _():
                x_copy(way, 1, part).start()
                if part == 0:
                    shift_copy(way, 1).start()
    for i in delta_kinds:
        for side in range(2):
            w_copy(side, i).start()
    for part in range(parts):
        forward(0, 0, part).start()

    def relay(i):
        for side in range(2):
            w_copy(side, i).wait_recv()
            w_relay(side, i).start()

    def arrive(step, part):
        for way in range(2):
            @pl.when(comes(way, step))
            def _():
                x_copy(way, step, part).wait_recv()
                forward(way, step, part).start()
                if step + 1 < sp:
                    @pl.when(onward(way))
                    def _():
                        x_copy(way, step + 1, part).start()
                if part == 0:
                    shift_copy(way, step).wait_recv()
                    if step + 1 < sp:
                        @pl.when(onward(way))
                        def _():
                            shift_copy(way, step + 1).start()

    early = [(step, part) for step in range(1, sp - 1) for part in range(parts)]
    relay(delta_kinds[0])
    arrive(*early[0])
    for i in delta_kinds[1:]:
        relay(i)
    for i in stick_kinds:
        for side in range(2):
            w_copy(side, i).start()
    for c in late:
        c.start()
    for step, part in early[1:parts]:
        arrive(step, part)
    for c in local:
        c.wait()
    own_w = ws.at[pl.ds(pl.multiple_of(f * depth, depth), depth), :]
    pltpu.make_async_copy(own_w, own_w, l_sem.at[10]).wait()
    gate_all[...] = jnp.concatenate(
        [gate_w[0].astype(jnp.float32), gate_w[1].astype(jnp.float32)], axis=0
    ).astype(jnp.bfloat16)
    def all_sent(ref, sem):
        remote(ref, ref, sem, sem, "tp", lax.rem(t + 1, tp)).wait_send()

    def all_came(ref, sem):
        remote(ref, ref, sem, sem, "tp", lax.rem(t + 1, tp)).wait_recv()

    def block_came(way, step):
        all_came(xs.at[z, :, slot], f_recv.at[way * (sp - 1) + step])

    block_came(0, 0)

    def relayed(kinds):
        first = kinds[0] * cols
        all_came(ws.at[pl.ds(0, depth), pl.ds(first, len(kinds) * cols)], r_recv.at[kinds[0] // 3])

    relayed(delta_kinds)

    size = offset_ref.shape[0] // sp
    sb_size = cols // size
    scale = sb_size ** (-0.5)
    tile = rows // 2
    below = lax.broadcasted_iota(jnp.int32, (rows, rows), 0)
    across = lax.broadcasted_iota(jnp.int32, (rows, rows), 1)
    after[:, :rows] = jnp.where(below > across, 1.0, 0.0).astype(jnp.bfloat16)
    after[:, rows:] = jnp.ones((rows, cols), jnp.bfloat16)

    def at_block(b, start=0, extent=rows):
        return pl.ds(pl.multiple_of(b * rows + start, extent), extent)

    def pair(i, j, masked, fresh):
        for part in range(rows // tile):
            span = (part + 1) * tile if fresh else rows
            mine = at_block(i, part * tile, tile)
            q = proj[0, mine, :]
            keys, values = proj[1, at_block(j), :], proj[2, at_block(j), :]
            keys, values = keys[:span], values[:span]
            lane = lax.broadcasted_iota(jnp.int32, (tile, cols), 1)
            query = jnp.concatenate(
                [jnp.where(lane // sb_size == h, q, jnp.zeros_like(q)) for h in range(size)], axis=0
            )
            score = dot_f32(query, keys, ((1,), (1,)))
            score = jnp.concatenate(
                [
                    score[h * tile : (h + 1) * tile] * scale + offset_ref[z * size + h]
                    for h in range(size)
                ],
                axis=0,
            )
            skip = jnp.maximum(score, jnp.log(1.0 + jnp.exp(jnp.minimum(score, 80.0))))
            weight = score - skip
            if masked:
                seen = across[:tile, :span] < below[:tile, :span] + part * tile + (i - j) * rows
                seen = jnp.concatenate([seen] * size, axis=0)
                skip = jnp.where(seen, skip, 0.0)
            suffix = after[:span, :]
            if span < rows:
                suffix = jnp.concatenate([suffix[:, :span], suffix[:, rows:]], axis=1)
            sums = dot_f32(skip.astype(jnp.bfloat16), suffix)
            weight = jnp.exp(weight - sums[:, :span])
            if masked:
                weight = jnp.where(seen, weight, 0.0)
            out = dot_f32(weight.astype(jnp.bfloat16), values)
            mixed, total = out[:tile], sums[:tile, span:]
            for h in range(1, size):
                at = slice(h * tile, (h + 1) * tile)
                mixed = jnp.where(lane // sb_size == h, out[at], mixed)
                total = jnp.where(lane // sb_size == h, sums[at, span:], total)
            if fresh:
                acc[mine, :] = mixed
                later[mine, :] = total
            else:
                passed = later[mine, :]
                acc[mine, :] = acc[mine, :] + mixed * jnp.exp(-passed)
                later[mine, :] = passed + total

    span = BLOCK
    duo = 2 * span
    blocks = rows // span
    width = GDN_DIM
    seg_row = lax.broadcasted_iota(jnp.int32, (rows, rows), 0)
    seg_col = lax.broadcasted_iota(jnp.int32, (rows, rows), 1)
    together = seg_row // span == seg_col // span
    upto = jnp.where(jnp.logical_and(together, seg_row <= seg_col), 1.0, 0.0).astype(jnp.bfloat16)
    beyond_it = jnp.where(jnp.logical_and(together, seg_row > seg_col), 1.0, 0.0).astype(
        jnp.bfloat16
    )
    prow = lax.broadcasted_iota(jnp.int32, (span, duo), 0)
    plane = lax.broadcasted_iota(jnp.int32, (span, duo), 1)
    first = plane < span
    pcol = jnp.where(first, plane, plane - span)
    inclusive, strictly = pcol <= prow, pcol < prow
    unit = jnp.where(pcol == prow, 1.0, 0.0)
    diagonal = lax.broadcasted_iota(jnp.int32, (width, width), 0) == lax.broadcasted_iota(
        jnp.int32, (width, width), 1
    )
    eighth = lax.broadcasted_iota(jnp.int32, (8, rows), 0)

    def silu(a):
        return a * (1.0 / (1.0 + jnp.exp(-a)))

    def unit_of(a):
        return a * lax.rsqrt(jnp.sum(a * a, axis=-1, keepdims=True) + NORM_EPS)

    def apart(a):
        lanes = lax.broadcasted_iota(jnp.int32, a.shape, 1) < span
        zero = jnp.zeros_like(a)
        return jnp.concatenate([jnp.where(lanes, a, zero), jnp.where(lanes, zero, a)], axis=0)

    def squared(left, power):
        high, low = halves(power)
        lhigh, llow = halves(left)
        return folded(
            dot_f32(
                jnp.concatenate([lhigh, llow], axis=1), wide_rhs(apart(high), apart(low), 1)
            )
        )

    def prepare(b, dq, dk, dv):
        gates[...] = dot_f32(gate_all[...], xs[b], ((1,), (1,)))
        pre = gates[pl.ds(z, 1), :]
        write = gates[pl.ds(heads + z, 1), :] + write_bias_ref[z]
        rate = jnp.exp(jnp.full((1, rows), decay_scale_ref[z], jnp.float32))
        soft = jnp.maximum(pre, 0.0) + jnp.log(1.0 + jnp.exp(-jnp.abs(pre)))
        decay = shifts_ref[b, pl.ds(z, 1), :] - rate * soft
        strength = 1.0 / (1.0 + jnp.exp(-write))
        d1 = decay.astype(jnp.bfloat16).astype(jnp.float32)
        d2 = (decay - d1).astype(jnp.bfloat16).astype(jnp.float32)
        d3 = decay - d1 - d2
        three = jnp.where(
            eighth == 0, d1, jnp.where(eighth == 1, d2, jnp.where(eighth == 2, d3, 0.0))
        ).astype(jnp.bfloat16)
        cum_row = jnp.sum(dot_f32(three, upto), axis=0, keepdims=True)
        rest_row = jnp.sum(dot_f32(three, beyond_it), axis=0, keepdims=True)
        stack = jnp.where(
            eighth == 0, strength,
            jnp.where(
                eighth == 1, jnp.exp(cum_row),
                jnp.where(eighth == 2, jnp.exp(rest_row), cum_row),
            ),
        )
        columns = stack.T
        s_col, grow, damp, cum = (columns[:, n : n + 1] for n in range(4))
        q = unit_of(silu(dq)) * width ** (-0.5)
        k = unit_of(silu(dk))
        v = silu(dv)
        boosted = q * grow
        damped = k * damp
        right = jnp.concatenate([v * s_col, k * (s_col * grow)], axis=1)
        kh, kl = halves(k)
        qh, ql = halves(q)
        work = []
        for duo_at in range(rows // duo):
            lo = duo_at * duo
            here = slice(lo, lo + duo)
            left = jnp.concatenate(
                [
                    jnp.concatenate([kh[here], kl[here]], axis=1),
                    jnp.concatenate([qh[here], ql[here]], axis=1),
                ],
                axis=0,
            )
            gram = folded(
                dot_f32(left, wide_rhs(kh[here], kl[here], 0), ((1,), (1,)))
            )
            spread = (
                jnp.where(first, cum[lo : lo + span], cum[lo + span : lo + duo])
                - cum_row[:, here]
            )
            table = jnp.where(inclusive, jnp.exp(jnp.where(inclusive, spread, 0.0)), 0.0)
            scale_col = jnp.where(first, s_col[lo : lo + span], s_col[lo + span : lo + duo])
            near_k = jnp.where(first, gram[:span], gram[span:duo])
            near_q = jnp.where(first, gram[duo : duo + span], gram[duo + span :])
            strict = jnp.where(strictly, near_k * table * scale_col, 0.0)
            work.append([unit - strict, strict, near_q * table])
        for w in work:
            w[1] = squared(w[1], w[1])
        levels = max(1, (span - 1).bit_length()) - 1
        for level in range(levels):
            for w in work:
                if level + 1 < levels:
                    both = squared(jnp.concatenate([w[1], w[0]], axis=0), w[1])
                    w[1], w[0] = both[:span], w[0] + both[span:]
                else:
                    w[0] = w[0] + squared(w[0], w[1])
        for duo_at, (inverse, _, inside) in enumerate(work):
            lo = duo_at * duo
            here = slice(lo, lo + duo)
            ih, il = (apart(a) for a in halves(inverse))
            rh, rl = halves(right[here])
            solved = dot_f32(
                jnp.concatenate([ih, il], axis=1), jnp.concatenate([rh, rh], axis=0)
            ) + dot_f32(ih, rl)
            lh, ll = (
                apart(a) for a in halves(jnp.concatenate([damped[here].T, inside], axis=0))
            )
            sh, sl = halves(solved)
            made = dot_f32(
                jnp.concatenate([lh, ll], axis=1), jnp.concatenate([sh, sh], axis=0)
            ) + dot_f32(lh, sl)
            for side in range(2):
                at = lo + side * span
                mine = made[side * (width + span) : (side + 1) * (width + span)]
                n = b * blocks + 2 * duo_at + side
                keep = grow[at + span - 1 : at + span]
                step_map = jnp.where(diagonal, keep, 0.0) - mine[:width, width:]
                query = boosted[at : at + span] - mine[width:, width:]
                high, low = halves(jnp.concatenate([step_map, query], axis=0))
                maps[n, :, :width] = high
                maps[n, :, width:] = low
                adds[n] = mine[:, :width]

    def wait_x(way, step):
        block_came(way, step)

    def give(which, out, target):
        here = target.at[:, pl.ds(pl.multiple_of(z * cols, cols), cols)]

        def send(g, k):
            return remote(
                out.at[at_block(g), :], here,
                a_send.at[which], a_recv.at[which], "sp", g,
            )

        def started(g):
            for k in range(1, sp):
                @pl.when(lax.rem(z + k, sp) == g)
                def _():
                    send(lax.rem(z + k, sp), k).start()

        def came():
            all_came(out.at[pl.ds(0, (sp - 1) * rows), :], a_recv.at[which])

        return started, came

    stick_started, stick_came = give(0, stick_out, sticks)
    delta_started, delta_came = give(1, delta_out, deltas)

    shorter = jnp.minimum(z, sp - 1 - z)
    down_last = z > sp - 1 - z

    def place(n):
        both = n <= 2 * shorter
        way_n = jnp.where(both, lax.rem(n + 1, 2), jnp.where(down_last, 0, 1))
        step_n = jnp.where(n == 0, 0, jnp.where(both, (n + 1) // 2, n - shorter))
        down = jnp.logical_and(way_n == 0, n > 0)
        return way_n, step_n, down, jnp.where(down, z - step_n, z + step_n)

    last_way = jnp.logical_or(z == 0, z == sp - 1)

    def delta_event(n):
        way_n, step_n, down, b = place(n)
        for step in range(1, sp):
            for way in range(2):
                @pl.when(jnp.logical_and(step_n == step, way_n == way))
                def _():
                    wait_x(way, step)
        delta_block(b)

    def delta_block(b):
        drows = dot_f32(xs[b], ws[:, 3 * cols :]).astype(jnp.bfloat16).astype(jnp.float32)
        prepare(b, drows[:, :cols], drows[:, cols : 2 * cols], drows[:, 2 * cols :])

    def settle(i):
        stick_out[at_block(i), :] = acc[at_block(i), :].astype(jnp.bfloat16)

    def stick_project(b):
        out = dot_f32(xs[b], ws[:, : 3 * cols]).astype(jnp.bfloat16)
        for i in range(3):
            proj[i, at_block(b), :] = out[:, i * cols : (i + 1) * cols]

    def stick_place(n):
        down = n > sp - 1 - z
        return down, jnp.where(down, sp - 1 - n, z + n)

    def stick_event(n, reach):
        lowest, highest = reach
        down, b = stick_place(n)
        lowest = jnp.minimum(lowest, b)
        highest = jnp.maximum(highest, b)

        @pl.when(last_way)
        def _():
            for part in range(2):
                @pl.when(n == sp - 3 + part)
                def _():
                    arrive(sp - 1, part)

        stick_project(b)
        pair(b, b, True, True)
        first_key = b == 0

        @pl.when(first_key)
        def _():
            settle(b)

        @pl.when(jnp.logical_and(last_way, n == sp - 2))
        def _():
            arrive(sp - 1, 2)

        def off(m, c):
            i = jnp.where(down, highest - m, b)
            j = jnp.where(down, b, b - 1 - m)
            pair(i, j, False, False)

            @pl.when(first_key)
            def _():
                stick_started(jnp.where(m == 0, b, i + 1))
                settle(i)
            return c

        lax.fori_loop(0, highest - lowest, off, 0)

        @pl.when(jnp.logical_and(lowest == 0, b > 0))
        def _():
            settle(b)

        @pl.when(lowest == 0)
        def _():
            stick_started(jnp.where(jnp.logical_and(first_key, highest > b), b + 1, b))
        return lowest, highest

    def early_delta(n, carry):
        @pl.when(n == 1)
        def _():
            relay(stick_kinds[0])

        @pl.when(n == sp - 2)
        def _():
            for c in early[parts:-1]:
                arrive(*c)
            for i in stick_kinds[1:]:
                relay(i)
            arrive(*early[-1])
        delta_event(n)
        return carry

    events = jnp.where(last_way, sp - 1, sp)
    lax.fori_loop(0, events, early_delta, 0)

    def walk(n, memory):
        high, low = halves(memory)
        new = folded(dot_f32(maps[n], wide_rhs(high, low, 1))) + adds[n]
        made = new[width:]
        made = made * lax.rsqrt(jnp.mean(made * made, axis=-1, keepdims=True) + NORM_EPS)
        at = pl.ds(pl.multiple_of(n * span, span), span)
        delta_out[at, :] = (made * gain_ref[...]).astype(delta_out.dtype)
        return new[:width]

    def walk_groups(start, stop):
        def group(g, c):
            @pl.when(g > start)
            def _():
                delta_started(g - 1)
            memory = memory_ref[...]
            for n in range(blocks):
                memory = walk(g * blocks + n, memory)
            memory_ref[...] = memory
            return c

        lax.fori_loop(start, stop, group, 0)
        delta_started(stop - 1)

    memory_ref[...] = jnp.zeros((width, width), jnp.float32)

    @pl.when(jnp.logical_not(last_way))
    def _():
        walk_groups(0, sp)

    relayed(stick_kinds)
    lax.fori_loop(0, events, stick_event, (z, z))

    @pl.when(last_way)
    def _():
        for part in range(3, parts):
            arrive(sp - 1, part)
        walked = jnp.where(z == 0, sp - 1, 0)

        @pl.when(z == 0)
        def _():
            walk_groups(0, sp - 1)
        for way in range(2):
            @pl.when(comes(way, sp - 1))
            def _():
                block_came(way, sp - 1)
        down, b = stick_place(sp - 1)
        stick_project(b)
        acc[at_block(b), :] = jnp.zeros((rows, cols), jnp.float32)
        later[at_block(b), :] = jnp.zeros((rows, cols), jnp.float32)

        def last_pairs(m, c):
            i = jnp.where(down, m, b)
            j = jnp.where(down, b, b - m)

            @pl.when(down)
            def _():
                stick_started(m - 1)
            pair(i, j, True, False)

            @pl.when(down)
            def _():
                settle(i)
            return c

        lax.fori_loop(0, sp, last_pairs, 0)

        @pl.when(jnp.logical_not(down))
        def _():
            settle(b)
            stick_started(b)
        delta_block(b)
        walk_groups(walked, sp)

    mine_z = pl.ds(pl.multiple_of(z * rows, rows), rows)
    lanes = pl.ds(pl.multiple_of(z * cols, cols), cols)
    sticks[:, lanes] = stick_out[mine_z, :]
    deltas[:, lanes] = delta_out[mine_z, :]
    for c in late:
        c.wait()
    stick_came()
    chunks, wide = outgoing.shape[0], outgoing.shape[2]
    share = rows // tp
    for c in range(chunks):
        columns = slice(c * wide, (c + 1) * wide)
        partial[:, columns] = dot_f32(sticks[...], sw_ref[:, columns])
    delta_came()
    mine = pl.ds(pl.multiple_of(t * share, share), share)
    partner = lax.rem(t + 1, tp)
    theirs = pl.ds(pl.multiple_of(partner * share, share), share)

    def finish(which, c):
        columns = slice(c * wide, (c + 1) * wide)
        return (
            partial[which, columns] + dot_f32(deltas[which, :], dw_ref[:, columns])
        ).astype(jnp.bfloat16)

    swaps = [
        remote(
            outgoing.at[c], incoming.at[:, c * wide : (c + 1) * wide],
            c_sem.at[0], c_sem.at[1], "tp", partner,
        )
        for c in range(chunks)
    ]
    for c in range(chunks):
        outgoing[c] = finish(theirs, c)
        if c > 0:
            swaps[c - 1].start()
    for c in range(chunks):
        own[:, c * wide : (c + 1) * wide] = finish(mine, c)
        if c == 0:
            swaps[chunks - 1].start()
    all_came(incoming, c_sem.at[1])
    all_sent(incoming, c_sem.at[0])
    all_sent(ws.at[pl.ds(0, 3 * depth), :], w_send.at[0])
    all_sent(xs.at[:, :, slot], f_send.at[0])
    for which, out in enumerate((stick_out, delta_out)):
        all_sent(out.at[pl.ds(0, (sp - 1) * rows), :], a_send.at[which])
    for c in range(sp):
        @pl.when(z == c)
        def _():
            for way, passed in enumerate((c + 1 if c + 1 < sp else 0, sp - c if c > 0 else 0)):
                if passed:
                    all_sent(xs.at[pl.ds(0, passed), :, slot], x_send.at[way])
                    all_sent(shifts_ref.at[pl.ds(0, passed)], s_send.at[way])


ANYWHERE = pl.BlockSpec(memory_space=pltpu.HBM)
ON_CORE = pl.BlockSpec(memory_space=pltpu.VMEM)


def on_device_heads(
    hidden_in, sb_query_w, sb_key_w, sb_value_w, sb_offset,
    delta_query_w, delta_key_w, delta_value_w, decay_w, write_w, write_bias,
    decay_log_scale, decay_shift, head_gain, sb_out_w, delta_out_w,
):
    sp, fs, tp = lax.axis_size("sp"), lax.axis_size("fs"), lax.axis_size("tp")
    rows, half = hidden_in.shape[1:]
    width = half * tp
    length = rows * sp
    heads = decay_log_scale.shape[0]
    cols = sb_query_w.shape[1] // sp
    parts, chunks = 4, 4
    share = rows // tp
    blocks = length // BLOCK
    dma = pltpu.SemaphoreType.DMA
    bf16, f32 = jnp.bfloat16, jnp.float32
    own, incoming = pl.pallas_call(
        layer_kernel,
        name="layer",
        out_shape=(pltpu.VMEM((share, width), bf16),) * 2,
        in_specs=[ANYWHERE] * 16,
        out_specs=(ON_CORE,) * 2,
        scratch_shapes=[
            pltpu.SMEM(sb_offset.shape, f32),
            pltpu.SMEM(decay_log_scale.shape, f32),
            pltpu.SMEM(write_bias.shape, f32),
            pltpu.VMEM((1, head_gain.shape[0]), f32),
            pltpu.VMEM((sp, rows, width), bf16),
            pltpu.VMEM((width, 6 * cols), bf16),
            pltpu.VMEM((2, heads, width), bf16),
            pltpu.VMEM((2 * heads, width), bf16),
            pltpu.VMEM((2 * heads, rows), f32),
            pltpu.VMEM((sp, heads, rows), f32),
            pltpu.VMEM((rows, rows + cols), bf16),
            pltpu.VMEM((3, length, cols), bf16),
            pltpu.VMEM((length, cols), f32),
            pltpu.VMEM((length, cols), f32),
            pltpu.VMEM((cols, cols), f32),
            pltpu.VMEM((blocks, cols + BLOCK, 2 * cols), bf16),
            pltpu.VMEM((blocks, cols + BLOCK, cols), f32),
            pltpu.VMEM((length, cols), bf16),
            pltpu.VMEM((length, cols), bf16),
            pltpu.VMEM((rows, cols * sp), bf16),
            pltpu.VMEM((rows, cols * sp), bf16),
            pltpu.VMEM(sb_out_w.shape, bf16),
            pltpu.VMEM(delta_out_w.shape, bf16),
            pltpu.VMEM((rows, width), f32),
            pltpu.VMEM((chunks, share, width // chunks), bf16),
            dma((2,)), dma((2, sp - 1, parts)), dma((1,)), dma((2 * sp - 1,)),
            dma((1,)), dma((2, 6)), dma((2,)), dma((2,)), dma((2, sp - 1)), dma((11,)),
            dma((2,)), dma((2,)), dma((2,)),
        ],
        compiler_params=pltpu.CompilerParams(
            collective_id=0, has_side_effects=True,
            vmem_limit_bytes=ALL_VMEM - 5 * share * width,
        ),
    )(
        sb_offset, decay_log_scale, write_bias,
        hidden_in.reshape(rows, half), sb_query_w, sb_key_w, sb_value_w,
        delta_query_w, delta_key_w, delta_value_w, decay_w.T, write_w.T,
        decay_shift.reshape(heads, rows), head_gain.reshape(1, -1), sb_out_w, delta_out_w,
    )
    result = (own.astype(f32) + incoming.astype(f32)).astype(bf16)
    return result.reshape(1, share, width)


def on_device(*inputs):
    delta_heads = inputs[11].shape[0]
    square = lax.axis_size("fs") == 4 and lax.axis_size("tp") == 2
    if square and delta_heads == lax.axis_size("sp") and inputs[4].shape[0] % delta_heads == 0:
        return on_device_heads(*inputs)
    return on_device_split(*inputs)


def solution(mesh):
    return jax.shard_map(
        on_device,
        mesh=mesh,
        in_specs=(
            P("fs", "sp", "tp"),
            P("fs", "tp"),
            P("fs", "tp"),
            P("fs", "tp"),
            P("tp"),
            P("fs", "tp"),
            P("fs", "tp"),
            P("fs", "tp"),
            P(None, "tp"),
            P(None, "tp"),
            P("tp"),
            P("tp"),
            P("fs", "tp", "sp"),
            P(),
            P("tp", None),
            P("tp", None),
        ),
        out_specs=P("fs", ("sp", "tp"), None),
        check_vma=False,
    )
```

```python
import jax
import jax.numpy as jnp
from jax import lax
from jax.experimental import pallas as pl
from jax.experimental.pallas import tpu as pltpu
from jax.sharding import PartitionSpec as P

MESH = pl.DeviceIdType.MESH
ALL_VMEM = 67043328

SB_DIM = 64
GDN_DIM = 128
BLOCK = 64


EXACT_MATMUL = lax.Precision.HIGHEST
NORM_EPS = 1e-06


def carried_in(value, axis, combine, identity):
    devices, index = (lax.axis_size(axis), lax.axis_index(axis))
    everything = jax.tree.map(
        lambda part, kind: lax.all_gather(part.astype(kind), axis),
        value,
        (jnp.bfloat16, jnp.bfloat16),
    )
    start = jax.tree.map(
        lambda part, zero: jnp.broadcast_to(jnp.asarray(zero, part.dtype), part.shape),
        value,
        identity,
    )

    def lap(k, before):
        reached = k < index
        new = combine(
            before, jax.tree.map(lambda part, own: part[k].astype(own.dtype), everything, value)
        )
        return jax.tree.map(lambda a, b: jnp.where(reached, a, b), new, before)

    return lax.fori_loop(0, devices, lap, start)


def unit_lower_inverse(strict_part):
    order_size = strict_part.shape[-1]
    powered = strict_part
    inverse = jnp.eye(order_size, dtype=strict_part.dtype) - strict_part
    for repeat_number in range(max(1, (order_size - 1).bit_length()) - 1):
        powered = jnp.einsum("...ij,...jk->...ik", powered, powered, precision=EXACT_MATMUL)
        inverse = inverse + jnp.einsum(
            "...ij,...jk->...ik", inverse, powered, precision=EXACT_MATMUL
        )
    return inverse


def to_blocks(row_data, block_span):
    blocks_count = row_data.shape[0] // block_span
    shaped = row_data.reshape((blocks_count, block_span) + row_data.shape[1:])
    return jnp.swapaxes(shaped, 1, 2)


def from_blocks(blocked):
    swapped = jnp.swapaxes(blocked, 1, 2)
    return swapped.reshape((-1,) + swapped.shape[2:])


def unit_rows(vectors):
    return vectors * lax.rsqrt(jnp.sum(vectors * vectors, axis=-1, keepdims=True) + NORM_EPS)


def delta_inputs(
    query_proj,
    key_proj,
    value_proj,
    decay_pre,
    write_pre,
    write_bias,
    decay_log_scale,
    shift_rows,
    head_count,
    head_size,
):
    query_act = jax.nn.silu(query_proj.astype(jnp.float32)).reshape(-1, head_count, head_size)
    key_act = jax.nn.silu(key_proj.astype(jnp.float32)).reshape(-1, head_count, head_size)
    value_rows = jax.nn.silu(value_proj.astype(jnp.float32)).reshape(-1, head_count, head_size)
    queries = unit_rows(query_act) * head_size ** (-0.5)
    key_rows = unit_rows(key_act)
    log_decay = -jnp.exp(decay_log_scale) * jax.nn.softplus(decay_pre) + shift_rows
    strength = jax.nn.sigmoid(write_pre + write_bias)
    return (queries, key_rows, value_rows, log_decay, strength)


def delta_prepare(queries, key_rows, value_rows, log_decay, strength):
    block_span = queries.shape[2]
    cumulative = jnp.cumsum(log_decay, axis=-1)
    row_place = lax.broadcasted_iota(jnp.int32, (block_span, block_span), 0)
    col_place = lax.broadcasted_iota(jnp.int32, (block_span, block_span), 1)
    inclusive = col_place <= row_place
    strictly = col_place < row_place
    spread = cumulative[..., :, None] - cumulative[..., None, :]
    decay_table = jnp.where(inclusive, jnp.exp(jnp.where(inclusive, spread, 0.0)), 0.0)
    keys_beta = key_rows * strength[..., None]
    lower_part = jnp.where(
        strictly,
        jnp.einsum("nhik,nhjk->nhij", keys_beta, key_rows, precision=EXACT_MATMUL) * decay_table,
        0.0,
    )
    inverse = unit_lower_inverse(lower_part)
    growth = jnp.exp(cumulative)
    state_updates = jnp.einsum(
        "nhij,nhjv->nhiv", inverse, value_rows * strength[..., None], precision=EXACT_MATMUL
    )
    erase_term = jnp.einsum(
        "nhij,nhjk->nhik", inverse, keys_beta * growth[..., None], precision=EXACT_MATMUL
    )
    inside_block = (
        jnp.einsum("nhik,nhjk->nhij", queries, key_rows, precision=EXACT_MATMUL) * decay_table
    )
    boosted_query = queries * growth[..., None]
    damped_keys = key_rows * jnp.exp(cumulative[..., -1:] - cumulative)[..., None]
    decay_per_block = jnp.exp(cumulative[..., -1])
    return (state_updates, erase_term, inside_block, boosted_query, damped_keys, decay_per_block)


def delta_step(memory_state, inputs):
    state_updates, erase_term, inside_block, boosted_query, damped_keys, decay_per_block = inputs
    fixed_values = state_updates - jnp.einsum(
        "mzq,mqc->mzc", erase_term, memory_state, precision=EXACT_MATMUL
    )
    produced_rows = jnp.einsum(
        "mzq,mqc->mzc", boosted_query, memory_state, precision=EXACT_MATMUL
    ) + jnp.einsum("efq,eqn->efn", inside_block, fixed_values, precision=EXACT_MATMUL)
    memory_state = memory_state * decay_per_block[:, None, None] + jnp.einsum(
        "wam,waz->wmz", damped_keys, fixed_values, precision=EXACT_MATMUL
    )
    return (memory_state, produced_rows)


def transition_step(carried, inputs):
    memory_state, transfer = carried
    state_updates, erase_term, inside_block, boosted_query, damped_keys, decay_per_block = inputs
    fixed_values = state_updates - jnp.einsum(
        "mzq,mqc->mzc", erase_term, memory_state, precision=EXACT_MATMUL
    )
    coupling = jnp.einsum("hik,hil->hkl", damped_keys, erase_term, precision=EXACT_MATMUL)
    memory_state = memory_state * decay_per_block[:, None, None] + jnp.einsum(
        "wam,waz->wmz", damped_keys, fixed_values, precision=EXACT_MATMUL
    )
    transfer = transfer * decay_per_block[:, None, None] - jnp.einsum(
        "hkl,hlm->hkm", coupling, transfer, precision=EXACT_MATMUL
    )
    return ((memory_state, transfer), None)


def compose(prior_blocks, following_blocks):
    joined_map = jnp.einsum(
        "hkl,hlm->hkm", following_blocks[0], prior_blocks[0], precision=EXACT_MATMUL
    )
    joined_state = (
        jnp.einsum("djo,dog->djg", following_blocks[0], prior_blocks[1], precision=EXACT_MATMUL)
        + following_blocks[1]
    )
    return (joined_map, joined_state)


def stick_block(queries, key_rows, value_rows, query_place, key_place, offsets):
    scale_factor = queries.shape[-1] ** (-0.5)
    scores = (
        jnp.einsum("qhd,khd->hqk", queries, key_rows, preferred_element_type=jnp.float32)
        * scale_factor
        + offsets[:, None, None]
    )
    visible = key_place[None, :] < query_place[:, None]
    skipped = jnp.where(visible, jax.nn.log_sigmoid(-scores), 0.0)
    beyond = lax.cumsum(skipped, axis=2, reverse=True) - skipped
    weights = jnp.where(visible, jnp.exp(jax.nn.log_sigmoid(scores) + beyond), 0.0).astype(
        jnp.bfloat16
    )
    partial_value = jnp.einsum(
        "hqk,khd->qhd", weights, value_rows, preferred_element_type=jnp.float32
    )
    return (partial_value, jnp.sum(skipped, axis=2).T)


def stick_combine(partials, totals):
    beyond = jnp.cumsum(totals[::-1], axis=0)[::-1] - totals
    return jnp.sum(partials * jnp.exp(beyond)[..., None], axis=0)


def on_device_split(
    hidden_in,
    sb_query_w,
    sb_key_w,
    sb_value_w,
    sb_offset,
    delta_query_w,
    delta_key_w,
    delta_value_w,
    decay_w,
    write_w,
    write_bias,
    decay_log_scale,
    decay_shift,
    head_gain,
    sb_out_w,
    delta_out_w,
):
    token_rows = hidden_in.shape[1]
    local_in = hidden_in.reshape(token_rows, hidden_in.shape[2])
    gathered = (
        lax.all_gather(sb_query_w, "fs", axis=0, tiled=True),
        lax.all_gather(sb_key_w, "fs", axis=0, tiled=True),
        lax.all_gather(sb_value_w, "fs", axis=0, tiled=True),
        lax.all_gather(delta_query_w, "fs", axis=0, tiled=True),
        lax.all_gather(delta_key_w, "fs", axis=0, tiled=True),
        lax.all_gather(delta_value_w, "fs", axis=0, tiled=True),
    )
    in_weights = tuple(gathered) + (decay_w, write_w)
    portion = lax.all_gather(local_in, "tp", axis=1, tiled=True)
    projected = tuple(
        (jnp.dot(portion, weight, preferred_element_type=jnp.float32) for weight in in_weights)
    )
    sb_heads = sb_offset.shape[0]
    delta_heads = decay_log_scale.shape[0]
    sb_query = projected[0].astype(jnp.bfloat16).reshape(token_rows, sb_heads, SB_DIM)
    sb_keys = projected[1].astype(jnp.bfloat16)
    sb_values = projected[2].astype(jnp.bfloat16)
    shift_rows = decay_shift.reshape(delta_heads, token_rows).T
    queries, key_rows, value_rows, log_decay, strength = delta_inputs(
        projected[3].astype(jnp.bfloat16),
        projected[4].astype(jnp.bfloat16),
        projected[5].astype(jnp.bfloat16),
        projected[6],
        projected[7],
        write_bias,
        decay_log_scale,
        shift_rows,
        delta_heads,
        GDN_DIM,
    )
    prepared = delta_prepare(
        to_blocks(queries, BLOCK),
        to_blocks(key_rows, BLOCK),
        to_blocks(value_rows, BLOCK),
        to_blocks(log_decay, BLOCK),
        to_blocks(strength, BLOCK),
    )
    identity_map = jnp.broadcast_to(
        jnp.eye(GDN_DIM, dtype=jnp.float32), (delta_heads, GDN_DIM, GDN_DIM)
    )
    empty_state = jnp.zeros((delta_heads, GDN_DIM, GDN_DIM), jnp.float32)
    (local_end, local_map), unused_out = lax.scan(
        transition_step, (empty_state, identity_map), prepared
    )
    own_first = lax.axis_index("sp") * token_rows
    query_place = own_first + lax.iota(jnp.int32, token_rows)
    sp_count = lax.axis_size("sp")
    slot_out = jnp.zeros((sp_count, token_rows, sb_heads, SB_DIM), jnp.float32)
    slot_total = jnp.zeros((sp_count, token_rows, sb_heads), jnp.float32)

    def absorb(slot_arrays, address_portion, value_part, shard_first):

        def active(current):
            partial_value, totals = stick_block(
                sb_query,
                address_portion.reshape(token_rows, sb_heads, SB_DIM),
                value_part.reshape(token_rows, sb_heads, SB_DIM),
                query_place,
                shard_first + lax.iota(jnp.int32, token_rows),
                sb_offset,
            )
            slot_index = shard_first // token_rows
            return (
                lax.dynamic_update_index_in_dim(current[0], partial_value, slot_index, 0),
                lax.dynamic_update_index_in_dim(current[1], totals, slot_index, 0),
            )

        def inactive(current):
            return current

        usable = jnp.logical_and(shard_first >= 0, shard_first <= own_first)
        return lax.cond(usable, active, inactive, slot_arrays)

    key_block = lax.all_gather(sb_keys, "sp", axis=0, tiled=True)
    value_block = lax.all_gather(sb_values, "sp", axis=0, tiled=True)

    def per_shard(shard_number, current):
        row_begin = shard_number * token_rows
        return absorb(
            current,
            lax.dynamic_slice_in_dim(key_block, row_begin, token_rows, 0),
            lax.dynamic_slice_in_dim(value_block, row_begin, token_rows, 0),
            row_begin,
        )

    slot_arrays = lax.fori_loop(
        0, key_block.shape[0] // token_rows, per_shard, (slot_out, slot_total)
    )
    unused_map, incoming = carried_in(
        (local_map, local_end), "sp", compose, (identity_map, empty_state)
    )
    sb_mixed = (
        stick_combine(slot_arrays[0], slot_arrays[1])
        .astype(jnp.bfloat16)
        .reshape(token_rows, sb_heads * SB_DIM)
    )
    unused_end, produced_rows = lax.scan(delta_step, incoming, prepared)
    produced_rows = from_blocks(produced_rows)
    normed = (
        produced_rows
        * lax.rsqrt(jnp.mean(produced_rows * produced_rows, axis=-1, keepdims=True) + NORM_EPS)
        * head_gain
    )
    delta_mixed = normed.astype(jnp.bfloat16).reshape(token_rows, delta_heads * GDN_DIM)
    result = lax.psum_scatter(
        (
            jnp.dot(sb_mixed, sb_out_w, preferred_element_type=jnp.float32)
            + jnp.dot(delta_mixed, delta_out_w, preferred_element_type=jnp.float32)
        ).astype(jnp.bfloat16),
        "tp",
        scatter_dimension=0,
        tiled=True,
    ).astype(jnp.float32)
    return result.astype(jnp.bfloat16).reshape(1, result.shape[0], result.shape[1])


def remote(src, dst, send, recv, axis, index):
    return pltpu.make_async_remote_copy(
        src_ref=src, dst_ref=dst, send_sem=send, recv_sem=recv,
        device_id={axis: index}, device_id_type=MESH,
    )


def greet(axes):
    barrier = pltpu.get_barrier_semaphore()
    count = 0
    for axis in axes:
        size, me = lax.axis_size(axis), lax.axis_index(axis)
        for k in range(1, size):
            pl.semaphore_signal(
                barrier, inc=1, device_id={axis: lax.rem(me + k, size)}, device_id_type=MESH
            )
            count += 1
    pl.semaphore_wait(barrier, count)


def halves(a):
    high = a.astype(jnp.bfloat16)
    return high, (a - high.astype(jnp.float32)).astype(jnp.bfloat16)


def dot_f32(a, b, dims=((1,), (0,))):
    return lax.dot_general(a, b, (dims, ((), ())), preferred_element_type=jnp.float32)


def wide_rhs(high, low, axis):
    top = jnp.concatenate([high, low], axis=axis)
    bottom = jnp.concatenate([high, jnp.zeros_like(low)], axis=axis)
    return jnp.concatenate([top, bottom], axis=1 - axis)


def folded(a):
    half = a.shape[1] // 2
    return a[:, :half] + a[:, half:]


def layer_kernel(
    offset_hbm, decay_scale_hbm, write_bias_hbm,
    x_ref, w0, w1, w2, w3, w4, w5, decay_w_ref, write_w_ref, shift_ref, gain_hbm, sw_hbm, dw_hbm,
    own, incoming,
    offset_ref, decay_scale_ref, write_bias_ref, gain_ref,
    xs, ws, gate_w, gate_all, gates, shifts_ref, after,
    proj, acc, later, memory_ref, maps, adds, stick_out, delta_out,
    sticks, deltas, sw_ref, dw_ref, partial, outgoing,
    x_send, x_recv, f_send, f_recv, w_send, w_recv, r_recv, s_send, s_recv, l_sem,
    a_send, a_recv, c_sem,
):
    weights = (w0, w1, w2, w3, w4, w5)
    sp, tp = lax.axis_size("sp"), lax.axis_size("tp")
    z, f, t = lax.axis_index("sp"), lax.axis_index("fs"), lax.axis_index("tp")
    rows, half = x_ref.shape
    depth = w0.shape[0]
    cols = ws.shape[1] // len(weights)
    parts = x_recv.shape[2]
    heads = decay_w_ref.shape[0]
    slot = pl.ds(pl.multiple_of(t * half, half), half)
    local = [
        pltpu.make_async_copy(x_ref, xs.at[z, :, slot], l_sem.at[0]),
        pltpu.make_async_copy(shift_ref, shifts_ref.at[z], l_sem.at[1]),
        pltpu.make_async_copy(decay_w_ref, gate_w.at[0], l_sem.at[2]),
        pltpu.make_async_copy(write_w_ref, gate_w.at[1], l_sem.at[3]),
        pltpu.make_async_copy(offset_hbm, offset_ref, l_sem.at[6]),
        pltpu.make_async_copy(decay_scale_hbm, decay_scale_ref, l_sem.at[7]),
        pltpu.make_async_copy(write_bias_hbm, write_bias_ref, l_sem.at[8]),
        pltpu.make_async_copy(gain_hbm, gain_ref, l_sem.at[9]),
    ]
    late = [
        pltpu.make_async_copy(sw_hbm, sw_ref, l_sem.at[4]),
        pltpu.make_async_copy(dw_hbm, dw_ref, l_sem.at[5]),
    ]

    def w_src(i):
        return weights[i].at[:, pl.ds(pl.multiple_of(z * cols, cols), cols)]

    def w_at(i, who):
        return ws.at[pl.ds(pl.multiple_of(who * depth, depth), depth), pl.ds(i * cols, cols)]

    local_w = [
        pltpu.make_async_copy(w_src(i), w_at(i, f), l_sem.at[10]) for i in range(len(weights))
    ]
    near = (f + 1 - 2 * (f % 2), f + 2 - 4 * (f // 2))
    count = len(weights)
    delta_kinds, stick_kinds = (3, 4, 5), (0, 1, 2)

    def onward(way):
        return z + 1 < sp if way == 0 else z > 0

    def ahead(way):
        return z + 1 if way == 0 else z - 1

    barrier = pltpu.get_barrier_semaphore()
    for way in range(2):
        @pl.when(onward(way))
        def _():
            pl.semaphore_signal(
                barrier, inc=1, device_id={"sp": ahead(way)}, device_id_type=MESH
            )
    for side in range(2):
        pl.semaphore_signal(barrier, inc=1, device_id={"fs": near[side]}, device_id_type=MESH)
    pl.semaphore_signal(
        barrier, inc=1, device_id={"tp": lax.rem(t + 1, tp)}, device_id_type=MESH
    )
    for c in local + local_w:
        c.start()
    peers = onward(0).astype(jnp.int32) + onward(1).astype(jnp.int32) + 3
    pl.semaphore_wait(barrier, peers)

    def x_copy(way, step, part):
        block = z - (step - 1) if way == 0 else z + (step - 1)
        piece = pl.ds(part * (rows // parts), rows // parts)
        there = xs.at[block, piece, slot]
        return remote(
            x_ref.at[piece, :] if step == 1 else there, there,
            x_send.at[way], x_recv.at[way, step - 1, part], "sp", ahead(way),
        )

    def shift_copy(way, step):
        block = z - (step - 1) if way == 0 else z + (step - 1)
        there = shifts_ref.at[block]
        return remote(
            shift_ref if step == 1 else there, there,
            s_send.at[way], s_recv.at[way, step - 1], "sp", ahead(way),
        )

    def comes(way, step):
        return z >= step if way == 0 else z + step < sp

    def sends(way, step):
        return jnp.logical_and(onward(way), comes(way, step - 1))

    def forward(way, step, part):
        block = z - step if way == 0 else z + step
        piece = pl.ds(part * (rows // parts), rows // parts)
        there = xs.at[block, piece, slot]
        return remote(
            x_ref.at[piece, :] if step == 0 else there, there,
            f_send.at[0], f_recv.at[way * (sp - 1) + step], "tp", lax.rem(t + 1, tp),
        )

    def w_copy(side, i):
        return remote(
            w_src(i), w_at(i, f), w_send.at[0], w_recv.at[side, i], "fs", near[side]
        )

    def w_relay(side, i):
        part = depth // 2
        start = pl.multiple_of(near[side] * depth + side * part, part)
        there = ws.at[pl.ds(start, part), pl.ds(i * cols, cols)]
        return remote(
            there, there, w_send.at[0], r_recv.at[i // 3], "fs", near[1 - side]
        )

    for part in range(parts):
        for way in range(2):
            @pl.when(onward(way))
            def _():
                x_copy(way, 1, part).start()
                if part == 0:
                    shift_copy(way, 1).start()
    for i in delta_kinds:
        for side in range(2):
            w_copy(side, i).start()
    for part in range(parts):
        forward(0, 0, part).start()

    def relay(i):
        for side in range(2):
            w_copy(side, i).wait_recv()
            w_relay(side, i).start()

    def arrive(step, part):
        for way in range(2):
            @pl.when(comes(way, step))
            def _():
                x_copy(way, step, part).wait_recv()
                forward(way, step, part).start()
                if step + 1 < sp:
                    @pl.when(onward(way))
                    def _():
                        x_copy(way, step + 1, part).start()
                if part == 0:
                    shift_copy(way, step).wait_recv()
                    if step + 1 < sp:
                        @pl.when(onward(way))
                        def _():
                            shift_copy(way, step + 1).start()

    below = lax.broadcasted_iota(jnp.int32, (rows, rows), 0)
    across = lax.broadcasted_iota(jnp.int32, (rows, rows), 1)
    after[:, :rows] = jnp.where(below > across, 1.0, 0.0).astype(jnp.bfloat16)
    after[:, rows:] = jnp.ones((rows, cols), jnp.bfloat16)
    acc[...] = jnp.zeros_like(acc)
    later[...] = jnp.zeros_like(later)
    memory_ref[...] = jnp.zeros_like(memory_ref)
    early = [(step, part) for step in range(1, sp - 1) for part in range(parts)]
    relay(delta_kinds[0])
    arrive(*early[0])
    for i in delta_kinds[1:]:
        relay(i)
    for i in stick_kinds:
        for side in range(2):
            w_copy(side, i).start()
    for c in late:
        c.start()
    for step, part in early[1:parts]:
        arrive(step, part)
    for c in local:
        c.wait()
    own_w = ws.at[pl.ds(pl.multiple_of(f * depth, depth), depth), :]
    pltpu.make_async_copy(own_w, own_w, l_sem.at[10]).wait()
    gate_all[...] = jnp.concatenate(
        [gate_w[0].astype(jnp.float32), gate_w[1].astype(jnp.float32)], axis=0
    ).astype(jnp.bfloat16)
    def all_sent(ref, sem):
        remote(ref, ref, sem, sem, "tp", lax.rem(t + 1, tp)).wait_send()

    def all_came(ref, sem):
        remote(ref, ref, sem, sem, "tp", lax.rem(t + 1, tp)).wait_recv()

    def block_came(way, step):
        all_came(xs.at[z, :, slot], f_recv.at[way * (sp - 1) + step])

    block_came(0, 0)

    def relayed(kinds):
        first = kinds[0] * cols
        all_came(ws.at[pl.ds(0, depth), pl.ds(first, len(kinds) * cols)], r_recv.at[kinds[0] // 3])

    relayed(delta_kinds)

    size = offset_ref.shape[0] // sp
    sb_size = cols // size
    scale = sb_size ** (-0.5)
    tile = rows // 2

    def at_block(b, start=0, extent=rows):
        return pl.ds(pl.multiple_of(b * rows + start, extent), extent)

    def pair(i, j):
        for part in range(rows // tile):
            mine = at_block(i, part * tile, tile)
            q = proj[0, mine, :]
            keys, values = proj[1, at_block(j), :], proj[2, at_block(j), :]
            lane = lax.broadcasted_iota(jnp.int32, (tile, cols), 1)
            query = jnp.concatenate(
                [jnp.where(lane // sb_size == h, q, jnp.zeros_like(q)) for h in range(size)], axis=0
            )
            score = dot_f32(query, keys, ((1,), (1,)))
            score = jnp.concatenate(
                [
                    score[h * tile : (h + 1) * tile] * scale + offset_ref[z * size + h]
                    for h in range(size)
                ],
                axis=0,
            )
            skip = jnp.maximum(score, jnp.log(1.0 + jnp.exp(jnp.minimum(score, 80.0))))
            weight = score - skip
            seen = across[:tile] < below[:tile] + (part * tile + (i - j) * rows)
            seen = jnp.concatenate([seen] * size, axis=0)
            skip = jnp.where(seen, skip, 0.0)
            sums = dot_f32(skip.astype(jnp.bfloat16), after[...])
            weight = jnp.where(seen, jnp.exp(weight - sums[:, :rows]), 0.0)
            out = dot_f32(weight.astype(jnp.bfloat16), values)
            mixed, total = out[:tile], sums[:tile, rows:]
            for h in range(1, size):
                at = slice(h * tile, (h + 1) * tile)
                mixed = jnp.where(lane // sb_size == h, out[at], mixed)
                total = jnp.where(lane // sb_size == h, sums[at, rows:], total)
            passed = later[mine, :]
            acc[mine, :] = acc[mine, :] + mixed * jnp.exp(-passed)
            later[mine, :] = passed + total

    span = BLOCK
    duo = 2 * span
    blocks = rows // span
    width = GDN_DIM
    seg_row = lax.broadcasted_iota(jnp.int32, (rows, rows), 0)
    seg_col = lax.broadcasted_iota(jnp.int32, (rows, rows), 1)
    together = seg_row // span == seg_col // span
    upto = jnp.where(jnp.logical_and(together, seg_row <= seg_col), 1.0, 0.0).astype(jnp.bfloat16)
    beyond_it = jnp.where(jnp.logical_and(together, seg_row > seg_col), 1.0, 0.0).astype(
        jnp.bfloat16
    )
    prow = lax.broadcasted_iota(jnp.int32, (span, duo), 0)
    plane = lax.broadcasted_iota(jnp.int32, (span, duo), 1)
    first = plane < span
    pcol = jnp.where(first, plane, plane - span)
    inclusive, strictly = pcol <= prow, pcol < prow
    unit = jnp.where(pcol == prow, 1.0, 0.0)
    diagonal = lax.broadcasted_iota(jnp.int32, (width, width), 0) == lax.broadcasted_iota(
        jnp.int32, (width, width), 1
    )
    eighth = lax.broadcasted_iota(jnp.int32, (8, rows), 0)

    def silu(a):
        return a * (1.0 / (1.0 + jnp.exp(-a)))

    def unit_of(a):
        return a * lax.rsqrt(jnp.sum(a * a, axis=-1, keepdims=True) + NORM_EPS)

    def apart(a):
        lanes = lax.broadcasted_iota(jnp.int32, a.shape, 1) < span
        zero = jnp.zeros_like(a)
        return jnp.concatenate([jnp.where(lanes, a, zero), jnp.where(lanes, zero, a)], axis=0)

    def squared(left, power):
        high, low = halves(power)
        lhigh, llow = halves(left)
        return folded(
            dot_f32(
                jnp.concatenate([lhigh, llow], axis=1), wide_rhs(apart(high), apart(low), 1)
            )
        )

    def prepare(b, dq, dk, dv):
        gates[...] = dot_f32(gate_all[...], xs[b], ((1,), (1,)))
        pre = gates[pl.ds(z, 1), :]
        write = gates[pl.ds(heads + z, 1), :] + write_bias_ref[z]
        rate = jnp.exp(jnp.full((1, rows), decay_scale_ref[z], jnp.float32))
        soft = jnp.maximum(pre, 0.0) + jnp.log(1.0 + jnp.exp(-jnp.abs(pre)))
        decay = shifts_ref[b, pl.ds(z, 1), :] - rate * soft
        strength = 1.0 / (1.0 + jnp.exp(-write))
        d1 = decay.astype(jnp.bfloat16).astype(jnp.float32)
        d2 = (decay - d1).astype(jnp.bfloat16).astype(jnp.float32)
        d3 = decay - d1 - d2
        three = jnp.where(
            eighth == 0, d1, jnp.where(eighth == 1, d2, jnp.where(eighth == 2, d3, 0.0))
        ).astype(jnp.bfloat16)
        cum_row = jnp.sum(dot_f32(three, upto), axis=0, keepdims=True)
        rest_row = jnp.sum(dot_f32(three, beyond_it), axis=0, keepdims=True)
        stack = jnp.where(
            eighth == 0, strength,
            jnp.where(
                eighth == 1, jnp.exp(cum_row),
                jnp.where(eighth == 2, jnp.exp(rest_row), cum_row),
            ),
        )
        columns = stack.T
        s_col, grow, damp, cum = (columns[:, n : n + 1] for n in range(4))
        q = unit_of(silu(dq)) * width ** (-0.5)
        k = unit_of(silu(dk))
        v = silu(dv)
        boosted = q * grow
        damped = k * damp
        right = jnp.concatenate([v * s_col, k * (s_col * grow)], axis=1)
        kh, kl = halves(k)
        qh, ql = halves(q)
        work = []
        for duo_at in range(rows // duo):
            lo = duo_at * duo
            here = slice(lo, lo + duo)
            left = jnp.concatenate(
                [
                    jnp.concatenate([kh[here], kl[here]], axis=1),
                    jnp.concatenate([qh[here], ql[here]], axis=1),
                ],
                axis=0,
            )
            gram = folded(
                dot_f32(left, wide_rhs(kh[here], kl[here], 0), ((1,), (1,)))
            )
            spread = (
                jnp.where(first, cum[lo : lo + span], cum[lo + span : lo + duo])
                - cum_row[:, here]
            )
            table = jnp.where(inclusive, jnp.exp(jnp.where(inclusive, spread, 0.0)), 0.0)
            scale_col = jnp.where(first, s_col[lo : lo + span], s_col[lo + span : lo + duo])
            near_k = jnp.where(first, gram[:span], gram[span:duo])
            near_q = jnp.where(first, gram[duo : duo + span], gram[duo + span :])
            strict = jnp.where(strictly, near_k * table * scale_col, 0.0)
            work.append([unit - strict, strict, near_q * table])
        yield
        for w in work:
            w[1] = squared(w[1], w[1])
        levels = max(1, (span - 1).bit_length()) - 1
        for level in range(levels):
            if level == levels // 2:
                yield
            for w in work:
                if level + 1 < levels:
                    both = squared(jnp.concatenate([w[1], w[0]], axis=0), w[1])
                    w[1], w[0] = both[:span], w[0] + both[span:]
                else:
                    w[0] = w[0] + squared(w[0], w[1])
        yield
        for duo_at, (inverse, _, inside) in enumerate(work):
            lo = duo_at * duo
            here = slice(lo, lo + duo)
            ih, il = (apart(a) for a in halves(inverse))
            rh, rl = halves(right[here])
            solved = dot_f32(
                jnp.concatenate([ih, il], axis=1), jnp.concatenate([rh, rh], axis=0)
            ) + dot_f32(ih, rl)
            lh, ll = (
                apart(a) for a in halves(jnp.concatenate([damped[here].T, inside], axis=0))
            )
            sh, sl = halves(solved)
            made = dot_f32(
                jnp.concatenate([lh, ll], axis=1), jnp.concatenate([sh, sh], axis=0)
            ) + dot_f32(lh, sl)
            for side in range(2):
                at = lo + side * span
                mine = made[side * (width + span) : (side + 1) * (width + span)]
                n = b * blocks + 2 * duo_at + side
                keep = grow[at + span - 1 : at + span]
                step_map = jnp.where(diagonal, keep, 0.0) - mine[:width, width:]
                query = boosted[at : at + span] - mine[width:, width:]
                high, low = halves(jnp.concatenate([step_map, query], axis=0))
                maps[n, :, :width] = high
                maps[n, :, width:] = low
                adds[n] = mine[:, :width]

    def give(which, out, target):
        here = target.at[:, pl.ds(pl.multiple_of(z * cols, cols), cols)]

        def send(g, k):
            return remote(
                out.at[at_block(g), :], here,
                a_send.at[which], a_recv.at[which], "sp", g,
            )

        def started(g):
            for k in range(1, sp):
                @pl.when(lax.rem(z + k, sp) == g)
                def _():
                    send(lax.rem(z + k, sp), k).start()

        def came():
            all_came(out.at[pl.ds(0, (sp - 1) * rows), :], a_recv.at[which])

        return started, came

    stick_started, stick_came = give(0, stick_out, sticks)
    delta_started, delta_came = give(1, delta_out, deltas)

    shorter = jnp.minimum(z, sp - 1 - z)
    down_last = z > sp - 1 - z

    def place(n):
        both = n <= 2 * shorter
        way_n = jnp.where(both, lax.rem(n + 1, 2), jnp.where(down_last, 0, 1))
        step_n = jnp.where(n == 0, 0, jnp.where(both, (n + 1) // 2, n - shorter))
        down = jnp.logical_and(way_n == 0, n > 0)
        return way_n, step_n, down, jnp.where(down, z - step_n, z + step_n)

    last_way = jnp.logical_or(z == 0, z == sp - 1)

    def block_ready(n):
        way_n, step_n, down, b = place(n)
        for step in range(1, sp):
            for way in range(2):
                @pl.when(jnp.logical_and(step_n == step, way_n == way))
                def _():
                    block_came(way, step)
        return b

    def delta_block(b):
        drows = dot_f32(xs[b], ws[:, 3 * cols :]).astype(jnp.bfloat16).astype(jnp.float32)
        return prepare(b, drows[:, :cols], drows[:, cols : 2 * cols], drows[:, 2 * cols :])

    def stick_project(n):
        b = stick_place(n)[1]
        out = dot_f32(xs[b], ws[:, : 3 * cols]).astype(jnp.bfloat16)
        for i in range(3):
            proj[i, at_block(b), :] = out[:, i * cols : (i + 1) * cols]

    def stick_place(n):
        down = n > sp - 1 - z
        return down, jnp.where(down, sp - 1 - n, z + n)

    def settle(i):
        stick_out[at_block(i), :] = acc[at_block(i), :].astype(jnp.bfloat16)

    def stick_pair(p):
        n = sum(((p >= e * (e + 1) // 2) * 1 for e in range(1, sp)), 0)
        r = p - n * (n + 1) // 2
        down, b = stick_place(n)
        other = jnp.where(z == sp - 1, b + r, sp - r)
        i = jnp.where(jnp.logical_and(down, r > 0), other, b)
        j = jnp.where(down, b, b - r)
        pair(i, j)

        @pl.when(j == 0)
        def _():
            settle(i)
            stick_started(i)

    def plain_delta(n, c):
        @pl.when(n == 1)
        def _():
            relay(stick_kinds[0])
        for _ in delta_block(block_ready(n)):
            pass
        return c

    def walk_groups(start, stop):
        def group(g, c):
            @pl.when(g > start)
            def _():
                delta_started(g - 1)
            memory = memory_ref[...]
            for n in range(blocks):
                memory = walk(g * blocks + n, memory)
            memory_ref[...] = memory
            return c

        lax.fori_loop(start, stop, group, 0)
        delta_started(stop - 1)

    def walk(n, memory):
        high, low = halves(memory)
        new = folded(dot_f32(maps[n], wide_rhs(high, low, 1))) + adds[n]
        made = new[width:]
        made = made * lax.rsqrt(jnp.mean(made * made, axis=-1, keepdims=True) + NORM_EPS)
        at = pl.ds(pl.multiple_of(n * span, span), span)
        delta_out[at, :] = (made * gain_ref[...]).astype(delta_out.dtype)
        return new[:width]

    last_way = jnp.logical_or(z == 0, z == sp - 1)

    lax.fori_loop(0, 2, plain_delta, 0)
    for c in early[parts:-1]:
        arrive(*c)
    for i in stick_kinds[1:]:
        relay(i)
    arrive(*early[-1])
    block_ready(2)
    relayed(stick_kinds)

    @pl.when(jnp.logical_not(last_way))
    def _():
        block_ready(sp - 1)

    def project_each(n, c):
        stick_project(n)
        return c

    lax.fori_loop(0, jnp.where(last_way, sp - 1, sp), project_each, 0)
    before = sp * (sp - 1) // 2

    def stream(start, stop):
        def one(p, c):
            stick_pair(p)
            return c

        lax.fori_loop(start, stop, one, 0)

    def both(n, c):
        final = jnp.logical_and(last_way, n == sp - 1)

        @pl.when(final)
        def _():
            arrive(sp - 1, 0)
            stream(sp * (sp - 3), before - 1)
            arrive(sp - 1, 1)
            arrive(sp - 1, 2)
            stream(before - 1, before)

            @pl.when(z == 0)
            def _():
                walk_groups(0, sp - 2)
            for part in range(3, parts):
                arrive(sp - 1, part)

            @pl.when(z == 0)
            def _():
                walk_groups(sp - 2, sp - 1)
            for way in range(2):
                @pl.when(comes(way, sp - 1))
                def _():
                    block_came(way, sp - 1)
            stick_project(sp - 1)
        stages = delta_block(place(n)[3])
        first = jnp.where(final, before, (n - 2) * sp)
        for u in range(sp):
            next(stages, None)
            stick_pair(first + u)
        return c

    lax.fori_loop(2, sp, both, 0)

    @pl.when(jnp.logical_not(last_way))
    def _():
        stream(sp * (sp - 2), before + sp)

    walk_groups(jnp.where(z == 0, sp - 1, 0), sp)

    mine_z = pl.ds(pl.multiple_of(z * rows, rows), rows)
    lanes = pl.ds(pl.multiple_of(z * cols, cols), cols)
    sticks[:, lanes] = stick_out[mine_z, :]
    deltas[:, lanes] = delta_out[mine_z, :]
    for c in late:
        c.wait()
    stick_came()
    chunks, wide = outgoing.shape[0], outgoing.shape[2]
    share = rows // tp
    for c in range(chunks):
        columns = slice(c * wide, (c + 1) * wide)
        partial[:, columns] = dot_f32(sticks[...], sw_ref[:, columns])
    delta_came()
    mine = pl.ds(pl.multiple_of(t * share, share), share)
    partner = lax.rem(t + 1, tp)
    theirs = pl.ds(pl.multiple_of(partner * share, share), share)

    def finish(which, c):
        columns = slice(c * wide, (c + 1) * wide)
        return (
            partial[which, columns] + dot_f32(deltas[which, :], dw_ref[:, columns])
        ).astype(jnp.bfloat16)

    swaps = [
        remote(
            outgoing.at[c], incoming.at[:, c * wide : (c + 1) * wide],
            c_sem.at[0], c_sem.at[1], "tp", partner,
        )
        for c in range(chunks)
    ]
    for c in range(chunks):
        outgoing[c] = finish(theirs, c)
        if c > 0:
            swaps[c - 1].start()
    for c in range(chunks):
        own[:, c * wide : (c + 1) * wide] = finish(mine, c)
        if c == 0:
            swaps[chunks - 1].start()
    all_came(incoming, c_sem.at[1])
    all_sent(incoming, c_sem.at[0])
    all_sent(ws.at[pl.ds(0, 3 * depth), :], w_send.at[0])
    all_sent(xs.at[:, :, slot], f_send.at[0])
    for which, out in enumerate((stick_out, delta_out)):
        all_sent(out.at[pl.ds(0, (sp - 1) * rows), :], a_send.at[which])
    for c in range(sp):
        @pl.when(z == c)
        def _():
            for way, passed in enumerate((c + 1 if c + 1 < sp else 0, sp - c if c > 0 else 0)):
                if passed:
                    all_sent(xs.at[pl.ds(0, passed), :, slot], x_send.at[way])
                    all_sent(shifts_ref.at[pl.ds(0, passed)], s_send.at[way])


ANYWHERE = pl.BlockSpec(memory_space=pltpu.HBM)
ON_CORE = pl.BlockSpec(memory_space=pltpu.VMEM)


def on_device_heads(
    hidden_in, sb_query_w, sb_key_w, sb_value_w, sb_offset,
    delta_query_w, delta_key_w, delta_value_w, decay_w, write_w, write_bias,
    decay_log_scale, decay_shift, head_gain, sb_out_w, delta_out_w,
):
    sp, fs, tp = lax.axis_size("sp"), lax.axis_size("fs"), lax.axis_size("tp")
    rows, half = hidden_in.shape[1:]
    width = half * tp
    length = rows * sp
    heads = decay_log_scale.shape[0]
    cols = sb_query_w.shape[1] // sp
    parts, chunks = 4, 4
    share = rows // tp
    blocks = length // BLOCK
    dma = pltpu.SemaphoreType.DMA
    bf16, f32 = jnp.bfloat16, jnp.float32
    own, incoming = pl.pallas_call(
        layer_kernel,
        name="layer",
        out_shape=(pltpu.VMEM((share, width), bf16),) * 2,
        in_specs=[ANYWHERE] * 16,
        out_specs=(ON_CORE,) * 2,
        scratch_shapes=[
            pltpu.SMEM(sb_offset.shape, f32),
            pltpu.SMEM(decay_log_scale.shape, f32),
            pltpu.SMEM(write_bias.shape, f32),
            pltpu.VMEM((1, head_gain.shape[0]), f32),
            pltpu.VMEM((sp, rows, width), bf16),
            pltpu.VMEM((width, 6 * cols), bf16),
            pltpu.VMEM((2, heads, width), bf16),
            pltpu.VMEM((2 * heads, width), bf16),
            pltpu.VMEM((2 * heads, rows), f32),
            pltpu.VMEM((sp, heads, rows), f32),
            pltpu.VMEM((rows, rows + cols), bf16),
            pltpu.VMEM((3, length, cols), bf16),
            pltpu.VMEM((length, cols), f32),
            pltpu.VMEM((length, cols), f32),
            pltpu.VMEM((cols, cols), f32),
            pltpu.VMEM((blocks, cols + BLOCK, 2 * cols), bf16),
            pltpu.VMEM((blocks, cols + BLOCK, cols), f32),
            pltpu.VMEM((length, cols), bf16),
            pltpu.VMEM((length, cols), bf16),
            pltpu.VMEM((rows, cols * sp), bf16),
            pltpu.VMEM((rows, cols * sp), bf16),
            pltpu.VMEM(sb_out_w.shape, bf16),
            pltpu.VMEM(delta_out_w.shape, bf16),
            pltpu.VMEM((rows, width), f32),
            pltpu.VMEM((chunks, share, width // chunks), bf16),
            dma((2,)), dma((2, sp - 1, parts)), dma((1,)), dma((2 * sp - 1,)),
            dma((1,)), dma((2, 6)), dma((2,)), dma((2,)), dma((2, sp - 1)), dma((11,)),
            dma((2,)), dma((2,)), dma((2,)),
        ],
        compiler_params=pltpu.CompilerParams(
            collective_id=0, has_side_effects=True,
            vmem_limit_bytes=ALL_VMEM - 5 * share * width,
        ),
    )(
        sb_offset, decay_log_scale, write_bias,
        hidden_in.reshape(rows, half), sb_query_w, sb_key_w, sb_value_w,
        delta_query_w, delta_key_w, delta_value_w, decay_w.T, write_w.T,
        decay_shift.reshape(heads, rows), head_gain.reshape(1, -1), sb_out_w, delta_out_w,
    )
    result = (own.astype(f32) + incoming.astype(f32)).astype(bf16)
    return result.reshape(1, share, width)


def on_device(*inputs):
    delta_heads = inputs[11].shape[0]
    square = lax.axis_size("sp") == lax.axis_size("fs") == 4 and lax.axis_size("tp") == 2
    if square and delta_heads == lax.axis_size("sp") and inputs[4].shape[0] % delta_heads == 0:
        return on_device_heads(*inputs)
    return on_device_split(*inputs)


def solution(mesh):
    return jax.shard_map(
        on_device,
        mesh=mesh,
        in_specs=(
            P("fs", "sp", "tp"),
            P("fs", "tp"),
            P("fs", "tp"),
            P("fs", "tp"),
            P("tp"),
            P("fs", "tp"),
            P("fs", "tp"),
            P("fs", "tp"),
            P(None, "tp"),
            P(None, "tp"),
            P("tp"),
            P("tp"),
            P("fs", "tp", "sp"),
            P(),
            P("tp", None),
            P("tp", None),
        ),
        out_specs=P("fs", ("sp", "tp"), None),
        check_vma=False,
    )
```

```python
import jax
import jax.numpy as jnp
from jax import lax
from jax.experimental import pallas as pl
from jax.experimental.pallas import tpu as pltpu
from jax.sharding import PartitionSpec as P

MESH = pl.DeviceIdType.MESH
ALL_VMEM = 67043328

SB_DIM = 64
GDN_DIM = 128
BLOCK = 64


EXACT_MATMUL = lax.Precision.HIGHEST
NORM_EPS = 1e-06


def carried_in(value, axis, combine, identity):
    devices, index = (lax.axis_size(axis), lax.axis_index(axis))
    everything = jax.tree.map(
        lambda part, kind: lax.all_gather(part.astype(kind), axis),
        value,
        (jnp.bfloat16, jnp.bfloat16),
    )
    start = jax.tree.map(
        lambda part, zero: jnp.broadcast_to(jnp.asarray(zero, part.dtype), part.shape),
        value,
        identity,
    )

    def lap(k, before):
        reached = k < index
        new = combine(
            before, jax.tree.map(lambda part, own: part[k].astype(own.dtype), everything, value)
        )
        return jax.tree.map(lambda a, b: jnp.where(reached, a, b), new, before)

    return lax.fori_loop(0, devices, lap, start)


def unit_lower_inverse(strict_part):
    order_size = strict_part.shape[-1]
    powered = strict_part
    inverse = jnp.eye(order_size, dtype=strict_part.dtype) - strict_part
    for repeat_number in range(max(1, (order_size - 1).bit_length()) - 1):
        powered = jnp.einsum("...ij,...jk->...ik", powered, powered, precision=EXACT_MATMUL)
        inverse = inverse + jnp.einsum(
            "...ij,...jk->...ik", inverse, powered, precision=EXACT_MATMUL
        )
    return inverse


def to_blocks(row_data, block_span):
    blocks_count = row_data.shape[0] // block_span
    shaped = row_data.reshape((blocks_count, block_span) + row_data.shape[1:])
    return jnp.swapaxes(shaped, 1, 2)


def from_blocks(blocked):
    swapped = jnp.swapaxes(blocked, 1, 2)
    return swapped.reshape((-1,) + swapped.shape[2:])


def unit_rows(vectors):
    return vectors * lax.rsqrt(jnp.sum(vectors * vectors, axis=-1, keepdims=True) + NORM_EPS)


def delta_inputs(
    query_proj,
    key_proj,
    value_proj,
    decay_pre,
    write_pre,
    write_bias,
    decay_log_scale,
    shift_rows,
    head_count,
    head_size,
):
    query_act = jax.nn.silu(query_proj.astype(jnp.float32)).reshape(-1, head_count, head_size)
    key_act = jax.nn.silu(key_proj.astype(jnp.float32)).reshape(-1, head_count, head_size)
    value_rows = jax.nn.silu(value_proj.astype(jnp.float32)).reshape(-1, head_count, head_size)
    queries = unit_rows(query_act) * head_size ** (-0.5)
    key_rows = unit_rows(key_act)
    log_decay = -jnp.exp(decay_log_scale) * jax.nn.softplus(decay_pre) + shift_rows
    strength = jax.nn.sigmoid(write_pre + write_bias)
    return (queries, key_rows, value_rows, log_decay, strength)


def delta_prepare(queries, key_rows, value_rows, log_decay, strength):
    block_span = queries.shape[2]
    cumulative = jnp.cumsum(log_decay, axis=-1)
    row_place = lax.broadcasted_iota(jnp.int32, (block_span, block_span), 0)
    col_place = lax.broadcasted_iota(jnp.int32, (block_span, block_span), 1)
    inclusive = col_place <= row_place
    strictly = col_place < row_place
    spread = cumulative[..., :, None] - cumulative[..., None, :]
    decay_table = jnp.where(inclusive, jnp.exp(jnp.where(inclusive, spread, 0.0)), 0.0)
    keys_beta = key_rows * strength[..., None]
    lower_part = jnp.where(
        strictly,
        jnp.einsum("nhik,nhjk->nhij", keys_beta, key_rows, precision=EXACT_MATMUL) * decay_table,
        0.0,
    )
    inverse = unit_lower_inverse(lower_part)
    growth = jnp.exp(cumulative)
    state_updates = jnp.einsum(
        "nhij,nhjv->nhiv", inverse, value_rows * strength[..., None], precision=EXACT_MATMUL
    )
    erase_term = jnp.einsum(
        "nhij,nhjk->nhik", inverse, keys_beta * growth[..., None], precision=EXACT_MATMUL
    )
    inside_block = (
        jnp.einsum("nhik,nhjk->nhij", queries, key_rows, precision=EXACT_MATMUL) * decay_table
    )
    boosted_query = queries * growth[..., None]
    damped_keys = key_rows * jnp.exp(cumulative[..., -1:] - cumulative)[..., None]
    decay_per_block = jnp.exp(cumulative[..., -1])
    return (state_updates, erase_term, inside_block, boosted_query, damped_keys, decay_per_block)


def delta_step(memory_state, inputs):
    state_updates, erase_term, inside_block, boosted_query, damped_keys, decay_per_block = inputs
    fixed_values = state_updates - jnp.einsum(
        "mzq,mqc->mzc", erase_term, memory_state, precision=EXACT_MATMUL
    )
    produced_rows = jnp.einsum(
        "mzq,mqc->mzc", boosted_query, memory_state, precision=EXACT_MATMUL
    ) + jnp.einsum("efq,eqn->efn", inside_block, fixed_values, precision=EXACT_MATMUL)
    memory_state = memory_state * decay_per_block[:, None, None] + jnp.einsum(
        "wam,waz->wmz", damped_keys, fixed_values, precision=EXACT_MATMUL
    )
    return (memory_state, produced_rows)


def transition_step(carried, inputs):
    memory_state, transfer = carried
    state_updates, erase_term, inside_block, boosted_query, damped_keys, decay_per_block = inputs
    fixed_values = state_updates - jnp.einsum(
        "mzq,mqc->mzc", erase_term, memory_state, precision=EXACT_MATMUL
    )
    coupling = jnp.einsum("hik,hil->hkl", damped_keys, erase_term, precision=EXACT_MATMUL)
    memory_state = memory_state * decay_per_block[:, None, None] + jnp.einsum(
        "wam,waz->wmz", damped_keys, fixed_values, precision=EXACT_MATMUL
    )
    transfer = transfer * decay_per_block[:, None, None] - jnp.einsum(
        "hkl,hlm->hkm", coupling, transfer, precision=EXACT_MATMUL
    )
    return ((memory_state, transfer), None)


def compose(prior_blocks, following_blocks):
    joined_map = jnp.einsum(
        "hkl,hlm->hkm", following_blocks[0], prior_blocks[0], precision=EXACT_MATMUL
    )
    joined_state = (
        jnp.einsum("djo,dog->djg", following_blocks[0], prior_blocks[1], precision=EXACT_MATMUL)
        + following_blocks[1]
    )
    return (joined_map, joined_state)


def stick_block(queries, key_rows, value_rows, query_place, key_place, offsets):
    scale_factor = queries.shape[-1] ** (-0.5)
    scores = (
        jnp.einsum("qhd,khd->hqk", queries, key_rows, preferred_element_type=jnp.float32)
        * scale_factor
        + offsets[:, None, None]
    )
    visible = key_place[None, :] < query_place[:, None]
    skipped = jnp.where(visible, jax.nn.log_sigmoid(-scores), 0.0)
    beyond = lax.cumsum(skipped, axis=2, reverse=True) - skipped
    weights = jnp.where(visible, jnp.exp(jax.nn.log_sigmoid(scores) + beyond), 0.0).astype(
        jnp.bfloat16
    )
    partial_value = jnp.einsum(
        "hqk,khd->qhd", weights, value_rows, preferred_element_type=jnp.float32
    )
    return (partial_value, jnp.sum(skipped, axis=2).T)


def stick_combine(partials, totals):
    beyond = jnp.cumsum(totals[::-1], axis=0)[::-1] - totals
    return jnp.sum(partials * jnp.exp(beyond)[..., None], axis=0)


def on_device_split(
    hidden_in,
    sb_query_w,
    sb_key_w,
    sb_value_w,
    sb_offset,
    delta_query_w,
    delta_key_w,
    delta_value_w,
    decay_w,
    write_w,
    write_bias,
    decay_log_scale,
    decay_shift,
    head_gain,
    sb_out_w,
    delta_out_w,
):
    token_rows = hidden_in.shape[1]
    local_in = hidden_in.reshape(token_rows, hidden_in.shape[2])
    gathered = (
        lax.all_gather(sb_query_w, "fs", axis=0, tiled=True),
        lax.all_gather(sb_key_w, "fs", axis=0, tiled=True),
        lax.all_gather(sb_value_w, "fs", axis=0, tiled=True),
        lax.all_gather(delta_query_w, "fs", axis=0, tiled=True),
        lax.all_gather(delta_key_w, "fs", axis=0, tiled=True),
        lax.all_gather(delta_value_w, "fs", axis=0, tiled=True),
    )
    in_weights = tuple(gathered) + (decay_w, write_w)
    portion = lax.all_gather(local_in, "tp", axis=1, tiled=True)
    projected = tuple(
        (jnp.dot(portion, weight, preferred_element_type=jnp.float32) for weight in in_weights)
    )
    sb_heads = sb_offset.shape[0]
    delta_heads = decay_log_scale.shape[0]
    sb_query = projected[0].astype(jnp.bfloat16).reshape(token_rows, sb_heads, SB_DIM)
    sb_keys = projected[1].astype(jnp.bfloat16)
    sb_values = projected[2].astype(jnp.bfloat16)
    shift_rows = decay_shift.reshape(delta_heads, token_rows).T
    queries, key_rows, value_rows, log_decay, strength = delta_inputs(
        projected[3].astype(jnp.bfloat16),
        projected[4].astype(jnp.bfloat16),
        projected[5].astype(jnp.bfloat16),
        projected[6],
        projected[7],
        write_bias,
        decay_log_scale,
        shift_rows,
        delta_heads,
        GDN_DIM,
    )
    prepared = delta_prepare(
        to_blocks(queries, BLOCK),
        to_blocks(key_rows, BLOCK),
        to_blocks(value_rows, BLOCK),
        to_blocks(log_decay, BLOCK),
        to_blocks(strength, BLOCK),
    )
    identity_map = jnp.broadcast_to(
        jnp.eye(GDN_DIM, dtype=jnp.float32), (delta_heads, GDN_DIM, GDN_DIM)
    )
    empty_state = jnp.zeros((delta_heads, GDN_DIM, GDN_DIM), jnp.float32)
    (local_end, local_map), unused_out = lax.scan(
        transition_step, (empty_state, identity_map), prepared
    )
    own_first = lax.axis_index("sp") * token_rows
    query_place = own_first + lax.iota(jnp.int32, token_rows)
    sp_count = lax.axis_size("sp")
    slot_out = jnp.zeros((sp_count, token_rows, sb_heads, SB_DIM), jnp.float32)
    slot_total = jnp.zeros((sp_count, token_rows, sb_heads), jnp.float32)

    def absorb(slot_arrays, address_portion, value_part, shard_first):

        def active(current):
            partial_value, totals = stick_block(
                sb_query,
                address_portion.reshape(token_rows, sb_heads, SB_DIM),
                value_part.reshape(token_rows, sb_heads, SB_DIM),
                query_place,
                shard_first + lax.iota(jnp.int32, token_rows),
                sb_offset,
            )
            slot_index = shard_first // token_rows
            return (
                lax.dynamic_update_index_in_dim(current[0], partial_value, slot_index, 0),
                lax.dynamic_update_index_in_dim(current[1], totals, slot_index, 0),
            )

        def inactive(current):
            return current

        usable = jnp.logical_and(shard_first >= 0, shard_first <= own_first)
        return lax.cond(usable, active, inactive, slot_arrays)

    key_block = lax.all_gather(sb_keys, "sp", axis=0, tiled=True)
    value_block = lax.all_gather(sb_values, "sp", axis=0, tiled=True)

    def per_shard(shard_number, current):
        row_begin = shard_number * token_rows
        return absorb(
            current,
            lax.dynamic_slice_in_dim(key_block, row_begin, token_rows, 0),
            lax.dynamic_slice_in_dim(value_block, row_begin, token_rows, 0),
            row_begin,
        )

    slot_arrays = lax.fori_loop(
        0, key_block.shape[0] // token_rows, per_shard, (slot_out, slot_total)
    )
    unused_map, incoming = carried_in(
        (local_map, local_end), "sp", compose, (identity_map, empty_state)
    )
    sb_mixed = (
        stick_combine(slot_arrays[0], slot_arrays[1])
        .astype(jnp.bfloat16)
        .reshape(token_rows, sb_heads * SB_DIM)
    )
    unused_end, produced_rows = lax.scan(delta_step, incoming, prepared)
    produced_rows = from_blocks(produced_rows)
    normed = (
        produced_rows
        * lax.rsqrt(jnp.mean(produced_rows * produced_rows, axis=-1, keepdims=True) + NORM_EPS)
        * head_gain
    )
    delta_mixed = normed.astype(jnp.bfloat16).reshape(token_rows, delta_heads * GDN_DIM)
    result = lax.psum_scatter(
        (
            jnp.dot(sb_mixed, sb_out_w, preferred_element_type=jnp.float32)
            + jnp.dot(delta_mixed, delta_out_w, preferred_element_type=jnp.float32)
        ).astype(jnp.bfloat16),
        "tp",
        scatter_dimension=0,
        tiled=True,
    ).astype(jnp.float32)
    return result.astype(jnp.bfloat16).reshape(1, result.shape[0], result.shape[1])


def remote(src, dst, send, recv, axis, index):
    return pltpu.make_async_remote_copy(
        src_ref=src, dst_ref=dst, send_sem=send, recv_sem=recv,
        device_id={axis: index}, device_id_type=MESH,
    )


def greet(axes):
    barrier = pltpu.get_barrier_semaphore()
    count = 0
    for axis in axes:
        size, me = lax.axis_size(axis), lax.axis_index(axis)
        for k in range(1, size):
            pl.semaphore_signal(
                barrier, inc=1, device_id={axis: lax.rem(me + k, size)}, device_id_type=MESH
            )
            count += 1
    pl.semaphore_wait(barrier, count)


def halves(a):
    high = a.astype(jnp.bfloat16)
    return high, (a - high.astype(jnp.float32)).astype(jnp.bfloat16)


def dot_f32(a, b, dims=((1,), (0,))):
    return lax.dot_general(a, b, (dims, ((), ())), preferred_element_type=jnp.float32)


def wide_rhs(high, low, axis):
    top = jnp.concatenate([high, low], axis=axis)
    bottom = jnp.concatenate([high, jnp.zeros_like(low)], axis=axis)
    return jnp.concatenate([top, bottom], axis=1 - axis)


def folded(a):
    half = a.shape[1] // 2
    return a[:, :half] + a[:, half:]


def layer_kernel(
    offset_hbm, decay_scale_hbm, write_bias_hbm,
    x_ref, w0, w1, w2, w3, w4, w5, decay_w_ref, write_w_ref, shift_ref, gain_hbm, sw_hbm, dw_hbm,
    own, incoming,
    offset_ref, decay_scale_ref, write_bias_ref, gain_ref,
    xs, ws, gate_w, gate_all, gates, shifts_ref, after,
    proj, acc, later, memory_ref, maps, adds, stick_out, delta_out,
    sticks, deltas, sw_ref, dw_ref, partial, outgoing,
    x_send, x_recv, f_send, f_recv, w_send, w_recv, r_recv, s_send, s_recv, l_sem,
    a_send, a_recv, c_sem,
):
    weights = (w0, w1, w2, w3, w4, w5)
    sp, tp = lax.axis_size("sp"), lax.axis_size("tp")
    z, f, t = lax.axis_index("sp"), lax.axis_index("fs"), lax.axis_index("tp")
    rows, half = x_ref.shape
    depth = w0.shape[0]
    cols = ws.shape[1] // len(weights)
    parts = x_recv.shape[2]
    heads = decay_w_ref.shape[0]
    slot = pl.ds(pl.multiple_of(t * half, half), half)
    local = [
        pltpu.make_async_copy(x_ref, xs.at[z, :, slot], l_sem.at[0]),
        pltpu.make_async_copy(shift_ref, shifts_ref.at[z], l_sem.at[1]),
        pltpu.make_async_copy(decay_w_ref, gate_w.at[0], l_sem.at[2]),
        pltpu.make_async_copy(write_w_ref, gate_w.at[1], l_sem.at[3]),
        pltpu.make_async_copy(offset_hbm, offset_ref, l_sem.at[6]),
        pltpu.make_async_copy(decay_scale_hbm, decay_scale_ref, l_sem.at[7]),
        pltpu.make_async_copy(write_bias_hbm, write_bias_ref, l_sem.at[8]),
        pltpu.make_async_copy(gain_hbm, gain_ref, l_sem.at[9]),
    ]
    late = [
        pltpu.make_async_copy(sw_hbm, sw_ref, l_sem.at[4]),
        pltpu.make_async_copy(dw_hbm, dw_ref, l_sem.at[5]),
    ]

    def w_src(i):
        return weights[i].at[:, pl.ds(pl.multiple_of(z * cols, cols), cols)]

    def w_at(i, who):
        return ws.at[pl.ds(pl.multiple_of(who * depth, depth), depth), pl.ds(i * cols, cols)]

    local_w = [
        pltpu.make_async_copy(w_src(i), w_at(i, f), l_sem.at[10]) for i in range(len(weights))
    ]
    near = (f + 1 - 2 * (f % 2), f + 2 - 4 * (f // 2))
    count = len(weights)
    delta_kinds, stick_kinds = (3, 4, 5), (0, 1, 2)

    def onward(way):
        return z + 1 < sp if way == 0 else z > 0

    def ahead(way):
        return z + 1 if way == 0 else z - 1

    barrier = pltpu.get_barrier_semaphore()
    for way in range(2):
        @pl.when(onward(way))
        def _():
            pl.semaphore_signal(
                barrier, inc=1, device_id={"sp": ahead(way)}, device_id_type=MESH
            )
    for side in range(2):
        pl.semaphore_signal(barrier, inc=1, device_id={"fs": near[side]}, device_id_type=MESH)
    pl.semaphore_signal(
        barrier, inc=1, device_id={"tp": lax.rem(t + 1, tp)}, device_id_type=MESH
    )
    for c in local + local_w:
        c.start()
    peers = onward(0).astype(jnp.int32) + onward(1).astype(jnp.int32) + 3
    pl.semaphore_wait(barrier, peers)

    def x_copy(way, step, part):
        block = z - (step - 1) if way == 0 else z + (step - 1)
        piece = pl.ds(part * (rows // parts), rows // parts)
        there = xs.at[block, piece, slot]
        return remote(
            x_ref.at[piece, :] if step == 1 else there, there,
            x_send.at[way], x_recv.at[way, step - 1, part], "sp", ahead(way),
        )

    def shift_copy(way, step):
        block = z - (step - 1) if way == 0 else z + (step - 1)
        there = shifts_ref.at[block]
        return remote(
            shift_ref if step == 1 else there, there,
            s_send.at[way], s_recv.at[way, step - 1], "sp", ahead(way),
        )

    def comes(way, step):
        return z >= step if way == 0 else z + step < sp

    def sends(way, step):
        return jnp.logical_and(onward(way), comes(way, step - 1))

    def forward(way, step, part):
        block = z - step if way == 0 else z + step
        piece = pl.ds(part * (rows // parts), rows // parts)
        there = xs.at[block, piece, slot]
        return remote(
            x_ref.at[piece, :] if step == 0 else there, there,
            f_send.at[0], f_recv.at[way * (sp - 1) + step], "tp", lax.rem(t + 1, tp),
        )

    def w_copy(side, i):
        return remote(
            w_src(i), w_at(i, f), w_send.at[0], w_recv.at[side, i], "fs", near[side]
        )

    def w_relay(side, i):
        part = depth // 2
        start = pl.multiple_of(near[side] * depth + side * part, part)
        there = ws.at[pl.ds(start, part), pl.ds(i * cols, cols)]
        return remote(
            there, there, w_send.at[0], r_recv.at[i // 3], "fs", near[1 - side]
        )

    for part in range(parts):
        for way in range(2):
            @pl.when(onward(way))
            def _():
                x_copy(way, 1, part).start()
                if part == 0:
                    shift_copy(way, 1).start()
    for i in delta_kinds:
        for side in range(2):
            w_copy(side, i).start()
    for part in range(parts):
        forward(0, 0, part).start()

    def relay(i):
        for side in range(2):
            w_copy(side, i).wait_recv()
            w_relay(side, i).start()

    def arrive(step, part):
        for way in range(2):
            @pl.when(comes(way, step))
            def _():
                x_copy(way, step, part).wait_recv()
                forward(way, step, part).start()
                if step + 1 < sp:
                    @pl.when(onward(way))
                    def _():
                        x_copy(way, step + 1, part).start()
                if part == 0:
                    shift_copy(way, step).wait_recv()
                    if step + 1 < sp:
                        @pl.when(onward(way))
                        def _():
                            shift_copy(way, step + 1).start()

    below = lax.broadcasted_iota(jnp.int32, (rows, rows), 0)
    across = lax.broadcasted_iota(jnp.int32, (rows, rows), 1)
    after[:, :rows] = jnp.where(below > across, 1.0, 0.0).astype(jnp.bfloat16)
    after[:, rows:] = jnp.ones((rows, cols), jnp.bfloat16)
    acc[...] = jnp.zeros_like(acc)
    later[...] = jnp.zeros_like(later)
    memory_ref[...] = jnp.zeros_like(memory_ref)
    early = [(step, part) for step in range(1, sp - 1) for part in range(parts)]
    relay(delta_kinds[0])
    arrive(*early[0])
    for i in delta_kinds[1:]:
        relay(i)
    for i in stick_kinds:
        for side in range(2):
            w_copy(side, i).start()
    for c in late:
        c.start()
    for step, part in early[1:parts]:
        arrive(step, part)
    for c in local:
        c.wait()
    own_w = ws.at[pl.ds(pl.multiple_of(f * depth, depth), depth), :]
    pltpu.make_async_copy(own_w, own_w, l_sem.at[10]).wait()
    gate_all[...] = jnp.concatenate(
        [gate_w[0].astype(jnp.float32), gate_w[1].astype(jnp.float32)], axis=0
    ).astype(jnp.bfloat16)
    def all_sent(ref, sem):
        remote(ref, ref, sem, sem, "tp", lax.rem(t + 1, tp)).wait_send()

    def all_came(ref, sem):
        remote(ref, ref, sem, sem, "tp", lax.rem(t + 1, tp)).wait_recv()

    def block_came(way, step):
        all_came(xs.at[z, :, slot], f_recv.at[way * (sp - 1) + step])

    block_came(0, 0)

    def relayed(kinds):
        first = kinds[0] * cols
        all_came(ws.at[pl.ds(0, depth), pl.ds(first, len(kinds) * cols)], r_recv.at[kinds[0] // 3])

    relayed(delta_kinds)

    size = offset_ref.shape[0] // sp
    sb_size = cols // size
    scale = sb_size ** (-0.5)
    tile = rows // 2

    def at_block(b, start=0, extent=rows):
        return pl.ds(pl.multiple_of(b * rows + start, extent), extent)

    def pair(i, j):
        for part in range(rows // tile):
            mine = at_block(i, part * tile, tile)
            q = proj[0, mine, :]
            keys, values = proj[1, at_block(j), :], proj[2, at_block(j), :]
            lane = lax.broadcasted_iota(jnp.int32, (tile, cols), 1)
            query = jnp.concatenate(
                [jnp.where(lane // sb_size == h, q, jnp.zeros_like(q)) for h in range(size)], axis=0
            )
            score = dot_f32(query, keys, ((1,), (1,)))
            score = jnp.concatenate(
                [
                    score[h * tile : (h + 1) * tile] * scale + offset_ref[z * size + h]
                    for h in range(size)
                ],
                axis=0,
            )
            skip = jnp.maximum(score, jnp.log(1.0 + jnp.exp(jnp.minimum(score, 80.0))))
            weight = score - skip
            seen = across[:tile] < below[:tile] + (part * tile + (i - j) * rows)
            seen = jnp.concatenate([seen] * size, axis=0)
            skip = jnp.where(seen, skip, 0.0)
            sums = dot_f32(skip.astype(jnp.bfloat16), after[...])
            weight = jnp.where(seen, jnp.exp(weight - sums[:, :rows]), 0.0)
            out = dot_f32(weight.astype(jnp.bfloat16), values)
            mixed, total = out[:tile], sums[:tile, rows:]
            for h in range(1, size):
                at = slice(h * tile, (h + 1) * tile)
                mixed = jnp.where(lane // sb_size == h, out[at], mixed)
                total = jnp.where(lane // sb_size == h, sums[at, rows:], total)
            passed = later[mine, :]
            acc[mine, :] = acc[mine, :] + mixed * jnp.exp(-passed)
            later[mine, :] = passed + total

    span = BLOCK
    duo = 2 * span
    blocks = rows // span
    width = GDN_DIM
    seg_row = lax.broadcasted_iota(jnp.int32, (rows, rows), 0)
    seg_col = lax.broadcasted_iota(jnp.int32, (rows, rows), 1)
    together = seg_row // span == seg_col // span
    upto = jnp.where(jnp.logical_and(together, seg_row <= seg_col), 1.0, 0.0).astype(jnp.bfloat16)
    beyond_it = jnp.where(jnp.logical_and(together, seg_row > seg_col), 1.0, 0.0).astype(
        jnp.bfloat16
    )
    prow = lax.broadcasted_iota(jnp.int32, (span, duo), 0)
    plane = lax.broadcasted_iota(jnp.int32, (span, duo), 1)
    first = plane < span
    pcol = jnp.where(first, plane, plane - span)
    inclusive, strictly = pcol <= prow, pcol < prow
    unit = jnp.where(pcol == prow, 1.0, 0.0)
    diagonal = lax.broadcasted_iota(jnp.int32, (width, width), 0) == lax.broadcasted_iota(
        jnp.int32, (width, width), 1
    )
    eighth = lax.broadcasted_iota(jnp.int32, (8, rows), 0)

    def silu(a):
        return a * (1.0 / (1.0 + jnp.exp(-a)))

    def unit_of(a):
        return a * lax.rsqrt(jnp.sum(a * a, axis=-1, keepdims=True) + NORM_EPS)

    def apart(a):
        lanes = lax.broadcasted_iota(jnp.int32, a.shape, 1) < span
        zero = jnp.zeros_like(a)
        return jnp.concatenate([jnp.where(lanes, a, zero), jnp.where(lanes, zero, a)], axis=0)

    def squared(left, power):
        high, low = halves(power)
        lhigh, llow = halves(left)
        return folded(
            dot_f32(
                jnp.concatenate([lhigh, llow], axis=1), wide_rhs(apart(high), apart(low), 1)
            )
        )

    def prepare(b, dq, dk, dv):
        gates[...] = dot_f32(gate_all[...], xs[b], ((1,), (1,)))
        pre = gates[pl.ds(z, 1), :]
        write = gates[pl.ds(heads + z, 1), :] + write_bias_ref[z]
        rate = jnp.exp(jnp.full((1, rows), decay_scale_ref[z], jnp.float32))
        soft = jnp.maximum(pre, 0.0) + jnp.log(1.0 + jnp.exp(-jnp.abs(pre)))
        decay = shifts_ref[b, pl.ds(z, 1), :] - rate * soft
        strength = 1.0 / (1.0 + jnp.exp(-write))
        d1 = decay.astype(jnp.bfloat16).astype(jnp.float32)
        d2 = (decay - d1).astype(jnp.bfloat16).astype(jnp.float32)
        d3 = decay - d1 - d2
        three = jnp.where(
            eighth == 0, d1, jnp.where(eighth == 1, d2, jnp.where(eighth == 2, d3, 0.0))
        ).astype(jnp.bfloat16)
        cum_row = jnp.sum(dot_f32(three, upto), axis=0, keepdims=True)
        rest_row = jnp.sum(dot_f32(three, beyond_it), axis=0, keepdims=True)
        stack = jnp.where(
            eighth == 0, strength,
            jnp.where(
                eighth == 1, jnp.exp(cum_row),
                jnp.where(eighth == 2, jnp.exp(rest_row), cum_row),
            ),
        )
        columns = stack.T
        s_col, grow, damp, cum = (columns[:, n : n + 1] for n in range(4))
        q = unit_of(silu(dq)) * width ** (-0.5)
        k = unit_of(silu(dk))
        v = silu(dv)
        boosted = q * grow
        damped = k * damp
        right = jnp.concatenate([v * s_col, k * (s_col * grow)], axis=1)
        kh, kl = halves(k)
        qh, ql = halves(q)
        work = []
        for duo_at in range(rows // duo):
            lo = duo_at * duo
            here = slice(lo, lo + duo)
            left = jnp.concatenate(
                [
                    jnp.concatenate([kh[here], kl[here]], axis=1),
                    jnp.concatenate([qh[here], ql[here]], axis=1),
                ],
                axis=0,
            )
            gram = folded(
                dot_f32(left, wide_rhs(kh[here], kl[here], 0), ((1,), (1,)))
            )
            spread = (
                jnp.where(first, cum[lo : lo + span], cum[lo + span : lo + duo])
                - cum_row[:, here]
            )
            table = jnp.where(inclusive, jnp.exp(jnp.where(inclusive, spread, 0.0)), 0.0)
            scale_col = jnp.where(first, s_col[lo : lo + span], s_col[lo + span : lo + duo])
            near_k = jnp.where(first, gram[:span], gram[span:duo])
            near_q = jnp.where(first, gram[duo : duo + span], gram[duo + span :])
            strict = jnp.where(strictly, near_k * table * scale_col, 0.0)
            work.append([unit - strict, strict, near_q * table])
        yield
        for w in work:
            w[1] = squared(w[1], w[1])
        levels = max(1, (span - 1).bit_length()) - 1
        for level in range(levels):
            if level == levels // 2:
                yield
            for w in work:
                if level + 1 < levels:
                    both = squared(jnp.concatenate([w[1], w[0]], axis=0), w[1])
                    w[1], w[0] = both[:span], w[0] + both[span:]
                else:
                    w[0] = w[0] + squared(w[0], w[1])
        yield
        for duo_at, (inverse, _, inside) in enumerate(work):
            lo = duo_at * duo
            here = slice(lo, lo + duo)
            ih, il = (apart(a) for a in halves(inverse))
            rh, rl = halves(right[here])
            solved = dot_f32(
                jnp.concatenate([ih, il], axis=1), jnp.concatenate([rh, rh], axis=0)
            ) + dot_f32(ih, rl)
            lh, ll = (
                apart(a) for a in halves(jnp.concatenate([damped[here].T, inside], axis=0))
            )
            sh, sl = halves(solved)
            made = dot_f32(
                jnp.concatenate([lh, ll], axis=1), jnp.concatenate([sh, sh], axis=0)
            ) + dot_f32(lh, sl)
            for side in range(2):
                at = lo + side * span
                mine = made[side * (width + span) : (side + 1) * (width + span)]
                n = b * blocks + 2 * duo_at + side
                keep = grow[at + span - 1 : at + span]
                step_map = jnp.where(diagonal, keep, 0.0) - mine[:width, width:]
                query = boosted[at : at + span] - mine[width:, width:]
                high, low = halves(jnp.concatenate([step_map, query], axis=0))
                maps[n, :, :width] = high
                maps[n, :, width:] = low
                adds[n] = mine[:, :width]

    def give(which, out, target):
        here = target.at[:, pl.ds(pl.multiple_of(z * cols, cols), cols)]

        def send(g, k):
            return remote(
                out.at[at_block(g), :], here,
                a_send.at[which], a_recv.at[which], "sp", g,
            )

        def started(g):
            for k in range(1, sp):
                @pl.when(lax.rem(z + k, sp) == g)
                def _():
                    send(lax.rem(z + k, sp), k).start()

        def came():
            all_came(out.at[pl.ds(0, (sp - 1) * rows), :], a_recv.at[which])

        return started, came

    stick_started, stick_came = give(0, stick_out, sticks)
    delta_started, delta_came = give(1, delta_out, deltas)

    shorter = jnp.minimum(z, sp - 1 - z)
    down_last = z > sp - 1 - z

    def place(n):
        both = n <= 2 * shorter
        way_n = jnp.where(both, lax.rem(n + 1, 2), jnp.where(down_last, 0, 1))
        step_n = jnp.where(n == 0, 0, jnp.where(both, (n + 1) // 2, n - shorter))
        down = jnp.logical_and(way_n == 0, n > 0)
        return way_n, step_n, down, jnp.where(down, z - step_n, z + step_n)

    last_way = jnp.logical_or(z == 0, z == sp - 1)

    def block_ready(n):
        way_n, step_n, down, b = place(n)
        for step in range(1, sp):
            for way in range(2):
                @pl.when(jnp.logical_and(step_n == step, way_n == way))
                def _():
                    block_came(way, step)
        return b

    def delta_block(b):
        drows = dot_f32(xs[b], ws[:, 3 * cols :]).astype(jnp.bfloat16).astype(jnp.float32)
        return prepare(b, drows[:, :cols], drows[:, cols : 2 * cols], drows[:, 2 * cols :])

    def stick_project(n):
        b = stick_place(n)[1]
        out = dot_f32(xs[b], ws[:, : 3 * cols]).astype(jnp.bfloat16)
        for i in range(3):
            proj[i, at_block(b), :] = out[:, i * cols : (i + 1) * cols]

    def stick_place(n):
        down = z == sp - 1
        return down, jnp.where(down, sp - 1 - n, n)

    def settle(i):
        stick_out[at_block(i), :] = acc[at_block(i), :].astype(jnp.bfloat16)

    def stick_pair(p):
        n = sum(((p >= e * (e + 1) // 2) * 1 for e in range(1, sp)), 0)
        r = p - n * (n + 1) // 2
        down, b = stick_place(n)
        i = jnp.where(down, b + r, b)
        j = jnp.where(down, b, b - r)
        pair(i, j)

        @pl.when(j == 0)
        def _():
            settle(i)
            stick_started(i)

    def plain_delta(n, c):
        @pl.when(n == 1)
        def _():
            relay(stick_kinds[0])

        @pl.when(n == sp - 2)
        def _():
            for c in early[parts:-1]:
                arrive(*c)
            for i in stick_kinds[1:]:
                relay(i)
            arrive(*early[-1])
        for _ in delta_block(block_ready(n)):
            pass
        return c

    def walk_groups(start, stop, held=False):
        def group(g, c):
            @pl.when(g > start + held)
            def _():
                delta_started(g - 1)
            memory = memory_ref[...]
            for n in range(blocks):
                memory = walk(g * blocks + n, memory)
            memory_ref[...] = memory
            return c

        lax.fori_loop(start, stop, group, 0)
        delta_started(stop - 1)

    def walk(n, memory):
        high, low = halves(memory)
        new = folded(dot_f32(maps[n], wide_rhs(high, low, 1))) + adds[n]
        made = new[width:]
        made = made * lax.rsqrt(jnp.mean(made * made, axis=-1, keepdims=True) + NORM_EPS)
        at = pl.ds(pl.multiple_of(n * span, span), span)
        delta_out[at, :] = (made * gain_ref[...]).astype(delta_out.dtype)
        return new[:width]

    last_way = jnp.logical_or(z == 0, z == sp - 1)

    before = sp * (sp - 1) // 2
    events = jnp.where(last_way, sp - 1, sp)
    lax.fori_loop(0, events, plain_delta, 0)

    @pl.when(jnp.logical_not(last_way))
    def _():
        walk_groups(0, sp, held=True)

    relayed(stick_kinds)

    def stick_event(n, c):
        for part in range(2):
            @pl.when(jnp.logical_and(last_way, n == part + 1))
            def _():
                arrive(sp - 1, part)

        @pl.when(jnp.logical_and(jnp.logical_not(last_way), n == 1))
        def _():
            delta_started(0)
        stick_project(n)

        def one(p, c):
            for part in range(2, parts):
                @pl.when(jnp.logical_and(last_way, p == before - parts + part))
                def _():
                    arrive(sp - 1, part)
            stick_pair(p)
            return c

        first = n * (n + 1) // 2
        return lax.fori_loop(first, first + n + 1, one, c)

    lax.fori_loop(0, events, stick_event, 0)

    @pl.when(last_way)
    def _():
        @pl.when(z == 0)
        def _():
            walk_groups(0, sp - 1)
        for way in range(2):
            @pl.when(comes(way, sp - 1))
            def _():
                block_came(way, sp - 1)
        stick_project(sp - 1)
        stages = delta_block(stick_place(sp - 1)[1])
        for u in range(sp):
            next(stages, None)
            stick_pair(before + u)
        walk_groups(jnp.where(z == 0, sp - 1, 0), sp)

    mine_z = pl.ds(pl.multiple_of(z * rows, rows), rows)
    lanes = pl.ds(pl.multiple_of(z * cols, cols), cols)
    sticks[:, lanes] = stick_out[mine_z, :]
    deltas[:, lanes] = delta_out[mine_z, :]
    for c in late:
        c.wait()
    stick_came()
    chunks, wide = outgoing.shape[0], outgoing.shape[2]
    share = rows // tp
    for c in range(chunks):
        columns = slice(c * wide, (c + 1) * wide)
        partial[:, columns] = dot_f32(sticks[...], sw_ref[:, columns])
    delta_came()
    mine = pl.ds(pl.multiple_of(t * share, share), share)
    partner = lax.rem(t + 1, tp)
    theirs = pl.ds(pl.multiple_of(partner * share, share), share)

    def finish(which, c):
        columns = slice(c * wide, (c + 1) * wide)
        return (
            partial[which, columns] + dot_f32(deltas[which, :], dw_ref[:, columns])
        ).astype(jnp.bfloat16)

    swaps = [
        remote(
            outgoing.at[c], incoming.at[:, c * wide : (c + 1) * wide],
            c_sem.at[0], c_sem.at[1], "tp", partner,
        )
        for c in range(chunks)
    ]
    for c in range(chunks):
        outgoing[c] = finish(theirs, c)
        if c > 0:
            swaps[c - 1].start()
    for c in range(chunks):
        own[:, c * wide : (c + 1) * wide] = finish(mine, c)
        if c == 0:
            swaps[chunks - 1].start()
    all_came(incoming, c_sem.at[1])
    all_sent(incoming, c_sem.at[0])
    all_sent(ws.at[pl.ds(0, 3 * depth), :], w_send.at[0])
    all_sent(xs.at[:, :, slot], f_send.at[0])
    for which, out in enumerate((stick_out, delta_out)):
        all_sent(out.at[pl.ds(0, (sp - 1) * rows), :], a_send.at[which])
    for c in range(sp):
        @pl.when(z == c)
        def _():
            for way, passed in enumerate((c + 1 if c + 1 < sp else 0, sp - c if c > 0 else 0)):
                if passed:
                    all_sent(xs.at[pl.ds(0, passed), :, slot], x_send.at[way])
                    all_sent(shifts_ref.at[pl.ds(0, passed)], s_send.at[way])


ANYWHERE = pl.BlockSpec(memory_space=pltpu.HBM)
ON_CORE = pl.BlockSpec(memory_space=pltpu.VMEM)


def on_device_heads(
    hidden_in, sb_query_w, sb_key_w, sb_value_w, sb_offset,
    delta_query_w, delta_key_w, delta_value_w, decay_w, write_w, write_bias,
    decay_log_scale, decay_shift, head_gain, sb_out_w, delta_out_w,
):
    sp, fs, tp = lax.axis_size("sp"), lax.axis_size("fs"), lax.axis_size("tp")
    rows, half = hidden_in.shape[1:]
    width = half * tp
    length = rows * sp
    heads = decay_log_scale.shape[0]
    cols = sb_query_w.shape[1] // sp
    parts, chunks = 4, 4
    share = rows // tp
    blocks = length // BLOCK
    dma = pltpu.SemaphoreType.DMA
    bf16, f32 = jnp.bfloat16, jnp.float32
    own, incoming = pl.pallas_call(
        layer_kernel,
        name="layer",
        out_shape=(pltpu.VMEM((share, width), bf16),) * 2,
        in_specs=[ANYWHERE] * 16,
        out_specs=(ON_CORE,) * 2,
        scratch_shapes=[
            pltpu.SMEM(sb_offset.shape, f32),
            pltpu.SMEM(decay_log_scale.shape, f32),
            pltpu.SMEM(write_bias.shape, f32),
            pltpu.VMEM((1, head_gain.shape[0]), f32),
            pltpu.VMEM((sp, rows, width), bf16),
            pltpu.VMEM((width, 6 * cols), bf16),
            pltpu.VMEM((2, heads, width), bf16),
            pltpu.VMEM((2 * heads, width), bf16),
            pltpu.VMEM((2 * heads, rows), f32),
            pltpu.VMEM((sp, heads, rows), f32),
            pltpu.VMEM((rows, rows + cols), bf16),
            pltpu.VMEM((3, length, cols), bf16),
            pltpu.VMEM((length, cols), f32),
            pltpu.VMEM((length, cols), f32),
            pltpu.VMEM((cols, cols), f32),
            pltpu.VMEM((blocks, cols + BLOCK, 2 * cols), bf16),
            pltpu.VMEM((blocks, cols + BLOCK, cols), f32),
            pltpu.VMEM((length, cols), bf16),
            pltpu.VMEM((length, cols), bf16),
            pltpu.VMEM((rows, cols * sp), bf16),
            pltpu.VMEM((rows, cols * sp), bf16),
            pltpu.VMEM(sb_out_w.shape, bf16),
            pltpu.VMEM(delta_out_w.shape, bf16),
            pltpu.VMEM((rows, width), f32),
            pltpu.VMEM((chunks, share, width // chunks), bf16),
            dma((2,)), dma((2, sp - 1, parts)), dma((1,)), dma((2 * sp - 1,)),
            dma((1,)), dma((2, 6)), dma((2,)), dma((2,)), dma((2, sp - 1)), dma((11,)),
            dma((2,)), dma((2,)), dma((2,)),
        ],
        compiler_params=pltpu.CompilerParams(
            collective_id=0, has_side_effects=True,
            vmem_limit_bytes=ALL_VMEM - 5 * share * width,
        ),
    )(
        sb_offset, decay_log_scale, write_bias,
        hidden_in.reshape(rows, half), sb_query_w, sb_key_w, sb_value_w,
        delta_query_w, delta_key_w, delta_value_w, decay_w.T, write_w.T,
        decay_shift.reshape(heads, rows), head_gain.reshape(1, -1), sb_out_w, delta_out_w,
    )
    result = (own.astype(f32) + incoming.astype(f32)).astype(bf16)
    return result.reshape(1, share, width)


def on_device(*inputs):
    delta_heads = inputs[11].shape[0]
    square = lax.axis_size("sp") == lax.axis_size("fs") == 4 and lax.axis_size("tp") == 2
    if square and delta_heads == lax.axis_size("sp") and inputs[4].shape[0] % delta_heads == 0:
        return on_device_heads(*inputs)
    return on_device_split(*inputs)


def solution(mesh):
    return jax.shard_map(
        on_device,
        mesh=mesh,
        in_specs=(
            P("fs", "sp", "tp"),
            P("fs", "tp"),
            P("fs", "tp"),
            P("fs", "tp"),
            P("tp"),
            P("fs", "tp"),
            P("fs", "tp"),
            P("fs", "tp"),
            P(None, "tp"),
            P(None, "tp"),
            P("tp"),
            P("tp"),
            P("fs", "tp", "sp"),
            P(),
            P("tp", None),
            P("tp", None),
        ),
        out_specs=P("fs", ("sp", "tp"), None),
        check_vma=False,
    )
```

```python
import jax
import jax.numpy as jnp
from jax import lax
from jax.experimental import pallas as pl
from jax.experimental.pallas import tpu as pltpu
from jax.sharding import PartitionSpec as P

MESH = pl.DeviceIdType.MESH
ALL_VMEM = 67043328

SB_DIM = 64
GDN_DIM = 128
BLOCK = 64


EXACT_MATMUL = lax.Precision.HIGHEST
NORM_EPS = 1e-06


def carried_in(value, axis, combine, identity):
    devices, index = (lax.axis_size(axis), lax.axis_index(axis))
    everything = jax.tree.map(
        lambda part, kind: lax.all_gather(part.astype(kind), axis),
        value,
        (jnp.bfloat16, jnp.bfloat16),
    )
    start = jax.tree.map(
        lambda part, zero: jnp.broadcast_to(jnp.asarray(zero, part.dtype), part.shape),
        value,
        identity,
    )

    def lap(k, before):
        reached = k < index
        new = combine(
            before, jax.tree.map(lambda part, own: part[k].astype(own.dtype), everything, value)
        )
        return jax.tree.map(lambda a, b: jnp.where(reached, a, b), new, before)

    return lax.fori_loop(0, devices, lap, start)


def unit_lower_inverse(strict_part):
    order_size = strict_part.shape[-1]
    powered = strict_part
    inverse = jnp.eye(order_size, dtype=strict_part.dtype) - strict_part
    for repeat_number in range(max(1, (order_size - 1).bit_length()) - 1):
        powered = jnp.einsum("...ij,...jk->...ik", powered, powered, precision=EXACT_MATMUL)
        inverse = inverse + jnp.einsum(
            "...ij,...jk->...ik", inverse, powered, precision=EXACT_MATMUL
        )
    return inverse


def to_blocks(row_data, block_span):
    blocks_count = row_data.shape[0] // block_span
    shaped = row_data.reshape((blocks_count, block_span) + row_data.shape[1:])
    return jnp.swapaxes(shaped, 1, 2)


def from_blocks(blocked):
    swapped = jnp.swapaxes(blocked, 1, 2)
    return swapped.reshape((-1,) + swapped.shape[2:])


def unit_rows(vectors):
    return vectors * lax.rsqrt(jnp.sum(vectors * vectors, axis=-1, keepdims=True) + NORM_EPS)


def delta_inputs(
    query_proj,
    key_proj,
    value_proj,
    decay_pre,
    write_pre,
    write_bias,
    decay_log_scale,
    shift_rows,
    head_count,
    head_size,
):
    query_act = jax.nn.silu(query_proj.astype(jnp.float32)).reshape(-1, head_count, head_size)
    key_act = jax.nn.silu(key_proj.astype(jnp.float32)).reshape(-1, head_count, head_size)
    value_rows = jax.nn.silu(value_proj.astype(jnp.float32)).reshape(-1, head_count, head_size)
    queries = unit_rows(query_act) * head_size ** (-0.5)
    key_rows = unit_rows(key_act)
    log_decay = -jnp.exp(decay_log_scale) * jax.nn.softplus(decay_pre) + shift_rows
    strength = jax.nn.sigmoid(write_pre + write_bias)
    return (queries, key_rows, value_rows, log_decay, strength)


def delta_prepare(queries, key_rows, value_rows, log_decay, strength):
    block_span = queries.shape[2]
    cumulative = jnp.cumsum(log_decay, axis=-1)
    row_place = lax.broadcasted_iota(jnp.int32, (block_span, block_span), 0)
    col_place = lax.broadcasted_iota(jnp.int32, (block_span, block_span), 1)
    inclusive = col_place <= row_place
    strictly = col_place < row_place
    spread = cumulative[..., :, None] - cumulative[..., None, :]
    decay_table = jnp.where(inclusive, jnp.exp(jnp.where(inclusive, spread, 0.0)), 0.0)
    keys_beta = key_rows * strength[..., None]
    lower_part = jnp.where(
        strictly,
        jnp.einsum("nhik,nhjk->nhij", keys_beta, key_rows, precision=EXACT_MATMUL) * decay_table,
        0.0,
    )
    inverse = unit_lower_inverse(lower_part)
    growth = jnp.exp(cumulative)
    state_updates = jnp.einsum(
        "nhij,nhjv->nhiv", inverse, value_rows * strength[..., None], precision=EXACT_MATMUL
    )
    erase_term = jnp.einsum(
        "nhij,nhjk->nhik", inverse, keys_beta * growth[..., None], precision=EXACT_MATMUL
    )
    inside_block = (
        jnp.einsum("nhik,nhjk->nhij", queries, key_rows, precision=EXACT_MATMUL) * decay_table
    )
    boosted_query = queries * growth[..., None]
    damped_keys = key_rows * jnp.exp(cumulative[..., -1:] - cumulative)[..., None]
    decay_per_block = jnp.exp(cumulative[..., -1])
    return (state_updates, erase_term, inside_block, boosted_query, damped_keys, decay_per_block)


def delta_step(memory_state, inputs):
    state_updates, erase_term, inside_block, boosted_query, damped_keys, decay_per_block = inputs
    fixed_values = state_updates - jnp.einsum(
        "mzq,mqc->mzc", erase_term, memory_state, precision=EXACT_MATMUL
    )
    produced_rows = jnp.einsum(
        "mzq,mqc->mzc", boosted_query, memory_state, precision=EXACT_MATMUL
    ) + jnp.einsum("efq,eqn->efn", inside_block, fixed_values, precision=EXACT_MATMUL)
    memory_state = memory_state * decay_per_block[:, None, None] + jnp.einsum(
        "wam,waz->wmz", damped_keys, fixed_values, precision=EXACT_MATMUL
    )
    return (memory_state, produced_rows)


def transition_step(carried, inputs):
    memory_state, transfer = carried
    state_updates, erase_term, inside_block, boosted_query, damped_keys, decay_per_block = inputs
    fixed_values = state_updates - jnp.einsum(
        "mzq,mqc->mzc", erase_term, memory_state, precision=EXACT_MATMUL
    )
    coupling = jnp.einsum("hik,hil->hkl", damped_keys, erase_term, precision=EXACT_MATMUL)
    memory_state = memory_state * decay_per_block[:, None, None] + jnp.einsum(
        "wam,waz->wmz", damped_keys, fixed_values, precision=EXACT_MATMUL
    )
    transfer = transfer * decay_per_block[:, None, None] - jnp.einsum(
        "hkl,hlm->hkm", coupling, transfer, precision=EXACT_MATMUL
    )
    return ((memory_state, transfer), None)


def compose(prior_blocks, following_blocks):
    joined_map = jnp.einsum(
        "hkl,hlm->hkm", following_blocks[0], prior_blocks[0], precision=EXACT_MATMUL
    )
    joined_state = (
        jnp.einsum("djo,dog->djg", following_blocks[0], prior_blocks[1], precision=EXACT_MATMUL)
        + following_blocks[1]
    )
    return (joined_map, joined_state)


def stick_block(queries, key_rows, value_rows, query_place, key_place, offsets):
    scale_factor = queries.shape[-1] ** (-0.5)
    scores = (
        jnp.einsum("qhd,khd->hqk", queries, key_rows, preferred_element_type=jnp.float32)
        * scale_factor
        + offsets[:, None, None]
    )
    visible = key_place[None, :] < query_place[:, None]
    skipped = jnp.where(visible, jax.nn.log_sigmoid(-scores), 0.0)
    beyond = lax.cumsum(skipped, axis=2, reverse=True) - skipped
    weights = jnp.where(visible, jnp.exp(jax.nn.log_sigmoid(scores) + beyond), 0.0).astype(
        jnp.bfloat16
    )
    partial_value = jnp.einsum(
        "hqk,khd->qhd", weights, value_rows, preferred_element_type=jnp.float32
    )
    return (partial_value, jnp.sum(skipped, axis=2).T)


def stick_combine(partials, totals):
    beyond = jnp.cumsum(totals[::-1], axis=0)[::-1] - totals
    return jnp.sum(partials * jnp.exp(beyond)[..., None], axis=0)


def on_device_split(
    hidden_in,
    sb_query_w,
    sb_key_w,
    sb_value_w,
    sb_offset,
    delta_query_w,
    delta_key_w,
    delta_value_w,
    decay_w,
    write_w,
    write_bias,
    decay_log_scale,
    decay_shift,
    head_gain,
    sb_out_w,
    delta_out_w,
):
    token_rows = hidden_in.shape[1]
    local_in = hidden_in.reshape(token_rows, hidden_in.shape[2])
    gathered = (
        lax.all_gather(sb_query_w, "fs", axis=0, tiled=True),
        lax.all_gather(sb_key_w, "fs", axis=0, tiled=True),
        lax.all_gather(sb_value_w, "fs", axis=0, tiled=True),
        lax.all_gather(delta_query_w, "fs", axis=0, tiled=True),
        lax.all_gather(delta_key_w, "fs", axis=0, tiled=True),
        lax.all_gather(delta_value_w, "fs", axis=0, tiled=True),
    )
    in_weights = tuple(gathered) + (decay_w, write_w)
    portion = lax.all_gather(local_in, "tp", axis=1, tiled=True)
    projected = tuple(
        (jnp.dot(portion, weight, preferred_element_type=jnp.float32) for weight in in_weights)
    )
    sb_heads = sb_offset.shape[0]
    delta_heads = decay_log_scale.shape[0]
    sb_query = projected[0].astype(jnp.bfloat16).reshape(token_rows, sb_heads, SB_DIM)
    sb_keys = projected[1].astype(jnp.bfloat16)
    sb_values = projected[2].astype(jnp.bfloat16)
    shift_rows = decay_shift.reshape(delta_heads, token_rows).T
    queries, key_rows, value_rows, log_decay, strength = delta_inputs(
        projected[3].astype(jnp.bfloat16),
        projected[4].astype(jnp.bfloat16),
        projected[5].astype(jnp.bfloat16),
        projected[6],
        projected[7],
        write_bias,
        decay_log_scale,
        shift_rows,
        delta_heads,
        GDN_DIM,
    )
    prepared = delta_prepare(
        to_blocks(queries, BLOCK),
        to_blocks(key_rows, BLOCK),
        to_blocks(value_rows, BLOCK),
        to_blocks(log_decay, BLOCK),
        to_blocks(strength, BLOCK),
    )
    identity_map = jnp.broadcast_to(
        jnp.eye(GDN_DIM, dtype=jnp.float32), (delta_heads, GDN_DIM, GDN_DIM)
    )
    empty_state = jnp.zeros((delta_heads, GDN_DIM, GDN_DIM), jnp.float32)
    (local_end, local_map), unused_out = lax.scan(
        transition_step, (empty_state, identity_map), prepared
    )
    own_first = lax.axis_index("sp") * token_rows
    query_place = own_first + lax.iota(jnp.int32, token_rows)
    sp_count = lax.axis_size("sp")
    slot_out = jnp.zeros((sp_count, token_rows, sb_heads, SB_DIM), jnp.float32)
    slot_total = jnp.zeros((sp_count, token_rows, sb_heads), jnp.float32)

    def absorb(slot_arrays, address_portion, value_part, shard_first):

        def active(current):
            partial_value, totals = stick_block(
                sb_query,
                address_portion.reshape(token_rows, sb_heads, SB_DIM),
                value_part.reshape(token_rows, sb_heads, SB_DIM),
                query_place,
                shard_first + lax.iota(jnp.int32, token_rows),
                sb_offset,
            )
            slot_index = shard_first // token_rows
            return (
                lax.dynamic_update_index_in_dim(current[0], partial_value, slot_index, 0),
                lax.dynamic_update_index_in_dim(current[1], totals, slot_index, 0),
            )

        def inactive(current):
            return current

        usable = jnp.logical_and(shard_first >= 0, shard_first <= own_first)
        return lax.cond(usable, active, inactive, slot_arrays)

    key_block = lax.all_gather(sb_keys, "sp", axis=0, tiled=True)
    value_block = lax.all_gather(sb_values, "sp", axis=0, tiled=True)

    def per_shard(shard_number, current):
        row_begin = shard_number * token_rows
        return absorb(
            current,
            lax.dynamic_slice_in_dim(key_block, row_begin, token_rows, 0),
            lax.dynamic_slice_in_dim(value_block, row_begin, token_rows, 0),
            row_begin,
        )

    slot_arrays = lax.fori_loop(
        0, key_block.shape[0] // token_rows, per_shard, (slot_out, slot_total)
    )
    unused_map, incoming = carried_in(
        (local_map, local_end), "sp", compose, (identity_map, empty_state)
    )
    sb_mixed = (
        stick_combine(slot_arrays[0], slot_arrays[1])
        .astype(jnp.bfloat16)
        .reshape(token_rows, sb_heads * SB_DIM)
    )
    unused_end, produced_rows = lax.scan(delta_step, incoming, prepared)
    produced_rows = from_blocks(produced_rows)
    normed = (
        produced_rows
        * lax.rsqrt(jnp.mean(produced_rows * produced_rows, axis=-1, keepdims=True) + NORM_EPS)
        * head_gain
    )
    delta_mixed = normed.astype(jnp.bfloat16).reshape(token_rows, delta_heads * GDN_DIM)
    result = lax.psum_scatter(
        (
            jnp.dot(sb_mixed, sb_out_w, preferred_element_type=jnp.float32)
            + jnp.dot(delta_mixed, delta_out_w, preferred_element_type=jnp.float32)
        ).astype(jnp.bfloat16),
        "tp",
        scatter_dimension=0,
        tiled=True,
    ).astype(jnp.float32)
    return result.astype(jnp.bfloat16).reshape(1, result.shape[0], result.shape[1])


def remote(src, dst, send, recv, axis, index):
    return pltpu.make_async_remote_copy(
        src_ref=src, dst_ref=dst, send_sem=send, recv_sem=recv,
        device_id={axis: index}, device_id_type=MESH,
    )


def greet(axes):
    barrier = pltpu.get_barrier_semaphore()
    count = 0
    for axis in axes:
        size, me = lax.axis_size(axis), lax.axis_index(axis)
        for k in range(1, size):
            pl.semaphore_signal(
                barrier, inc=1, device_id={axis: lax.rem(me + k, size)}, device_id_type=MESH
            )
            count += 1
    pl.semaphore_wait(barrier, count)


def halves(a):
    high = a.astype(jnp.bfloat16)
    return high, (a - high.astype(jnp.float32)).astype(jnp.bfloat16)


def dot_f32(a, b, dims=((1,), (0,))):
    return lax.dot_general(a, b, (dims, ((), ())), preferred_element_type=jnp.float32)


def wide_rhs(high, low, axis):
    top = jnp.concatenate([high, low], axis=axis)
    bottom = jnp.concatenate([high, jnp.zeros_like(low)], axis=axis)
    return jnp.concatenate([top, bottom], axis=1 - axis)


def folded(a):
    half = a.shape[1] // 2
    return a[:, :half] + a[:, half:]


def layer_kernel(
    offset_hbm, decay_scale_hbm, write_bias_hbm,
    x_ref, w0, w1, w2, w3, w4, w5, decay_w_ref, write_w_ref, shift_ref, gain_hbm, sw_hbm, dw_hbm,
    own, incoming,
    offset_ref, decay_scale_ref, write_bias_ref, gain_ref,
    xs, ws, gate_w, gate_all, gates, shifts_ref, after,
    proj, acc, later, memory_ref, maps, adds, stick_out, delta_out,
    sticks, deltas, sw_ref, dw_ref, partial, outgoing,
    x_send, x_recv, f_send, f_recv, w_send, w_recv, r_recv, s_send, s_recv, l_sem,
    a_send, a_recv, c_sem,
):
    weights = (w0, w1, w2, w3, w4, w5)
    sp, tp = lax.axis_size("sp"), lax.axis_size("tp")
    z, f, t = lax.axis_index("sp"), lax.axis_index("fs"), lax.axis_index("tp")
    rows, half = x_ref.shape
    depth = w0.shape[0]
    cols = ws.shape[1] // len(weights)
    parts = x_recv.shape[2]
    heads = decay_w_ref.shape[0]
    slot = pl.ds(pl.multiple_of(t * half, half), half)
    local = [
        pltpu.make_async_copy(x_ref, xs.at[z, :, slot], l_sem.at[0]),
        pltpu.make_async_copy(shift_ref, shifts_ref.at[z], l_sem.at[1]),
        pltpu.make_async_copy(decay_w_ref, gate_w.at[0], l_sem.at[2]),
        pltpu.make_async_copy(write_w_ref, gate_w.at[1], l_sem.at[3]),
        pltpu.make_async_copy(offset_hbm, offset_ref, l_sem.at[6]),
        pltpu.make_async_copy(decay_scale_hbm, decay_scale_ref, l_sem.at[7]),
        pltpu.make_async_copy(write_bias_hbm, write_bias_ref, l_sem.at[8]),
        pltpu.make_async_copy(gain_hbm, gain_ref, l_sem.at[9]),
    ]
    late = [
        pltpu.make_async_copy(sw_hbm, sw_ref, l_sem.at[4]),
        pltpu.make_async_copy(dw_hbm, dw_ref, l_sem.at[5]),
    ]

    def w_src(i):
        return weights[i].at[:, pl.ds(pl.multiple_of(z * cols, cols), cols)]

    def w_at(i, who):
        return ws.at[pl.ds(pl.multiple_of(who * depth, depth), depth), pl.ds(i * cols, cols)]

    local_w = [
        pltpu.make_async_copy(w_src(i), w_at(i, f), l_sem.at[10]) for i in range(len(weights))
    ]
    near = (f + 1 - 2 * (f % 2), f + 2 - 4 * (f // 2))
    count = len(weights)
    delta_kinds, stick_kinds = (3, 4, 5), (0, 1, 2)

    def onward(way):
        return z + 1 < sp if way == 0 else z > 0

    def ahead(way):
        return z + 1 if way == 0 else z - 1

    barrier = pltpu.get_barrier_semaphore()
    for way in range(2):
        @pl.when(onward(way))
        def _():
            pl.semaphore_signal(
                barrier, inc=1, device_id={"sp": ahead(way)}, device_id_type=MESH
            )
    for side in range(2):
        pl.semaphore_signal(barrier, inc=1, device_id={"fs": near[side]}, device_id_type=MESH)
    pl.semaphore_signal(
        barrier, inc=1, device_id={"tp": lax.rem(t + 1, tp)}, device_id_type=MESH
    )
    for c in local + local_w:
        c.start()
    peers = onward(0).astype(jnp.int32) + onward(1).astype(jnp.int32) + 3
    pl.semaphore_wait(barrier, peers)

    def x_copy(way, step, part):
        block = z - (step - 1) if way == 0 else z + (step - 1)
        piece = pl.ds(part * (rows // parts), rows // parts)
        there = xs.at[block, piece, slot]
        return remote(
            x_ref.at[piece, :] if step == 1 else there, there,
            x_send.at[way], x_recv.at[way, step - 1, part], "sp", ahead(way),
        )

    def shift_copy(way, step):
        block = z - (step - 1) if way == 0 else z + (step - 1)
        there = shifts_ref.at[block]
        return remote(
            shift_ref if step == 1 else there, there,
            s_send.at[way], s_recv.at[way, step - 1], "sp", ahead(way),
        )

    def comes(way, step):
        return z >= step if way == 0 else z + step < sp

    def sends(way, step):
        return jnp.logical_and(onward(way), comes(way, step - 1))

    def forward(way, step, part):
        block = z - step if way == 0 else z + step
        piece = pl.ds(part * (rows // parts), rows // parts)
        there = xs.at[block, piece, slot]
        return remote(
            x_ref.at[piece, :] if step == 0 else there, there,
            f_send.at[0], f_recv.at[way * (sp - 1) + step], "tp", lax.rem(t + 1, tp),
        )

    def w_copy(side, i):
        return remote(
            w_src(i), w_at(i, f), w_send.at[0], w_recv.at[side, i], "fs", near[side]
        )

    def w_relay(side, i):
        part = depth // 2
        start = pl.multiple_of(near[side] * depth + side * part, part)
        there = ws.at[pl.ds(start, part), pl.ds(i * cols, cols)]
        return remote(
            there, there, w_send.at[0], r_recv.at[i // 3], "fs", near[1 - side]
        )

    for part in range(parts):
        for way in range(2):
            @pl.when(onward(way))
            def _():
                x_copy(way, 1, part).start()
                if part == 0:
                    shift_copy(way, 1).start()
    for i in delta_kinds:
        for side in range(2):
            w_copy(side, i).start()
    for part in range(parts):
        forward(0, 0, part).start()

    def relay(i):
        for side in range(2):
            w_copy(side, i).wait_recv()
            w_relay(side, i).start()

    def arrive(step, part):
        for way in range(2):
            @pl.when(comes(way, step))
            def _():
                x_copy(way, step, part).wait_recv()
                forward(way, step, part).start()
                if step + 1 < sp:
                    @pl.when(onward(way))
                    def _():
                        x_copy(way, step + 1, part).start()
                if part == 0:
                    shift_copy(way, step).wait_recv()
                    if step + 1 < sp:
                        @pl.when(onward(way))
                        def _():
                            shift_copy(way, step + 1).start()

    below = lax.broadcasted_iota(jnp.int32, (rows, rows), 0)
    across = lax.broadcasted_iota(jnp.int32, (rows, rows), 1)
    after[:, :rows] = jnp.where(below > across, 1.0, 0.0).astype(jnp.bfloat16)
    after[:, rows:] = jnp.ones((rows, cols), jnp.bfloat16)
    acc[...] = jnp.zeros_like(acc)
    later[...] = jnp.zeros_like(later)
    memory_ref[...] = jnp.zeros_like(memory_ref)
    early = [(step, part) for step in range(1, sp - 1) for part in range(parts)]
    relay(delta_kinds[0])
    arrive(*early[0])
    for i in delta_kinds[1:]:
        relay(i)
    for i in stick_kinds:
        for side in range(2):
            w_copy(side, i).start()
    for c in late:
        c.start()
    for step, part in early[1:parts]:
        arrive(step, part)
    for c in local:
        c.wait()
    own_w = ws.at[pl.ds(pl.multiple_of(f * depth, depth), depth), :]
    pltpu.make_async_copy(own_w, own_w, l_sem.at[10]).wait()
    gate_all[...] = jnp.concatenate(
        [gate_w[0].astype(jnp.float32), gate_w[1].astype(jnp.float32)], axis=0
    ).astype(jnp.bfloat16)
    def all_sent(ref, sem):
        remote(ref, ref, sem, sem, "tp", lax.rem(t + 1, tp)).wait_send()

    def all_came(ref, sem):
        remote(ref, ref, sem, sem, "tp", lax.rem(t + 1, tp)).wait_recv()

    def block_came(way, step):
        all_came(xs.at[z, :, slot], f_recv.at[way * (sp - 1) + step])

    block_came(0, 0)

    def relayed(kinds):
        first = kinds[0] * cols
        all_came(ws.at[pl.ds(0, depth), pl.ds(first, len(kinds) * cols)], r_recv.at[kinds[0] // 3])

    relayed(delta_kinds)

    size = offset_ref.shape[0] // sp
    sb_size = cols // size
    scale = sb_size ** (-0.5)
    tile = rows // 2

    def at_block(b, start=0, extent=rows):
        return pl.ds(pl.multiple_of(b * rows + start, extent), extent)

    def pair(i, j):
        for part in range(rows // tile):
            mine = at_block(i, part * tile, tile)
            q = proj[0, mine, :]
            keys, values = proj[1, at_block(j), :], proj[2, at_block(j), :]
            lane = lax.broadcasted_iota(jnp.int32, (tile, cols), 1)
            query = jnp.concatenate(
                [jnp.where(lane // sb_size == h, q, jnp.zeros_like(q)) for h in range(size)], axis=0
            )
            score = dot_f32(query, keys, ((1,), (1,)))
            score = jnp.concatenate(
                [
                    score[h * tile : (h + 1) * tile] * scale + offset_ref[z * size + h]
                    for h in range(size)
                ],
                axis=0,
            )
            skip = jnp.maximum(score, jnp.log(1.0 + jnp.exp(jnp.minimum(score, 80.0))))
            weight = score - skip
            seen = across[:tile] < below[:tile] + (part * tile + (i - j) * rows)
            seen = jnp.concatenate([seen] * size, axis=0)
            skip = jnp.where(seen, skip, 0.0)
            sums = dot_f32(skip.astype(jnp.bfloat16), after[...])
            weight = jnp.where(seen, jnp.exp(weight - sums[:, :rows]), 0.0)
            out = dot_f32(weight.astype(jnp.bfloat16), values)
            mixed, total = out[:tile], sums[:tile, rows:]
            for h in range(1, size):
                at = slice(h * tile, (h + 1) * tile)
                mixed = jnp.where(lane // sb_size == h, out[at], mixed)
                total = jnp.where(lane // sb_size == h, sums[at, rows:], total)
            passed = later[mine, :]
            acc[mine, :] = acc[mine, :] + mixed * jnp.exp(-passed)
            later[mine, :] = passed + total

    span = BLOCK
    duo = 2 * span
    blocks = rows // span
    width = GDN_DIM
    seg_row = lax.broadcasted_iota(jnp.int32, (rows, rows), 0)
    seg_col = lax.broadcasted_iota(jnp.int32, (rows, rows), 1)
    together = seg_row // span == seg_col // span
    upto = jnp.where(jnp.logical_and(together, seg_row <= seg_col), 1.0, 0.0).astype(jnp.bfloat16)
    beyond_it = jnp.where(jnp.logical_and(together, seg_row > seg_col), 1.0, 0.0).astype(
        jnp.bfloat16
    )
    prow = lax.broadcasted_iota(jnp.int32, (span, duo), 0)
    plane = lax.broadcasted_iota(jnp.int32, (span, duo), 1)
    first = plane < span
    pcol = jnp.where(first, plane, plane - span)
    inclusive, strictly = pcol <= prow, pcol < prow
    unit = jnp.where(pcol == prow, 1.0, 0.0)
    diagonal = lax.broadcasted_iota(jnp.int32, (width, width), 0) == lax.broadcasted_iota(
        jnp.int32, (width, width), 1
    )
    eighth = lax.broadcasted_iota(jnp.int32, (8, rows), 0)

    def silu(a):
        return a * (1.0 / (1.0 + jnp.exp(-a)))

    def unit_of(a):
        return a * lax.rsqrt(jnp.sum(a * a, axis=-1, keepdims=True) + NORM_EPS)

    def apart(a):
        lanes = lax.broadcasted_iota(jnp.int32, a.shape, 1) < span
        zero = jnp.zeros_like(a)
        return jnp.concatenate([jnp.where(lanes, a, zero), jnp.where(lanes, zero, a)], axis=0)

    def squared(left, power):
        high, low = halves(power)
        lhigh, llow = halves(left)
        return folded(
            dot_f32(
                jnp.concatenate([lhigh, llow], axis=1), wide_rhs(apart(high), apart(low), 1)
            )
        )

    def prepare(b, dq, dk, dv):
        gates[...] = dot_f32(gate_all[...], xs[b], ((1,), (1,)))
        pre = gates[pl.ds(z, 1), :]
        write = gates[pl.ds(heads + z, 1), :] + write_bias_ref[z]
        rate = jnp.exp(jnp.full((1, rows), decay_scale_ref[z], jnp.float32))
        soft = jnp.maximum(pre, 0.0) + jnp.log(1.0 + jnp.exp(-jnp.abs(pre)))
        decay = shifts_ref[b, pl.ds(z, 1), :] - rate * soft
        strength = 1.0 / (1.0 + jnp.exp(-write))
        d1 = decay.astype(jnp.bfloat16).astype(jnp.float32)
        d2 = (decay - d1).astype(jnp.bfloat16).astype(jnp.float32)
        d3 = decay - d1 - d2
        three = jnp.where(
            eighth == 0, d1, jnp.where(eighth == 1, d2, jnp.where(eighth == 2, d3, 0.0))
        ).astype(jnp.bfloat16)
        cum_row = jnp.sum(dot_f32(three, upto), axis=0, keepdims=True)
        rest_row = jnp.sum(dot_f32(three, beyond_it), axis=0, keepdims=True)
        stack = jnp.where(
            eighth == 0, strength,
            jnp.where(
                eighth == 1, jnp.exp(cum_row),
                jnp.where(eighth == 2, jnp.exp(rest_row), cum_row),
            ),
        )
        columns = stack.T
        s_col, grow, damp, cum = (columns[:, n : n + 1] for n in range(4))
        q = unit_of(silu(dq)) * width ** (-0.5)
        k = unit_of(silu(dk))
        v = silu(dv)
        boosted = q * grow
        damped = k * damp
        right = jnp.concatenate([v * s_col, k * (s_col * grow)], axis=1)
        kh, kl = halves(k)
        qh, ql = halves(q)
        work = []
        for duo_at in range(rows // duo):
            lo = duo_at * duo
            here = slice(lo, lo + duo)
            left = jnp.concatenate(
                [
                    jnp.concatenate([kh[here], kl[here]], axis=1),
                    jnp.concatenate([qh[here], ql[here]], axis=1),
                ],
                axis=0,
            )
            gram = folded(
                dot_f32(left, wide_rhs(kh[here], kl[here], 0), ((1,), (1,)))
            )
            spread = (
                jnp.where(first, cum[lo : lo + span], cum[lo + span : lo + duo])
                - cum_row[:, here]
            )
            table = jnp.where(inclusive, jnp.exp(jnp.where(inclusive, spread, 0.0)), 0.0)
            scale_col = jnp.where(first, s_col[lo : lo + span], s_col[lo + span : lo + duo])
            near_k = jnp.where(first, gram[:span], gram[span:duo])
            near_q = jnp.where(first, gram[duo : duo + span], gram[duo + span :])
            strict = jnp.where(strictly, near_k * table * scale_col, 0.0)
            work.append([unit - strict, strict, near_q * table])
        yield
        for w in work:
            w[1] = squared(w[1], w[1])
        levels = max(1, (span - 1).bit_length()) - 1
        for level in range(levels):
            if level == levels // 2:
                yield
            for w in work:
                if level + 1 < levels:
                    both = squared(jnp.concatenate([w[1], w[0]], axis=0), w[1])
                    w[1], w[0] = both[:span], w[0] + both[span:]
                else:
                    w[0] = w[0] + squared(w[0], w[1])
        yield
        for duo_at, (inverse, _, inside) in enumerate(work):
            lo = duo_at * duo
            here = slice(lo, lo + duo)
            ih, il = (apart(a) for a in halves(inverse))
            rh, rl = halves(right[here])
            solved = dot_f32(
                jnp.concatenate([ih, il], axis=1), jnp.concatenate([rh, rh], axis=0)
            ) + dot_f32(ih, rl)
            lh, ll = (
                apart(a) for a in halves(jnp.concatenate([damped[here].T, inside], axis=0))
            )
            sh, sl = halves(solved)
            made = dot_f32(
                jnp.concatenate([lh, ll], axis=1), jnp.concatenate([sh, sh], axis=0)
            ) + dot_f32(lh, sl)
            for side in range(2):
                at = lo + side * span
                mine = made[side * (width + span) : (side + 1) * (width + span)]
                n = b * blocks + 2 * duo_at + side
                keep = grow[at + span - 1 : at + span]
                step_map = jnp.where(diagonal, keep, 0.0) - mine[:width, width:]
                query = boosted[at : at + span] - mine[width:, width:]
                high, low = halves(jnp.concatenate([step_map, query], axis=0))
                maps[n, :, :width] = high
                maps[n, :, width:] = low
                adds[n] = mine[:, :width]

    def give(which, out, target):
        here = target.at[:, pl.ds(pl.multiple_of(z * cols, cols), cols)]

        def send(g, k, sem):
            return remote(
                out.at[at_block(g), :], here,
                a_send.at[which], a_recv.at[sem], "sp", g,
            )

        def started(g):
            for k in range(1, sp):
                there = lax.rem(z + k, sp)
                if which == 0:
                    @pl.when(there == g)
                    def _():
                        send(there, k, 0).start()
                else:
                    slow = jnp.logical_or(
                        z == sp - 1, jnp.logical_and(z == 0, there == sp - 1)
                    )

                    @pl.when(jnp.logical_and(there == g, slow))
                    def _():
                        send(there, k, 2).start()

                    @pl.when(jnp.logical_and(there == g, jnp.logical_not(slow)))
                    def _():
                        send(there, k, 1).start()

        return started

    stick_started = give(0, stick_out, sticks)
    delta_started = give(1, delta_out, deltas)

    shorter = jnp.minimum(z, sp - 1 - z)
    down_last = z > sp - 1 - z

    def place(n):
        both = n <= 2 * shorter
        way_n = jnp.where(both, lax.rem(n + 1, 2), jnp.where(down_last, 0, 1))
        step_n = jnp.where(n == 0, 0, jnp.where(both, (n + 1) // 2, n - shorter))
        down = jnp.logical_and(way_n == 0, n > 0)
        return way_n, step_n, down, jnp.where(down, z - step_n, z + step_n)

    last_way = jnp.logical_or(z == 0, z == sp - 1)

    def block_ready(n):
        way_n, step_n, down, b = place(n)
        for step in range(1, sp):
            for way in range(2):
                @pl.when(jnp.logical_and(step_n == step, way_n == way))
                def _():
                    block_came(way, step)
        return b

    def delta_block(b):
        drows = dot_f32(xs[b], ws[:, 3 * cols :]).astype(jnp.bfloat16).astype(jnp.float32)
        return prepare(b, drows[:, :cols], drows[:, cols : 2 * cols], drows[:, 2 * cols :])

    last_way = jnp.logical_or(z == 0, z == sp - 1)
    from_top = z == sp - 1

    def stick_project(n):
        b = jnp.where(from_top, sp - 1 - n, n)
        out = dot_f32(xs[b], ws[:, : 3 * cols]).astype(jnp.bfloat16)
        for i in range(3):
            proj[i, at_block(b), :] = out[:, i * cols : (i + 1) * cols]

    def stick_place(n):
        between = jnp.where(
            n == 0, sp - 1, jnp.where(n == 1, 0, jnp.where(n == 2, sp - 1 - z, z))
        )
        return jnp.where(from_top, sp - 1 - n, jnp.where(last_way, n, between))

    def settle(i):
        stick_out[at_block(i), :] = acc[at_block(i), :].astype(jnp.bfloat16)

    def stick_pair(n, r):
        b = stick_place(n)
        i = jnp.where(from_top, b + r, b)
        j = jnp.where(from_top, b, b - r)
        pair(i, j)

        @pl.when(j == 0)
        def _():
            settle(i)
            stick_started(i)

    def walk_groups(start, stop, held=False):
        def group(g, c):
            @pl.when(g > start + held)
            def _():
                delta_started(g - 1)
            memory = memory_ref[...]
            for n in range(blocks):
                memory = walk(g * blocks + n, memory)
            memory_ref[...] = memory
            return c

        lax.fori_loop(start, stop, group, 0)
        delta_started(stop - 1)

    def walk(n, memory):
        high, low = halves(memory)
        new = folded(dot_f32(maps[n], wide_rhs(high, low, 1))) + adds[n]
        made = new[width:]
        made = made * lax.rsqrt(jnp.mean(made * made, axis=-1, keepdims=True) + NORM_EPS)
        at = pl.ds(pl.multiple_of(n * span, span), span)
        delta_out[at, :] = (made * gain_ref[...]).astype(delta_out.dtype)
        return new[:width]

    def plain_delta(n, c):
        @pl.when(n == 1)
        def _():
            relay(stick_kinds[0])

        @pl.when(n == sp - 2)
        def _():
            for c in early[parts:-1]:
                arrive(*c)
            relay(stick_kinds[1])

            @pl.when(z == 0)
            def _():
                walk_groups(0, 2)
            relay(stick_kinds[2])
            arrive(*early[-1])
        for _ in delta_block(block_ready(n)):
            pass
        return c

    events = jnp.where(last_way, sp - 1, sp)
    lax.fori_loop(0, events, plain_delta, 0)

    @pl.when(jnp.logical_not(last_way))
    def _():
        walk_groups(0, sp, held=True)

    relayed(stick_kinds)

    def stick_event(n, c):
        for part in range(2):
            @pl.when(jnp.logical_and(last_way, n == part + 1))
            def _():
                arrive(sp - 1, part)

        def project_one(m, c):
            stick_project(m)
            return c

        all_now = jnp.where(n == 0, sp, 0)
        lax.fori_loop(
            jnp.where(last_way, n, 0), jnp.where(last_way, n + 1, all_now), project_one, 0
        )

        @pl.when(jnp.logical_and(jnp.logical_not(last_way), n == 0))
        def _():
            delta_started(0)

        def one(r, c):
            for part in range(2, parts):
                @pl.when(
                    jnp.logical_and(
                        last_way, jnp.logical_and(n == sp - 2, r == sp - 1 - parts + part)
                    )
                )
                def _():
                    arrive(sp - 1, part)
            stick_pair(n, r)
            return c

        return lax.fori_loop(0, jnp.where(last_way, n, stick_place(n)) + 1, one, c)

    lax.fori_loop(0, events, stick_event, 0)

    @pl.when(last_way)
    def _():
        @pl.when(z == 0)
        def _():
            walk_groups(2, sp - 1)
        for way in range(2):
            @pl.when(comes(way, sp - 1))
            def _():
                block_came(way, sp - 1)
        stick_project(sp - 1)
        stages = delta_block(stick_place(sp - 1))
        for u in range(sp):
            next(stages, None)
            stick_pair(sp - 1, u)
        walk_groups(jnp.where(z == 0, sp - 1, 0), sp)

    mine_z = pl.ds(pl.multiple_of(z * rows, rows), rows)
    lanes = pl.ds(pl.multiple_of(z * cols, cols), cols)
    sticks[:, lanes] = stick_out[mine_z, :]
    deltas[:, lanes] = delta_out[mine_z, :]
    for c in late:
        c.wait()
    all_sent(ws.at[pl.ds(0, 3 * depth), :], w_send.at[0])
    all_sent(xs.at[:, :, slot], f_send.at[0])
    for c in range(sp):
        @pl.when(z == c)
        def _():
            for way, passed in enumerate((c + 1 if c + 1 < sp else 0, sp - c if c > 0 else 0)):
                if passed:
                    all_sent(xs.at[pl.ds(0, passed), :, slot], x_send.at[way])
                    all_sent(shifts_ref.at[pl.ds(0, passed)], s_send.at[way])
    all_came(stick_out.at[pl.ds(0, (sp - 1) * rows), :], a_recv.at[0])
    chunks, wide = outgoing.shape[0], outgoing.shape[2]
    share = rows // tp
    for c in range(chunks):
        columns = slice(c * wide, (c + 1) * wide)
        partial[:, columns] = dot_f32(sticks[...], sw_ref[:, columns])
    all_came(delta_out.at[pl.ds(0, (sp - 2) * rows), :], a_recv.at[1])
    soon = pl.ds(pl.multiple_of(jnp.where(from_top, 1, 0) * cols, cols), (sp - 1) * cols)
    for c in range(chunks):
        columns = slice(c * wide, (c + 1) * wide)
        partial[:, columns] += dot_f32(deltas[:, soon], dw_ref[soon, columns])
    all_came(delta_out.at[pl.ds(0, rows), :], a_recv.at[2])
    final = pl.ds(pl.multiple_of(jnp.where(from_top, 0, sp - 1) * cols, cols), cols)
    mine = pl.ds(pl.multiple_of(t * share, share), share)
    partner = lax.rem(t + 1, tp)
    theirs = pl.ds(pl.multiple_of(partner * share, share), share)

    def finish(which, c):
        columns = slice(c * wide, (c + 1) * wide)
        return (
            partial[which, columns] + dot_f32(deltas[which, final], dw_ref[final, columns])
        ).astype(jnp.bfloat16)

    swaps = [
        remote(
            outgoing.at[c], incoming.at[:, c * wide : (c + 1) * wide],
            c_sem.at[0], c_sem.at[1], "tp", partner,
        )
        for c in range(chunks)
    ]
    for c in range(chunks):
        outgoing[c] = finish(theirs, c)
        if c > 0:
            swaps[c - 1].start()
    for c in range(chunks):
        own[:, c * wide : (c + 1) * wide] = finish(mine, c)
        if c == 0:
            swaps[chunks - 1].start()
    all_came(incoming, c_sem.at[1])
    all_sent(incoming, c_sem.at[0])
    for which, out in enumerate((stick_out, delta_out)):
        all_sent(out.at[pl.ds(0, (sp - 1) * rows), :], a_send.at[which])


ANYWHERE = pl.BlockSpec(memory_space=pltpu.HBM)
ON_CORE = pl.BlockSpec(memory_space=pltpu.VMEM)


def on_device_heads(
    hidden_in, sb_query_w, sb_key_w, sb_value_w, sb_offset,
    delta_query_w, delta_key_w, delta_value_w, decay_w, write_w, write_bias,
    decay_log_scale, decay_shift, head_gain, sb_out_w, delta_out_w,
):
    sp, fs, tp = lax.axis_size("sp"), lax.axis_size("fs"), lax.axis_size("tp")
    rows, half = hidden_in.shape[1:]
    width = half * tp
    length = rows * sp
    heads = decay_log_scale.shape[0]
    cols = sb_query_w.shape[1] // sp
    parts, chunks = 4, 4
    share = rows // tp
    blocks = length // BLOCK
    dma = pltpu.SemaphoreType.DMA
    bf16, f32 = jnp.bfloat16, jnp.float32
    own, incoming = pl.pallas_call(
        layer_kernel,
        name="layer",
        out_shape=(pltpu.VMEM((share, width), bf16),) * 2,
        in_specs=[ANYWHERE] * 16,
        out_specs=(ON_CORE,) * 2,
        scratch_shapes=[
            pltpu.SMEM(sb_offset.shape, f32),
            pltpu.SMEM(decay_log_scale.shape, f32),
            pltpu.SMEM(write_bias.shape, f32),
            pltpu.VMEM((1, head_gain.shape[0]), f32),
            pltpu.VMEM((sp, rows, width), bf16),
            pltpu.VMEM((width, 6 * cols), bf16),
            pltpu.VMEM((2, heads, width), bf16),
            pltpu.VMEM((2 * heads, width), bf16),
            pltpu.VMEM((2 * heads, rows), f32),
            pltpu.VMEM((sp, heads, rows), f32),
            pltpu.VMEM((rows, rows + cols), bf16),
            pltpu.VMEM((3, length, cols), bf16),
            pltpu.VMEM((length, cols), f32),
            pltpu.VMEM((length, cols), f32),
            pltpu.VMEM((cols, cols), f32),
            pltpu.VMEM((blocks, cols + BLOCK, 2 * cols), bf16),
            pltpu.VMEM((blocks, cols + BLOCK, cols), f32),
            pltpu.VMEM((length, cols), bf16),
            pltpu.VMEM((length, cols), bf16),
            pltpu.VMEM((rows, cols * sp), bf16),
            pltpu.VMEM((rows, cols * sp), bf16),
            pltpu.VMEM(sb_out_w.shape, bf16),
            pltpu.VMEM(delta_out_w.shape, bf16),
            pltpu.VMEM((rows, width), f32),
            pltpu.VMEM((chunks, share, width // chunks), bf16),
            dma((2,)), dma((2, sp - 1, parts)), dma((1,)), dma((2 * sp - 1,)),
            dma((1,)), dma((2, 6)), dma((2,)), dma((2,)), dma((2, sp - 1)), dma((11,)),
            dma((2,)), dma((3,)), dma((2,)),
        ],
        compiler_params=pltpu.CompilerParams(
            collective_id=0, has_side_effects=True,
            vmem_limit_bytes=ALL_VMEM - 5 * share * width,
        ),
    )(
        sb_offset, decay_log_scale, write_bias,
        hidden_in.reshape(rows, half), sb_query_w, sb_key_w, sb_value_w,
        delta_query_w, delta_key_w, delta_value_w, decay_w.T, write_w.T,
        decay_shift.reshape(heads, rows), head_gain.reshape(1, -1), sb_out_w, delta_out_w,
    )
    result = (own.astype(f32) + incoming.astype(f32)).astype(bf16)
    return result.reshape(1, share, width)


def on_device(*inputs):
    delta_heads = inputs[11].shape[0]
    square = lax.axis_size("sp") == lax.axis_size("fs") == 4 and lax.axis_size("tp") == 2
    if square and delta_heads == lax.axis_size("sp") and inputs[4].shape[0] % delta_heads == 0:
        return on_device_heads(*inputs)
    return on_device_split(*inputs)


def solution(mesh):
    return jax.shard_map(
        on_device,
        mesh=mesh,
        in_specs=(
            P("fs", "sp", "tp"),
            P("fs", "tp"),
            P("fs", "tp"),
            P("fs", "tp"),
            P("tp"),
            P("fs", "tp"),
            P("fs", "tp"),
            P("fs", "tp"),
            P(None, "tp"),
            P(None, "tp"),
            P("tp"),
            P("tp"),
            P("fs", "tp", "sp"),
            P(),
            P("tp", None),
            P("tp", None),
        ),
        out_specs=P("fs", ("sp", "tp"), None),
        check_vma=False,
    )
```

```python
import jax
import jax.numpy as jnp
from jax import lax
from jax.experimental import pallas as pl
from jax.experimental.pallas import tpu as pltpu
from jax.sharding import PartitionSpec as P

MESH = pl.DeviceIdType.MESH
ALL_VMEM = 67043328

SB_DIM = 64
GDN_DIM = 128
BLOCK = 64


EXACT_MATMUL = lax.Precision.HIGHEST
NORM_EPS = 1e-06


def carried_in(value, axis, combine, identity):
    devices, index = (lax.axis_size(axis), lax.axis_index(axis))
    everything = jax.tree.map(
        lambda part, kind: lax.all_gather(part.astype(kind), axis),
        value,
        (jnp.bfloat16, jnp.bfloat16),
    )
    start = jax.tree.map(
        lambda part, zero: jnp.broadcast_to(jnp.asarray(zero, part.dtype), part.shape),
        value,
        identity,
    )

    def lap(k, before):
        reached = k < index
        new = combine(
            before, jax.tree.map(lambda part, own: part[k].astype(own.dtype), everything, value)
        )
        return jax.tree.map(lambda a, b: jnp.where(reached, a, b), new, before)

    return lax.fori_loop(0, devices, lap, start)


def unit_lower_inverse(strict_part):
    order_size = strict_part.shape[-1]
    powered = strict_part
    inverse = jnp.eye(order_size, dtype=strict_part.dtype) - strict_part
    for repeat_number in range(max(1, (order_size - 1).bit_length()) - 1):
        powered = jnp.einsum("...ij,...jk->...ik", powered, powered, precision=EXACT_MATMUL)
        inverse = inverse + jnp.einsum(
            "...ij,...jk->...ik", inverse, powered, precision=EXACT_MATMUL
        )
    return inverse


def to_blocks(row_data, block_span):
    blocks_count = row_data.shape[0] // block_span
    shaped = row_data.reshape((blocks_count, block_span) + row_data.shape[1:])
    return jnp.swapaxes(shaped, 1, 2)


def from_blocks(blocked):
    swapped = jnp.swapaxes(blocked, 1, 2)
    return swapped.reshape((-1,) + swapped.shape[2:])


def unit_rows(vectors):
    return vectors * lax.rsqrt(jnp.sum(vectors * vectors, axis=-1, keepdims=True) + NORM_EPS)


def delta_inputs(
    query_proj,
    key_proj,
    value_proj,
    decay_pre,
    write_pre,
    write_bias,
    decay_log_scale,
    shift_rows,
    head_count,
    head_size,
):
    query_act = jax.nn.silu(query_proj.astype(jnp.float32)).reshape(-1, head_count, head_size)
    key_act = jax.nn.silu(key_proj.astype(jnp.float32)).reshape(-1, head_count, head_size)
    value_rows = jax.nn.silu(value_proj.astype(jnp.float32)).reshape(-1, head_count, head_size)
    queries = unit_rows(query_act) * head_size ** (-0.5)
    key_rows = unit_rows(key_act)
    log_decay = -jnp.exp(decay_log_scale) * jax.nn.softplus(decay_pre) + shift_rows
    strength = jax.nn.sigmoid(write_pre + write_bias)
    return (queries, key_rows, value_rows, log_decay, strength)


def delta_prepare(queries, key_rows, value_rows, log_decay, strength):
    block_span = queries.shape[2]
    cumulative = jnp.cumsum(log_decay, axis=-1)
    row_place = lax.broadcasted_iota(jnp.int32, (block_span, block_span), 0)
    col_place = lax.broadcasted_iota(jnp.int32, (block_span, block_span), 1)
    inclusive = col_place <= row_place
    strictly = col_place < row_place
    spread = cumulative[..., :, None] - cumulative[..., None, :]
    decay_table = jnp.where(inclusive, jnp.exp(jnp.where(inclusive, spread, 0.0)), 0.0)
    keys_beta = key_rows * strength[..., None]
    lower_part = jnp.where(
        strictly,
        jnp.einsum("nhik,nhjk->nhij", keys_beta, key_rows, precision=EXACT_MATMUL) * decay_table,
        0.0,
    )
    inverse = unit_lower_inverse(lower_part)
    growth = jnp.exp(cumulative)
    state_updates = jnp.einsum(
        "nhij,nhjv->nhiv", inverse, value_rows * strength[..., None], precision=EXACT_MATMUL
    )
    erase_term = jnp.einsum(
        "nhij,nhjk->nhik", inverse, keys_beta * growth[..., None], precision=EXACT_MATMUL
    )
    inside_block = (
        jnp.einsum("nhik,nhjk->nhij", queries, key_rows, precision=EXACT_MATMUL) * decay_table
    )
    boosted_query = queries * growth[..., None]
    damped_keys = key_rows * jnp.exp(cumulative[..., -1:] - cumulative)[..., None]
    decay_per_block = jnp.exp(cumulative[..., -1])
    return (state_updates, erase_term, inside_block, boosted_query, damped_keys, decay_per_block)


def delta_step(memory_state, inputs):
    state_updates, erase_term, inside_block, boosted_query, damped_keys, decay_per_block = inputs
    fixed_values = state_updates - jnp.einsum(
        "mzq,mqc->mzc", erase_term, memory_state, precision=EXACT_MATMUL
    )
    produced_rows = jnp.einsum(
        "mzq,mqc->mzc", boosted_query, memory_state, precision=EXACT_MATMUL
    ) + jnp.einsum("efq,eqn->efn", inside_block, fixed_values, precision=EXACT_MATMUL)
    memory_state = memory_state * decay_per_block[:, None, None] + jnp.einsum(
        "wam,waz->wmz", damped_keys, fixed_values, precision=EXACT_MATMUL
    )
    return (memory_state, produced_rows)


def transition_step(carried, inputs):
    memory_state, transfer = carried
    state_updates, erase_term, inside_block, boosted_query, damped_keys, decay_per_block = inputs
    fixed_values = state_updates - jnp.einsum(
        "mzq,mqc->mzc", erase_term, memory_state, precision=EXACT_MATMUL
    )
    coupling = jnp.einsum("hik,hil->hkl", damped_keys, erase_term, precision=EXACT_MATMUL)
    memory_state = memory_state * decay_per_block[:, None, None] + jnp.einsum(
        "wam,waz->wmz", damped_keys, fixed_values, precision=EXACT_MATMUL
    )
    transfer = transfer * decay_per_block[:, None, None] - jnp.einsum(
        "hkl,hlm->hkm", coupling, transfer, precision=EXACT_MATMUL
    )
    return ((memory_state, transfer), None)


def compose(prior_blocks, following_blocks):
    joined_map = jnp.einsum(
        "hkl,hlm->hkm", following_blocks[0], prior_blocks[0], precision=EXACT_MATMUL
    )
    joined_state = (
        jnp.einsum("djo,dog->djg", following_blocks[0], prior_blocks[1], precision=EXACT_MATMUL)
        + following_blocks[1]
    )
    return (joined_map, joined_state)


def stick_block(queries, key_rows, value_rows, query_place, key_place, offsets):
    scale_factor = queries.shape[-1] ** (-0.5)
    scores = (
        jnp.einsum("qhd,khd->hqk", queries, key_rows, preferred_element_type=jnp.float32)
        * scale_factor
        + offsets[:, None, None]
    )
    visible = key_place[None, :] < query_place[:, None]
    skipped = jnp.where(visible, jax.nn.log_sigmoid(-scores), 0.0)
    beyond = lax.cumsum(skipped, axis=2, reverse=True) - skipped
    weights = jnp.where(visible, jnp.exp(jax.nn.log_sigmoid(scores) + beyond), 0.0).astype(
        jnp.bfloat16
    )
    partial_value = jnp.einsum(
        "hqk,khd->qhd", weights, value_rows, preferred_element_type=jnp.float32
    )
    return (partial_value, jnp.sum(skipped, axis=2).T)


def stick_combine(partials, totals):
    beyond = jnp.cumsum(totals[::-1], axis=0)[::-1] - totals
    return jnp.sum(partials * jnp.exp(beyond)[..., None], axis=0)


def on_device_split(
    hidden_in,
    sb_query_w,
    sb_key_w,
    sb_value_w,
    sb_offset,
    delta_query_w,
    delta_key_w,
    delta_value_w,
    decay_w,
    write_w,
    write_bias,
    decay_log_scale,
    decay_shift,
    head_gain,
    sb_out_w,
    delta_out_w,
):
    token_rows = hidden_in.shape[1]
    local_in = hidden_in.reshape(token_rows, hidden_in.shape[2])
    gathered = (
        lax.all_gather(sb_query_w, "fs", axis=0, tiled=True),
        lax.all_gather(sb_key_w, "fs", axis=0, tiled=True),
        lax.all_gather(sb_value_w, "fs", axis=0, tiled=True),
        lax.all_gather(delta_query_w, "fs", axis=0, tiled=True),
        lax.all_gather(delta_key_w, "fs", axis=0, tiled=True),
        lax.all_gather(delta_value_w, "fs", axis=0, tiled=True),
    )
    in_weights = tuple(gathered) + (decay_w, write_w)
    portion = lax.all_gather(local_in, "tp", axis=1, tiled=True)
    projected = tuple(
        (jnp.dot(portion, weight, preferred_element_type=jnp.float32) for weight in in_weights)
    )
    sb_heads = sb_offset.shape[0]
    delta_heads = decay_log_scale.shape[0]
    sb_query = projected[0].astype(jnp.bfloat16).reshape(token_rows, sb_heads, SB_DIM)
    sb_keys = projected[1].astype(jnp.bfloat16)
    sb_values = projected[2].astype(jnp.bfloat16)
    shift_rows = decay_shift.reshape(delta_heads, token_rows).T
    queries, key_rows, value_rows, log_decay, strength = delta_inputs(
        projected[3].astype(jnp.bfloat16),
        projected[4].astype(jnp.bfloat16),
        projected[5].astype(jnp.bfloat16),
        projected[6],
        projected[7],
        write_bias,
        decay_log_scale,
        shift_rows,
        delta_heads,
        GDN_DIM,
    )
    prepared = delta_prepare(
        to_blocks(queries, BLOCK),
        to_blocks(key_rows, BLOCK),
        to_blocks(value_rows, BLOCK),
        to_blocks(log_decay, BLOCK),
        to_blocks(strength, BLOCK),
    )
    identity_map = jnp.broadcast_to(
        jnp.eye(GDN_DIM, dtype=jnp.float32), (delta_heads, GDN_DIM, GDN_DIM)
    )
    empty_state = jnp.zeros((delta_heads, GDN_DIM, GDN_DIM), jnp.float32)
    (local_end, local_map), unused_out = lax.scan(
        transition_step, (empty_state, identity_map), prepared
    )
    own_first = lax.axis_index("sp") * token_rows
    query_place = own_first + lax.iota(jnp.int32, token_rows)
    sp_count = lax.axis_size("sp")
    slot_out = jnp.zeros((sp_count, token_rows, sb_heads, SB_DIM), jnp.float32)
    slot_total = jnp.zeros((sp_count, token_rows, sb_heads), jnp.float32)

    def absorb(slot_arrays, address_portion, value_part, shard_first):

        def active(current):
            partial_value, totals = stick_block(
                sb_query,
                address_portion.reshape(token_rows, sb_heads, SB_DIM),
                value_part.reshape(token_rows, sb_heads, SB_DIM),
                query_place,
                shard_first + lax.iota(jnp.int32, token_rows),
                sb_offset,
            )
            slot_index = shard_first // token_rows
            return (
                lax.dynamic_update_index_in_dim(current[0], partial_value, slot_index, 0),
                lax.dynamic_update_index_in_dim(current[1], totals, slot_index, 0),
            )

        def inactive(current):
            return current

        usable = jnp.logical_and(shard_first >= 0, shard_first <= own_first)
        return lax.cond(usable, active, inactive, slot_arrays)

    key_block = lax.all_gather(sb_keys, "sp", axis=0, tiled=True)
    value_block = lax.all_gather(sb_values, "sp", axis=0, tiled=True)

    def per_shard(shard_number, current):
        row_begin = shard_number * token_rows
        return absorb(
            current,
            lax.dynamic_slice_in_dim(key_block, row_begin, token_rows, 0),
            lax.dynamic_slice_in_dim(value_block, row_begin, token_rows, 0),
            row_begin,
        )

    slot_arrays = lax.fori_loop(
        0, key_block.shape[0] // token_rows, per_shard, (slot_out, slot_total)
    )
    unused_map, incoming = carried_in(
        (local_map, local_end), "sp", compose, (identity_map, empty_state)
    )
    sb_mixed = (
        stick_combine(slot_arrays[0], slot_arrays[1])
        .astype(jnp.bfloat16)
        .reshape(token_rows, sb_heads * SB_DIM)
    )
    unused_end, produced_rows = lax.scan(delta_step, incoming, prepared)
    produced_rows = from_blocks(produced_rows)
    normed = (
        produced_rows
        * lax.rsqrt(jnp.mean(produced_rows * produced_rows, axis=-1, keepdims=True) + NORM_EPS)
        * head_gain
    )
    delta_mixed = normed.astype(jnp.bfloat16).reshape(token_rows, delta_heads * GDN_DIM)
    result = lax.psum_scatter(
        (
            jnp.dot(sb_mixed, sb_out_w, preferred_element_type=jnp.float32)
            + jnp.dot(delta_mixed, delta_out_w, preferred_element_type=jnp.float32)
        ).astype(jnp.bfloat16),
        "tp",
        scatter_dimension=0,
        tiled=True,
    ).astype(jnp.float32)
    return result.astype(jnp.bfloat16).reshape(1, result.shape[0], result.shape[1])


def remote(src, dst, send, recv, axis, index):
    return pltpu.make_async_remote_copy(
        src_ref=src, dst_ref=dst, send_sem=send, recv_sem=recv,
        device_id={axis: index}, device_id_type=MESH,
    )


def greet(axes):
    barrier = pltpu.get_barrier_semaphore()
    count = 0
    for axis in axes:
        size, me = lax.axis_size(axis), lax.axis_index(axis)
        for k in range(1, size):
            pl.semaphore_signal(
                barrier, inc=1, device_id={axis: lax.rem(me + k, size)}, device_id_type=MESH
            )
            count += 1
    pl.semaphore_wait(barrier, count)


def halves(a):
    high = a.astype(jnp.bfloat16)
    return high, (a - high.astype(jnp.float32)).astype(jnp.bfloat16)


def dot_f32(a, b, dims=((1,), (0,))):
    return lax.dot_general(a, b, (dims, ((), ())), preferred_element_type=jnp.float32)


def wide_rhs(high, low, axis):
    top = jnp.concatenate([high, low], axis=axis)
    bottom = jnp.concatenate([high, jnp.zeros_like(low)], axis=axis)
    return jnp.concatenate([top, bottom], axis=1 - axis)


def folded(a):
    half = a.shape[1] // 2
    return a[:, :half] + a[:, half:]


def layer_kernel(
    offset_hbm, decay_scale_hbm, write_bias_hbm,
    x_ref, w0, w1, w2, w3, w4, w5, decay_w_ref, write_w_ref, shift_ref, gain_hbm, sw_hbm, dw_hbm,
    own, incoming,
    offset_ref, decay_scale_ref, write_bias_ref, gain_ref,
    xs, ws, gate_w, gate_all, gates, shifts_ref, after,
    proj, acc, later, memory_ref, maps, adds, stick_out, delta_out,
    sticks, deltas, sw_ref, dw_ref, partial, outgoing,
    x_send, x_recv, f_send, f_recv, w_send, w_recv, r_recv, s_send, s_recv, l_sem,
    a_send, a_recv, c_sem,
):
    weights = (w0, w1, w2, w3, w4, w5)
    sp, tp = lax.axis_size("sp"), lax.axis_size("tp")
    z, f, t = lax.axis_index("sp"), lax.axis_index("fs"), lax.axis_index("tp")
    rows, half = x_ref.shape
    depth = w0.shape[0]
    cols = ws.shape[1] // len(weights)
    parts = x_recv.shape[2]
    heads = decay_w_ref.shape[0]
    slot = pl.ds(pl.multiple_of(t * half, half), half)
    local = [
        pltpu.make_async_copy(x_ref, xs.at[z, :, slot], l_sem.at[0]),
        pltpu.make_async_copy(shift_ref, shifts_ref.at[z], l_sem.at[1]),
        pltpu.make_async_copy(decay_w_ref, gate_w.at[0], l_sem.at[2]),
        pltpu.make_async_copy(write_w_ref, gate_w.at[1], l_sem.at[3]),
        pltpu.make_async_copy(offset_hbm, offset_ref, l_sem.at[6]),
        pltpu.make_async_copy(decay_scale_hbm, decay_scale_ref, l_sem.at[7]),
        pltpu.make_async_copy(write_bias_hbm, write_bias_ref, l_sem.at[8]),
        pltpu.make_async_copy(gain_hbm, gain_ref, l_sem.at[9]),
    ]
    late = [
        pltpu.make_async_copy(sw_hbm, sw_ref, l_sem.at[4]),
        pltpu.make_async_copy(dw_hbm, dw_ref, l_sem.at[5]),
    ]

    def w_src(i):
        return weights[i].at[:, pl.ds(pl.multiple_of(z * cols, cols), cols)]

    def w_at(i, who):
        return ws.at[pl.ds(pl.multiple_of(who * depth, depth), depth), pl.ds(i * cols, cols)]

    local_w = [
        pltpu.make_async_copy(w_src(i), w_at(i, f), l_sem.at[10]) for i in range(len(weights))
    ]
    near = (f + 1 - 2 * (f % 2), f + 2 - 4 * (f // 2))
    count = len(weights)
    delta_kinds, stick_kinds = (3, 4, 5), (0, 1, 2)

    def onward(way):
        return z + 1 < sp if way == 0 else z > 0

    def ahead(way):
        return z + 1 if way == 0 else z - 1

    barrier = pltpu.get_barrier_semaphore()
    for way in range(2):
        @pl.when(onward(way))
        def _():
            pl.semaphore_signal(
                barrier, inc=1, device_id={"sp": ahead(way)}, device_id_type=MESH
            )
    for side in range(2):
        pl.semaphore_signal(barrier, inc=1, device_id={"fs": near[side]}, device_id_type=MESH)
    pl.semaphore_signal(
        barrier, inc=1, device_id={"tp": lax.rem(t + 1, tp)}, device_id_type=MESH
    )
    for c in local + local_w:
        c.start()
    peers = onward(0).astype(jnp.int32) + onward(1).astype(jnp.int32) + 3
    pl.semaphore_wait(barrier, peers)

    def x_copy(way, step, part):
        block = z - (step - 1) if way == 0 else z + (step - 1)
        piece = pl.ds(part * (rows // parts), rows // parts)
        there = xs.at[block, piece, slot]
        return remote(
            x_ref.at[piece, :] if step == 1 else there, there,
            x_send.at[way], x_recv.at[way, step - 1, part], "sp", ahead(way),
        )

    def shift_copy(way, step):
        block = z - (step - 1) if way == 0 else z + (step - 1)
        there = shifts_ref.at[block]
        return remote(
            shift_ref if step == 1 else there, there,
            s_send.at[way], s_recv.at[way, step - 1], "sp", ahead(way),
        )

    def comes(way, step):
        return z >= step if way == 0 else z + step < sp

    def sends(way, step):
        return jnp.logical_and(onward(way), comes(way, step - 1))

    def forward(way, step, part):
        block = z - step if way == 0 else z + step
        piece = pl.ds(part * (rows // parts), rows // parts)
        there = xs.at[block, piece, slot]
        return remote(
            x_ref.at[piece, :] if step == 0 else there, there,
            f_send.at[0], f_recv.at[way * (sp - 1) + step], "tp", lax.rem(t + 1, tp),
        )

    def w_copy(side, i):
        return remote(
            w_src(i), w_at(i, f), w_send.at[0], w_recv.at[side, i], "fs", near[side]
        )

    def w_relay(side, i):
        part = depth // 2
        start = pl.multiple_of(near[side] * depth + side * part, part)
        there = ws.at[pl.ds(start, part), pl.ds(i * cols, cols)]
        return remote(
            there, there, w_send.at[0], r_recv.at[i // 3], "fs", near[1 - side]
        )

    for part in range(parts):
        for way in range(2):
            @pl.when(onward(way))
            def _():
                x_copy(way, 1, part).start()
                if part == 0:
                    shift_copy(way, 1).start()
    for i in delta_kinds:
        for side in range(2):
            w_copy(side, i).start()
    for part in range(parts):
        forward(0, 0, part).start()

    def relay(i):
        for side in range(2):
            w_copy(side, i).wait_recv()
            w_relay(side, i).start()

    def arrive(step, part):
        for way in range(2):
            @pl.when(comes(way, step))
            def _():
                x_copy(way, step, part).wait_recv()
                forward(way, step, part).start()
                if step + 1 < sp:
                    @pl.when(onward(way))
                    def _():
                        x_copy(way, step + 1, part).start()
                if part == 0:
                    shift_copy(way, step).wait_recv()
                    if step + 1 < sp:
                        @pl.when(onward(way))
                        def _():
                            shift_copy(way, step + 1).start()

    below = lax.broadcasted_iota(jnp.int32, (rows, rows), 0)
    across = lax.broadcasted_iota(jnp.int32, (rows, rows), 1)
    after[:, :rows] = jnp.where(below > across, 1.0, 0.0).astype(jnp.bfloat16)
    after[:, rows:] = jnp.ones((rows, cols), jnp.bfloat16)
    acc[...] = jnp.zeros_like(acc)
    later[...] = jnp.zeros_like(later)
    memory_ref[...] = jnp.zeros_like(memory_ref)
    early = [(step, part) for step in range(1, sp - 1) for part in range(parts)]
    relay(delta_kinds[0])
    arrive(*early[0])
    for i in delta_kinds[1:]:
        relay(i)
    for i in stick_kinds:
        for side in range(2):
            w_copy(side, i).start()
    for c in late:
        c.start()
    for step, part in early[1:parts]:
        arrive(step, part)
    for c in local:
        c.wait()
    own_w = ws.at[pl.ds(pl.multiple_of(f * depth, depth), depth), :]
    pltpu.make_async_copy(own_w, own_w, l_sem.at[10]).wait()
    gate_all[...] = jnp.concatenate(
        [gate_w[0].astype(jnp.float32), gate_w[1].astype(jnp.float32)], axis=0
    ).astype(jnp.bfloat16)
    def all_sent(ref, sem):
        remote(ref, ref, sem, sem, "tp", lax.rem(t + 1, tp)).wait_send()

    def all_came(ref, sem):
        remote(ref, ref, sem, sem, "tp", lax.rem(t + 1, tp)).wait_recv()

    def block_came(way, step):
        all_came(xs.at[z, :, slot], f_recv.at[way * (sp - 1) + step])

    block_came(0, 0)

    def relayed(kinds):
        first = kinds[0] * cols
        all_came(ws.at[pl.ds(0, depth), pl.ds(first, len(kinds) * cols)], r_recv.at[kinds[0] // 3])

    relayed(delta_kinds)

    size = offset_ref.shape[0] // sp
    sb_size = cols // size
    scale = sb_size ** (-0.5)
    tile = rows // 2

    def at_block(b, start=0, extent=rows):
        return pl.ds(pl.multiple_of(b * rows + start, extent), extent)

    def pair(i, j):
        for part in range(rows // tile):
            mine = at_block(i, part * tile, tile)
            q = proj[0, mine, :]
            keys, values = proj[1, at_block(j), :], proj[2, at_block(j), :]
            lane = lax.broadcasted_iota(jnp.int32, (tile, cols), 1)
            query = jnp.concatenate(
                [jnp.where(lane // sb_size == h, q, jnp.zeros_like(q)) for h in range(size)], axis=0
            )
            score = dot_f32(query, keys, ((1,), (1,)))
            score = jnp.concatenate(
                [
                    score[h * tile : (h + 1) * tile] * scale + offset_ref[z * size + h]
                    for h in range(size)
                ],
                axis=0,
            )
            skip = jnp.maximum(score, jnp.log(1.0 + jnp.exp(jnp.minimum(score, 80.0))))
            weight = score - skip
            seen = across[:tile] < below[:tile] + (part * tile + (i - j) * rows)
            seen = jnp.concatenate([seen] * size, axis=0)
            skip = jnp.where(seen, skip, 0.0)
            sums = dot_f32(skip.astype(jnp.bfloat16), after[...])
            weight = jnp.where(seen, jnp.exp(weight - sums[:, :rows]), 0.0)
            out = dot_f32(weight.astype(jnp.bfloat16), values)
            mixed, total = out[:tile], sums[:tile, rows:]
            for h in range(1, size):
                at = slice(h * tile, (h + 1) * tile)
                mixed = jnp.where(lane // sb_size == h, out[at], mixed)
                total = jnp.where(lane // sb_size == h, sums[at, rows:], total)
            passed = later[mine, :]
            acc[mine, :] = acc[mine, :] + mixed * jnp.exp(-passed)
            later[mine, :] = passed + total

    span = BLOCK
    duo = 2 * span
    blocks = rows // span
    width = GDN_DIM
    seg_row = lax.broadcasted_iota(jnp.int32, (rows, rows), 0)
    seg_col = lax.broadcasted_iota(jnp.int32, (rows, rows), 1)
    together = seg_row // span == seg_col // span
    upto = jnp.where(jnp.logical_and(together, seg_row <= seg_col), 1.0, 0.0).astype(jnp.bfloat16)
    beyond_it = jnp.where(jnp.logical_and(together, seg_row > seg_col), 1.0, 0.0).astype(
        jnp.bfloat16
    )
    prow = lax.broadcasted_iota(jnp.int32, (span, duo), 0)
    plane = lax.broadcasted_iota(jnp.int32, (span, duo), 1)
    first = plane < span
    pcol = jnp.where(first, plane, plane - span)
    inclusive, strictly = pcol <= prow, pcol < prow
    unit = jnp.where(pcol == prow, 1.0, 0.0)
    diagonal = lax.broadcasted_iota(jnp.int32, (width, width), 0) == lax.broadcasted_iota(
        jnp.int32, (width, width), 1
    )
    eighth = lax.broadcasted_iota(jnp.int32, (8, rows), 0)

    def silu(a):
        return a * (1.0 / (1.0 + jnp.exp(-a)))

    def unit_of(a):
        return a * lax.rsqrt(jnp.sum(a * a, axis=-1, keepdims=True) + NORM_EPS)

    def apart(a):
        lanes = lax.broadcasted_iota(jnp.int32, a.shape, 1) < span
        zero = jnp.zeros_like(a)
        return jnp.concatenate([jnp.where(lanes, a, zero), jnp.where(lanes, zero, a)], axis=0)

    def squared(left, power):
        high, low = halves(power)
        lhigh, llow = halves(left)
        return folded(
            dot_f32(
                jnp.concatenate([lhigh, llow], axis=1), wide_rhs(apart(high), apart(low), 1)
            )
        )

    def prepare(b, dq, dk, dv):
        gates[...] = dot_f32(gate_all[...], xs[b], ((1,), (1,)))
        pre = gates[pl.ds(z, 1), :]
        write = gates[pl.ds(heads + z, 1), :] + write_bias_ref[z]
        rate = jnp.exp(jnp.full((1, rows), decay_scale_ref[z], jnp.float32))
        soft = jnp.maximum(pre, 0.0) + jnp.log(1.0 + jnp.exp(-jnp.abs(pre)))
        decay = shifts_ref[b, pl.ds(z, 1), :] - rate * soft
        strength = 1.0 / (1.0 + jnp.exp(-write))
        d1 = decay.astype(jnp.bfloat16).astype(jnp.float32)
        d2 = (decay - d1).astype(jnp.bfloat16).astype(jnp.float32)
        d3 = decay - d1 - d2
        three = jnp.where(
            eighth == 0, d1, jnp.where(eighth == 1, d2, jnp.where(eighth == 2, d3, 0.0))
        ).astype(jnp.bfloat16)
        cum_row = jnp.sum(dot_f32(three, upto), axis=0, keepdims=True)
        rest_row = jnp.sum(dot_f32(three, beyond_it), axis=0, keepdims=True)
        stack = jnp.where(
            eighth == 0, strength,
            jnp.where(
                eighth == 1, jnp.exp(cum_row),
                jnp.where(eighth == 2, jnp.exp(rest_row), cum_row),
            ),
        )
        columns = stack.T
        s_col, grow, damp, cum = (columns[:, n : n + 1] for n in range(4))
        q = unit_of(silu(dq)) * width ** (-0.5)
        k = unit_of(silu(dk))
        v = silu(dv)
        boosted = q * grow
        damped = k * damp
        right = jnp.concatenate([v * s_col, k * (s_col * grow)], axis=1)
        kh, kl = halves(k)
        qh, ql = halves(q)
        work = []
        for duo_at in range(rows // duo):
            lo = duo_at * duo
            here = slice(lo, lo + duo)
            left = jnp.concatenate(
                [
                    jnp.concatenate([kh[here], kl[here]], axis=1),
                    jnp.concatenate([qh[here], ql[here]], axis=1),
                ],
                axis=0,
            )
            gram = folded(
                dot_f32(left, wide_rhs(kh[here], kl[here], 0), ((1,), (1,)))
            )
            spread = (
                jnp.where(first, cum[lo : lo + span], cum[lo + span : lo + duo])
                - cum_row[:, here]
            )
            table = jnp.where(inclusive, jnp.exp(jnp.where(inclusive, spread, 0.0)), 0.0)
            scale_col = jnp.where(first, s_col[lo : lo + span], s_col[lo + span : lo + duo])
            near_k = jnp.where(first, gram[:span], gram[span:duo])
            near_q = jnp.where(first, gram[duo : duo + span], gram[duo + span :])
            strict = jnp.where(strictly, near_k * table * scale_col, 0.0)
            work.append([unit - strict, strict, near_q * table])
        yield
        for w in work:
            w[1] = squared(w[1], w[1])
        levels = max(1, (span - 1).bit_length()) - 1
        for level in range(levels):
            if level == levels // 2:
                yield
            for w in work:
                if level + 1 < levels:
                    both = squared(jnp.concatenate([w[1], w[0]], axis=0), w[1])
                    w[1], w[0] = both[:span], w[0] + both[span:]
                else:
                    w[0] = w[0] + squared(w[0], w[1])
        yield
        for duo_at, (inverse, _, inside) in enumerate(work):
            lo = duo_at * duo
            here = slice(lo, lo + duo)
            ih, il = (apart(a) for a in halves(inverse))
            rh, rl = halves(right[here])
            solved = dot_f32(
                jnp.concatenate([ih, il], axis=1), jnp.concatenate([rh, rh], axis=0)
            ) + dot_f32(ih, rl)
            lh, ll = (
                apart(a) for a in halves(jnp.concatenate([damped[here].T, inside], axis=0))
            )
            sh, sl = halves(solved)
            made = dot_f32(
                jnp.concatenate([lh, ll], axis=1), jnp.concatenate([sh, sh], axis=0)
            ) + dot_f32(lh, sl)
            for side in range(2):
                at = lo + side * span
                mine = made[side * (width + span) : (side + 1) * (width + span)]
                n = b * blocks + 2 * duo_at + side
                keep = grow[at + span - 1 : at + span]
                step_map = jnp.where(diagonal, keep, 0.0) - mine[:width, width:]
                query = boosted[at : at + span] - mine[width:, width:]
                high, low = halves(jnp.concatenate([step_map, query], axis=0))
                maps[n, :, :width] = high
                maps[n, :, width:] = low
                adds[n] = mine[:, :width]

    def give(which, out, target):
        here = target.at[:, pl.ds(pl.multiple_of(z * cols, cols), cols)]

        def send(g, k, sem):
            return remote(
                out.at[at_block(g), :], here,
                a_send.at[which], a_recv.at[sem], "sp", g,
            )

        def started(g):
            for k in range(1, sp):
                there = lax.rem(z + k, sp)
                if which == 0:
                    @pl.when(there == g)
                    def _():
                        send(there, k, 0).start()
                else:
                    slow = jnp.logical_or(
                        z == sp - 1, jnp.logical_and(z == 0, there == sp - 1)
                    )

                    @pl.when(jnp.logical_and(there == g, slow))
                    def _():
                        send(there, k, 2).start()

                    @pl.when(jnp.logical_and(there == g, jnp.logical_not(slow)))
                    def _():
                        send(there, k, 1).start()

        return started

    stick_started = give(0, stick_out, sticks)
    delta_started = give(1, delta_out, deltas)

    shorter = jnp.minimum(z, sp - 1 - z)
    down_last = z > sp - 1 - z

    def place(n):
        both = n <= 2 * shorter
        way_n = jnp.where(both, lax.rem(n + 1, 2), jnp.where(down_last, 0, 1))
        step_n = jnp.where(n == 0, 0, jnp.where(both, (n + 1) // 2, n - shorter))
        down = jnp.logical_and(way_n == 0, n > 0)
        return way_n, step_n, down, jnp.where(down, z - step_n, z + step_n)

    last_way = jnp.logical_or(z == 0, z == sp - 1)

    def block_ready(n):
        way_n, step_n, down, b = place(n)
        for step in range(1, sp):
            for way in range(2):
                @pl.when(jnp.logical_and(step_n == step, way_n == way))
                def _():
                    block_came(way, step)
        return b

    def delta_block(b):
        drows = dot_f32(xs[b], ws[:, 3 * cols :]).astype(jnp.bfloat16).astype(jnp.float32)
        return prepare(b, drows[:, :cols], drows[:, cols : 2 * cols], drows[:, 2 * cols :])

    last_way = jnp.logical_or(z == 0, z == sp - 1)
    from_top = z == sp - 1

    def stick_project(n):
        b = jnp.where(from_top, sp - 1 - n, n)
        out = dot_f32(xs[b], ws[:, : 3 * cols]).astype(jnp.bfloat16)
        for i in range(3):
            proj[i, at_block(b), :] = out[:, i * cols : (i + 1) * cols]

    def stick_place(n):
        lower = z < sp // 2
        between = jnp.where(
            n == 0,
            jnp.where(lower, sp - 1, 0),
            jnp.where(
                n == 1,
                jnp.where(lower, sp - 2, 1),
                jnp.where(n == 2, jnp.where(lower, 0, sp - 1), z),
            ),
        )
        return jnp.where(from_top, sp - 1 - n, jnp.where(last_way, n, between))

    def settle(i):
        stick_out[at_block(i), :] = acc[at_block(i), :].astype(jnp.bfloat16)

    def stick_pair(n, r):
        b = stick_place(n)
        i = jnp.where(from_top, b + r, b)
        j = jnp.where(from_top, b, b - r)
        pair(i, j)

        @pl.when(j == 0)
        def _():
            settle(i)
            stick_started(i)

    def walk_groups(start, stop, held=False):
        def group(g, c):
            @pl.when(g > start + held)
            def _():
                delta_started(g - 1)
            memory = memory_ref[...]
            for n in range(blocks):
                memory = walk(g * blocks + n, memory)
            memory_ref[...] = memory
            return c

        lax.fori_loop(start, stop, group, 0)
        delta_started(stop - 1)

    def walk(n, memory):
        high, low = halves(memory)
        new = folded(dot_f32(maps[n], wide_rhs(high, low, 1))) + adds[n]
        made = new[width:]
        made = made * lax.rsqrt(jnp.mean(made * made, axis=-1, keepdims=True) + NORM_EPS)
        at = pl.ds(pl.multiple_of(n * span, span), span)
        delta_out[at, :] = (made * gain_ref[...]).astype(delta_out.dtype)
        return new[:width]

    def plain_delta(n, c):
        @pl.when(n == 1)
        def _():
            relay(stick_kinds[0])

        @pl.when(n == sp - 2)
        def _():
            for c in early[parts:-1]:
                arrive(*c)
            relay(stick_kinds[1])

            @pl.when(z == 0)
            def _():
                walk_groups(0, 2)
            relay(stick_kinds[2])
            arrive(*early[-1])
        for _ in delta_block(block_ready(n)):
            pass
        return c

    events = jnp.where(last_way, sp - 1, sp)
    lax.fori_loop(0, events, plain_delta, 0)

    @pl.when(jnp.logical_not(last_way))
    def _():
        walk_groups(0, sp, held=True)

    relayed(stick_kinds)

    def stick_event(n, c):
        for part in range(2):
            @pl.when(jnp.logical_and(last_way, n == part + 1))
            def _():
                arrive(sp - 1, part)

        def project_one(m, c):
            stick_project(m)
            return c

        needed = jnp.where(from_top, n, stick_place(n)) + 1
        lax.fori_loop(c, needed, project_one, 0)

        @pl.when(jnp.logical_and(jnp.logical_not(last_way), n == 0))
        def _():
            delta_started(0)

        def one(r, c):
            for part in range(2, parts):
                @pl.when(
                    jnp.logical_and(
                        last_way, jnp.logical_and(n == sp - 2, r == sp - 1 - parts + part)
                    )
                )
                def _():
                    arrive(sp - 1, part)
            stick_pair(n, r)
            return c

        lax.fori_loop(0, jnp.where(last_way, n, stick_place(n)) + 1, one, 0)
        return jnp.maximum(c, needed)

    lax.fori_loop(0, events, stick_event, 0)

    @pl.when(last_way)
    def _():
        @pl.when(z == 0)
        def _():
            walk_groups(2, sp - 1)
        for way in range(2):
            @pl.when(comes(way, sp - 1))
            def _():
                block_came(way, sp - 1)
        stick_project(sp - 1)
        stages = delta_block(stick_place(sp - 1))
        for u in range(sp):
            next(stages, None)
            stick_pair(sp - 1, u)
        walk_groups(jnp.where(z == 0, sp - 1, 0), sp)

    mine_z = pl.ds(pl.multiple_of(z * rows, rows), rows)
    lanes = pl.ds(pl.multiple_of(z * cols, cols), cols)
    sticks[:, lanes] = stick_out[mine_z, :]
    deltas[:, lanes] = delta_out[mine_z, :]
    for c in late:
        c.wait()
    all_sent(ws.at[pl.ds(0, 3 * depth), :], w_send.at[0])
    all_sent(xs.at[:, :, slot], f_send.at[0])
    for c in range(sp):
        @pl.when(z == c)
        def _():
            for way, passed in enumerate((c + 1 if c + 1 < sp else 0, sp - c if c > 0 else 0)):
                if passed:
                    all_sent(xs.at[pl.ds(0, passed), :, slot], x_send.at[way])
                    all_sent(shifts_ref.at[pl.ds(0, passed)], s_send.at[way])
    all_came(stick_out.at[pl.ds(0, (sp - 1) * rows), :], a_recv.at[0])
    chunks, wide = outgoing.shape[0], outgoing.shape[2]
    share = rows // tp
    for c in range(chunks):
        columns = slice(c * wide, (c + 1) * wide)
        partial[:, columns] = dot_f32(sticks[...], sw_ref[:, columns])
    all_came(delta_out.at[pl.ds(0, (sp - 2) * rows), :], a_recv.at[1])
    soon = pl.ds(pl.multiple_of(jnp.where(from_top, 1, 0) * cols, cols), (sp - 1) * cols)
    for c in range(chunks):
        columns = slice(c * wide, (c + 1) * wide)
        partial[:, columns] += dot_f32(deltas[:, soon], dw_ref[soon, columns])
    all_came(delta_out.at[pl.ds(0, rows), :], a_recv.at[2])
    final = pl.ds(pl.multiple_of(jnp.where(from_top, 0, sp - 1) * cols, cols), cols)
    mine = pl.ds(pl.multiple_of(t * share, share), share)
    partner = lax.rem(t + 1, tp)
    theirs = pl.ds(pl.multiple_of(partner * share, share), share)

    def finish(which, c):
        columns = slice(c * wide, (c + 1) * wide)
        return (
            partial[which, columns] + dot_f32(deltas[which, final], dw_ref[final, columns])
        ).astype(jnp.bfloat16)

    swaps = [
        remote(
            outgoing.at[c], incoming.at[:, c * wide : (c + 1) * wide],
            c_sem.at[0], c_sem.at[1], "tp", partner,
        )
        for c in range(chunks)
    ]
    for c in range(chunks):
        outgoing[c] = finish(theirs, c)
        if c > 0:
            swaps[c - 1].start()
    for c in range(chunks):
        own[:, c * wide : (c + 1) * wide] = finish(mine, c)
        if c == 0:
            swaps[chunks - 1].start()
    all_came(incoming, c_sem.at[1])
    all_sent(incoming, c_sem.at[0])
    for which, out in enumerate((stick_out, delta_out)):
        all_sent(out.at[pl.ds(0, (sp - 1) * rows), :], a_send.at[which])


ANYWHERE = pl.BlockSpec(memory_space=pltpu.HBM)
ON_CORE = pl.BlockSpec(memory_space=pltpu.VMEM)


def on_device_heads(
    hidden_in, sb_query_w, sb_key_w, sb_value_w, sb_offset,
    delta_query_w, delta_key_w, delta_value_w, decay_w, write_w, write_bias,
    decay_log_scale, decay_shift, head_gain, sb_out_w, delta_out_w,
):
    sp, fs, tp = lax.axis_size("sp"), lax.axis_size("fs"), lax.axis_size("tp")
    rows, half = hidden_in.shape[1:]
    width = half * tp
    length = rows * sp
    heads = decay_log_scale.shape[0]
    cols = sb_query_w.shape[1] // sp
    parts, chunks = 4, 4
    share = rows // tp
    blocks = length // BLOCK
    dma = pltpu.SemaphoreType.DMA
    bf16, f32 = jnp.bfloat16, jnp.float32
    own, incoming = pl.pallas_call(
        layer_kernel,
        name="layer",
        out_shape=(pltpu.VMEM((share, width), bf16),) * 2,
        in_specs=[ANYWHERE] * 16,
        out_specs=(ON_CORE,) * 2,
        scratch_shapes=[
            pltpu.SMEM(sb_offset.shape, f32),
            pltpu.SMEM(decay_log_scale.shape, f32),
            pltpu.SMEM(write_bias.shape, f32),
            pltpu.VMEM((1, head_gain.shape[0]), f32),
            pltpu.VMEM((sp, rows, width), bf16),
            pltpu.VMEM((width, 6 * cols), bf16),
            pltpu.VMEM((2, heads, width), bf16),
            pltpu.VMEM((2 * heads, width), bf16),
            pltpu.VMEM((2 * heads, rows), f32),
            pltpu.VMEM((sp, heads, rows), f32),
            pltpu.VMEM((rows, rows + cols), bf16),
            pltpu.VMEM((3, length, cols), bf16),
            pltpu.VMEM((length, cols), f32),
            pltpu.VMEM((length, cols), f32),
            pltpu.VMEM((cols, cols), f32),
            pltpu.VMEM((blocks, cols + BLOCK, 2 * cols), bf16),
            pltpu.VMEM((blocks, cols + BLOCK, cols), f32),
            pltpu.VMEM((length, cols), bf16),
            pltpu.VMEM((length, cols), bf16),
            pltpu.VMEM((rows, cols * sp), bf16),
            pltpu.VMEM((rows, cols * sp), bf16),
            pltpu.VMEM(sb_out_w.shape, bf16),
            pltpu.VMEM(delta_out_w.shape, bf16),
            pltpu.VMEM((rows, width), f32),
            pltpu.VMEM((chunks, share, width // chunks), bf16),
            dma((2,)), dma((2, sp - 1, parts)), dma((1,)), dma((2 * sp - 1,)),
            dma((1,)), dma((2, 6)), dma((2,)), dma((2,)), dma((2, sp - 1)), dma((11,)),
            dma((2,)), dma((3,)), dma((2,)),
        ],
        compiler_params=pltpu.CompilerParams(
            collective_id=0, has_side_effects=True,
            vmem_limit_bytes=ALL_VMEM - 5 * share * width,
        ),
    )(
        sb_offset, decay_log_scale, write_bias,
        hidden_in.reshape(rows, half), sb_query_w, sb_key_w, sb_value_w,
        delta_query_w, delta_key_w, delta_value_w, decay_w.T, write_w.T,
        decay_shift.reshape(heads, rows), head_gain.reshape(1, -1), sb_out_w, delta_out_w,
    )
    result = (own.astype(f32) + incoming.astype(f32)).astype(bf16)
    return result.reshape(1, share, width)


def on_device(*inputs):
    delta_heads = inputs[11].shape[0]
    square = lax.axis_size("sp") == lax.axis_size("fs") == 4 and lax.axis_size("tp") == 2
    if square and delta_heads == lax.axis_size("sp") and inputs[4].shape[0] % delta_heads == 0:
        return on_device_heads(*inputs)
    return on_device_split(*inputs)


def solution(mesh):
    return jax.shard_map(
        on_device,
        mesh=mesh,
        in_specs=(
            P("fs", "sp", "tp"),
            P("fs", "tp"),
            P("fs", "tp"),
            P("fs", "tp"),
            P("tp"),
            P("fs", "tp"),
            P("fs", "tp"),
            P("fs", "tp"),
            P(None, "tp"),
            P(None, "tp"),
            P("tp"),
            P("tp"),
            P("fs", "tp", "sp"),
            P(),
            P("tp", None),
            P("tp", None),
        ),
        out_specs=P("fs", ("sp", "tp"), None),
        check_vma=False,
    )
```

```python
import jax
import jax.numpy as jnp
from jax import lax
from jax.experimental import pallas as pl
from jax.experimental.pallas import tpu as pltpu
from jax.sharding import PartitionSpec as P

MESH = pl.DeviceIdType.MESH
ALL_VMEM = 67043328

SB_DIM = 64
GDN_DIM = 128
BLOCK = 64


EXACT_MATMUL = lax.Precision.HIGHEST
NORM_EPS = 1e-06


def carried_in(value, axis, combine, identity):
    devices, index = (lax.axis_size(axis), lax.axis_index(axis))
    everything = jax.tree.map(
        lambda part, kind: lax.all_gather(part.astype(kind), axis),
        value,
        (jnp.bfloat16, jnp.bfloat16),
    )
    start = jax.tree.map(
        lambda part, zero: jnp.broadcast_to(jnp.asarray(zero, part.dtype), part.shape),
        value,
        identity,
    )

    def lap(k, before):
        reached = k < index
        new = combine(
            before, jax.tree.map(lambda part, own: part[k].astype(own.dtype), everything, value)
        )
        return jax.tree.map(lambda a, b: jnp.where(reached, a, b), new, before)

    return lax.fori_loop(0, devices, lap, start)


def unit_lower_inverse(strict_part):
    order_size = strict_part.shape[-1]
    powered = strict_part
    inverse = jnp.eye(order_size, dtype=strict_part.dtype) - strict_part
    for repeat_number in range(max(1, (order_size - 1).bit_length()) - 1):
        powered = jnp.einsum("...ij,...jk->...ik", powered, powered, precision=EXACT_MATMUL)
        inverse = inverse + jnp.einsum(
            "...ij,...jk->...ik", inverse, powered, precision=EXACT_MATMUL
        )
    return inverse


def to_blocks(row_data, block_span):
    blocks_count = row_data.shape[0] // block_span
    shaped = row_data.reshape((blocks_count, block_span) + row_data.shape[1:])
    return jnp.swapaxes(shaped, 1, 2)


def from_blocks(blocked):
    swapped = jnp.swapaxes(blocked, 1, 2)
    return swapped.reshape((-1,) + swapped.shape[2:])


def unit_rows(vectors):
    return vectors * lax.rsqrt(jnp.sum(vectors * vectors, axis=-1, keepdims=True) + NORM_EPS)


def delta_inputs(
    query_proj,
    key_proj,
    value_proj,
    decay_pre,
    write_pre,
    write_bias,
    decay_log_scale,
    shift_rows,
    head_count,
    head_size,
):
    query_act = jax.nn.silu(query_proj.astype(jnp.float32)).reshape(-1, head_count, head_size)
    key_act = jax.nn.silu(key_proj.astype(jnp.float32)).reshape(-1, head_count, head_size)
    value_rows = jax.nn.silu(value_proj.astype(jnp.float32)).reshape(-1, head_count, head_size)
    queries = unit_rows(query_act) * head_size ** (-0.5)
    key_rows = unit_rows(key_act)
    log_decay = -jnp.exp(decay_log_scale) * jax.nn.softplus(decay_pre) + shift_rows
    strength = jax.nn.sigmoid(write_pre + write_bias)
    return (queries, key_rows, value_rows, log_decay, strength)


def delta_prepare(queries, key_rows, value_rows, log_decay, strength):
    block_span = queries.shape[2]
    cumulative = jnp.cumsum(log_decay, axis=-1)
    row_place = lax.broadcasted_iota(jnp.int32, (block_span, block_span), 0)
    col_place = lax.broadcasted_iota(jnp.int32, (block_span, block_span), 1)
    inclusive = col_place <= row_place
    strictly = col_place < row_place
    spread = cumulative[..., :, None] - cumulative[..., None, :]
    decay_table = jnp.where(inclusive, jnp.exp(jnp.where(inclusive, spread, 0.0)), 0.0)
    keys_beta = key_rows * strength[..., None]
    lower_part = jnp.where(
        strictly,
        jnp.einsum("nhik,nhjk->nhij", keys_beta, key_rows, precision=EXACT_MATMUL) * decay_table,
        0.0,
    )
    inverse = unit_lower_inverse(lower_part)
    growth = jnp.exp(cumulative)
    state_updates = jnp.einsum(
        "nhij,nhjv->nhiv", inverse, value_rows * strength[..., None], precision=EXACT_MATMUL
    )
    erase_term = jnp.einsum(
        "nhij,nhjk->nhik", inverse, keys_beta * growth[..., None], precision=EXACT_MATMUL
    )
    inside_block = (
        jnp.einsum("nhik,nhjk->nhij", queries, key_rows, precision=EXACT_MATMUL) * decay_table
    )
    boosted_query = queries * growth[..., None]
    damped_keys = key_rows * jnp.exp(cumulative[..., -1:] - cumulative)[..., None]
    decay_per_block = jnp.exp(cumulative[..., -1])
    return (state_updates, erase_term, inside_block, boosted_query, damped_keys, decay_per_block)


def delta_step(memory_state, inputs):
    state_updates, erase_term, inside_block, boosted_query, damped_keys, decay_per_block = inputs
    fixed_values = state_updates - jnp.einsum(
        "mzq,mqc->mzc", erase_term, memory_state, precision=EXACT_MATMUL
    )
    produced_rows = jnp.einsum(
        "mzq,mqc->mzc", boosted_query, memory_state, precision=EXACT_MATMUL
    ) + jnp.einsum("efq,eqn->efn", inside_block, fixed_values, precision=EXACT_MATMUL)
    memory_state = memory_state * decay_per_block[:, None, None] + jnp.einsum(
        "wam,waz->wmz", damped_keys, fixed_values, precision=EXACT_MATMUL
    )
    return (memory_state, produced_rows)


def transition_step(carried, inputs):
    memory_state, transfer = carried
    state_updates, erase_term, inside_block, boosted_query, damped_keys, decay_per_block = inputs
    fixed_values = state_updates - jnp.einsum(
        "mzq,mqc->mzc", erase_term, memory_state, precision=EXACT_MATMUL
    )
    coupling = jnp.einsum("hik,hil->hkl", damped_keys, erase_term, precision=EXACT_MATMUL)
    memory_state = memory_state * decay_per_block[:, None, None] + jnp.einsum(
        "wam,waz->wmz", damped_keys, fixed_values, precision=EXACT_MATMUL
    )
    transfer = transfer * decay_per_block[:, None, None] - jnp.einsum(
        "hkl,hlm->hkm", coupling, transfer, precision=EXACT_MATMUL
    )
    return ((memory_state, transfer), None)


def compose(prior_blocks, following_blocks):
    joined_map = jnp.einsum(
        "hkl,hlm->hkm", following_blocks[0], prior_blocks[0], precision=EXACT_MATMUL
    )
    joined_state = (
        jnp.einsum("djo,dog->djg", following_blocks[0], prior_blocks[1], precision=EXACT_MATMUL)
        + following_blocks[1]
    )
    return (joined_map, joined_state)


def stick_block(queries, key_rows, value_rows, query_place, key_place, offsets):
    scale_factor = queries.shape[-1] ** (-0.5)
    scores = (
        jnp.einsum("qhd,khd->hqk", queries, key_rows, preferred_element_type=jnp.float32)
        * scale_factor
        + offsets[:, None, None]
    )
    visible = key_place[None, :] < query_place[:, None]
    skipped = jnp.where(visible, jax.nn.log_sigmoid(-scores), 0.0)
    beyond = lax.cumsum(skipped, axis=2, reverse=True) - skipped
    weights = jnp.where(visible, jnp.exp(jax.nn.log_sigmoid(scores) + beyond), 0.0).astype(
        jnp.bfloat16
    )
    partial_value = jnp.einsum(
        "hqk,khd->qhd", weights, value_rows, preferred_element_type=jnp.float32
    )
    return (partial_value, jnp.sum(skipped, axis=2).T)


def stick_combine(partials, totals):
    beyond = jnp.cumsum(totals[::-1], axis=0)[::-1] - totals
    return jnp.sum(partials * jnp.exp(beyond)[..., None], axis=0)


def on_device_split(
    hidden_in,
    sb_query_w,
    sb_key_w,
    sb_value_w,
    sb_offset,
    delta_query_w,
    delta_key_w,
    delta_value_w,
    decay_w,
    write_w,
    write_bias,
    decay_log_scale,
    decay_shift,
    head_gain,
    sb_out_w,
    delta_out_w,
):
    token_rows = hidden_in.shape[1]
    local_in = hidden_in.reshape(token_rows, hidden_in.shape[2])
    gathered = (
        lax.all_gather(sb_query_w, "fs", axis=0, tiled=True),
        lax.all_gather(sb_key_w, "fs", axis=0, tiled=True),
        lax.all_gather(sb_value_w, "fs", axis=0, tiled=True),
        lax.all_gather(delta_query_w, "fs", axis=0, tiled=True),
        lax.all_gather(delta_key_w, "fs", axis=0, tiled=True),
        lax.all_gather(delta_value_w, "fs", axis=0, tiled=True),
    )
    in_weights = tuple(gathered) + (decay_w, write_w)
    portion = lax.all_gather(local_in, "tp", axis=1, tiled=True)
    projected = tuple(
        (jnp.dot(portion, weight, preferred_element_type=jnp.float32) for weight in in_weights)
    )
    sb_heads = sb_offset.shape[0]
    delta_heads = decay_log_scale.shape[0]
    sb_query = projected[0].astype(jnp.bfloat16).reshape(token_rows, sb_heads, SB_DIM)
    sb_keys = projected[1].astype(jnp.bfloat16)
    sb_values = projected[2].astype(jnp.bfloat16)
    shift_rows = decay_shift.reshape(delta_heads, token_rows).T
    queries, key_rows, value_rows, log_decay, strength = delta_inputs(
        projected[3].astype(jnp.bfloat16),
        projected[4].astype(jnp.bfloat16),
        projected[5].astype(jnp.bfloat16),
        projected[6],
        projected[7],
        write_bias,
        decay_log_scale,
        shift_rows,
        delta_heads,
        GDN_DIM,
    )
    prepared = delta_prepare(
        to_blocks(queries, BLOCK),
        to_blocks(key_rows, BLOCK),
        to_blocks(value_rows, BLOCK),
        to_blocks(log_decay, BLOCK),
        to_blocks(strength, BLOCK),
    )
    identity_map = jnp.broadcast_to(
        jnp.eye(GDN_DIM, dtype=jnp.float32), (delta_heads, GDN_DIM, GDN_DIM)
    )
    empty_state = jnp.zeros((delta_heads, GDN_DIM, GDN_DIM), jnp.float32)
    (local_end, local_map), unused_out = lax.scan(
        transition_step, (empty_state, identity_map), prepared
    )
    own_first = lax.axis_index("sp") * token_rows
    query_place = own_first + lax.iota(jnp.int32, token_rows)
    sp_count = lax.axis_size("sp")
    slot_out = jnp.zeros((sp_count, token_rows, sb_heads, SB_DIM), jnp.float32)
    slot_total = jnp.zeros((sp_count, token_rows, sb_heads), jnp.float32)

    def absorb(slot_arrays, address_portion, value_part, shard_first):

        def active(current):
            partial_value, totals = stick_block(
                sb_query,
                address_portion.reshape(token_rows, sb_heads, SB_DIM),
                value_part.reshape(token_rows, sb_heads, SB_DIM),
                query_place,
                shard_first + lax.iota(jnp.int32, token_rows),
                sb_offset,
            )
            slot_index = shard_first // token_rows
            return (
                lax.dynamic_update_index_in_dim(current[0], partial_value, slot_index, 0),
                lax.dynamic_update_index_in_dim(current[1], totals, slot_index, 0),
            )

        def inactive(current):
            return current

        usable = jnp.logical_and(shard_first >= 0, shard_first <= own_first)
        return lax.cond(usable, active, inactive, slot_arrays)

    key_block = lax.all_gather(sb_keys, "sp", axis=0, tiled=True)
    value_block = lax.all_gather(sb_values, "sp", axis=0, tiled=True)

    def per_shard(shard_number, current):
        row_begin = shard_number * token_rows
        return absorb(
            current,
            lax.dynamic_slice_in_dim(key_block, row_begin, token_rows, 0),
            lax.dynamic_slice_in_dim(value_block, row_begin, token_rows, 0),
            row_begin,
        )

    slot_arrays = lax.fori_loop(
        0, key_block.shape[0] // token_rows, per_shard, (slot_out, slot_total)
    )
    unused_map, incoming = carried_in(
        (local_map, local_end), "sp", compose, (identity_map, empty_state)
    )
    sb_mixed = (
        stick_combine(slot_arrays[0], slot_arrays[1])
        .astype(jnp.bfloat16)
        .reshape(token_rows, sb_heads * SB_DIM)
    )
    unused_end, produced_rows = lax.scan(delta_step, incoming, prepared)
    produced_rows = from_blocks(produced_rows)
    normed = (
        produced_rows
        * lax.rsqrt(jnp.mean(produced_rows * produced_rows, axis=-1, keepdims=True) + NORM_EPS)
        * head_gain
    )
    delta_mixed = normed.astype(jnp.bfloat16).reshape(token_rows, delta_heads * GDN_DIM)
    result = lax.psum_scatter(
        (
            jnp.dot(sb_mixed, sb_out_w, preferred_element_type=jnp.float32)
            + jnp.dot(delta_mixed, delta_out_w, preferred_element_type=jnp.float32)
        ).astype(jnp.bfloat16),
        "tp",
        scatter_dimension=0,
        tiled=True,
    ).astype(jnp.float32)
    return result.astype(jnp.bfloat16).reshape(1, result.shape[0], result.shape[1])


def remote(src, dst, send, recv, axis, index):
    return pltpu.make_async_remote_copy(
        src_ref=src, dst_ref=dst, send_sem=send, recv_sem=recv,
        device_id={axis: index}, device_id_type=MESH,
    )


def greet(axes):
    barrier = pltpu.get_barrier_semaphore()
    count = 0
    for axis in axes:
        size, me = lax.axis_size(axis), lax.axis_index(axis)
        for k in range(1, size):
            pl.semaphore_signal(
                barrier, inc=1, device_id={axis: lax.rem(me + k, size)}, device_id_type=MESH
            )
            count += 1
    pl.semaphore_wait(barrier, count)


def halves(a):
    high = a.astype(jnp.bfloat16)
    return high, (a - high.astype(jnp.float32)).astype(jnp.bfloat16)


def dot_f32(a, b, dims=((1,), (0,))):
    return lax.dot_general(a, b, (dims, ((), ())), preferred_element_type=jnp.float32)


def wide_rhs(high, low, axis):
    top = jnp.concatenate([high, low], axis=axis)
    bottom = jnp.concatenate([high, jnp.zeros_like(low)], axis=axis)
    return jnp.concatenate([top, bottom], axis=1 - axis)


def folded(a):
    half = a.shape[1] // 2
    return a[:, :half] + a[:, half:]


def layer_kernel(
    offset_hbm, decay_scale_hbm, write_bias_hbm,
    x_ref, w0, w1, w2, w3, w4, w5, decay_w_ref, write_w_ref, shift_ref, gain_hbm, sw_hbm, dw_hbm,
    own, incoming,
    offset_ref, decay_scale_ref, write_bias_ref, gain_ref,
    xs, ws, gate_w, gate_all, gates, shifts_ref, after,
    proj, acc, later, memory_ref, maps, adds, stick_out, delta_out,
    sticks, deltas, sw_ref, dw_ref, partial, outgoing,
    x_send, x_recv, f_send, f_recv, w_send, w_recv, r_recv, s_send, s_recv, l_sem,
    a_send, a_recv, c_sem,
):
    weights = (w0, w1, w2, w3, w4, w5)
    sp, tp = lax.axis_size("sp"), lax.axis_size("tp")
    z, f, t = lax.axis_index("sp"), lax.axis_index("fs"), lax.axis_index("tp")
    rows, half = x_ref.shape
    depth = w0.shape[0]
    cols = ws.shape[1] // len(weights)
    parts = x_recv.shape[2]
    heads = decay_w_ref.shape[0]
    slot = pl.ds(pl.multiple_of(t * half, half), half)
    local = [
        pltpu.make_async_copy(x_ref, xs.at[z, :, slot], l_sem.at[0]),
        pltpu.make_async_copy(shift_ref, shifts_ref.at[z], l_sem.at[1]),
        pltpu.make_async_copy(decay_w_ref, gate_w.at[0], l_sem.at[2]),
        pltpu.make_async_copy(write_w_ref, gate_w.at[1], l_sem.at[3]),
        pltpu.make_async_copy(offset_hbm, offset_ref, l_sem.at[6]),
        pltpu.make_async_copy(decay_scale_hbm, decay_scale_ref, l_sem.at[7]),
        pltpu.make_async_copy(write_bias_hbm, write_bias_ref, l_sem.at[8]),
        pltpu.make_async_copy(gain_hbm, gain_ref, l_sem.at[9]),
    ]
    late = [
        pltpu.make_async_copy(sw_hbm, sw_ref, l_sem.at[4]),
        pltpu.make_async_copy(dw_hbm, dw_ref, l_sem.at[5]),
    ]

    def w_src(i):
        return weights[i].at[:, pl.ds(pl.multiple_of(z * cols, cols), cols)]

    def w_at(i, who):
        return ws.at[pl.ds(pl.multiple_of(who * depth, depth), depth), pl.ds(i * cols, cols)]

    local_w = [
        pltpu.make_async_copy(w_src(i), w_at(i, f), l_sem.at[10]) for i in range(len(weights))
    ]
    near = (f + 1 - 2 * (f % 2), f + 2 - 4 * (f // 2))
    count = len(weights)
    delta_kinds, stick_kinds = (3, 4, 5), (0, 1, 2)

    def onward(way):
        return z + 1 < sp if way == 0 else z > 0

    def ahead(way):
        return z + 1 if way == 0 else z - 1

    barrier = pltpu.get_barrier_semaphore()
    for way in range(2):
        @pl.when(onward(way))
        def _():
            pl.semaphore_signal(
                barrier, inc=1, device_id={"sp": ahead(way)}, device_id_type=MESH
            )
    for side in range(2):
        pl.semaphore_signal(barrier, inc=1, device_id={"fs": near[side]}, device_id_type=MESH)
    pl.semaphore_signal(
        barrier, inc=1, device_id={"tp": lax.rem(t + 1, tp)}, device_id_type=MESH
    )
    for c in local + local_w:
        c.start()
    peers = onward(0).astype(jnp.int32) + onward(1).astype(jnp.int32) + 3
    pl.semaphore_wait(barrier, peers)

    def x_copy(way, step, part):
        block = z - (step - 1) if way == 0 else z + (step - 1)
        piece = pl.ds(part * (rows // parts), rows // parts)
        there = xs.at[block, piece, slot]
        return remote(
            x_ref.at[piece, :] if step == 1 else there, there,
            x_send.at[way], x_recv.at[way, step - 1, part], "sp", ahead(way),
        )

    def shift_copy(way, step):
        block = z - (step - 1) if way == 0 else z + (step - 1)
        there = shifts_ref.at[block]
        return remote(
            shift_ref if step == 1 else there, there,
            s_send.at[way], s_recv.at[way, step - 1], "sp", ahead(way),
        )

    def comes(way, step):
        return z >= step if way == 0 else z + step < sp

    def sends(way, step):
        return jnp.logical_and(onward(way), comes(way, step - 1))

    def f_slot(way, step, part):
        if step == sp - 1 and part < parts // 2:
            return 2 * sp - 1 + way
        return way * (sp - 1) + step

    def forward(way, step, part):
        block = z - step if way == 0 else z + step
        piece = pl.ds(part * (rows // parts), rows // parts)
        there = xs.at[block, piece, slot]
        return remote(
            x_ref.at[piece, :] if step == 0 else there, there,
            f_send.at[0], f_recv.at[f_slot(way, step, part)], "tp", lax.rem(t + 1, tp),
        )

    def w_copy(side, i):
        return remote(
            w_src(i), w_at(i, f), w_send.at[0], w_recv.at[side, i], "fs", near[side]
        )

    def w_relay(side, i):
        part = depth // 2
        start = pl.multiple_of(near[side] * depth + side * part, part)
        there = ws.at[pl.ds(start, part), pl.ds(i * cols, cols)]
        return remote(
            there, there, w_send.at[0], r_recv.at[i // 3], "fs", near[1 - side]
        )

    for part in range(parts):
        for way in range(2):
            @pl.when(onward(way))
            def _():
                x_copy(way, 1, part).start()
                if part == 0:
                    shift_copy(way, 1).start()
    for i in delta_kinds:
        for side in range(2):
            w_copy(side, i).start()
    for part in range(parts):
        forward(0, 0, part).start()

    def relay(i):
        for side in range(2):
            w_copy(side, i).wait_recv()
            w_relay(side, i).start()

    def arrive(step, part):
        for way in range(2):
            @pl.when(comes(way, step))
            def _():
                x_copy(way, step, part).wait_recv()
                forward(way, step, part).start()
                if step + 1 < sp:
                    @pl.when(onward(way))
                    def _():
                        x_copy(way, step + 1, part).start()
                if part == 0:
                    shift_copy(way, step).wait_recv()
                    if step + 1 < sp:
                        @pl.when(onward(way))
                        def _():
                            shift_copy(way, step + 1).start()

    below = lax.broadcasted_iota(jnp.int32, (rows, rows), 0)
    across = lax.broadcasted_iota(jnp.int32, (rows, rows), 1)
    after[:, :rows] = jnp.where(below > across, 1.0, 0.0).astype(jnp.bfloat16)
    after[:, rows:] = jnp.ones((rows, cols), jnp.bfloat16)
    acc[...] = jnp.zeros_like(acc)
    later[...] = jnp.zeros_like(later)
    memory_ref[...] = jnp.zeros_like(memory_ref)
    early = [(step, part) for step in range(1, sp - 1) for part in range(parts)]
    relay(delta_kinds[0])
    arrive(*early[0])
    for i in delta_kinds[1:]:
        relay(i)
    for i in stick_kinds:
        for side in range(2):
            w_copy(side, i).start()
    for c in late:
        c.start()
    for step, part in early[1:parts]:
        arrive(step, part)
    for c in local:
        c.wait()
    own_w = ws.at[pl.ds(pl.multiple_of(f * depth, depth), depth), :]
    pltpu.make_async_copy(own_w, own_w, l_sem.at[10]).wait()
    gate_all[...] = jnp.concatenate(
        [gate_w[0].astype(jnp.float32), gate_w[1].astype(jnp.float32)], axis=0
    ).astype(jnp.bfloat16)
    def all_sent(ref, sem):
        remote(ref, ref, sem, sem, "tp", lax.rem(t + 1, tp)).wait_send()

    def all_came(ref, sem):
        remote(ref, ref, sem, sem, "tp", lax.rem(t + 1, tp)).wait_recv()

    def block_came(way, step):
        extent = rows // 2 if step == sp - 1 else rows
        all_came(xs.at[z, pl.ds(0, extent), slot], f_recv.at[way * (sp - 1) + step])

    def half_came(way):
        all_came(xs.at[z, pl.ds(0, rows // 2), slot], f_recv.at[2 * sp - 1 + way])

    block_came(0, 0)

    def relayed(kinds):
        first = kinds[0] * cols
        all_came(ws.at[pl.ds(0, depth), pl.ds(first, len(kinds) * cols)], r_recv.at[kinds[0] // 3])

    relayed(delta_kinds)

    size = offset_ref.shape[0] // sp
    sb_size = cols // size
    scale = sb_size ** (-0.5)
    tile = rows // 2

    def at_block(b, start=0, extent=rows):
        return pl.ds(pl.multiple_of(b * rows + start, extent), extent)

    def pair(i, j):
        for part in range(rows // tile):
            mine = at_block(i, part * tile, tile)
            q = proj[0, mine, :]
            keys, values = proj[1, at_block(j), :], proj[2, at_block(j), :]
            lane = lax.broadcasted_iota(jnp.int32, (tile, cols), 1)
            query = jnp.concatenate(
                [jnp.where(lane // sb_size == h, q, jnp.zeros_like(q)) for h in range(size)], axis=0
            )
            score = dot_f32(query, keys, ((1,), (1,)))
            score = jnp.concatenate(
                [
                    score[h * tile : (h + 1) * tile] * scale + offset_ref[z * size + h]
                    for h in range(size)
                ],
                axis=0,
            )
            skip = jnp.maximum(score, jnp.log(1.0 + jnp.exp(jnp.minimum(score, 80.0))))
            weight = score - skip
            seen = across[:tile] < below[:tile] + (part * tile + (i - j) * rows)
            seen = jnp.concatenate([seen] * size, axis=0)
            skip = jnp.where(seen, skip, 0.0)
            sums = dot_f32(skip.astype(jnp.bfloat16), after[...])
            weight = jnp.where(seen, jnp.exp(weight - sums[:, :rows]), 0.0)
            out = dot_f32(weight.astype(jnp.bfloat16), values)
            mixed, total = out[:tile], sums[:tile, rows:]
            for h in range(1, size):
                at = slice(h * tile, (h + 1) * tile)
                mixed = jnp.where(lane // sb_size == h, out[at], mixed)
                total = jnp.where(lane // sb_size == h, sums[at, rows:], total)
            passed = later[mine, :]
            acc[mine, :] = acc[mine, :] + mixed * jnp.exp(-passed)
            later[mine, :] = passed + total

    span = BLOCK
    duo = 2 * span
    blocks = rows // span
    width = GDN_DIM
    seg_row = lax.broadcasted_iota(jnp.int32, (rows, rows), 0)
    seg_col = lax.broadcasted_iota(jnp.int32, (rows, rows), 1)
    together = seg_row // span == seg_col // span
    upto = jnp.where(jnp.logical_and(together, seg_row <= seg_col), 1.0, 0.0).astype(jnp.bfloat16)
    beyond_it = jnp.where(jnp.logical_and(together, seg_row > seg_col), 1.0, 0.0).astype(
        jnp.bfloat16
    )
    prow = lax.broadcasted_iota(jnp.int32, (span, duo), 0)
    plane = lax.broadcasted_iota(jnp.int32, (span, duo), 1)
    first = plane < span
    pcol = jnp.where(first, plane, plane - span)
    inclusive, strictly = pcol <= prow, pcol < prow
    unit = jnp.where(pcol == prow, 1.0, 0.0)
    diagonal = lax.broadcasted_iota(jnp.int32, (width, width), 0) == lax.broadcasted_iota(
        jnp.int32, (width, width), 1
    )
    eighth = lax.broadcasted_iota(jnp.int32, (8, rows), 0)

    def silu(a):
        return a * (1.0 / (1.0 + jnp.exp(-a)))

    def unit_of(a):
        return a * lax.rsqrt(jnp.sum(a * a, axis=-1, keepdims=True) + NORM_EPS)

    def apart(a):
        lanes = lax.broadcasted_iota(jnp.int32, a.shape, 1) < span
        zero = jnp.zeros_like(a)
        return jnp.concatenate([jnp.where(lanes, a, zero), jnp.where(lanes, zero, a)], axis=0)

    def squared(left, power):
        high, low = halves(power)
        lhigh, llow = halves(left)
        return folded(
            dot_f32(
                jnp.concatenate([lhigh, llow], axis=1), wide_rhs(apart(high), apart(low), 1)
            )
        )

    def prepare(b, dq, dk, dv, begin, extent):
        lanes_at = slice(begin, begin + extent)
        order = eighth[:, :extent]
        gates[:, lanes_at] = dot_f32(gate_all[...], xs[b, lanes_at, :], ((1,), (1,)))
        pre = gates[pl.ds(z, 1), :][:, lanes_at]
        write = gates[pl.ds(heads + z, 1), :][:, lanes_at] + write_bias_ref[z]
        rate = jnp.exp(jnp.full((1, extent), decay_scale_ref[z], jnp.float32))
        soft = jnp.maximum(pre, 0.0) + jnp.log(1.0 + jnp.exp(-jnp.abs(pre)))
        decay = shifts_ref[b, pl.ds(z, 1), :][:, lanes_at] - rate * soft
        strength = 1.0 / (1.0 + jnp.exp(-write))
        d1 = decay.astype(jnp.bfloat16).astype(jnp.float32)
        d2 = (decay - d1).astype(jnp.bfloat16).astype(jnp.float32)
        d3 = decay - d1 - d2
        three = jnp.where(
            order == 0, d1, jnp.where(order == 1, d2, jnp.where(order == 2, d3, 0.0))
        ).astype(jnp.bfloat16)
        cum_row = jnp.sum(dot_f32(three, upto[:extent, :extent]), axis=0, keepdims=True)
        rest_row = jnp.sum(dot_f32(three, beyond_it[:extent, :extent]), axis=0, keepdims=True)
        stack = jnp.where(
            order == 0, strength,
            jnp.where(
                order == 1, jnp.exp(cum_row),
                jnp.where(order == 2, jnp.exp(rest_row), cum_row),
            ),
        )
        columns = stack.T
        s_col, grow, damp, cum = (columns[:, n : n + 1] for n in range(4))
        q = unit_of(silu(dq)) * width ** (-0.5)
        k = unit_of(silu(dk))
        v = silu(dv)
        boosted = q * grow
        damped = k * damp
        right = jnp.concatenate([v * s_col, k * (s_col * grow)], axis=1)
        kh, kl = halves(k)
        qh, ql = halves(q)
        work = []
        for duo_at in range(extent // duo):
            lo = duo_at * duo
            here = slice(lo, lo + duo)
            left = jnp.concatenate(
                [
                    jnp.concatenate([kh[here], kl[here]], axis=1),
                    jnp.concatenate([qh[here], ql[here]], axis=1),
                ],
                axis=0,
            )
            gram = folded(
                dot_f32(left, wide_rhs(kh[here], kl[here], 0), ((1,), (1,)))
            )
            spread = (
                jnp.where(first, cum[lo : lo + span], cum[lo + span : lo + duo])
                - cum_row[:, here]
            )
            table = jnp.where(inclusive, jnp.exp(jnp.where(inclusive, spread, 0.0)), 0.0)
            scale_col = jnp.where(first, s_col[lo : lo + span], s_col[lo + span : lo + duo])
            near_k = jnp.where(first, gram[:span], gram[span:duo])
            near_q = jnp.where(first, gram[duo : duo + span], gram[duo + span :])
            strict = jnp.where(strictly, near_k * table * scale_col, 0.0)
            work.append([unit - strict, strict, near_q * table])
        yield
        for w in work:
            w[1] = squared(w[1], w[1])
        levels = max(1, (span - 1).bit_length()) - 1
        for level in range(levels):
            if level == levels // 2:
                yield
            for w in work:
                if level + 1 < levels:
                    both = squared(jnp.concatenate([w[1], w[0]], axis=0), w[1])
                    w[1], w[0] = both[:span], w[0] + both[span:]
                else:
                    w[0] = w[0] + squared(w[0], w[1])
        yield
        for duo_at, (inverse, _, inside) in enumerate(work):
            lo = duo_at * duo
            here = slice(lo, lo + duo)
            ih, il = (apart(a) for a in halves(inverse))
            rh, rl = halves(right[here])
            solved = dot_f32(
                jnp.concatenate([ih, il], axis=1), jnp.concatenate([rh, rh], axis=0)
            ) + dot_f32(ih, rl)
            lh, ll = (
                apart(a) for a in halves(jnp.concatenate([damped[here].T, inside], axis=0))
            )
            sh, sl = halves(solved)
            made = dot_f32(
                jnp.concatenate([lh, ll], axis=1), jnp.concatenate([sh, sh], axis=0)
            ) + dot_f32(lh, sl)
            for side in range(2):
                at = lo + side * span
                mine = made[side * (width + span) : (side + 1) * (width + span)]
                n = b * blocks + begin // span + 2 * duo_at + side
                keep = grow[at + span - 1 : at + span]
                step_map = jnp.where(diagonal, keep, 0.0) - mine[:width, width:]
                query = boosted[at : at + span] - mine[width:, width:]
                high, low = halves(jnp.concatenate([step_map, query], axis=0))
                maps[n, :, :width] = high
                maps[n, :, width:] = low
                adds[n] = mine[:, :width]

    def give(which, out, target):
        here = target.at[:, pl.ds(pl.multiple_of(z * cols, cols), cols)]

        def send(g, k, sem):
            return remote(
                out.at[at_block(g), :], here,
                a_send.at[which], a_recv.at[sem], "sp", g,
            )

        def started(g):
            for k in range(1, sp):
                there = lax.rem(z + k, sp)
                if which == 0:
                    @pl.when(there == g)
                    def _():
                        send(there, k, 0).start()
                else:
                    slow = jnp.logical_or(
                        z == sp - 1, jnp.logical_and(z == 0, there == sp - 1)
                    )

                    @pl.when(jnp.logical_and(there == g, slow))
                    def _():
                        send(there, k, 2).start()

                    @pl.when(jnp.logical_and(there == g, jnp.logical_not(slow)))
                    def _():
                        send(there, k, 1).start()

        return started

    stick_started = give(0, stick_out, sticks)
    delta_started = give(1, delta_out, deltas)

    shorter = jnp.minimum(z, sp - 1 - z)
    down_last = z > sp - 1 - z

    def place(n):
        both = n <= 2 * shorter
        way_n = jnp.where(both, lax.rem(n + 1, 2), jnp.where(down_last, 0, 1))
        step_n = jnp.where(n == 0, 0, jnp.where(both, (n + 1) // 2, n - shorter))
        down = jnp.logical_and(way_n == 0, n > 0)
        return way_n, step_n, down, jnp.where(down, z - step_n, z + step_n)

    last_way = jnp.logical_or(z == 0, z == sp - 1)

    def block_ready(n):
        way_n, step_n, down, b = place(n)
        for step in range(1, sp):
            for way in range(2):
                @pl.when(jnp.logical_and(step_n == step, way_n == way))
                def _():
                    block_came(way, step)
        return b

    def delta_block(b, begin=0, extent=rows):
        drows = dot_f32(xs[b, begin : begin + extent, :], ws[:, 3 * cols :])
        drows = drows.astype(jnp.bfloat16).astype(jnp.float32)
        return prepare(
            b, drows[:, :cols], drows[:, cols : 2 * cols], drows[:, 2 * cols :], begin, extent
        )

    last_way = jnp.logical_or(z == 0, z == sp - 1)
    from_top = z == sp - 1

    def stick_project(n, begin=0, extent=rows):
        b = jnp.where(from_top, sp - 1 - n, n)
        out = dot_f32(xs[b, begin : begin + extent, :], ws[:, : 3 * cols]).astype(jnp.bfloat16)
        for i in range(3):
            proj[i, at_block(b, begin, extent), :] = out[:, i * cols : (i + 1) * cols]

    def stick_place(n):
        lower = z < sp // 2
        between = jnp.where(
            n == 0,
            jnp.where(lower, sp - 1, 0),
            jnp.where(
                n == 1,
                jnp.where(lower, sp - 2, 1),
                jnp.where(n == 2, jnp.where(lower, 0, sp - 1), z),
            ),
        )
        return jnp.where(from_top, sp - 1 - n, jnp.where(last_way, n, between))

    def settle(i):
        stick_out[at_block(i), :] = acc[at_block(i), :].astype(jnp.bfloat16)

    def stick_pair(n, r):
        b = stick_place(n)
        i = jnp.where(from_top, b + r, b)
        j = jnp.where(from_top, b, b - r)
        pair(i, j)

        @pl.when(j == 0)
        def _():
            settle(i)
            stick_started(i)

    def walk_groups(start, stop, held=False):
        def group(g, c):
            @pl.when(g > start + held)
            def _():
                delta_started(g - 1)
            memory = memory_ref[...]
            for n in range(blocks):
                memory = walk(g * blocks + n, memory)
            memory_ref[...] = memory
            return c

        lax.fori_loop(start, stop, group, 0)
        delta_started(stop - 1)

    def walk(n, memory):
        high, low = halves(memory)
        new = folded(dot_f32(maps[n], wide_rhs(high, low, 1))) + adds[n]
        made = new[width:]
        made = made * lax.rsqrt(jnp.mean(made * made, axis=-1, keepdims=True) + NORM_EPS)
        at = pl.ds(pl.multiple_of(n * span, span), span)
        delta_out[at, :] = (made * gain_ref[...]).astype(delta_out.dtype)
        return new[:width]

    def plain_delta(n, c):
        @pl.when(n == 1)
        def _():
            relay(stick_kinds[0])

        @pl.when(n == sp - 2)
        def _():
            for c in early[parts:-1]:
                arrive(*c)
            relay(stick_kinds[1])

            @pl.when(z == 0)
            def _():
                walk_groups(0, 2)
            relay(stick_kinds[2])
            arrive(*early[-1])
        for _ in delta_block(block_ready(n)):
            pass
        return c

    events = jnp.where(last_way, sp - 1, sp)
    lax.fori_loop(0, events, plain_delta, 0)

    @pl.when(jnp.logical_not(last_way))
    def _():
        walk_groups(0, sp, held=True)

    relayed(stick_kinds)

    def stick_event(n, c):
        for part in range(2):
            @pl.when(jnp.logical_and(last_way, n == part + 1))
            def _():
                arrive(sp - 1, part)

        def project_one(m, c):
            stick_project(m)
            return c

        needed = jnp.where(from_top, n, stick_place(n)) + 1
        lax.fori_loop(c, needed, project_one, 0)

        @pl.when(jnp.logical_and(jnp.logical_not(last_way), n == 0))
        def _():
            delta_started(0)

        def one(r, c):
            for part in range(2, parts):
                @pl.when(
                    jnp.logical_and(
                        last_way, jnp.logical_and(n == sp - 2, r == sp - 1 - parts + part)
                    )
                )
                def _():
                    if part == parts - 1:
                        for way in range(2):
                            @pl.when(comes(way, sp - 1))
                            def _():
                                half_came(way)
                        for _ in delta_block(stick_place(sp - 1), 0, rows // 2):
                            pass
                        stick_project(sp - 1, 0, rows // 2)
                    arrive(sp - 1, part)
            stick_pair(n, r)
            return c

        lax.fori_loop(0, jnp.where(last_way, n, stick_place(n)) + 1, one, 0)
        return jnp.maximum(c, needed)

    lax.fori_loop(0, events, stick_event, 0)

    @pl.when(last_way)
    def _():
        @pl.when(z == 0)
        def _():
            walk_groups(2, sp - 1)
        for way in range(2):
            @pl.when(comes(way, sp - 1))
            def _():
                block_came(way, sp - 1)
        stick_project(sp - 1, rows // 2, rows // 2)
        stages = delta_block(stick_place(sp - 1), rows // 2, rows // 2)
        for u in range(sp):
            next(stages, None)
            stick_pair(sp - 1, u)
        walk_groups(jnp.where(z == 0, sp - 1, 0), sp)

    mine_z = pl.ds(pl.multiple_of(z * rows, rows), rows)
    lanes = pl.ds(pl.multiple_of(z * cols, cols), cols)
    sticks[:, lanes] = stick_out[mine_z, :]
    deltas[:, lanes] = delta_out[mine_z, :]
    for c in late:
        c.wait()
    all_sent(ws.at[pl.ds(0, 3 * depth), :], w_send.at[0])
    all_sent(xs.at[:, :, slot], f_send.at[0])
    for c in range(sp):
        @pl.when(z == c)
        def _():
            for way, passed in enumerate((c + 1 if c + 1 < sp else 0, sp - c if c > 0 else 0)):
                if passed:
                    all_sent(xs.at[pl.ds(0, passed), :, slot], x_send.at[way])
                    all_sent(shifts_ref.at[pl.ds(0, passed)], s_send.at[way])
    all_came(stick_out.at[pl.ds(0, (sp - 1) * rows), :], a_recv.at[0])
    chunks, wide = outgoing.shape[0], outgoing.shape[2]
    share = rows // tp
    for c in range(chunks):
        columns = slice(c * wide, (c + 1) * wide)
        partial[:, columns] = dot_f32(sticks[...], sw_ref[:, columns])
    all_came(delta_out.at[pl.ds(0, (sp - 2) * rows), :], a_recv.at[1])
    soon = pl.ds(pl.multiple_of(jnp.where(from_top, 1, 0) * cols, cols), (sp - 1) * cols)
    for c in range(chunks):
        columns = slice(c * wide, (c + 1) * wide)
        partial[:, columns] += dot_f32(deltas[:, soon], dw_ref[soon, columns])
    all_came(delta_out.at[pl.ds(0, rows), :], a_recv.at[2])
    final = pl.ds(pl.multiple_of(jnp.where(from_top, 0, sp - 1) * cols, cols), cols)
    mine = pl.ds(pl.multiple_of(t * share, share), share)
    partner = lax.rem(t + 1, tp)
    theirs = pl.ds(pl.multiple_of(partner * share, share), share)

    def finish(which, c):
        columns = slice(c * wide, (c + 1) * wide)
        return (
            partial[which, columns] + dot_f32(deltas[which, final], dw_ref[final, columns])
        ).astype(jnp.bfloat16)

    swaps = [
        remote(
            outgoing.at[c], incoming.at[:, c * wide : (c + 1) * wide],
            c_sem.at[0], c_sem.at[1], "tp", partner,
        )
        for c in range(chunks)
    ]
    for c in range(chunks):
        outgoing[c] = finish(theirs, c)
        if c > 0:
            swaps[c - 1].start()
    for c in range(chunks):
        own[:, c * wide : (c + 1) * wide] = finish(mine, c)
        if c == 0:
            swaps[chunks - 1].start()
    all_came(incoming, c_sem.at[1])
    all_sent(incoming, c_sem.at[0])
    for which, out in enumerate((stick_out, delta_out)):
        all_sent(out.at[pl.ds(0, (sp - 1) * rows), :], a_send.at[which])


ANYWHERE = pl.BlockSpec(memory_space=pltpu.HBM)
ON_CORE = pl.BlockSpec(memory_space=pltpu.VMEM)


def on_device_heads(
    hidden_in, sb_query_w, sb_key_w, sb_value_w, sb_offset,
    delta_query_w, delta_key_w, delta_value_w, decay_w, write_w, write_bias,
    decay_log_scale, decay_shift, head_gain, sb_out_w, delta_out_w,
):
    sp, fs, tp = lax.axis_size("sp"), lax.axis_size("fs"), lax.axis_size("tp")
    rows, half = hidden_in.shape[1:]
    width = half * tp
    length = rows * sp
    heads = decay_log_scale.shape[0]
    cols = sb_query_w.shape[1] // sp
    parts, chunks = 4, 4
    share = rows // tp
    blocks = length // BLOCK
    dma = pltpu.SemaphoreType.DMA
    bf16, f32 = jnp.bfloat16, jnp.float32
    own, incoming = pl.pallas_call(
        layer_kernel,
        name="layer",
        out_shape=(pltpu.VMEM((share, width), bf16),) * 2,
        in_specs=[ANYWHERE] * 16,
        out_specs=(ON_CORE,) * 2,
        scratch_shapes=[
            pltpu.SMEM(sb_offset.shape, f32),
            pltpu.SMEM(decay_log_scale.shape, f32),
            pltpu.SMEM(write_bias.shape, f32),
            pltpu.VMEM((1, head_gain.shape[0]), f32),
            pltpu.VMEM((sp, rows, width), bf16),
            pltpu.VMEM((width, 6 * cols), bf16),
            pltpu.VMEM((2, heads, width), bf16),
            pltpu.VMEM((2 * heads, width), bf16),
            pltpu.VMEM((2 * heads, rows), f32),
            pltpu.VMEM((sp, heads, rows), f32),
            pltpu.VMEM((rows, rows + cols), bf16),
            pltpu.VMEM((3, length, cols), bf16),
            pltpu.VMEM((length, cols), f32),
            pltpu.VMEM((length, cols), f32),
            pltpu.VMEM((cols, cols), f32),
            pltpu.VMEM((blocks, cols + BLOCK, 2 * cols), bf16),
            pltpu.VMEM((blocks, cols + BLOCK, cols), f32),
            pltpu.VMEM((length, cols), bf16),
            pltpu.VMEM((length, cols), bf16),
            pltpu.VMEM((rows, cols * sp), bf16),
            pltpu.VMEM((rows, cols * sp), bf16),
            pltpu.VMEM(sb_out_w.shape, bf16),
            pltpu.VMEM(delta_out_w.shape, bf16),
            pltpu.VMEM((rows, width), f32),
            pltpu.VMEM((chunks, share, width // chunks), bf16),
            dma((2,)), dma((2, sp - 1, parts)), dma((1,)), dma((2 * sp + 1,)),
            dma((1,)), dma((2, 6)), dma((2,)), dma((2,)), dma((2, sp - 1)), dma((11,)),
            dma((2,)), dma((3,)), dma((2,)),
        ],
        compiler_params=pltpu.CompilerParams(
            collective_id=0, has_side_effects=True,
            vmem_limit_bytes=ALL_VMEM - 5 * share * width,
        ),
    )(
        sb_offset, decay_log_scale, write_bias,
        hidden_in.reshape(rows, half), sb_query_w, sb_key_w, sb_value_w,
        delta_query_w, delta_key_w, delta_value_w, decay_w.T, write_w.T,
        decay_shift.reshape(heads, rows), head_gain.reshape(1, -1), sb_out_w, delta_out_w,
    )
    result = (own.astype(f32) + incoming.astype(f32)).astype(bf16)
    return result.reshape(1, share, width)


def on_device(*inputs):
    delta_heads = inputs[11].shape[0]
    square = lax.axis_size("sp") == lax.axis_size("fs") == 4 and lax.axis_size("tp") == 2
    if square and delta_heads == lax.axis_size("sp") and inputs[4].shape[0] % delta_heads == 0:
        return on_device_heads(*inputs)
    return on_device_split(*inputs)


def solution(mesh):
    return jax.shard_map(
        on_device,
        mesh=mesh,
        in_specs=(
            P("fs", "sp", "tp"),
            P("fs", "tp"),
            P("fs", "tp"),
            P("fs", "tp"),
            P("tp"),
            P("fs", "tp"),
            P("fs", "tp"),
            P("fs", "tp"),
            P(None, "tp"),
            P(None, "tp"),
            P("tp"),
            P("tp"),
            P("fs", "tp", "sp"),
            P(),
            P("tp", None),
            P("tp", None),
        ),
        out_specs=P("fs", ("sp", "tp"), None),
        check_vma=False,
    )
```

```python
import jax
import jax.numpy as jnp
from jax import lax
from jax.experimental import pallas as pl
from jax.experimental.pallas import tpu as pltpu
from jax.sharding import PartitionSpec as P

MESH = pl.DeviceIdType.MESH
ALL_VMEM = 67043328

SB_DIM = 64
GDN_DIM = 128
BLOCK = 64


EXACT_MATMUL = lax.Precision.HIGHEST
NORM_EPS = 1e-06


def carried_in(value, axis, combine, identity):
    devices, index = (lax.axis_size(axis), lax.axis_index(axis))
    everything = jax.tree.map(
        lambda part, kind: lax.all_gather(part.astype(kind), axis),
        value,
        (jnp.bfloat16, jnp.bfloat16),
    )
    start = jax.tree.map(
        lambda part, zero: jnp.broadcast_to(jnp.asarray(zero, part.dtype), part.shape),
        value,
        identity,
    )

    def lap(k, before):
        reached = k < index
        new = combine(
            before, jax.tree.map(lambda part, own: part[k].astype(own.dtype), everything, value)
        )
        return jax.tree.map(lambda a, b: jnp.where(reached, a, b), new, before)

    return lax.fori_loop(0, devices, lap, start)


def unit_lower_inverse(strict_part):
    order_size = strict_part.shape[-1]
    powered = strict_part
    inverse = jnp.eye(order_size, dtype=strict_part.dtype) - strict_part
    for repeat_number in range(max(1, (order_size - 1).bit_length()) - 1):
        powered = jnp.einsum("...ij,...jk->...ik", powered, powered, precision=EXACT_MATMUL)
        inverse = inverse + jnp.einsum(
            "...ij,...jk->...ik", inverse, powered, precision=EXACT_MATMUL
        )
    return inverse


def to_blocks(row_data, block_span):
    blocks_count = row_data.shape[0] // block_span
    shaped = row_data.reshape((blocks_count, block_span) + row_data.shape[1:])
    return jnp.swapaxes(shaped, 1, 2)


def from_blocks(blocked):
    swapped = jnp.swapaxes(blocked, 1, 2)
    return swapped.reshape((-1,) + swapped.shape[2:])


def unit_rows(vectors):
    return vectors * lax.rsqrt(jnp.sum(vectors * vectors, axis=-1, keepdims=True) + NORM_EPS)


def delta_inputs(
    query_proj,
    key_proj,
    value_proj,
    decay_pre,
    write_pre,
    write_bias,
    decay_log_scale,
    shift_rows,
    head_count,
    head_size,
):
    query_act = jax.nn.silu(query_proj.astype(jnp.float32)).reshape(-1, head_count, head_size)
    key_act = jax.nn.silu(key_proj.astype(jnp.float32)).reshape(-1, head_count, head_size)
    value_rows = jax.nn.silu(value_proj.astype(jnp.float32)).reshape(-1, head_count, head_size)
    queries = unit_rows(query_act) * head_size ** (-0.5)
    key_rows = unit_rows(key_act)
    log_decay = -jnp.exp(decay_log_scale) * jax.nn.softplus(decay_pre) + shift_rows
    strength = jax.nn.sigmoid(write_pre + write_bias)
    return (queries, key_rows, value_rows, log_decay, strength)


def delta_prepare(queries, key_rows, value_rows, log_decay, strength):
    block_span = queries.shape[2]
    cumulative = jnp.cumsum(log_decay, axis=-1)
    row_place = lax.broadcasted_iota(jnp.int32, (block_span, block_span), 0)
    col_place = lax.broadcasted_iota(jnp.int32, (block_span, block_span), 1)
    inclusive = col_place <= row_place
    strictly = col_place < row_place
    spread = cumulative[..., :, None] - cumulative[..., None, :]
    decay_table = jnp.where(inclusive, jnp.exp(jnp.where(inclusive, spread, 0.0)), 0.0)
    keys_beta = key_rows * strength[..., None]
    lower_part = jnp.where(
        strictly,
        jnp.einsum("nhik,nhjk->nhij", keys_beta, key_rows, precision=EXACT_MATMUL) * decay_table,
        0.0,
    )
    inverse = unit_lower_inverse(lower_part)
    growth = jnp.exp(cumulative)
    state_updates = jnp.einsum(
        "nhij,nhjv->nhiv", inverse, value_rows * strength[..., None], precision=EXACT_MATMUL
    )
    erase_term = jnp.einsum(
        "nhij,nhjk->nhik", inverse, keys_beta * growth[..., None], precision=EXACT_MATMUL
    )
    inside_block = (
        jnp.einsum("nhik,nhjk->nhij", queries, key_rows, precision=EXACT_MATMUL) * decay_table
    )
    boosted_query = queries * growth[..., None]
    damped_keys = key_rows * jnp.exp(cumulative[..., -1:] - cumulative)[..., None]
    decay_per_block = jnp.exp(cumulative[..., -1])
    return (state_updates, erase_term, inside_block, boosted_query, damped_keys, decay_per_block)


def delta_step(memory_state, inputs):
    state_updates, erase_term, inside_block, boosted_query, damped_keys, decay_per_block = inputs
    fixed_values = state_updates - jnp.einsum(
        "mzq,mqc->mzc", erase_term, memory_state, precision=EXACT_MATMUL
    )
    produced_rows = jnp.einsum(
        "mzq,mqc->mzc", boosted_query, memory_state, precision=EXACT_MATMUL
    ) + jnp.einsum("efq,eqn->efn", inside_block, fixed_values, precision=EXACT_MATMUL)
    memory_state = memory_state * decay_per_block[:, None, None] + jnp.einsum(
        "wam,waz->wmz", damped_keys, fixed_values, precision=EXACT_MATMUL
    )
    return (memory_state, produced_rows)


def transition_step(carried, inputs):
    memory_state, transfer = carried
    state_updates, erase_term, inside_block, boosted_query, damped_keys, decay_per_block = inputs
    fixed_values = state_updates - jnp.einsum(
        "mzq,mqc->mzc", erase_term, memory_state, precision=EXACT_MATMUL
    )
    coupling = jnp.einsum("hik,hil->hkl", damped_keys, erase_term, precision=EXACT_MATMUL)
    memory_state = memory_state * decay_per_block[:, None, None] + jnp.einsum(
        "wam,waz->wmz", damped_keys, fixed_values, precision=EXACT_MATMUL
    )
    transfer = transfer * decay_per_block[:, None, None] - jnp.einsum(
        "hkl,hlm->hkm", coupling, transfer, precision=EXACT_MATMUL
    )
    return ((memory_state, transfer), None)


def compose(prior_blocks, following_blocks):
    joined_map = jnp.einsum(
        "hkl,hlm->hkm", following_blocks[0], prior_blocks[0], precision=EXACT_MATMUL
    )
    joined_state = (
        jnp.einsum("djo,dog->djg", following_blocks[0], prior_blocks[1], precision=EXACT_MATMUL)
        + following_blocks[1]
    )
    return (joined_map, joined_state)


def stick_block(queries, key_rows, value_rows, query_place, key_place, offsets):
    scale_factor = queries.shape[-1] ** (-0.5)
    scores = (
        jnp.einsum("qhd,khd->hqk", queries, key_rows, preferred_element_type=jnp.float32)
        * scale_factor
        + offsets[:, None, None]
    )
    visible = key_place[None, :] < query_place[:, None]
    skipped = jnp.where(visible, jax.nn.log_sigmoid(-scores), 0.0)
    beyond = lax.cumsum(skipped, axis=2, reverse=True) - skipped
    weights = jnp.where(visible, jnp.exp(jax.nn.log_sigmoid(scores) + beyond), 0.0).astype(
        jnp.bfloat16
    )
    partial_value = jnp.einsum(
        "hqk,khd->qhd", weights, value_rows, preferred_element_type=jnp.float32
    )
    return (partial_value, jnp.sum(skipped, axis=2).T)


def stick_combine(partials, totals):
    beyond = jnp.cumsum(totals[::-1], axis=0)[::-1] - totals
    return jnp.sum(partials * jnp.exp(beyond)[..., None], axis=0)


def on_device_split(
    hidden_in,
    sb_query_w,
    sb_key_w,
    sb_value_w,
    sb_offset,
    delta_query_w,
    delta_key_w,
    delta_value_w,
    decay_w,
    write_w,
    write_bias,
    decay_log_scale,
    decay_shift,
    head_gain,
    sb_out_w,
    delta_out_w,
):
    token_rows = hidden_in.shape[1]
    local_in = hidden_in.reshape(token_rows, hidden_in.shape[2])
    gathered = (
        lax.all_gather(sb_query_w, "fs", axis=0, tiled=True),
        lax.all_gather(sb_key_w, "fs", axis=0, tiled=True),
        lax.all_gather(sb_value_w, "fs", axis=0, tiled=True),
        lax.all_gather(delta_query_w, "fs", axis=0, tiled=True),
        lax.all_gather(delta_key_w, "fs", axis=0, tiled=True),
        lax.all_gather(delta_value_w, "fs", axis=0, tiled=True),
    )
    in_weights = tuple(gathered) + (decay_w, write_w)
    portion = lax.all_gather(local_in, "tp", axis=1, tiled=True)
    projected = tuple(
        (jnp.dot(portion, weight, preferred_element_type=jnp.float32) for weight in in_weights)
    )
    sb_heads = sb_offset.shape[0]
    delta_heads = decay_log_scale.shape[0]
    sb_query = projected[0].astype(jnp.bfloat16).reshape(token_rows, sb_heads, SB_DIM)
    sb_keys = projected[1].astype(jnp.bfloat16)
    sb_values = projected[2].astype(jnp.bfloat16)
    shift_rows = decay_shift.reshape(delta_heads, token_rows).T
    queries, key_rows, value_rows, log_decay, strength = delta_inputs(
        projected[3].astype(jnp.bfloat16),
        projected[4].astype(jnp.bfloat16),
        projected[5].astype(jnp.bfloat16),
        projected[6],
        projected[7],
        write_bias,
        decay_log_scale,
        shift_rows,
        delta_heads,
        GDN_DIM,
    )
    prepared = delta_prepare(
        to_blocks(queries, BLOCK),
        to_blocks(key_rows, BLOCK),
        to_blocks(value_rows, BLOCK),
        to_blocks(log_decay, BLOCK),
        to_blocks(strength, BLOCK),
    )
    identity_map = jnp.broadcast_to(
        jnp.eye(GDN_DIM, dtype=jnp.float32), (delta_heads, GDN_DIM, GDN_DIM)
    )
    empty_state = jnp.zeros((delta_heads, GDN_DIM, GDN_DIM), jnp.float32)
    (local_end, local_map), unused_out = lax.scan(
        transition_step, (empty_state, identity_map), prepared
    )
    own_first = lax.axis_index("sp") * token_rows
    query_place = own_first + lax.iota(jnp.int32, token_rows)
    sp_count = lax.axis_size("sp")
    slot_out = jnp.zeros((sp_count, token_rows, sb_heads, SB_DIM), jnp.float32)
    slot_total = jnp.zeros((sp_count, token_rows, sb_heads), jnp.float32)

    def absorb(slot_arrays, address_portion, value_part, shard_first):

        def active(current):
            partial_value, totals = stick_block(
                sb_query,
                address_portion.reshape(token_rows, sb_heads, SB_DIM),
                value_part.reshape(token_rows, sb_heads, SB_DIM),
                query_place,
                shard_first + lax.iota(jnp.int32, token_rows),
                sb_offset,
            )
            slot_index = shard_first // token_rows
            return (
                lax.dynamic_update_index_in_dim(current[0], partial_value, slot_index, 0),
                lax.dynamic_update_index_in_dim(current[1], totals, slot_index, 0),
            )

        def inactive(current):
            return current

        usable = jnp.logical_and(shard_first >= 0, shard_first <= own_first)
        return lax.cond(usable, active, inactive, slot_arrays)

    key_block = lax.all_gather(sb_keys, "sp", axis=0, tiled=True)
    value_block = lax.all_gather(sb_values, "sp", axis=0, tiled=True)

    def per_shard(shard_number, current):
        row_begin = shard_number * token_rows
        return absorb(
            current,
            lax.dynamic_slice_in_dim(key_block, row_begin, token_rows, 0),
            lax.dynamic_slice_in_dim(value_block, row_begin, token_rows, 0),
            row_begin,
        )

    slot_arrays = lax.fori_loop(
        0, key_block.shape[0] // token_rows, per_shard, (slot_out, slot_total)
    )
    unused_map, incoming = carried_in(
        (local_map, local_end), "sp", compose, (identity_map, empty_state)
    )
    sb_mixed = (
        stick_combine(slot_arrays[0], slot_arrays[1])
        .astype(jnp.bfloat16)
        .reshape(token_rows, sb_heads * SB_DIM)
    )
    unused_end, produced_rows = lax.scan(delta_step, incoming, prepared)
    produced_rows = from_blocks(produced_rows)
    normed = (
        produced_rows
        * lax.rsqrt(jnp.mean(produced_rows * produced_rows, axis=-1, keepdims=True) + NORM_EPS)
        * head_gain
    )
    delta_mixed = normed.astype(jnp.bfloat16).reshape(token_rows, delta_heads * GDN_DIM)
    result = lax.psum_scatter(
        (
            jnp.dot(sb_mixed, sb_out_w, preferred_element_type=jnp.float32)
            + jnp.dot(delta_mixed, delta_out_w, preferred_element_type=jnp.float32)
        ).astype(jnp.bfloat16),
        "tp",
        scatter_dimension=0,
        tiled=True,
    ).astype(jnp.float32)
    return result.astype(jnp.bfloat16).reshape(1, result.shape[0], result.shape[1])


def remote(src, dst, send, recv, axis, index):
    return pltpu.make_async_remote_copy(
        src_ref=src, dst_ref=dst, send_sem=send, recv_sem=recv,
        device_id={axis: index}, device_id_type=MESH,
    )


def greet(axes):
    barrier = pltpu.get_barrier_semaphore()
    count = 0
    for axis in axes:
        size, me = lax.axis_size(axis), lax.axis_index(axis)
        for k in range(1, size):
            pl.semaphore_signal(
                barrier, inc=1, device_id={axis: lax.rem(me + k, size)}, device_id_type=MESH
            )
            count += 1
    pl.semaphore_wait(barrier, count)


def halves(a):
    high = a.astype(jnp.bfloat16)
    return high, (a - high.astype(jnp.float32)).astype(jnp.bfloat16)


def dot_f32(a, b, dims=((1,), (0,))):
    return lax.dot_general(a, b, (dims, ((), ())), preferred_element_type=jnp.float32)


def wide_rhs(high, low, axis):
    top = jnp.concatenate([high, low], axis=axis)
    bottom = jnp.concatenate([high, jnp.zeros_like(low)], axis=axis)
    return jnp.concatenate([top, bottom], axis=1 - axis)


def folded(a):
    half = a.shape[1] // 2
    return a[:, :half] + a[:, half:]


def layer_kernel(
    offset_hbm, decay_scale_hbm, write_bias_hbm,
    x_ref, w0, w1, w2, w3, w4, w5, decay_w_ref, write_w_ref, shift_ref, gain_hbm, sw_hbm, dw_hbm,
    own, incoming,
    offset_ref, decay_scale_ref, write_bias_ref, gain_ref,
    xs, ws, gate_w, gate_all, gates, shifts_ref, after,
    proj, acc, later, memory_ref, maps, adds, stick_out, delta_out,
    sticks, deltas, sw_ref, dw_ref, partial, outgoing,
    x_send, x_recv, f_send, f_recv, w_send, w_recv, r_recv, s_send, s_recv, l_sem,
    a_send, a_recv, c_sem,
):
    weights = (w0, w1, w2, w3, w4, w5)
    sp, tp = lax.axis_size("sp"), lax.axis_size("tp")
    z, f, t = lax.axis_index("sp"), lax.axis_index("fs"), lax.axis_index("tp")
    rows, half = x_ref.shape
    depth = w0.shape[0]
    cols = ws.shape[1] // len(weights)
    parts = x_recv.shape[2]
    heads = decay_w_ref.shape[0]
    slot = pl.ds(pl.multiple_of(t * half, half), half)
    local = [
        pltpu.make_async_copy(x_ref, xs.at[z, :, slot], l_sem.at[0]),
        pltpu.make_async_copy(shift_ref, shifts_ref.at[z], l_sem.at[1]),
        pltpu.make_async_copy(decay_w_ref, gate_w.at[0], l_sem.at[2]),
        pltpu.make_async_copy(write_w_ref, gate_w.at[1], l_sem.at[3]),
        pltpu.make_async_copy(offset_hbm, offset_ref, l_sem.at[6]),
        pltpu.make_async_copy(decay_scale_hbm, decay_scale_ref, l_sem.at[7]),
        pltpu.make_async_copy(write_bias_hbm, write_bias_ref, l_sem.at[8]),
        pltpu.make_async_copy(gain_hbm, gain_ref, l_sem.at[9]),
    ]
    late = [
        pltpu.make_async_copy(sw_hbm, sw_ref, l_sem.at[4]),
        pltpu.make_async_copy(dw_hbm, dw_ref, l_sem.at[5]),
    ]

    def w_src(i):
        return weights[i].at[:, pl.ds(pl.multiple_of(z * cols, cols), cols)]

    def w_at(i, who):
        return ws.at[pl.ds(pl.multiple_of(who * depth, depth), depth), pl.ds(i * cols, cols)]

    local_w = [
        pltpu.make_async_copy(w_src(i), w_at(i, f), l_sem.at[10]) for i in range(len(weights))
    ]
    near = (f + 1 - 2 * (f % 2), f + 2 - 4 * (f // 2))
    count = len(weights)
    delta_kinds, stick_kinds = (3, 4, 5), (0, 1, 2)

    def onward(way):
        return z + 1 < sp if way == 0 else z > 0

    def ahead(way):
        return z + 1 if way == 0 else z - 1

    barrier = pltpu.get_barrier_semaphore()
    for way in range(2):
        @pl.when(onward(way))
        def _():
            pl.semaphore_signal(
                barrier, inc=1, device_id={"sp": ahead(way)}, device_id_type=MESH
            )
    for side in range(2):
        pl.semaphore_signal(barrier, inc=1, device_id={"fs": near[side]}, device_id_type=MESH)
    pl.semaphore_signal(
        barrier, inc=1, device_id={"tp": lax.rem(t + 1, tp)}, device_id_type=MESH
    )
    for c in local + local_w:
        c.start()
    peers = onward(0).astype(jnp.int32) + onward(1).astype(jnp.int32) + 3
    pl.semaphore_wait(barrier, peers)

    def x_copy(way, step, part):
        block = z - (step - 1) if way == 0 else z + (step - 1)
        piece = pl.ds(part * (rows // parts), rows // parts)
        there = xs.at[block, piece, slot]
        return remote(
            x_ref.at[piece, :] if step == 1 else there, there,
            x_send.at[way], x_recv.at[way, step - 1, part], "sp", ahead(way),
        )

    def shift_copy(way, step):
        block = z - (step - 1) if way == 0 else z + (step - 1)
        there = shifts_ref.at[block]
        return remote(
            shift_ref if step == 1 else there, there,
            s_send.at[way], s_recv.at[way, step - 1], "sp", ahead(way),
        )

    def comes(way, step):
        return z >= step if way == 0 else z + step < sp

    def sends(way, step):
        return jnp.logical_and(onward(way), comes(way, step - 1))

    def forward(way, step, part):
        block = z - step if way == 0 else z + step
        piece = pl.ds(part * (rows // parts), rows // parts)
        there = xs.at[block, piece, slot]
        return remote(
            x_ref.at[piece, :] if step == 0 else there, there,
            f_send.at[0], f_recv.at[way * (sp - 1) + step], "tp", lax.rem(t + 1, tp),
        )

    def w_copy(side, i):
        return remote(
            w_src(i), w_at(i, f), w_send.at[0], w_recv.at[side, i], "fs", near[side]
        )

    def w_relay(side, i):
        part = depth // 2
        start = pl.multiple_of(near[side] * depth + side * part, part)
        there = ws.at[pl.ds(start, part), pl.ds(i * cols, cols)]
        return remote(
            there, there, w_send.at[0], r_recv.at[i // 3], "fs", near[1 - side]
        )

    for part in range(parts):
        for way in range(2):
            @pl.when(onward(way))
            def _():
                x_copy(way, 1, part).start()
                if part == 0:
                    shift_copy(way, 1).start()
    for i in delta_kinds:
        for side in range(2):
            w_copy(side, i).start()
    for part in range(parts):
        forward(0, 0, part).start()

    def relay(i):
        for side in range(2):
            w_copy(side, i).wait_recv()
            w_relay(side, i).start()

    def arrive(step, part):
        for way in range(2):
            @pl.when(comes(way, step))
            def _():
                x_copy(way, step, part).wait_recv()
                forward(way, step, part).start()
                if step + 1 < sp:
                    @pl.when(onward(way))
                    def _():
                        x_copy(way, step + 1, part).start()
                if part == 0:
                    shift_copy(way, step).wait_recv()
                    if step + 1 < sp:
                        @pl.when(onward(way))
                        def _():
                            shift_copy(way, step + 1).start()

    below = lax.broadcasted_iota(jnp.int32, (rows, rows), 0)
    across = lax.broadcasted_iota(jnp.int32, (rows, rows), 1)
    after[:, :rows] = jnp.where(below > across, 1.0, 0.0).astype(jnp.bfloat16)
    after[:, rows:] = jnp.ones((rows, cols), jnp.bfloat16)
    acc[...] = jnp.zeros_like(acc)
    later[...] = jnp.zeros_like(later)
    memory_ref[...] = jnp.zeros_like(memory_ref)
    early = [(step, part) for step in range(1, sp - 1) for part in range(parts)]
    relay(delta_kinds[0])
    arrive(*early[0])
    for i in delta_kinds[1:]:
        relay(i)
    for i in stick_kinds:
        for side in range(2):
            w_copy(side, i).start()
    for c in late:
        c.start()
    for step, part in early[1:parts]:
        arrive(step, part)
    for c in local:
        c.wait()
    own_w = ws.at[pl.ds(pl.multiple_of(f * depth, depth), depth), :]
    pltpu.make_async_copy(own_w, own_w, l_sem.at[10]).wait()
    gate_all[...] = jnp.concatenate(
        [gate_w[0].astype(jnp.float32), gate_w[1].astype(jnp.float32)], axis=0
    ).astype(jnp.bfloat16)
    def all_sent(ref, sem):
        remote(ref, ref, sem, sem, "tp", lax.rem(t + 1, tp)).wait_send()

    def all_came(ref, sem):
        remote(ref, ref, sem, sem, "tp", lax.rem(t + 1, tp)).wait_recv()

    def block_came(way, step):
        all_came(xs.at[z, :, slot], f_recv.at[way * (sp - 1) + step])

    block_came(0, 0)

    def relayed(kinds):
        first = kinds[0] * cols
        all_came(ws.at[pl.ds(0, depth), pl.ds(first, len(kinds) * cols)], r_recv.at[kinds[0] // 3])

    relayed(delta_kinds)

    size = offset_ref.shape[0] // sp
    sb_size = cols // size
    scale = sb_size ** (-0.5)
    tile = rows // 2

    def at_block(b, start=0, extent=rows):
        return pl.ds(pl.multiple_of(b * rows + start, extent), extent)

    def pair(i, j):
        for part in range(rows // tile):
            mine = at_block(i, part * tile, tile)
            q = proj[0, mine, :]
            keys, values = proj[1, at_block(j), :], proj[2, at_block(j), :]
            lane = lax.broadcasted_iota(jnp.int32, (tile, cols), 1)
            query = jnp.concatenate(
                [jnp.where(lane // sb_size == h, q, jnp.zeros_like(q)) for h in range(size)], axis=0
            )
            score = dot_f32(query, keys, ((1,), (1,)))
            score = jnp.concatenate(
                [
                    score[h * tile : (h + 1) * tile] * scale + offset_ref[z * size + h]
                    for h in range(size)
                ],
                axis=0,
            )
            skip = jnp.maximum(score, jnp.log(1.0 + jnp.exp(jnp.minimum(score, 80.0))))
            weight = score - skip
            seen = across[:tile] < below[:tile] + (part * tile + (i - j) * rows)
            seen = jnp.concatenate([seen] * size, axis=0)
            skip = jnp.where(seen, skip, 0.0)
            sums = dot_f32(skip.astype(jnp.bfloat16), after[...])
            weight = jnp.where(seen, jnp.exp(weight - sums[:, :rows]), 0.0)
            out = dot_f32(weight.astype(jnp.bfloat16), values)
            mixed, total = out[:tile], sums[:tile, rows:]
            for h in range(1, size):
                at = slice(h * tile, (h + 1) * tile)
                mixed = jnp.where(lane // sb_size == h, out[at], mixed)
                total = jnp.where(lane // sb_size == h, sums[at, rows:], total)
            passed = later[mine, :]
            acc[mine, :] = acc[mine, :] + mixed * jnp.exp(-passed)
            later[mine, :] = passed + total

    span = BLOCK
    duo = 2 * span
    blocks = rows // span
    width = GDN_DIM
    seg_row = lax.broadcasted_iota(jnp.int32, (rows, rows), 0)
    seg_col = lax.broadcasted_iota(jnp.int32, (rows, rows), 1)
    together = seg_row // span == seg_col // span
    upto = jnp.where(jnp.logical_and(together, seg_row <= seg_col), 1.0, 0.0).astype(jnp.bfloat16)
    beyond_it = jnp.where(jnp.logical_and(together, seg_row > seg_col), 1.0, 0.0).astype(
        jnp.bfloat16
    )
    prow = lax.broadcasted_iota(jnp.int32, (span, duo), 0)
    plane = lax.broadcasted_iota(jnp.int32, (span, duo), 1)
    first = plane < span
    pcol = jnp.where(first, plane, plane - span)
    inclusive, strictly = pcol <= prow, pcol < prow
    unit = jnp.where(pcol == prow, 1.0, 0.0)
    diagonal = lax.broadcasted_iota(jnp.int32, (width, width), 0) == lax.broadcasted_iota(
        jnp.int32, (width, width), 1
    )
    eighth = lax.broadcasted_iota(jnp.int32, (8, rows), 0)

    def silu(a):
        return a * (1.0 / (1.0 + jnp.exp(-a)))

    def unit_of(a):
        return a * lax.rsqrt(jnp.sum(a * a, axis=-1, keepdims=True) + NORM_EPS)

    def apart(a):
        lanes = lax.broadcasted_iota(jnp.int32, a.shape, 1) < span
        zero = jnp.zeros_like(a)
        return jnp.concatenate([jnp.where(lanes, a, zero), jnp.where(lanes, zero, a)], axis=0)

    def squared(left, power):
        high, low = halves(power)
        lhigh, llow = halves(left)
        return folded(
            dot_f32(
                jnp.concatenate([lhigh, llow], axis=1), wide_rhs(apart(high), apart(low), 1)
            )
        )

    def prepare(b, dq, dk, dv):
        gates[...] = dot_f32(gate_all[...], xs[b], ((1,), (1,)))
        pre = gates[pl.ds(z, 1), :]
        write = gates[pl.ds(heads + z, 1), :] + write_bias_ref[z]
        rate = jnp.exp(jnp.full((1, rows), decay_scale_ref[z], jnp.float32))
        soft = jnp.maximum(pre, 0.0) + jnp.log(1.0 + jnp.exp(-jnp.abs(pre)))
        decay = shifts_ref[b, pl.ds(z, 1), :] - rate * soft
        strength = 1.0 / (1.0 + jnp.exp(-write))
        d1 = decay.astype(jnp.bfloat16).astype(jnp.float32)
        d2 = (decay - d1).astype(jnp.bfloat16).astype(jnp.float32)
        d3 = decay - d1 - d2
        three = jnp.where(
            eighth == 0, d1, jnp.where(eighth == 1, d2, jnp.where(eighth == 2, d3, 0.0))
        ).astype(jnp.bfloat16)
        cum_row = jnp.sum(dot_f32(three, upto), axis=0, keepdims=True)
        rest_row = jnp.sum(dot_f32(three, beyond_it), axis=0, keepdims=True)
        stack = jnp.where(
            eighth == 0, strength,
            jnp.where(
                eighth == 1, jnp.exp(cum_row),
                jnp.where(eighth == 2, jnp.exp(rest_row), cum_row),
            ),
        )
        columns = stack.T
        s_col, grow, damp, cum = (columns[:, n : n + 1] for n in range(4))
        q = unit_of(silu(dq)) * width ** (-0.5)
        k = unit_of(silu(dk))
        v = silu(dv)
        boosted = q * grow
        damped = k * damp
        right = jnp.concatenate([v * s_col, k * (s_col * grow)], axis=1)
        kh, kl = halves(k)
        qh, ql = halves(q)
        work = []
        for duo_at in range(rows // duo):
            lo = duo_at * duo
            here = slice(lo, lo + duo)
            left = jnp.concatenate(
                [
                    jnp.concatenate([kh[here], kl[here]], axis=1),
                    jnp.concatenate([qh[here], ql[here]], axis=1),
                ],
                axis=0,
            )
            gram = folded(
                dot_f32(left, wide_rhs(kh[here], kl[here], 0), ((1,), (1,)))
            )
            spread = (
                jnp.where(first, cum[lo : lo + span], cum[lo + span : lo + duo])
                - cum_row[:, here]
            )
            table = jnp.where(inclusive, jnp.exp(jnp.where(inclusive, spread, 0.0)), 0.0)
            scale_col = jnp.where(first, s_col[lo : lo + span], s_col[lo + span : lo + duo])
            near_k = jnp.where(first, gram[:span], gram[span:duo])
            near_q = jnp.where(first, gram[duo : duo + span], gram[duo + span :])
            strict = jnp.where(strictly, near_k * table * scale_col, 0.0)
            work.append([unit - strict, strict, near_q * table])
        yield
        for w in work:
            w[1] = squared(w[1], w[1])
        levels = max(1, (span - 1).bit_length()) - 1
        for level in range(levels):
            if level == levels // 2:
                yield
            for w in work:
                if level + 1 < levels:
                    both = squared(jnp.concatenate([w[1], w[0]], axis=0), w[1])
                    w[1], w[0] = both[:span], w[0] + both[span:]
                else:
                    w[0] = w[0] + squared(w[0], w[1])
        yield
        for duo_at, (inverse, _, inside) in enumerate(work):
            lo = duo_at * duo
            here = slice(lo, lo + duo)
            ih, il = (apart(a) for a in halves(inverse))
            rh, rl = halves(right[here])
            solved = dot_f32(
                jnp.concatenate([ih, il], axis=1), jnp.concatenate([rh, rh], axis=0)
            ) + dot_f32(ih, rl)
            lh, ll = (
                apart(a) for a in halves(jnp.concatenate([damped[here].T, inside], axis=0))
            )
            sh, sl = halves(solved)
            made = dot_f32(
                jnp.concatenate([lh, ll], axis=1), jnp.concatenate([sh, sh], axis=0)
            ) + dot_f32(lh, sl)
            for side in range(2):
                at = lo + side * span
                mine = made[side * (width + span) : (side + 1) * (width + span)]
                n = b * blocks + 2 * duo_at + side
                keep = grow[at + span - 1 : at + span]
                step_map = jnp.where(diagonal, keep, 0.0) - mine[:width, width:]
                query = boosted[at : at + span] - mine[width:, width:]
                high, low = halves(jnp.concatenate([step_map, query], axis=0))
                maps[n, :, :width] = high
                maps[n, :, width:] = low
                adds[n] = mine[:, :width]

    def give(which, out, target):
        here = target.at[:, pl.ds(pl.multiple_of(z * cols, cols), cols)]

        def send(g, k, sem):
            return remote(
                out.at[at_block(g), :], here,
                a_send.at[which], a_recv.at[sem], "sp", g,
            )

        def started(g):
            for k in range(1, sp):
                there = lax.rem(z + k, sp)
                if which == 0:
                    @pl.when(there == g)
                    def _():
                        send(there, k, 0).start()
                else:
                    slow = jnp.logical_or(
                        z == sp - 1, jnp.logical_and(z == 0, there == sp - 1)
                    )

                    @pl.when(jnp.logical_and(there == g, slow))
                    def _():
                        send(there, k, 2).start()

                    @pl.when(jnp.logical_and(there == g, jnp.logical_not(slow)))
                    def _():
                        send(there, k, 1).start()

        return started

    stick_started = give(0, stick_out, sticks)
    delta_started = give(1, delta_out, deltas)

    shorter = jnp.minimum(z, sp - 1 - z)
    down_last = z > sp - 1 - z

    def place(n):
        both = n <= 2 * shorter
        way_n = jnp.where(both, lax.rem(n + 1, 2), jnp.where(down_last, 0, 1))
        step_n = jnp.where(n == 0, 0, jnp.where(both, (n + 1) // 2, n - shorter))
        down = jnp.logical_and(way_n == 0, n > 0)
        return way_n, step_n, down, jnp.where(down, z - step_n, z + step_n)

    last_way = jnp.logical_or(z == 0, z == sp - 1)

    def block_ready(n):
        way_n, step_n, down, b = place(n)
        for step in range(1, sp):
            for way in range(2):
                @pl.when(jnp.logical_and(step_n == step, way_n == way))
                def _():
                    block_came(way, step)
        return b

    def delta_block(b):
        drows = dot_f32(xs[b], ws[:, 3 * cols :]).astype(jnp.bfloat16).astype(jnp.float32)
        return prepare(b, drows[:, :cols], drows[:, cols : 2 * cols], drows[:, 2 * cols :])

    last_way = jnp.logical_or(z == 0, z == sp - 1)
    from_top = z == sp - 1

    def stick_project(n):
        b = jnp.where(from_top, sp - 1 - n, n)
        out = dot_f32(xs[b], ws[:, : 3 * cols]).astype(jnp.bfloat16)
        for i in range(3):
            proj[i, at_block(b), :] = out[:, i * cols : (i + 1) * cols]

    def stick_place(n):
        lower = z < sp // 2
        between = jnp.where(
            n == 0,
            jnp.where(lower, sp - 1, 0),
            jnp.where(
                n == 1,
                jnp.where(lower, sp - 2, 1),
                jnp.where(n == 2, jnp.where(lower, 0, sp - 1), z),
            ),
        )
        return jnp.where(from_top, sp - 1 - n, jnp.where(last_way, n, between))

    def settle(i):
        stick_out[at_block(i), :] = acc[at_block(i), :].astype(jnp.bfloat16)

    def stick_pair(n, r):
        b = stick_place(n)
        i = jnp.where(from_top, b + r, b)
        j = jnp.where(from_top, b, b - r)
        pair(i, j)

        @pl.when(j == 0)
        def _():
            settle(i)
            stick_started(i)

    def walk_groups(start, stop, held=False):
        def group(g, c):
            @pl.when(g > start + held)
            def _():
                delta_started(g - 1)
            memory = memory_ref[...]
            for n in range(blocks):
                memory = walk(g * blocks + n, memory)
            memory_ref[...] = memory
            return c

        lax.fori_loop(start, stop, group, 0)
        delta_started(stop - 1)

    def walk(n, memory):
        high, low = halves(memory)
        new = folded(dot_f32(maps[n], wide_rhs(high, low, 1))) + adds[n]
        made = new[width:]
        made = made * lax.rsqrt(jnp.mean(made * made, axis=-1, keepdims=True) + NORM_EPS)
        at = pl.ds(pl.multiple_of(n * span, span), span)
        delta_out[at, :] = (made * gain_ref[...]).astype(delta_out.dtype)
        return new[:width]

    def plain_delta(n, c):
        @pl.when(n == 1)
        def _():
            relay(stick_kinds[0])

        @pl.when(n == sp - 2)
        def _():
            for c in early[parts:-1]:
                arrive(*c)
            relay(stick_kinds[1])

            @pl.when(z == 0)
            def _():
                walk_groups(0, 2)
            relay(stick_kinds[2])
            arrive(*early[-1])
        for _ in delta_block(block_ready(n)):
            pass
        return c

    events = jnp.where(last_way, sp - 1, sp)
    lax.fori_loop(0, events, plain_delta, 0)

    @pl.when(jnp.logical_not(last_way))
    def _():
        walk_groups(0, sp, held=True)

    relayed(stick_kinds)

    def stick_event(n, c):
        for part in range(2):
            @pl.when(jnp.logical_and(last_way, n == part + 1))
            def _():
                arrive(sp - 1, part)

        def project_one(m, c):
            stick_project(m)
            return c

        needed = jnp.where(from_top, n, stick_place(n)) + 1
        lax.fori_loop(c, needed, project_one, 0)

        @pl.when(jnp.logical_and(jnp.logical_not(last_way), n == 0))
        def _():
            delta_started(0)

        def one(r, c):
            for part in range(2, parts):
                @pl.when(
                    jnp.logical_and(
                        last_way, jnp.logical_and(n == sp - 2, r == sp - 1 - parts + part)
                    )
                )
                def _():
                    arrive(sp - 1, part)
            stick_pair(n, r)
            return c

        lax.fori_loop(0, jnp.where(last_way, n, stick_place(n)) + 1, one, 0)
        return jnp.maximum(c, needed)

    lax.fori_loop(0, events, stick_event, 0)

    @pl.when(last_way)
    def _():
        @pl.when(z == 0)
        def _():
            walk_groups(2, sp - 1)
        for way in range(2):
            @pl.when(comes(way, sp - 1))
            def _():
                block_came(way, sp - 1)
        stick_project(sp - 1)
        stick_pair(sp - 1, 0)
        stages = delta_block(stick_place(sp - 1))
        for u in range(1, sp):
            next(stages)
            stick_pair(sp - 1, u)
        for _ in stages:
            pass
        walk_groups(jnp.where(z == 0, sp - 1, 0), sp)

    mine_z = pl.ds(pl.multiple_of(z * rows, rows), rows)
    lanes = pl.ds(pl.multiple_of(z * cols, cols), cols)
    sticks[:, lanes] = stick_out[mine_z, :]
    deltas[:, lanes] = delta_out[mine_z, :]
    for c in late:
        c.wait()
    all_sent(ws.at[pl.ds(0, 3 * depth), :], w_send.at[0])
    all_sent(xs.at[:, :, slot], f_send.at[0])
    for c in range(sp):
        @pl.when(z == c)
        def _():
            for way, passed in enumerate((c + 1 if c + 1 < sp else 0, sp - c if c > 0 else 0)):
                if passed:
                    all_sent(xs.at[pl.ds(0, passed), :, slot], x_send.at[way])
                    all_sent(shifts_ref.at[pl.ds(0, passed)], s_send.at[way])
    all_came(stick_out.at[pl.ds(0, (sp - 1) * rows), :], a_recv.at[0])
    chunks, wide = outgoing.shape[0], outgoing.shape[2]
    share = rows // tp
    for c in range(chunks):
        columns = slice(c * wide, (c + 1) * wide)
        partial[:, columns] = dot_f32(sticks[...], sw_ref[:, columns])
    all_came(delta_out.at[pl.ds(0, (sp - 2) * rows), :], a_recv.at[1])
    soon = pl.ds(pl.multiple_of(jnp.where(from_top, 1, 0) * cols, cols), (sp - 1) * cols)
    for c in range(chunks):
        columns = slice(c * wide, (c + 1) * wide)
        partial[:, columns] += dot_f32(deltas[:, soon], dw_ref[soon, columns])
    all_came(delta_out.at[pl.ds(0, rows), :], a_recv.at[2])
    final = pl.ds(pl.multiple_of(jnp.where(from_top, 0, sp - 1) * cols, cols), cols)
    mine = pl.ds(pl.multiple_of(t * share, share), share)
    partner = lax.rem(t + 1, tp)
    theirs = pl.ds(pl.multiple_of(partner * share, share), share)

    def finish(which, c):
        columns = slice(c * wide, (c + 1) * wide)
        return (
            partial[which, columns] + dot_f32(deltas[which, final], dw_ref[final, columns])
        ).astype(jnp.bfloat16)

    swaps = [
        remote(
            outgoing.at[c], incoming.at[:, c * wide : (c + 1) * wide],
            c_sem.at[0], c_sem.at[1], "tp", partner,
        )
        for c in range(chunks)
    ]
    for c in range(chunks):
        outgoing[c] = finish(theirs, c)
        if c > 0:
            swaps[c - 1].start()
    for c in range(chunks):
        own[:, c * wide : (c + 1) * wide] = finish(mine, c)
        if c == 0:
            swaps[chunks - 1].start()
    all_came(incoming, c_sem.at[1])
    all_sent(incoming, c_sem.at[0])
    for which, out in enumerate((stick_out, delta_out)):
        all_sent(out.at[pl.ds(0, (sp - 1) * rows), :], a_send.at[which])


ANYWHERE = pl.BlockSpec(memory_space=pltpu.HBM)
ON_CORE = pl.BlockSpec(memory_space=pltpu.VMEM)


def on_device_heads(
    hidden_in, sb_query_w, sb_key_w, sb_value_w, sb_offset,
    delta_query_w, delta_key_w, delta_value_w, decay_w, write_w, write_bias,
    decay_log_scale, decay_shift, head_gain, sb_out_w, delta_out_w,
):
    sp, fs, tp = lax.axis_size("sp"), lax.axis_size("fs"), lax.axis_size("tp")
    rows, half = hidden_in.shape[1:]
    width = half * tp
    length = rows * sp
    heads = decay_log_scale.shape[0]
    cols = sb_query_w.shape[1] // sp
    parts, chunks = 4, 4
    share = rows // tp
    blocks = length // BLOCK
    dma = pltpu.SemaphoreType.DMA
    bf16, f32 = jnp.bfloat16, jnp.float32
    own, incoming = pl.pallas_call(
        layer_kernel,
        name="layer",
        out_shape=(pltpu.VMEM((share, width), bf16),) * 2,
        in_specs=[ANYWHERE] * 16,
        out_specs=(ON_CORE,) * 2,
        scratch_shapes=[
            pltpu.SMEM(sb_offset.shape, f32),
            pltpu.SMEM(decay_log_scale.shape, f32),
            pltpu.SMEM(write_bias.shape, f32),
            pltpu.VMEM((1, head_gain.shape[0]), f32),
            pltpu.VMEM((sp, rows, width), bf16),
            pltpu.VMEM((width, 6 * cols), bf16),
            pltpu.VMEM((2, heads, width), bf16),
            pltpu.VMEM((2 * heads, width), bf16),
            pltpu.VMEM((2 * heads, rows), f32),
            pltpu.VMEM((sp, heads, rows), f32),
            pltpu.VMEM((rows, rows + cols), bf16),
            pltpu.VMEM((3, length, cols), bf16),
            pltpu.VMEM((length, cols), f32),
            pltpu.VMEM((length, cols), f32),
            pltpu.VMEM((cols, cols), f32),
            pltpu.VMEM((blocks, cols + BLOCK, 2 * cols), bf16),
            pltpu.VMEM((blocks, cols + BLOCK, cols), f32),
            pltpu.VMEM((length, cols), bf16),
            pltpu.VMEM((length, cols), bf16),
            pltpu.VMEM((rows, cols * sp), bf16),
            pltpu.VMEM((rows, cols * sp), bf16),
            pltpu.VMEM(sb_out_w.shape, bf16),
            pltpu.VMEM(delta_out_w.shape, bf16),
            pltpu.VMEM((rows, width), f32),
            pltpu.VMEM((chunks, share, width // chunks), bf16),
            dma((2,)), dma((2, sp - 1, parts)), dma((1,)), dma((2 * sp - 1,)),
            dma((1,)), dma((2, 6)), dma((2,)), dma((2,)), dma((2, sp - 1)), dma((11,)),
            dma((2,)), dma((3,)), dma((2,)),
        ],
        compiler_params=pltpu.CompilerParams(
            collective_id=0, has_side_effects=True,
            vmem_limit_bytes=ALL_VMEM - 5 * share * width,
        ),
    )(
        sb_offset, decay_log_scale, write_bias,
        hidden_in.reshape(rows, half), sb_query_w, sb_key_w, sb_value_w,
        delta_query_w, delta_key_w, delta_value_w, decay_w.T, write_w.T,
        decay_shift.reshape(heads, rows), head_gain.reshape(1, -1), sb_out_w, delta_out_w,
    )
    result = (own.astype(f32) + incoming.astype(f32)).astype(bf16)
    return result.reshape(1, share, width)


def on_device(*inputs):
    delta_heads = inputs[11].shape[0]
    square = lax.axis_size("sp") == lax.axis_size("fs") == 4 and lax.axis_size("tp") == 2
    if square and delta_heads == lax.axis_size("sp") and inputs[4].shape[0] % delta_heads == 0:
        return on_device_heads(*inputs)
    return on_device_split(*inputs)


def solution(mesh):
    return jax.shard_map(
        on_device,
        mesh=mesh,
        in_specs=(
            P("fs", "sp", "tp"),
            P("fs", "tp"),
            P("fs", "tp"),
            P("fs", "tp"),
            P("tp"),
            P("fs", "tp"),
            P("fs", "tp"),
            P("fs", "tp"),
            P(None, "tp"),
            P(None, "tp"),
            P("tp"),
            P("tp"),
            P("fs", "tp", "sp"),
            P(),
            P("tp", None),
            P("tp", None),
        ),
        out_specs=P("fs", ("sp", "tp"), None),
        check_vma=False,
    )
```

```python
import jax
import jax.numpy as jnp
from jax import lax
from jax.experimental import pallas as pl
from jax.experimental.pallas import tpu as pltpu
from jax.sharding import PartitionSpec as P

MESH = pl.DeviceIdType.MESH
ALL_VMEM = 67043328

SB_DIM = 64
GDN_DIM = 128
BLOCK = 64


EXACT_MATMUL = lax.Precision.HIGHEST
NORM_EPS = 1e-06


def carried_in(value, axis, combine, identity):
    devices, index = (lax.axis_size(axis), lax.axis_index(axis))
    everything = jax.tree.map(
        lambda part, kind: lax.all_gather(part.astype(kind), axis),
        value,
        (jnp.bfloat16, jnp.bfloat16),
    )
    start = jax.tree.map(
        lambda part, zero: jnp.broadcast_to(jnp.asarray(zero, part.dtype), part.shape),
        value,
        identity,
    )

    def lap(k, before):
        reached = k < index
        new = combine(
            before, jax.tree.map(lambda part, own: part[k].astype(own.dtype), everything, value)
        )
        return jax.tree.map(lambda a, b: jnp.where(reached, a, b), new, before)

    return lax.fori_loop(0, devices, lap, start)


def unit_lower_inverse(strict_part):
    order_size = strict_part.shape[-1]
    powered = strict_part
    inverse = jnp.eye(order_size, dtype=strict_part.dtype) - strict_part
    for repeat_number in range(max(1, (order_size - 1).bit_length()) - 1):
        powered = jnp.einsum("...ij,...jk->...ik", powered, powered, precision=EXACT_MATMUL)
        inverse = inverse + jnp.einsum(
            "...ij,...jk->...ik", inverse, powered, precision=EXACT_MATMUL
        )
    return inverse


def to_blocks(row_data, block_span):
    blocks_count = row_data.shape[0] // block_span
    shaped = row_data.reshape((blocks_count, block_span) + row_data.shape[1:])
    return jnp.swapaxes(shaped, 1, 2)


def from_blocks(blocked):
    swapped = jnp.swapaxes(blocked, 1, 2)
    return swapped.reshape((-1,) + swapped.shape[2:])


def unit_rows(vectors):
    return vectors * lax.rsqrt(jnp.sum(vectors * vectors, axis=-1, keepdims=True) + NORM_EPS)


def delta_inputs(
    query_proj,
    key_proj,
    value_proj,
    decay_pre,
    write_pre,
    write_bias,
    decay_log_scale,
    shift_rows,
    head_count,
    head_size,
):
    query_act = jax.nn.silu(query_proj.astype(jnp.float32)).reshape(-1, head_count, head_size)
    key_act = jax.nn.silu(key_proj.astype(jnp.float32)).reshape(-1, head_count, head_size)
    value_rows = jax.nn.silu(value_proj.astype(jnp.float32)).reshape(-1, head_count, head_size)
    queries = unit_rows(query_act) * head_size ** (-0.5)
    key_rows = unit_rows(key_act)
    log_decay = -jnp.exp(decay_log_scale) * jax.nn.softplus(decay_pre) + shift_rows
    strength = jax.nn.sigmoid(write_pre + write_bias)
    return (queries, key_rows, value_rows, log_decay, strength)


def delta_prepare(queries, key_rows, value_rows, log_decay, strength):
    block_span = queries.shape[2]
    cumulative = jnp.cumsum(log_decay, axis=-1)
    row_place = lax.broadcasted_iota(jnp.int32, (block_span, block_span), 0)
    col_place = lax.broadcasted_iota(jnp.int32, (block_span, block_span), 1)
    inclusive = col_place <= row_place
    strictly = col_place < row_place
    spread = cumulative[..., :, None] - cumulative[..., None, :]
    decay_table = jnp.where(inclusive, jnp.exp(jnp.where(inclusive, spread, 0.0)), 0.0)
    keys_beta = key_rows * strength[..., None]
    lower_part = jnp.where(
        strictly,
        jnp.einsum("nhik,nhjk->nhij", keys_beta, key_rows, precision=EXACT_MATMUL) * decay_table,
        0.0,
    )
    inverse = unit_lower_inverse(lower_part)
    growth = jnp.exp(cumulative)
    state_updates = jnp.einsum(
        "nhij,nhjv->nhiv", inverse, value_rows * strength[..., None], precision=EXACT_MATMUL
    )
    erase_term = jnp.einsum(
        "nhij,nhjk->nhik", inverse, keys_beta * growth[..., None], precision=EXACT_MATMUL
    )
    inside_block = (
        jnp.einsum("nhik,nhjk->nhij", queries, key_rows, precision=EXACT_MATMUL) * decay_table
    )
    boosted_query = queries * growth[..., None]
    damped_keys = key_rows * jnp.exp(cumulative[..., -1:] - cumulative)[..., None]
    decay_per_block = jnp.exp(cumulative[..., -1])
    return (state_updates, erase_term, inside_block, boosted_query, damped_keys, decay_per_block)


def delta_step(memory_state, inputs):
    state_updates, erase_term, inside_block, boosted_query, damped_keys, decay_per_block = inputs
    fixed_values = state_updates - jnp.einsum(
        "mzq,mqc->mzc", erase_term, memory_state, precision=EXACT_MATMUL
    )
    produced_rows = jnp.einsum(
        "mzq,mqc->mzc", boosted_query, memory_state, precision=EXACT_MATMUL
    ) + jnp.einsum("efq,eqn->efn", inside_block, fixed_values, precision=EXACT_MATMUL)
    memory_state = memory_state * decay_per_block[:, None, None] + jnp.einsum(
        "wam,waz->wmz", damped_keys, fixed_values, precision=EXACT_MATMUL
    )
    return (memory_state, produced_rows)


def transition_step(carried, inputs):
    memory_state, transfer = carried
    state_updates, erase_term, inside_block, boosted_query, damped_keys, decay_per_block = inputs
    fixed_values = state_updates - jnp.einsum(
        "mzq,mqc->mzc", erase_term, memory_state, precision=EXACT_MATMUL
    )
    coupling = jnp.einsum("hik,hil->hkl", damped_keys, erase_term, precision=EXACT_MATMUL)
    memory_state = memory_state * decay_per_block[:, None, None] + jnp.einsum(
        "wam,waz->wmz", damped_keys, fixed_values, precision=EXACT_MATMUL
    )
    transfer = transfer * decay_per_block[:, None, None] - jnp.einsum(
        "hkl,hlm->hkm", coupling, transfer, precision=EXACT_MATMUL
    )
    return ((memory_state, transfer), None)


def compose(prior_blocks, following_blocks):
    joined_map = jnp.einsum(
        "hkl,hlm->hkm", following_blocks[0], prior_blocks[0], precision=EXACT_MATMUL
    )
    joined_state = (
        jnp.einsum("djo,dog->djg", following_blocks[0], prior_blocks[1], precision=EXACT_MATMUL)
        + following_blocks[1]
    )
    return (joined_map, joined_state)


def stick_block(queries, key_rows, value_rows, query_place, key_place, offsets):
    scale_factor = queries.shape[-1] ** (-0.5)
    scores = (
        jnp.einsum("qhd,khd->hqk", queries, key_rows, preferred_element_type=jnp.float32)
        * scale_factor
        + offsets[:, None, None]
    )
    visible = key_place[None, :] < query_place[:, None]
    skipped = jnp.where(visible, jax.nn.log_sigmoid(-scores), 0.0)
    beyond = lax.cumsum(skipped, axis=2, reverse=True) - skipped
    weights = jnp.where(visible, jnp.exp(jax.nn.log_sigmoid(scores) + beyond), 0.0).astype(
        jnp.bfloat16
    )
    partial_value = jnp.einsum(
        "hqk,khd->qhd", weights, value_rows, preferred_element_type=jnp.float32
    )
    return (partial_value, jnp.sum(skipped, axis=2).T)


def stick_combine(partials, totals):
    beyond = jnp.cumsum(totals[::-1], axis=0)[::-1] - totals
    return jnp.sum(partials * jnp.exp(beyond)[..., None], axis=0)


def on_device_split(
    hidden_in,
    sb_query_w,
    sb_key_w,
    sb_value_w,
    sb_offset,
    delta_query_w,
    delta_key_w,
    delta_value_w,
    decay_w,
    write_w,
    write_bias,
    decay_log_scale,
    decay_shift,
    head_gain,
    sb_out_w,
    delta_out_w,
):
    token_rows = hidden_in.shape[1]
    local_in = hidden_in.reshape(token_rows, hidden_in.shape[2])
    gathered = (
        lax.all_gather(sb_query_w, "fs", axis=0, tiled=True),
        lax.all_gather(sb_key_w, "fs", axis=0, tiled=True),
        lax.all_gather(sb_value_w, "fs", axis=0, tiled=True),
        lax.all_gather(delta_query_w, "fs", axis=0, tiled=True),
        lax.all_gather(delta_key_w, "fs", axis=0, tiled=True),
        lax.all_gather(delta_value_w, "fs", axis=0, tiled=True),
    )
    in_weights = tuple(gathered) + (decay_w, write_w)
    portion = lax.all_gather(local_in, "tp", axis=1, tiled=True)
    projected = tuple(
        (jnp.dot(portion, weight, preferred_element_type=jnp.float32) for weight in in_weights)
    )
    sb_heads = sb_offset.shape[0]
    delta_heads = decay_log_scale.shape[0]
    sb_query = projected[0].astype(jnp.bfloat16).reshape(token_rows, sb_heads, SB_DIM)
    sb_keys = projected[1].astype(jnp.bfloat16)
    sb_values = projected[2].astype(jnp.bfloat16)
    shift_rows = decay_shift.reshape(delta_heads, token_rows).T
    queries, key_rows, value_rows, log_decay, strength = delta_inputs(
        projected[3].astype(jnp.bfloat16),
        projected[4].astype(jnp.bfloat16),
        projected[5].astype(jnp.bfloat16),
        projected[6],
        projected[7],
        write_bias,
        decay_log_scale,
        shift_rows,
        delta_heads,
        GDN_DIM,
    )
    prepared = delta_prepare(
        to_blocks(queries, BLOCK),
        to_blocks(key_rows, BLOCK),
        to_blocks(value_rows, BLOCK),
        to_blocks(log_decay, BLOCK),
        to_blocks(strength, BLOCK),
    )
    identity_map = jnp.broadcast_to(
        jnp.eye(GDN_DIM, dtype=jnp.float32), (delta_heads, GDN_DIM, GDN_DIM)
    )
    empty_state = jnp.zeros((delta_heads, GDN_DIM, GDN_DIM), jnp.float32)
    (local_end, local_map), unused_out = lax.scan(
        transition_step, (empty_state, identity_map), prepared
    )
    own_first = lax.axis_index("sp") * token_rows
    query_place = own_first + lax.iota(jnp.int32, token_rows)
    sp_count = lax.axis_size("sp")
    slot_out = jnp.zeros((sp_count, token_rows, sb_heads, SB_DIM), jnp.float32)
    slot_total = jnp.zeros((sp_count, token_rows, sb_heads), jnp.float32)

    def absorb(slot_arrays, address_portion, value_part, shard_first):

        def active(current):
            partial_value, totals = stick_block(
                sb_query,
                address_portion.reshape(token_rows, sb_heads, SB_DIM),
                value_part.reshape(token_rows, sb_heads, SB_DIM),
                query_place,
                shard_first + lax.iota(jnp.int32, token_rows),
                sb_offset,
            )
            slot_index = shard_first // token_rows
            return (
                lax.dynamic_update_index_in_dim(current[0], partial_value, slot_index, 0),
                lax.dynamic_update_index_in_dim(current[1], totals, slot_index, 0),
            )

        def inactive(current):
            return current

        usable = jnp.logical_and(shard_first >= 0, shard_first <= own_first)
        return lax.cond(usable, active, inactive, slot_arrays)

    key_block = lax.all_gather(sb_keys, "sp", axis=0, tiled=True)
    value_block = lax.all_gather(sb_values, "sp", axis=0, tiled=True)

    def per_shard(shard_number, current):
        row_begin = shard_number * token_rows
        return absorb(
            current,
            lax.dynamic_slice_in_dim(key_block, row_begin, token_rows, 0),
            lax.dynamic_slice_in_dim(value_block, row_begin, token_rows, 0),
            row_begin,
        )

    slot_arrays = lax.fori_loop(
        0, key_block.shape[0] // token_rows, per_shard, (slot_out, slot_total)
    )
    unused_map, incoming = carried_in(
        (local_map, local_end), "sp", compose, (identity_map, empty_state)
    )
    sb_mixed = (
        stick_combine(slot_arrays[0], slot_arrays[1])
        .astype(jnp.bfloat16)
        .reshape(token_rows, sb_heads * SB_DIM)
    )
    unused_end, produced_rows = lax.scan(delta_step, incoming, prepared)
    produced_rows = from_blocks(produced_rows)
    normed = (
        produced_rows
        * lax.rsqrt(jnp.mean(produced_rows * produced_rows, axis=-1, keepdims=True) + NORM_EPS)
        * head_gain
    )
    delta_mixed = normed.astype(jnp.bfloat16).reshape(token_rows, delta_heads * GDN_DIM)
    result = lax.psum_scatter(
        (
            jnp.dot(sb_mixed, sb_out_w, preferred_element_type=jnp.float32)
            + jnp.dot(delta_mixed, delta_out_w, preferred_element_type=jnp.float32)
        ).astype(jnp.bfloat16),
        "tp",
        scatter_dimension=0,
        tiled=True,
    ).astype(jnp.float32)
    return result.astype(jnp.bfloat16).reshape(1, result.shape[0], result.shape[1])


def remote(src, dst, send, recv, axis, index):
    return pltpu.make_async_remote_copy(
        src_ref=src, dst_ref=dst, send_sem=send, recv_sem=recv,
        device_id={axis: index}, device_id_type=MESH,
    )


def greet(axes):
    barrier = pltpu.get_barrier_semaphore()
    count = 0
    for axis in axes:
        size, me = lax.axis_size(axis), lax.axis_index(axis)
        for k in range(1, size):
            pl.semaphore_signal(
                barrier, inc=1, device_id={axis: lax.rem(me + k, size)}, device_id_type=MESH
            )
            count += 1
    pl.semaphore_wait(barrier, count)


def halves(a):
    high = a.astype(jnp.bfloat16)
    return high, (a - high.astype(jnp.float32)).astype(jnp.bfloat16)


def dot_f32(a, b, dims=((1,), (0,))):
    return lax.dot_general(a, b, (dims, ((), ())), preferred_element_type=jnp.float32)


def wide_rhs(high, low, axis):
    top = jnp.concatenate([high, low], axis=axis)
    bottom = jnp.concatenate([high, jnp.zeros_like(low)], axis=axis)
    return jnp.concatenate([top, bottom], axis=1 - axis)


def folded(a):
    half = a.shape[1] // 2
    return a[:, :half] + a[:, half:]


def layer_kernel(
    offset_hbm, decay_scale_hbm, write_bias_hbm,
    x_ref, w0, w1, w2, w3, w4, w5, decay_w_ref, write_w_ref, shift_ref, gain_hbm, sw_hbm, dw_hbm,
    own, incoming,
    offset_ref, decay_scale_ref, write_bias_ref, gain_ref,
    xs, ws, gate_w, gate_all, gates, shifts_ref, after,
    proj, acc, later, memory_ref, maps, adds, stick_out, delta_out,
    sticks, deltas, sw_ref, dw_ref, partial, outgoing,
    x_send, x_recv, f_send, f_recv, w_send, w_recv, r_recv, s_send, s_recv, l_sem,
    a_send, a_recv, c_sem,
):
    weights = (w0, w1, w2, w3, w4, w5)
    sp, tp = lax.axis_size("sp"), lax.axis_size("tp")
    z, f, t = lax.axis_index("sp"), lax.axis_index("fs"), lax.axis_index("tp")
    rows, half = x_ref.shape
    depth = w0.shape[0]
    cols = ws.shape[1] // len(weights)
    parts = x_recv.shape[2]
    heads = decay_w_ref.shape[0]
    slot = pl.ds(pl.multiple_of(t * half, half), half)
    local = [
        pltpu.make_async_copy(x_ref, xs.at[z, :, slot], l_sem.at[0]),
        pltpu.make_async_copy(shift_ref, shifts_ref.at[z], l_sem.at[1]),
        pltpu.make_async_copy(decay_w_ref, gate_w.at[0], l_sem.at[2]),
        pltpu.make_async_copy(write_w_ref, gate_w.at[1], l_sem.at[3]),
        pltpu.make_async_copy(offset_hbm, offset_ref, l_sem.at[6]),
        pltpu.make_async_copy(decay_scale_hbm, decay_scale_ref, l_sem.at[7]),
        pltpu.make_async_copy(write_bias_hbm, write_bias_ref, l_sem.at[8]),
        pltpu.make_async_copy(gain_hbm, gain_ref, l_sem.at[9]),
    ]
    late = [
        pltpu.make_async_copy(sw_hbm, sw_ref, l_sem.at[4]),
        pltpu.make_async_copy(dw_hbm, dw_ref, l_sem.at[5]),
    ]

    def w_src(i):
        return weights[i].at[:, pl.ds(pl.multiple_of(z * cols, cols), cols)]

    def w_at(i, who):
        return ws.at[pl.ds(pl.multiple_of(who * depth, depth), depth), pl.ds(i * cols, cols)]

    local_w = [
        pltpu.make_async_copy(w_src(i), w_at(i, f), l_sem.at[10]) for i in range(len(weights))
    ]
    near = (f + 1 - 2 * (f % 2), f + 2 - 4 * (f // 2))
    count = len(weights)
    delta_kinds, stick_kinds = (3, 4, 5), (0, 1, 2)

    def onward(way):
        return z + 1 < sp if way == 0 else z > 0

    def ahead(way):
        return z + 1 if way == 0 else z - 1

    barrier = pltpu.get_barrier_semaphore()
    for way in range(2):
        @pl.when(onward(way))
        def _():
            pl.semaphore_signal(
                barrier, inc=1, device_id={"sp": ahead(way)}, device_id_type=MESH
            )
    for side in range(2):
        pl.semaphore_signal(barrier, inc=1, device_id={"fs": near[side]}, device_id_type=MESH)
    pl.semaphore_signal(
        barrier, inc=1, device_id={"tp": lax.rem(t + 1, tp)}, device_id_type=MESH
    )
    for c in local + local_w:
        c.start()
    peers = onward(0).astype(jnp.int32) + onward(1).astype(jnp.int32) + 3
    pl.semaphore_wait(barrier, peers)

    def x_copy(way, step, part):
        block = z - (step - 1) if way == 0 else z + (step - 1)
        piece = pl.ds(part * (rows // parts), rows // parts)
        there = xs.at[block, piece, slot]
        return remote(
            x_ref.at[piece, :] if step == 1 else there, there,
            x_send.at[way], x_recv.at[way, step - 1, part], "sp", ahead(way),
        )

    def shift_copy(way, step):
        block = z - (step - 1) if way == 0 else z + (step - 1)
        there = shifts_ref.at[block]
        return remote(
            shift_ref if step == 1 else there, there,
            s_send.at[way], s_recv.at[way, step - 1], "sp", ahead(way),
        )

    def comes(way, step):
        return z >= step if way == 0 else z + step < sp

    def sends(way, step):
        return jnp.logical_and(onward(way), comes(way, step - 1))

    def forward(way, step, part):
        block = z - step if way == 0 else z + step
        piece = pl.ds(part * (rows // parts), rows // parts)
        there = xs.at[block, piece, slot]
        return remote(
            x_ref.at[piece, :] if step == 0 else there, there,
            f_send.at[0], f_recv.at[way * (sp - 1) + step], "tp", lax.rem(t + 1, tp),
        )

    def w_copy(side, i):
        return remote(
            w_src(i), w_at(i, f), w_send.at[0], w_recv.at[side, i], "fs", near[side]
        )

    def w_relay(side, i):
        part = depth // 2
        start = pl.multiple_of(near[side] * depth + side * part, part)
        there = ws.at[pl.ds(start, part), pl.ds(i * cols, cols)]
        return remote(
            there, there, w_send.at[0], r_recv.at[i // 3], "fs", near[1 - side]
        )

    for part in range(parts):
        for way in range(2):
            @pl.when(onward(way))
            def _():
                x_copy(way, 1, part).start()
                if part == 0:
                    shift_copy(way, 1).start()
    for i in delta_kinds:
        for side in range(2):
            w_copy(side, i).start()
    for part in range(parts):
        forward(0, 0, part).start()

    def relay(i):
        for side in range(2):
            w_copy(side, i).wait_recv()
            w_relay(side, i).start()

    def arrive(step, part):
        for way in range(2):
            @pl.when(comes(way, step))
            def _():
                x_copy(way, step, part).wait_recv()
                forward(way, step, part).start()
                if step + 1 < sp:
                    @pl.when(onward(way))
                    def _():
                        x_copy(way, step + 1, part).start()
                if part == 0:
                    shift_copy(way, step).wait_recv()
                    if step + 1 < sp:
                        @pl.when(onward(way))
                        def _():
                            shift_copy(way, step + 1).start()

    below = lax.broadcasted_iota(jnp.int32, (rows, rows), 0)
    across = lax.broadcasted_iota(jnp.int32, (rows, rows), 1)
    after[:, :rows] = jnp.where(below > across, 1.0, 0.0).astype(jnp.bfloat16)
    after[:, rows:] = jnp.ones((rows, cols), jnp.bfloat16)
    acc[...] = jnp.zeros_like(acc)
    later[...] = jnp.zeros_like(later)
    memory_ref[...] = jnp.zeros_like(memory_ref)
    early = [(step, part) for step in range(1, sp - 1) for part in range(parts)]
    relay(delta_kinds[0])
    arrive(*early[0])
    for i in delta_kinds[1:]:
        relay(i)
    for i in stick_kinds:
        for side in range(2):
            w_copy(side, i).start()
    for c in late:
        c.start()
    for step, part in early[1:parts]:
        arrive(step, part)
    for c in local:
        c.wait()
    own_w = ws.at[pl.ds(pl.multiple_of(f * depth, depth), depth), :]
    pltpu.make_async_copy(own_w, own_w, l_sem.at[10]).wait()
    gate_all[...] = jnp.concatenate(
        [gate_w[0].astype(jnp.float32), gate_w[1].astype(jnp.float32)], axis=0
    ).astype(jnp.bfloat16)
    def all_sent(ref, sem):
        remote(ref, ref, sem, sem, "tp", lax.rem(t + 1, tp)).wait_send()

    def all_came(ref, sem):
        remote(ref, ref, sem, sem, "tp", lax.rem(t + 1, tp)).wait_recv()

    def block_came(way, step):
        all_came(xs.at[z, :, slot], f_recv.at[way * (sp - 1) + step])

    block_came(0, 0)

    def relayed(kinds):
        first = kinds[0] * cols
        all_came(ws.at[pl.ds(0, depth), pl.ds(first, len(kinds) * cols)], r_recv.at[kinds[0] // 3])

    relayed(delta_kinds)

    size = offset_ref.shape[0] // sp
    sb_size = cols // size
    scale = sb_size ** (-0.5)
    tile = rows // 2

    def at_block(b, start=0, extent=rows):
        return pl.ds(pl.multiple_of(b * rows + start, extent), extent)

    def pair(i, j):
        for part in range(rows // tile):
            mine = at_block(i, part * tile, tile)
            q = proj[0, mine, :]
            keys, values = proj[1, at_block(j), :], proj[2, at_block(j), :]
            lane = lax.broadcasted_iota(jnp.int32, (tile, cols), 1)
            query = jnp.concatenate(
                [jnp.where(lane // sb_size == h, q, jnp.zeros_like(q)) for h in range(size)], axis=0
            )
            score = dot_f32(query, keys, ((1,), (1,)))
            score = jnp.concatenate(
                [
                    score[h * tile : (h + 1) * tile] * scale + offset_ref[z * size + h]
                    for h in range(size)
                ],
                axis=0,
            )
            seen = across[:tile] < below[:tile] + (part * tile + (i - j) * rows)
            score = jnp.where(jnp.concatenate([seen] * size, axis=0), score, -1e30)
            skip = jnp.maximum(score, jnp.log(1.0 + jnp.exp(jnp.minimum(score, 80.0))))
            weight = score - skip
            sums = dot_f32(skip.astype(jnp.bfloat16), after[...])
            weight = jnp.exp(weight - sums[:, :rows])
            out = dot_f32(weight.astype(jnp.bfloat16), values)
            mixed, total = out[:tile], sums[:tile, rows:]
            for h in range(1, size):
                at = slice(h * tile, (h + 1) * tile)
                mixed = jnp.where(lane // sb_size == h, out[at], mixed)
                total = jnp.where(lane // sb_size == h, sums[at, rows:], total)
            passed = later[mine, :]
            acc[mine, :] = acc[mine, :] + mixed * jnp.exp(-passed)
            later[mine, :] = passed + total

    span = BLOCK
    duo = 2 * span
    blocks = rows // span
    width = GDN_DIM
    seg_row = lax.broadcasted_iota(jnp.int32, (rows, rows), 0)
    seg_col = lax.broadcasted_iota(jnp.int32, (rows, rows), 1)
    together = seg_row // span == seg_col // span
    upto = jnp.where(jnp.logical_and(together, seg_row <= seg_col), 1.0, 0.0).astype(jnp.bfloat16)
    beyond_it = jnp.where(jnp.logical_and(together, seg_row > seg_col), 1.0, 0.0).astype(
        jnp.bfloat16
    )
    prow = lax.broadcasted_iota(jnp.int32, (span, duo), 0)
    plane = lax.broadcasted_iota(jnp.int32, (span, duo), 1)
    first = plane < span
    pcol = jnp.where(first, plane, plane - span)
    inclusive, strictly = pcol <= prow, pcol < prow
    unit = jnp.where(pcol == prow, 1.0, 0.0)
    diagonal = lax.broadcasted_iota(jnp.int32, (width, width), 0) == lax.broadcasted_iota(
        jnp.int32, (width, width), 1
    )
    eighth = lax.broadcasted_iota(jnp.int32, (8, rows), 0)

    def silu(a):
        return a * (1.0 / (1.0 + jnp.exp(-a)))

    def unit_of(a):
        return a * lax.rsqrt(jnp.sum(a * a, axis=-1, keepdims=True) + NORM_EPS)

    def apart(a):
        lanes = lax.broadcasted_iota(jnp.int32, a.shape, 1) < span
        zero = jnp.zeros_like(a)
        return jnp.concatenate([jnp.where(lanes, a, zero), jnp.where(lanes, zero, a)], axis=0)

    def squared(left, power):
        high, low = halves(power)
        lhigh, llow = halves(left)
        return folded(
            dot_f32(
                jnp.concatenate([lhigh, llow], axis=1), wide_rhs(apart(high), apart(low), 1)
            )
        )

    def prepare(b, dq, dk, dv):
        gates[...] = dot_f32(gate_all[...], xs[b], ((1,), (1,)))
        pre = gates[pl.ds(z, 1), :]
        write = gates[pl.ds(heads + z, 1), :] + write_bias_ref[z]
        rate = jnp.exp(jnp.full((1, rows), decay_scale_ref[z], jnp.float32))
        soft = jnp.maximum(pre, 0.0) + jnp.log(1.0 + jnp.exp(-jnp.abs(pre)))
        decay = shifts_ref[b, pl.ds(z, 1), :] - rate * soft
        strength = 1.0 / (1.0 + jnp.exp(-write))
        d1 = decay.astype(jnp.bfloat16).astype(jnp.float32)
        d2 = (decay - d1).astype(jnp.bfloat16).astype(jnp.float32)
        d3 = decay - d1 - d2
        three = jnp.where(
            eighth == 0, d1, jnp.where(eighth == 1, d2, jnp.where(eighth == 2, d3, 0.0))
        ).astype(jnp.bfloat16)
        cum_row = jnp.sum(dot_f32(three, upto), axis=0, keepdims=True)
        rest_row = jnp.sum(dot_f32(three, beyond_it), axis=0, keepdims=True)
        stack = jnp.where(
            eighth == 0, strength,
            jnp.where(
                eighth == 1, jnp.exp(cum_row),
                jnp.where(eighth == 2, jnp.exp(rest_row), cum_row),
            ),
        )
        columns = stack.T
        s_col, grow, damp, cum = (columns[:, n : n + 1] for n in range(4))
        q = unit_of(silu(dq)) * width ** (-0.5)
        k = unit_of(silu(dk))
        v = silu(dv)
        boosted = q * grow
        damped = k * damp
        right = jnp.concatenate([v * s_col, k * (s_col * grow)], axis=1)
        kh, kl = halves(k)
        qh, ql = halves(q)
        work = []
        for duo_at in range(rows // duo):
            lo = duo_at * duo
            here = slice(lo, lo + duo)
            left = jnp.concatenate(
                [
                    jnp.concatenate([kh[here], kl[here]], axis=1),
                    jnp.concatenate([qh[here], ql[here]], axis=1),
                ],
                axis=0,
            )
            gram = folded(
                dot_f32(left, wide_rhs(kh[here], kl[here], 0), ((1,), (1,)))
            )
            spread = (
                jnp.where(first, cum[lo : lo + span], cum[lo + span : lo + duo])
                - cum_row[:, here]
            )
            table = jnp.where(inclusive, jnp.exp(jnp.where(inclusive, spread, 0.0)), 0.0)
            scale_col = jnp.where(first, s_col[lo : lo + span], s_col[lo + span : lo + duo])
            near_k = jnp.where(first, gram[:span], gram[span:duo])
            near_q = jnp.where(first, gram[duo : duo + span], gram[duo + span :])
            strict = jnp.where(strictly, near_k * table * scale_col, 0.0)
            work.append([unit - strict, strict, near_q * table])
        yield
        for w in work:
            w[1] = squared(w[1], w[1])
        levels = max(1, (span - 1).bit_length()) - 1
        for level in range(levels):
            if level == levels // 2:
                yield
            for w in work:
                if level + 1 < levels:
                    both = squared(jnp.concatenate([w[1], w[0]], axis=0), w[1])
                    w[1], w[0] = both[:span], w[0] + both[span:]
                else:
                    w[0] = w[0] + squared(w[0], w[1])
        yield
        for duo_at, (inverse, _, inside) in enumerate(work):
            lo = duo_at * duo
            here = slice(lo, lo + duo)
            ih, il = (apart(a) for a in halves(inverse))
            rh, rl = halves(right[here])
            solved = dot_f32(
                jnp.concatenate([ih, il], axis=1), jnp.concatenate([rh, rh], axis=0)
            ) + dot_f32(ih, rl)
            lh, ll = (
                apart(a) for a in halves(jnp.concatenate([damped[here].T, inside], axis=0))
            )
            sh, sl = halves(solved)
            made = dot_f32(
                jnp.concatenate([lh, ll], axis=1), jnp.concatenate([sh, sh], axis=0)
            ) + dot_f32(lh, sl)
            for side in range(2):
                at = lo + side * span
                mine = made[side * (width + span) : (side + 1) * (width + span)]
                n = b * blocks + 2 * duo_at + side
                keep = grow[at + span - 1 : at + span]
                step_map = jnp.where(diagonal, keep, 0.0) - mine[:width, width:]
                query = boosted[at : at + span] - mine[width:, width:]
                high, low = halves(jnp.concatenate([step_map, query], axis=0))
                maps[n, :, :width] = high
                maps[n, :, width:] = low
                adds[n] = mine[:, :width]

    def give(which, out, target):
        here = target.at[:, pl.ds(pl.multiple_of(z * cols, cols), cols)]

        def send(g, k, sem):
            return remote(
                out.at[at_block(g), :], here,
                a_send.at[which], a_recv.at[sem], "sp", g,
            )

        def started(g):
            for k in range(1, sp):
                there = lax.rem(z + k, sp)
                if which == 0:
                    @pl.when(there == g)
                    def _():
                        send(there, k, 0).start()
                else:
                    slow = jnp.logical_or(
                        z == sp - 1, jnp.logical_and(z == 0, there == sp - 1)
                    )

                    @pl.when(jnp.logical_and(there == g, slow))
                    def _():
                        send(there, k, 2).start()

                    @pl.when(jnp.logical_and(there == g, jnp.logical_not(slow)))
                    def _():
                        send(there, k, 1).start()

        return started

    stick_started = give(0, stick_out, sticks)
    delta_started = give(1, delta_out, deltas)

    shorter = jnp.minimum(z, sp - 1 - z)
    down_last = z > sp - 1 - z

    def place(n):
        both = n <= 2 * shorter
        way_n = jnp.where(both, lax.rem(n + 1, 2), jnp.where(down_last, 0, 1))
        step_n = jnp.where(n == 0, 0, jnp.where(both, (n + 1) // 2, n - shorter))
        down = jnp.logical_and(way_n == 0, n > 0)
        return way_n, step_n, down, jnp.where(down, z - step_n, z + step_n)

    last_way = jnp.logical_or(z == 0, z == sp - 1)

    def block_ready(n):
        way_n, step_n, down, b = place(n)
        for step in range(1, sp):
            for way in range(2):
                @pl.when(jnp.logical_and(step_n == step, way_n == way))
                def _():
                    block_came(way, step)
        return b

    def delta_block(b):
        drows = dot_f32(xs[b], ws[:, 3 * cols :]).astype(jnp.bfloat16).astype(jnp.float32)
        return prepare(b, drows[:, :cols], drows[:, cols : 2 * cols], drows[:, 2 * cols :])

    last_way = jnp.logical_or(z == 0, z == sp - 1)
    from_top = z == sp - 1

    def stick_project(n):
        b = jnp.where(from_top, sp - 1 - n, n)
        out = dot_f32(xs[b], ws[:, : 3 * cols]).astype(jnp.bfloat16)
        for i in range(3):
            proj[i, at_block(b), :] = out[:, i * cols : (i + 1) * cols]

    def stick_place(n):
        lower = z < sp // 2
        between = jnp.where(
            n == 0,
            jnp.where(lower, sp - 1, 0),
            jnp.where(
                n == 1,
                jnp.where(lower, sp - 2, 1),
                jnp.where(n == 2, jnp.where(lower, 0, sp - 1), z),
            ),
        )
        return jnp.where(from_top, sp - 1 - n, jnp.where(last_way, n, between))

    def settle(i):
        stick_out[at_block(i), :] = acc[at_block(i), :].astype(jnp.bfloat16)

    def stick_pair(n, r):
        b = stick_place(n)
        i = jnp.where(from_top, b + r, b)
        j = jnp.where(from_top, b, b - r)
        pair(i, j)

        @pl.when(j == 0)
        def _():
            settle(i)
            stick_started(i)

    def walk_groups(start, stop, held=False):
        def group(g, c):
            @pl.when(g > start + held)
            def _():
                delta_started(g - 1)
            memory = memory_ref[...]
            for n in range(blocks):
                memory = walk(g * blocks + n, memory)
            memory_ref[...] = memory
            return c

        lax.fori_loop(start, stop, group, 0)
        delta_started(stop - 1)

    def walk(n, memory):
        high, low = halves(memory)
        new = folded(dot_f32(maps[n], wide_rhs(high, low, 1))) + adds[n]
        made = new[width:]
        made = made * lax.rsqrt(jnp.mean(made * made, axis=-1, keepdims=True) + NORM_EPS)
        at = pl.ds(pl.multiple_of(n * span, span), span)
        delta_out[at, :] = (made * gain_ref[...]).astype(delta_out.dtype)
        return new[:width]

    def plain_delta(n, c):
        @pl.when(n == 1)
        def _():
            relay(stick_kinds[0])

        @pl.when(n == sp - 2)
        def _():
            for c in early[parts:-1]:
                arrive(*c)
            relay(stick_kinds[1])

            @pl.when(z == 0)
            def _():
                walk_groups(0, 2)
            relay(stick_kinds[2])
            arrive(*early[-1])
        for _ in delta_block(block_ready(n)):
            pass
        return c

    events = jnp.where(last_way, sp - 1, sp)
    lax.fori_loop(0, events, plain_delta, 0)

    @pl.when(jnp.logical_not(last_way))
    def _():
        walk_groups(0, sp, held=True)

    relayed(stick_kinds)

    def stick_event(n, c):
        for part in range(2):
            @pl.when(jnp.logical_and(last_way, n == part + 1))
            def _():
                arrive(sp - 1, part)

        def project_one(m, c):
            stick_project(m)
            return c

        needed = jnp.where(from_top, n, stick_place(n)) + 1
        lax.fori_loop(c, needed, project_one, 0)

        @pl.when(jnp.logical_and(jnp.logical_not(last_way), n == 0))
        def _():
            delta_started(0)

        def one(r, c):
            for part in range(2, parts):
                @pl.when(
                    jnp.logical_and(
                        last_way, jnp.logical_and(n == sp - 2, r == sp - 1 - parts + part)
                    )
                )
                def _():
                    arrive(sp - 1, part)
            stick_pair(n, r)
            return c

        lax.fori_loop(0, jnp.where(last_way, n, stick_place(n)) + 1, one, 0)
        return jnp.maximum(c, needed)

    lax.fori_loop(0, events, stick_event, 0)

    @pl.when(last_way)
    def _():
        @pl.when(z == 0)
        def _():
            walk_groups(2, sp - 1)
        for way in range(2):
            @pl.when(comes(way, sp - 1))
            def _():
                block_came(way, sp - 1)
        b = stick_place(sp - 1)
        pieces = []
        for i in range(0, count, 2):
            out = dot_f32(xs[b], ws[:, i * cols : (i + 2) * cols]).astype(jnp.bfloat16)
            pieces += [out[:, :cols], out[:, cols:]]
        for i in range(3):
            proj[i, at_block(b), :] = pieces[i]
        stages = prepare(b, *(piece.astype(jnp.float32) for piece in pieces[3:]))
        for u in range(sp):
            next(stages, None)
            stick_pair(sp - 1, u)
        walk_groups(jnp.where(z == 0, sp - 1, 0), sp)

    mine_z = pl.ds(pl.multiple_of(z * rows, rows), rows)
    lanes = pl.ds(pl.multiple_of(z * cols, cols), cols)
    sticks[:, lanes] = stick_out[mine_z, :]
    deltas[:, lanes] = delta_out[mine_z, :]
    for c in late:
        c.wait()
    all_sent(ws.at[pl.ds(0, 3 * depth), :], w_send.at[0])
    all_sent(xs.at[:, :, slot], f_send.at[0])
    for c in range(sp):
        @pl.when(z == c)
        def _():
            for way, passed in enumerate((c + 1 if c + 1 < sp else 0, sp - c if c > 0 else 0)):
                if passed:
                    all_sent(xs.at[pl.ds(0, passed), :, slot], x_send.at[way])
                    all_sent(shifts_ref.at[pl.ds(0, passed)], s_send.at[way])
    all_came(stick_out.at[pl.ds(0, (sp - 1) * rows), :], a_recv.at[0])
    chunks, wide = outgoing.shape[0], outgoing.shape[2]
    share = rows // tp
    for c in range(chunks):
        columns = slice(c * wide, (c + 1) * wide)
        partial[:, columns] = dot_f32(sticks[...], sw_ref[:, columns])
    all_came(delta_out.at[pl.ds(0, (sp - 2) * rows), :], a_recv.at[1])
    soon = pl.ds(pl.multiple_of(jnp.where(from_top, 1, 0) * cols, cols), (sp - 1) * cols)
    for c in range(chunks):
        columns = slice(c * wide, (c + 1) * wide)
        partial[:, columns] += dot_f32(deltas[:, soon], dw_ref[soon, columns])
    all_came(delta_out.at[pl.ds(0, rows), :], a_recv.at[2])
    final = pl.ds(pl.multiple_of(jnp.where(from_top, 0, sp - 1) * cols, cols), cols)
    mine = pl.ds(pl.multiple_of(t * share, share), share)
    partner = lax.rem(t + 1, tp)
    theirs = pl.ds(pl.multiple_of(partner * share, share), share)

    def finish(which, c):
        columns = slice(c * wide, (c + 1) * wide)
        return (
            partial[which, columns] + dot_f32(deltas[which, final], dw_ref[final, columns])
        ).astype(jnp.bfloat16)

    swaps = [
        remote(
            outgoing.at[c], incoming.at[:, c * wide : (c + 1) * wide],
            c_sem.at[0], c_sem.at[1], "tp", partner,
        )
        for c in range(chunks)
    ]
    for c in range(chunks):
        outgoing[c] = finish(theirs, c)
        if c > 0:
            swaps[c - 1].start()
    for c in range(chunks):
        own[:, c * wide : (c + 1) * wide] = finish(mine, c)
        if c == 0:
            swaps[chunks - 1].start()
    all_came(incoming, c_sem.at[1])
    all_sent(incoming, c_sem.at[0])
    for which, out in enumerate((stick_out, delta_out)):
        all_sent(out.at[pl.ds(0, (sp - 1) * rows), :], a_send.at[which])


ANYWHERE = pl.BlockSpec(memory_space=pltpu.HBM)
ON_CORE = pl.BlockSpec(memory_space=pltpu.VMEM)


def on_device_heads(
    hidden_in, sb_query_w, sb_key_w, sb_value_w, sb_offset,
    delta_query_w, delta_key_w, delta_value_w, decay_w, write_w, write_bias,
    decay_log_scale, decay_shift, head_gain, sb_out_w, delta_out_w,
):
    sp, fs, tp = lax.axis_size("sp"), lax.axis_size("fs"), lax.axis_size("tp")
    rows, half = hidden_in.shape[1:]
    width = half * tp
    length = rows * sp
    heads = decay_log_scale.shape[0]
    cols = sb_query_w.shape[1] // sp
    parts, chunks = 4, 4
    share = rows // tp
    blocks = length // BLOCK
    dma = pltpu.SemaphoreType.DMA
    bf16, f32 = jnp.bfloat16, jnp.float32
    own, incoming = pl.pallas_call(
        layer_kernel,
        name="layer",
        out_shape=(pltpu.VMEM((share, width), bf16),) * 2,
        in_specs=[ANYWHERE] * 16,
        out_specs=(ON_CORE,) * 2,
        scratch_shapes=[
            pltpu.SMEM(sb_offset.shape, f32),
            pltpu.SMEM(decay_log_scale.shape, f32),
            pltpu.SMEM(write_bias.shape, f32),
            pltpu.VMEM((1, head_gain.shape[0]), f32),
            pltpu.VMEM((sp, rows, width), bf16),
            pltpu.VMEM((width, 6 * cols), bf16),
            pltpu.VMEM((2, heads, width), bf16),
            pltpu.VMEM((2 * heads, width), bf16),
            pltpu.VMEM((2 * heads, rows), f32),
            pltpu.VMEM((sp, heads, rows), f32),
            pltpu.VMEM((rows, rows + cols), bf16),
            pltpu.VMEM((3, length, cols), bf16),
            pltpu.VMEM((length, cols), f32),
            pltpu.VMEM((length, cols), f32),
            pltpu.VMEM((cols, cols), f32),
            pltpu.VMEM((blocks, cols + BLOCK, 2 * cols), bf16),
            pltpu.VMEM((blocks, cols + BLOCK, cols), f32),
            pltpu.VMEM((length, cols), bf16),
            pltpu.VMEM((length, cols), bf16),
            pltpu.VMEM((rows, cols * sp), bf16),
            pltpu.VMEM((rows, cols * sp), bf16),
            pltpu.VMEM(sb_out_w.shape, bf16),
            pltpu.VMEM(delta_out_w.shape, bf16),
            pltpu.VMEM((rows, width), f32),
            pltpu.VMEM((chunks, share, width // chunks), bf16),
            dma((2,)), dma((2, sp - 1, parts)), dma((1,)), dma((2 * sp - 1,)),
            dma((1,)), dma((2, 6)), dma((2,)), dma((2,)), dma((2, sp - 1)), dma((11,)),
            dma((2,)), dma((3,)), dma((2,)),
        ],
        compiler_params=pltpu.CompilerParams(
            collective_id=0, has_side_effects=True,
            vmem_limit_bytes=ALL_VMEM - 5 * share * width,
        ),
    )(
        sb_offset, decay_log_scale, write_bias,
        hidden_in.reshape(rows, half), sb_query_w, sb_key_w, sb_value_w,
        delta_query_w, delta_key_w, delta_value_w, decay_w.T, write_w.T,
        decay_shift.reshape(heads, rows), head_gain.reshape(1, -1), sb_out_w, delta_out_w,
    )
    result = (own.astype(f32) + incoming.astype(f32)).astype(bf16)
    return result.reshape(1, share, width)


def on_device(*inputs):
    delta_heads = inputs[11].shape[0]
    square = lax.axis_size("sp") == lax.axis_size("fs") == 4 and lax.axis_size("tp") == 2
    if square and delta_heads == lax.axis_size("sp") and inputs[4].shape[0] % delta_heads == 0:
        return on_device_heads(*inputs)
    return on_device_split(*inputs)


def solution(mesh):
    return jax.shard_map(
        on_device,
        mesh=mesh,
        in_specs=(
            P("fs", "sp", "tp"),
            P("fs", "tp"),
            P("fs", "tp"),
            P("fs", "tp"),
            P("tp"),
            P("fs", "tp"),
            P("fs", "tp"),
            P("fs", "tp"),
            P(None, "tp"),
            P(None, "tp"),
            P("tp"),
            P("tp"),
            P("fs", "tp", "sp"),
            P(),
            P("tp", None),
            P("tp", None),
        ),
        out_specs=P("fs", ("sp", "tp"), None),
        check_vma=False,
    )
```

```python
import jax
import jax.numpy as jnp
from jax import lax
from jax.experimental import pallas as pl
from jax.experimental.pallas import tpu as pltpu
from jax.sharding import PartitionSpec as P

MESH = pl.DeviceIdType.MESH
ALL_VMEM = 67043328

SB_DIM = 64
GDN_DIM = 128
BLOCK = 64


EXACT_MATMUL = lax.Precision.HIGHEST
NORM_EPS = 1e-06


def carried_in(value, axis, combine, identity):
    devices, index = (lax.axis_size(axis), lax.axis_index(axis))
    everything = jax.tree.map(
        lambda part, kind: lax.all_gather(part.astype(kind), axis),
        value,
        (jnp.bfloat16, jnp.bfloat16),
    )
    start = jax.tree.map(
        lambda part, zero: jnp.broadcast_to(jnp.asarray(zero, part.dtype), part.shape),
        value,
        identity,
    )

    def lap(k, before):
        reached = k < index
        new = combine(
            before, jax.tree.map(lambda part, own: part[k].astype(own.dtype), everything, value)
        )
        return jax.tree.map(lambda a, b: jnp.where(reached, a, b), new, before)

    return lax.fori_loop(0, devices, lap, start)


def unit_lower_inverse(strict_part):
    order_size = strict_part.shape[-1]
    powered = strict_part
    inverse = jnp.eye(order_size, dtype=strict_part.dtype) - strict_part
    for repeat_number in range(max(1, (order_size - 1).bit_length()) - 1):
        powered = jnp.einsum("...ij,...jk->...ik", powered, powered, precision=EXACT_MATMUL)
        inverse = inverse + jnp.einsum(
            "...ij,...jk->...ik", inverse, powered, precision=EXACT_MATMUL
        )
    return inverse


def to_blocks(row_data, block_span):
    blocks_count = row_data.shape[0] // block_span
    shaped = row_data.reshape((blocks_count, block_span) + row_data.shape[1:])
    return jnp.swapaxes(shaped, 1, 2)


def from_blocks(blocked):
    swapped = jnp.swapaxes(blocked, 1, 2)
    return swapped.reshape((-1,) + swapped.shape[2:])


def unit_rows(vectors):
    return vectors * lax.rsqrt(jnp.sum(vectors * vectors, axis=-1, keepdims=True) + NORM_EPS)


def delta_inputs(
    query_proj,
    key_proj,
    value_proj,
    decay_pre,
    write_pre,
    write_bias,
    decay_log_scale,
    shift_rows,
    head_count,
    head_size,
):
    query_act = jax.nn.silu(query_proj.astype(jnp.float32)).reshape(-1, head_count, head_size)
    key_act = jax.nn.silu(key_proj.astype(jnp.float32)).reshape(-1, head_count, head_size)
    value_rows = jax.nn.silu(value_proj.astype(jnp.float32)).reshape(-1, head_count, head_size)
    queries = unit_rows(query_act) * head_size ** (-0.5)
    key_rows = unit_rows(key_act)
    log_decay = -jnp.exp(decay_log_scale) * jax.nn.softplus(decay_pre) + shift_rows
    strength = jax.nn.sigmoid(write_pre + write_bias)
    return (queries, key_rows, value_rows, log_decay, strength)


def delta_prepare(queries, key_rows, value_rows, log_decay, strength):
    block_span = queries.shape[2]
    cumulative = jnp.cumsum(log_decay, axis=-1)
    row_place = lax.broadcasted_iota(jnp.int32, (block_span, block_span), 0)
    col_place = lax.broadcasted_iota(jnp.int32, (block_span, block_span), 1)
    inclusive = col_place <= row_place
    strictly = col_place < row_place
    spread = cumulative[..., :, None] - cumulative[..., None, :]
    decay_table = jnp.where(inclusive, jnp.exp(jnp.where(inclusive, spread, 0.0)), 0.0)
    keys_beta = key_rows * strength[..., None]
    lower_part = jnp.where(
        strictly,
        jnp.einsum("nhik,nhjk->nhij", keys_beta, key_rows, precision=EXACT_MATMUL) * decay_table,
        0.0,
    )
    inverse = unit_lower_inverse(lower_part)
    growth = jnp.exp(cumulative)
    state_updates = jnp.einsum(
        "nhij,nhjv->nhiv", inverse, value_rows * strength[..., None], precision=EXACT_MATMUL
    )
    erase_term = jnp.einsum(
        "nhij,nhjk->nhik", inverse, keys_beta * growth[..., None], precision=EXACT_MATMUL
    )
    inside_block = (
        jnp.einsum("nhik,nhjk->nhij", queries, key_rows, precision=EXACT_MATMUL) * decay_table
    )
    boosted_query = queries * growth[..., None]
    damped_keys = key_rows * jnp.exp(cumulative[..., -1:] - cumulative)[..., None]
    decay_per_block = jnp.exp(cumulative[..., -1])
    return (state_updates, erase_term, inside_block, boosted_query, damped_keys, decay_per_block)


def delta_step(memory_state, inputs):
    state_updates, erase_term, inside_block, boosted_query, damped_keys, decay_per_block = inputs
    fixed_values = state_updates - jnp.einsum(
        "mzq,mqc->mzc", erase_term, memory_state, precision=EXACT_MATMUL
    )
    produced_rows = jnp.einsum(
        "mzq,mqc->mzc", boosted_query, memory_state, precision=EXACT_MATMUL
    ) + jnp.einsum("efq,eqn->efn", inside_block, fixed_values, precision=EXACT_MATMUL)
    memory_state = memory_state * decay_per_block[:, None, None] + jnp.einsum(
        "wam,waz->wmz", damped_keys, fixed_values, precision=EXACT_MATMUL
    )
    return (memory_state, produced_rows)


def transition_step(carried, inputs):
    memory_state, transfer = carried
    state_updates, erase_term, inside_block, boosted_query, damped_keys, decay_per_block = inputs
    fixed_values = state_updates - jnp.einsum(
        "mzq,mqc->mzc", erase_term, memory_state, precision=EXACT_MATMUL
    )
    coupling = jnp.einsum("hik,hil->hkl", damped_keys, erase_term, precision=EXACT_MATMUL)
    memory_state = memory_state * decay_per_block[:, None, None] + jnp.einsum(
        "wam,waz->wmz", damped_keys, fixed_values, precision=EXACT_MATMUL
    )
    transfer = transfer * decay_per_block[:, None, None] - jnp.einsum(
        "hkl,hlm->hkm", coupling, transfer, precision=EXACT_MATMUL
    )
    return ((memory_state, transfer), None)


def compose(prior_blocks, following_blocks):
    joined_map = jnp.einsum(
        "hkl,hlm->hkm", following_blocks[0], prior_blocks[0], precision=EXACT_MATMUL
    )
    joined_state = (
        jnp.einsum("djo,dog->djg", following_blocks[0], prior_blocks[1], precision=EXACT_MATMUL)
        + following_blocks[1]
    )
    return (joined_map, joined_state)


def stick_block(queries, key_rows, value_rows, query_place, key_place, offsets):
    scale_factor = queries.shape[-1] ** (-0.5)
    scores = (
        jnp.einsum("qhd,khd->hqk", queries, key_rows, preferred_element_type=jnp.float32)
        * scale_factor
        + offsets[:, None, None]
    )
    visible = key_place[None, :] < query_place[:, None]
    skipped = jnp.where(visible, jax.nn.log_sigmoid(-scores), 0.0)
    beyond = lax.cumsum(skipped, axis=2, reverse=True) - skipped
    weights = jnp.where(visible, jnp.exp(jax.nn.log_sigmoid(scores) + beyond), 0.0).astype(
        jnp.bfloat16
    )
    partial_value = jnp.einsum(
        "hqk,khd->qhd", weights, value_rows, preferred_element_type=jnp.float32
    )
    return (partial_value, jnp.sum(skipped, axis=2).T)


def stick_combine(partials, totals):
    beyond = jnp.cumsum(totals[::-1], axis=0)[::-1] - totals
    return jnp.sum(partials * jnp.exp(beyond)[..., None], axis=0)


def on_device_split(
    hidden_in,
    sb_query_w,
    sb_key_w,
    sb_value_w,
    sb_offset,
    delta_query_w,
    delta_key_w,
    delta_value_w,
    decay_w,
    write_w,
    write_bias,
    decay_log_scale,
    decay_shift,
    head_gain,
    sb_out_w,
    delta_out_w,
):
    token_rows = hidden_in.shape[1]
    local_in = hidden_in.reshape(token_rows, hidden_in.shape[2])
    gathered = (
        lax.all_gather(sb_query_w, "fs", axis=0, tiled=True),
        lax.all_gather(sb_key_w, "fs", axis=0, tiled=True),
        lax.all_gather(sb_value_w, "fs", axis=0, tiled=True),
        lax.all_gather(delta_query_w, "fs", axis=0, tiled=True),
        lax.all_gather(delta_key_w, "fs", axis=0, tiled=True),
        lax.all_gather(delta_value_w, "fs", axis=0, tiled=True),
    )
    in_weights = tuple(gathered) + (decay_w, write_w)
    portion = lax.all_gather(local_in, "tp", axis=1, tiled=True)
    projected = tuple(
        (jnp.dot(portion, weight, preferred_element_type=jnp.float32) for weight in in_weights)
    )
    sb_heads = sb_offset.shape[0]
    delta_heads = decay_log_scale.shape[0]
    sb_query = projected[0].astype(jnp.bfloat16).reshape(token_rows, sb_heads, SB_DIM)
    sb_keys = projected[1].astype(jnp.bfloat16)
    sb_values = projected[2].astype(jnp.bfloat16)
    shift_rows = decay_shift.reshape(delta_heads, token_rows).T
    queries, key_rows, value_rows, log_decay, strength = delta_inputs(
        projected[3].astype(jnp.bfloat16),
        projected[4].astype(jnp.bfloat16),
        projected[5].astype(jnp.bfloat16),
        projected[6],
        projected[7],
        write_bias,
        decay_log_scale,
        shift_rows,
        delta_heads,
        GDN_DIM,
    )
    prepared = delta_prepare(
        to_blocks(queries, BLOCK),
        to_blocks(key_rows, BLOCK),
        to_blocks(value_rows, BLOCK),
        to_blocks(log_decay, BLOCK),
        to_blocks(strength, BLOCK),
    )
    identity_map = jnp.broadcast_to(
        jnp.eye(GDN_DIM, dtype=jnp.float32), (delta_heads, GDN_DIM, GDN_DIM)
    )
    empty_state = jnp.zeros((delta_heads, GDN_DIM, GDN_DIM), jnp.float32)
    (local_end, local_map), unused_out = lax.scan(
        transition_step, (empty_state, identity_map), prepared
    )
    own_first = lax.axis_index("sp") * token_rows
    query_place = own_first + lax.iota(jnp.int32, token_rows)
    sp_count = lax.axis_size("sp")
    slot_out = jnp.zeros((sp_count, token_rows, sb_heads, SB_DIM), jnp.float32)
    slot_total = jnp.zeros((sp_count, token_rows, sb_heads), jnp.float32)

    def absorb(slot_arrays, address_portion, value_part, shard_first):

        def active(current):
            partial_value, totals = stick_block(
                sb_query,
                address_portion.reshape(token_rows, sb_heads, SB_DIM),
                value_part.reshape(token_rows, sb_heads, SB_DIM),
                query_place,
                shard_first + lax.iota(jnp.int32, token_rows),
                sb_offset,
            )
            slot_index = shard_first // token_rows
            return (
                lax.dynamic_update_index_in_dim(current[0], partial_value, slot_index, 0),
                lax.dynamic_update_index_in_dim(current[1], totals, slot_index, 0),
            )

        def inactive(current):
            return current

        usable = jnp.logical_and(shard_first >= 0, shard_first <= own_first)
        return lax.cond(usable, active, inactive, slot_arrays)

    key_block = lax.all_gather(sb_keys, "sp", axis=0, tiled=True)
    value_block = lax.all_gather(sb_values, "sp", axis=0, tiled=True)

    def per_shard(shard_number, current):
        row_begin = shard_number * token_rows
        return absorb(
            current,
            lax.dynamic_slice_in_dim(key_block, row_begin, token_rows, 0),
            lax.dynamic_slice_in_dim(value_block, row_begin, token_rows, 0),
            row_begin,
        )

    slot_arrays = lax.fori_loop(
        0, key_block.shape[0] // token_rows, per_shard, (slot_out, slot_total)
    )
    unused_map, incoming = carried_in(
        (local_map, local_end), "sp", compose, (identity_map, empty_state)
    )
    sb_mixed = (
        stick_combine(slot_arrays[0], slot_arrays[1])
        .astype(jnp.bfloat16)
        .reshape(token_rows, sb_heads * SB_DIM)
    )
    unused_end, produced_rows = lax.scan(delta_step, incoming, prepared)
    produced_rows = from_blocks(produced_rows)
    normed = (
        produced_rows
        * lax.rsqrt(jnp.mean(produced_rows * produced_rows, axis=-1, keepdims=True) + NORM_EPS)
        * head_gain
    )
    delta_mixed = normed.astype(jnp.bfloat16).reshape(token_rows, delta_heads * GDN_DIM)
    result = lax.psum_scatter(
        (
            jnp.dot(sb_mixed, sb_out_w, preferred_element_type=jnp.float32)
            + jnp.dot(delta_mixed, delta_out_w, preferred_element_type=jnp.float32)
        ).astype(jnp.bfloat16),
        "tp",
        scatter_dimension=0,
        tiled=True,
    ).astype(jnp.float32)
    return result.astype(jnp.bfloat16).reshape(1, result.shape[0], result.shape[1])


def remote(src, dst, send, recv, axis, index):
    return pltpu.make_async_remote_copy(
        src_ref=src, dst_ref=dst, send_sem=send, recv_sem=recv,
        device_id={axis: index}, device_id_type=MESH,
    )


def greet(axes):
    barrier = pltpu.get_barrier_semaphore()
    count = 0
    for axis in axes:
        size, me = lax.axis_size(axis), lax.axis_index(axis)
        for k in range(1, size):
            pl.semaphore_signal(
                barrier, inc=1, device_id={axis: lax.rem(me + k, size)}, device_id_type=MESH
            )
            count += 1
    pl.semaphore_wait(barrier, count)


def halves(a):
    high = a.astype(jnp.bfloat16)
    return high, (a - high.astype(jnp.float32)).astype(jnp.bfloat16)


def dot_f32(a, b, dims=((1,), (0,))):
    return lax.dot_general(a, b, (dims, ((), ())), preferred_element_type=jnp.float32)


def wide_rhs(high, low, axis):
    top = jnp.concatenate([high, low], axis=axis)
    bottom = jnp.concatenate([high, jnp.zeros_like(low)], axis=axis)
    return jnp.concatenate([top, bottom], axis=1 - axis)


def folded(a):
    half = a.shape[1] // 2
    return a[:, :half] + a[:, half:]


def layer_kernel(
    offset_hbm, decay_scale_hbm, write_bias_hbm,
    x_ref, w0, w1, w2, w3, w4, w5, decay_w_ref, write_w_ref, shift_ref, gain_hbm, sw_hbm, dw_hbm,
    own, incoming,
    offset_ref, decay_scale_ref, write_bias_ref, gain_ref,
    xs, ws, gate_w, gate_all, gates, shifts_ref, after,
    proj, acc, later, memory_ref, maps, adds, stick_out, delta_out,
    sticks, deltas, sw_ref, dw_ref, partial, outgoing,
    x_send, x_recv, f_send, f_recv, w_send, w_recv, r_recv, s_send, s_recv, l_sem,
    a_send, a_recv, c_sem,
):
    weights = (w0, w1, w2, w3, w4, w5)
    sp, tp = lax.axis_size("sp"), lax.axis_size("tp")
    z, f, t = lax.axis_index("sp"), lax.axis_index("fs"), lax.axis_index("tp")
    rows, half = x_ref.shape
    depth = w0.shape[0]
    cols = ws.shape[1] // len(weights)
    parts = x_recv.shape[2]
    heads = decay_w_ref.shape[0]
    slot = pl.ds(pl.multiple_of(t * half, half), half)
    local = [
        pltpu.make_async_copy(x_ref, xs.at[z, :, slot], l_sem.at[0]),
        pltpu.make_async_copy(shift_ref, shifts_ref.at[z], l_sem.at[1]),
        pltpu.make_async_copy(decay_w_ref, gate_w.at[0], l_sem.at[2]),
        pltpu.make_async_copy(write_w_ref, gate_w.at[1], l_sem.at[3]),
        pltpu.make_async_copy(offset_hbm, offset_ref, l_sem.at[6]),
        pltpu.make_async_copy(decay_scale_hbm, decay_scale_ref, l_sem.at[7]),
        pltpu.make_async_copy(write_bias_hbm, write_bias_ref, l_sem.at[8]),
        pltpu.make_async_copy(gain_hbm, gain_ref, l_sem.at[9]),
    ]
    late = [
        pltpu.make_async_copy(sw_hbm, sw_ref, l_sem.at[4]),
        pltpu.make_async_copy(dw_hbm, dw_ref, l_sem.at[5]),
    ]

    def w_src(i):
        return weights[i].at[:, pl.ds(pl.multiple_of(z * cols, cols), cols)]

    def w_at(i, who):
        return ws.at[pl.ds(pl.multiple_of(who * depth, depth), depth), pl.ds(i * cols, cols)]

    local_w = [
        pltpu.make_async_copy(w_src(i), w_at(i, f), l_sem.at[10]) for i in range(len(weights))
    ]
    near = (f + 1 - 2 * (f % 2), f + 2 - 4 * (f // 2))
    count = len(weights)
    delta_kinds, stick_kinds = (3, 4, 5), (0, 1, 2)

    def onward(way):
        return z + 1 < sp if way == 0 else z > 0

    def ahead(way):
        return z + 1 if way == 0 else z - 1

    barrier = pltpu.get_barrier_semaphore()
    for way in range(2):
        @pl.when(onward(way))
        def _():
            pl.semaphore_signal(
                barrier, inc=1, device_id={"sp": ahead(way)}, device_id_type=MESH
            )
    for side in range(2):
        pl.semaphore_signal(barrier, inc=1, device_id={"fs": near[side]}, device_id_type=MESH)
    pl.semaphore_signal(
        barrier, inc=1, device_id={"tp": lax.rem(t + 1, tp)}, device_id_type=MESH
    )
    for c in local + local_w:
        c.start()
    peers = onward(0).astype(jnp.int32) + onward(1).astype(jnp.int32) + 3
    pl.semaphore_wait(barrier, peers)

    def x_copy(way, step, part):
        block = z - (step - 1) if way == 0 else z + (step - 1)
        piece = pl.ds(part * (rows // parts), rows // parts)
        there = xs.at[block, piece, slot]
        return remote(
            x_ref.at[piece, :] if step == 1 else there, there,
            x_send.at[way], x_recv.at[way, step - 1, part], "sp", ahead(way),
        )

    def shift_copy(way, step):
        block = z - (step - 1) if way == 0 else z + (step - 1)
        there = shifts_ref.at[block]
        return remote(
            shift_ref if step == 1 else there, there,
            s_send.at[way], s_recv.at[way, step - 1], "sp", ahead(way),
        )

    def comes(way, step):
        return z >= step if way == 0 else z + step < sp

    def sends(way, step):
        return jnp.logical_and(onward(way), comes(way, step - 1))

    def forward(way, step, part):
        block = z - step if way == 0 else z + step
        piece = pl.ds(part * (rows // parts), rows // parts)
        there = xs.at[block, piece, slot]
        return remote(
            x_ref.at[piece, :] if step == 0 else there, there,
            f_send.at[0], f_recv.at[way * (sp - 1) + step], "tp", lax.rem(t + 1, tp),
        )

    def w_copy(side, i):
        return remote(
            w_src(i), w_at(i, f), w_send.at[0], w_recv.at[side, i], "fs", near[side]
        )

    def w_relay(side, i):
        part = depth // 2
        start = pl.multiple_of(near[side] * depth + side * part, part)
        there = ws.at[pl.ds(start, part), pl.ds(i * cols, cols)]
        return remote(
            there, there, w_send.at[0], r_recv.at[i // 3], "fs", near[1 - side]
        )

    for part in range(parts):
        for way in range(2):
            @pl.when(onward(way))
            def _():
                x_copy(way, 1, part).start()
                if part == 0:
                    shift_copy(way, 1).start()
    for i in delta_kinds:
        for side in range(2):
            w_copy(side, i).start()
    for part in range(parts):
        forward(0, 0, part).start()

    def relay(i):
        for side in range(2):
            w_copy(side, i).wait_recv()
            w_relay(side, i).start()

    def arrive(step, part):
        for way in range(2):
            @pl.when(comes(way, step))
            def _():
                x_copy(way, step, part).wait_recv()
                forward(way, step, part).start()
                if step + 1 < sp:
                    @pl.when(onward(way))
                    def _():
                        x_copy(way, step + 1, part).start()
                if part == 0:
                    shift_copy(way, step).wait_recv()
                    if step + 1 < sp:
                        @pl.when(onward(way))
                        def _():
                            shift_copy(way, step + 1).start()

    below = lax.broadcasted_iota(jnp.int32, (rows, rows), 0)
    across = lax.broadcasted_iota(jnp.int32, (rows, rows), 1)
    after[:, :rows] = jnp.where(below > across, 1.0, 0.0).astype(jnp.bfloat16)
    after[:, rows:] = jnp.ones((rows, cols), jnp.bfloat16)
    acc[...] = jnp.zeros_like(acc)
    later[...] = jnp.zeros_like(later)
    memory_ref[...] = jnp.zeros_like(memory_ref)
    early = [(step, part) for step in range(1, sp - 1) for part in range(parts)]
    relay(delta_kinds[0])
    arrive(*early[0])
    for i in delta_kinds[1:]:
        relay(i)
    for i in stick_kinds:
        for side in range(2):
            w_copy(side, i).start()
    for c in late:
        c.start()
    for step, part in early[1:parts]:
        arrive(step, part)
    for c in local:
        c.wait()
    own_w = ws.at[pl.ds(pl.multiple_of(f * depth, depth), depth), :]
    pltpu.make_async_copy(own_w, own_w, l_sem.at[10]).wait()
    gate_all[...] = jnp.concatenate(
        [gate_w[0].astype(jnp.float32), gate_w[1].astype(jnp.float32)], axis=0
    ).astype(jnp.bfloat16)
    def all_sent(ref, sem):
        remote(ref, ref, sem, sem, "tp", lax.rem(t + 1, tp)).wait_send()

    def all_came(ref, sem):
        remote(ref, ref, sem, sem, "tp", lax.rem(t + 1, tp)).wait_recv()

    def block_came(way, step):
        all_came(xs.at[z, :, slot], f_recv.at[way * (sp - 1) + step])

    block_came(0, 0)

    def relayed(kinds):
        first = kinds[0] * cols
        all_came(ws.at[pl.ds(0, depth), pl.ds(first, len(kinds) * cols)], r_recv.at[kinds[0] // 3])

    relayed(delta_kinds)

    size = offset_ref.shape[0] // sp
    sb_size = cols // size
    scale = sb_size ** (-0.5)
    tile = rows

    def at_block(b, start=0, extent=rows):
        return pl.ds(pl.multiple_of(b * rows + start, extent), extent)

    def pair(i, j):
        for part in range(rows // tile):
            mine = at_block(i, part * tile, tile)
            q = proj[0, mine, :]
            keys, values = proj[1, at_block(j), :], proj[2, at_block(j), :]
            lane = lax.broadcasted_iota(jnp.int32, (tile, cols), 1)
            query = jnp.concatenate(
                [jnp.where(lane // sb_size == h, q, jnp.zeros_like(q)) for h in range(size)], axis=0
            )
            score = dot_f32(query, keys, ((1,), (1,)))
            score = jnp.concatenate(
                [
                    score[h * tile : (h + 1) * tile] * scale + offset_ref[z * size + h]
                    for h in range(size)
                ],
                axis=0,
            )
            seen = across[:tile] < below[:tile] + (part * tile + (i - j) * rows)
            score = jnp.where(jnp.concatenate([seen] * size, axis=0), score, -1e30)
            skip = jnp.maximum(score, jnp.log(1.0 + jnp.exp(jnp.minimum(score, 80.0))))
            weight = score - skip
            sums = dot_f32(skip.astype(jnp.bfloat16), after[...])
            weight = jnp.exp(weight - sums[:, :rows])
            out = dot_f32(weight.astype(jnp.bfloat16), values)
            mixed, total = out[:tile], sums[:tile, rows:]
            for h in range(1, size):
                at = slice(h * tile, (h + 1) * tile)
                mixed = jnp.where(lane // sb_size == h, out[at], mixed)
                total = jnp.where(lane // sb_size == h, sums[at, rows:], total)
            passed = later[mine, :]
            acc[mine, :] = acc[mine, :] + mixed * jnp.exp(-passed)
            later[mine, :] = passed + total

    span = BLOCK
    duo = 2 * span
    blocks = rows // span
    width = GDN_DIM
    seg_row = lax.broadcasted_iota(jnp.int32, (rows, rows), 0)
    seg_col = lax.broadcasted_iota(jnp.int32, (rows, rows), 1)
    together = seg_row // span == seg_col // span
    upto = jnp.where(jnp.logical_and(together, seg_row <= seg_col), 1.0, 0.0).astype(jnp.bfloat16)
    beyond_it = jnp.where(jnp.logical_and(together, seg_row > seg_col), 1.0, 0.0).astype(
        jnp.bfloat16
    )
    prow = lax.broadcasted_iota(jnp.int32, (span, duo), 0)
    plane = lax.broadcasted_iota(jnp.int32, (span, duo), 1)
    first = plane < span
    pcol = jnp.where(first, plane, plane - span)
    inclusive, strictly = pcol <= prow, pcol < prow
    unit = jnp.where(pcol == prow, 1.0, 0.0)
    diagonal = lax.broadcasted_iota(jnp.int32, (width, width), 0) == lax.broadcasted_iota(
        jnp.int32, (width, width), 1
    )
    eighth = lax.broadcasted_iota(jnp.int32, (8, rows), 0)

    def silu(a):
        return a * (1.0 / (1.0 + jnp.exp(-a)))

    def unit_of(a):
        return a * lax.rsqrt(jnp.sum(a * a, axis=-1, keepdims=True) + NORM_EPS)

    def apart(a):
        lanes = lax.broadcasted_iota(jnp.int32, a.shape, 1) < span
        zero = jnp.zeros_like(a)
        return jnp.concatenate([jnp.where(lanes, a, zero), jnp.where(lanes, zero, a)], axis=0)

    def squared(left, power):
        high, low = halves(power)
        lhigh, llow = halves(left)
        return folded(
            dot_f32(
                jnp.concatenate([lhigh, llow], axis=1), wide_rhs(apart(high), apart(low), 1)
            )
        )

    def prepare(b, dq, dk, dv):
        gates[...] = dot_f32(gate_all[...], xs[b], ((1,), (1,)))
        pre = gates[pl.ds(z, 1), :]
        write = gates[pl.ds(heads + z, 1), :] + write_bias_ref[z]
        rate = jnp.exp(jnp.full((1, rows), decay_scale_ref[z], jnp.float32))
        soft = jnp.maximum(pre, 0.0) + jnp.log(1.0 + jnp.exp(-jnp.abs(pre)))
        decay = shifts_ref[b, pl.ds(z, 1), :] - rate * soft
        strength = 1.0 / (1.0 + jnp.exp(-write))
        d1 = decay.astype(jnp.bfloat16).astype(jnp.float32)
        d2 = (decay - d1).astype(jnp.bfloat16).astype(jnp.float32)
        d3 = decay - d1 - d2
        three = jnp.where(
            eighth == 0, d1, jnp.where(eighth == 1, d2, jnp.where(eighth == 2, d3, 0.0))
        ).astype(jnp.bfloat16)
        cum_row = jnp.sum(dot_f32(three, upto), axis=0, keepdims=True)
        rest_row = jnp.sum(dot_f32(three, beyond_it), axis=0, keepdims=True)
        stack = jnp.where(
            eighth == 0, strength,
            jnp.where(
                eighth == 1, jnp.exp(cum_row),
                jnp.where(eighth == 2, jnp.exp(rest_row), cum_row),
            ),
        )
        columns = stack.T
        s_col, grow, damp, cum = (columns[:, n : n + 1] for n in range(4))
        q = unit_of(silu(dq)) * width ** (-0.5)
        k = unit_of(silu(dk))
        v = silu(dv)
        boosted = q * grow
        damped = k * damp
        right = jnp.concatenate([v * s_col, k * (s_col * grow)], axis=1)
        kh, kl = halves(k)
        qh, ql = halves(q)
        work = []
        for duo_at in range(rows // duo):
            lo = duo_at * duo
            here = slice(lo, lo + duo)
            left = jnp.concatenate(
                [
                    jnp.concatenate([kh[here], kl[here]], axis=1),
                    jnp.concatenate([qh[here], ql[here]], axis=1),
                ],
                axis=0,
            )
            gram = folded(
                dot_f32(left, wide_rhs(kh[here], kl[here], 0), ((1,), (1,)))
            )
            spread = (
                jnp.where(first, cum[lo : lo + span], cum[lo + span : lo + duo])
                - cum_row[:, here]
            )
            table = jnp.where(inclusive, jnp.exp(jnp.where(inclusive, spread, 0.0)), 0.0)
            scale_col = jnp.where(first, s_col[lo : lo + span], s_col[lo + span : lo + duo])
            near_k = jnp.where(first, gram[:span], gram[span:duo])
            near_q = jnp.where(first, gram[duo : duo + span], gram[duo + span :])
            strict = jnp.where(strictly, near_k * table * scale_col, 0.0)
            work.append([unit - strict, strict, near_q * table])
        yield
        for w in work:
            w[1] = squared(w[1], w[1])
        levels = max(1, (span - 1).bit_length()) - 1
        for level in range(levels):
            if level == levels // 2:
                yield
            for w in work:
                if level + 1 < levels:
                    both = squared(jnp.concatenate([w[1], w[0]], axis=0), w[1])
                    w[1], w[0] = both[:span], w[0] + both[span:]
                else:
                    w[0] = w[0] + squared(w[0], w[1])
        yield
        for duo_at, (inverse, _, inside) in enumerate(work):
            lo = duo_at * duo
            here = slice(lo, lo + duo)
            ih, il = (apart(a) for a in halves(inverse))
            rh, rl = halves(right[here])
            solved = dot_f32(
                jnp.concatenate([ih, il], axis=1), jnp.concatenate([rh, rh], axis=0)
            ) + dot_f32(ih, rl)
            lh, ll = (
                apart(a) for a in halves(jnp.concatenate([damped[here].T, inside], axis=0))
            )
            sh, sl = halves(solved)
            made = dot_f32(
                jnp.concatenate([lh, ll], axis=1), jnp.concatenate([sh, sh], axis=0)
            ) + dot_f32(lh, sl)
            for side in range(2):
                at = lo + side * span
                mine = made[side * (width + span) : (side + 1) * (width + span)]
                n = b * blocks + 2 * duo_at + side
                keep = grow[at + span - 1 : at + span]
                step_map = jnp.where(diagonal, keep, 0.0) - mine[:width, width:]
                query = boosted[at : at + span] - mine[width:, width:]
                high, low = halves(jnp.concatenate([step_map, query], axis=0))
                maps[n, :, :width] = high
                maps[n, :, width:] = low
                adds[n] = mine[:, :width]

    def give(which, out, target):
        here = target.at[:, pl.ds(pl.multiple_of(z * cols, cols), cols)]

        def send(g, k, sem):
            return remote(
                out.at[at_block(g), :], here,
                a_send.at[which], a_recv.at[sem], "sp", g,
            )

        def started(g):
            for k in range(1, sp):
                there = lax.rem(z + k, sp)
                if which == 0:
                    @pl.when(there == g)
                    def _():
                        send(there, k, 0).start()
                else:
                    slow = jnp.logical_or(
                        z == sp - 1, jnp.logical_and(z == 0, there == sp - 1)
                    )

                    @pl.when(jnp.logical_and(there == g, slow))
                    def _():
                        send(there, k, 2).start()

                    @pl.when(jnp.logical_and(there == g, jnp.logical_not(slow)))
                    def _():
                        send(there, k, 1).start()

        return started

    stick_started = give(0, stick_out, sticks)
    delta_started = give(1, delta_out, deltas)

    shorter = jnp.minimum(z, sp - 1 - z)
    down_last = z > sp - 1 - z

    def place(n):
        both = n <= 2 * shorter
        way_n = jnp.where(both, lax.rem(n + 1, 2), jnp.where(down_last, 0, 1))
        step_n = jnp.where(n == 0, 0, jnp.where(both, (n + 1) // 2, n - shorter))
        down = jnp.logical_and(way_n == 0, n > 0)
        return way_n, step_n, down, jnp.where(down, z - step_n, z + step_n)

    last_way = jnp.logical_or(z == 0, z == sp - 1)

    def block_ready(n):
        way_n, step_n, down, b = place(n)
        for step in range(1, sp):
            for way in range(2):
                @pl.when(jnp.logical_and(step_n == step, way_n == way))
                def _():
                    block_came(way, step)
        return b

    def delta_block(b):
        drows = dot_f32(xs[b], ws[:, 3 * cols :]).astype(jnp.bfloat16).astype(jnp.float32)
        return prepare(b, drows[:, :cols], drows[:, cols : 2 * cols], drows[:, 2 * cols :])

    last_way = jnp.logical_or(z == 0, z == sp - 1)
    from_top = z == sp - 1

    def stick_project(n):
        b = jnp.where(from_top, sp - 1 - n, n)
        out = dot_f32(xs[b], ws[:, : 3 * cols]).astype(jnp.bfloat16)
        for i in range(3):
            proj[i, at_block(b), :] = out[:, i * cols : (i + 1) * cols]

    def stick_place(n):
        lower = z < sp // 2
        between = jnp.where(
            n == 0,
            jnp.where(lower, sp - 1, 0),
            jnp.where(
                n == 1,
                jnp.where(lower, sp - 2, 1),
                jnp.where(n == 2, jnp.where(lower, 0, sp - 1), z),
            ),
        )
        return jnp.where(from_top, sp - 1 - n, jnp.where(last_way, n, between))

    def settle(i):
        stick_out[at_block(i), :] = acc[at_block(i), :].astype(jnp.bfloat16)

    def stick_pair(n, r):
        b = stick_place(n)
        i = jnp.where(from_top, b + r, b)
        j = jnp.where(from_top, b, b - r)
        pair(i, j)

        @pl.when(j == 0)
        def _():
            settle(i)
            stick_started(i)

    def walk_groups(start, stop, held=False):
        def group(g, c):
            @pl.when(g > start + held)
            def _():
                delta_started(g - 1)
            memory = memory_ref[...]
            for n in range(blocks):
                memory = walk(g * blocks + n, memory)
            memory_ref[...] = memory
            return c

        lax.fori_loop(start, stop, group, 0)
        delta_started(stop - 1)

    def walk(n, memory):
        high, low = halves(memory)
        new = folded(dot_f32(maps[n], wide_rhs(high, low, 1))) + adds[n]
        made = new[width:]
        made = made * lax.rsqrt(jnp.mean(made * made, axis=-1, keepdims=True) + NORM_EPS)
        at = pl.ds(pl.multiple_of(n * span, span), span)
        delta_out[at, :] = (made * gain_ref[...]).astype(delta_out.dtype)
        return new[:width]

    def plain_delta(n, c):
        @pl.when(n == 1)
        def _():
            relay(stick_kinds[0])

        @pl.when(n == sp - 2)
        def _():
            for c in early[parts:-1]:
                arrive(*c)
            relay(stick_kinds[1])

            @pl.when(z == 0)
            def _():
                walk_groups(0, 2)
            relay(stick_kinds[2])
            arrive(*early[-1])
        for _ in delta_block(block_ready(n)):
            pass
        return c

    events = jnp.where(last_way, sp - 1, sp)
    lax.fori_loop(0, events, plain_delta, 0)

    @pl.when(jnp.logical_not(last_way))
    def _():
        walk_groups(0, sp, held=True)

    relayed(stick_kinds)

    def stick_event(n, c):
        for part in range(2):
            @pl.when(jnp.logical_and(last_way, n == part + 1))
            def _():
                arrive(sp - 1, part)

        def project_one(m, c):
            stick_project(m)
            return c

        needed = jnp.where(from_top, n, stick_place(n)) + 1
        lax.fori_loop(c, needed, project_one, 0)

        @pl.when(jnp.logical_and(jnp.logical_not(last_way), n == 0))
        def _():
            delta_started(0)

        def one(r, c):
            for part in range(2, parts):
                @pl.when(
                    jnp.logical_and(
                        last_way, jnp.logical_and(n == sp - 2, r == sp - 1 - parts + part)
                    )
                )
                def _():
                    arrive(sp - 1, part)
            stick_pair(n, r)
            return c

        lax.fori_loop(0, jnp.where(last_way, n, stick_place(n)) + 1, one, 0)
        return jnp.maximum(c, needed)

    lax.fori_loop(0, events, stick_event, 0)

    @pl.when(last_way)
    def _():
        @pl.when(z == 0)
        def _():
            walk_groups(2, sp - 1)
        for way in range(2):
            @pl.when(comes(way, sp - 1))
            def _():
                block_came(way, sp - 1)
        b = stick_place(sp - 1)
        pieces = []
        for i in range(0, count, 2):
            out = dot_f32(xs[b], ws[:, i * cols : (i + 2) * cols]).astype(jnp.bfloat16)
            pieces += [out[:, :cols], out[:, cols:]]
        for i in range(3):
            proj[i, at_block(b), :] = pieces[i]
        stages = prepare(b, *(piece.astype(jnp.float32) for piece in pieces[3:]))
        for u in range(sp):
            next(stages, None)
            stick_pair(sp - 1, u)
        walk_groups(jnp.where(z == 0, sp - 1, 0), sp)

    mine_z = pl.ds(pl.multiple_of(z * rows, rows), rows)
    lanes = pl.ds(pl.multiple_of(z * cols, cols), cols)
    sticks[:, lanes] = stick_out[mine_z, :]
    deltas[:, lanes] = delta_out[mine_z, :]
    for c in late:
        c.wait()
    all_sent(ws.at[pl.ds(0, 3 * depth), :], w_send.at[0])
    all_sent(xs.at[:, :, slot], f_send.at[0])
    for c in range(sp):
        @pl.when(z == c)
        def _():
            for way, passed in enumerate((c + 1 if c + 1 < sp else 0, sp - c if c > 0 else 0)):
                if passed:
                    all_sent(xs.at[pl.ds(0, passed), :, slot], x_send.at[way])
                    all_sent(shifts_ref.at[pl.ds(0, passed)], s_send.at[way])
    all_came(stick_out.at[pl.ds(0, (sp - 1) * rows), :], a_recv.at[0])
    chunks, wide = outgoing.shape[0], outgoing.shape[2]
    share = rows // tp
    for c in range(chunks):
        columns = slice(c * wide, (c + 1) * wide)
        partial[:, columns] = dot_f32(sticks[...], sw_ref[:, columns])
    all_came(delta_out.at[pl.ds(0, (sp - 2) * rows), :], a_recv.at[1])
    soon = pl.ds(pl.multiple_of(jnp.where(from_top, 1, 0) * cols, cols), (sp - 1) * cols)
    for c in range(chunks):
        columns = slice(c * wide, (c + 1) * wide)
        partial[:, columns] += dot_f32(deltas[:, soon], dw_ref[soon, columns])
    all_came(delta_out.at[pl.ds(0, rows), :], a_recv.at[2])
    final = pl.ds(pl.multiple_of(jnp.where(from_top, 0, sp - 1) * cols, cols), cols)
    mine = pl.ds(pl.multiple_of(t * share, share), share)
    partner = lax.rem(t + 1, tp)
    theirs = pl.ds(pl.multiple_of(partner * share, share), share)

    def finish(which, c):
        columns = slice(c * wide, (c + 1) * wide)
        return (
            partial[which, columns] + dot_f32(deltas[which, final], dw_ref[final, columns])
        ).astype(jnp.bfloat16)

    swaps = [
        remote(
            outgoing.at[c], incoming.at[:, c * wide : (c + 1) * wide],
            c_sem.at[0], c_sem.at[1], "tp", partner,
        )
        for c in range(chunks)
    ]
    for c in range(chunks):
        outgoing[c] = finish(theirs, c)
        if c > 0:
            swaps[c - 1].start()
    for c in range(chunks):
        own[:, c * wide : (c + 1) * wide] = finish(mine, c)
        if c == 0:
            swaps[chunks - 1].start()
    all_came(incoming, c_sem.at[1])
    all_sent(incoming, c_sem.at[0])
    for which, out in enumerate((stick_out, delta_out)):
        all_sent(out.at[pl.ds(0, (sp - 1) * rows), :], a_send.at[which])


ANYWHERE = pl.BlockSpec(memory_space=pltpu.HBM)
ON_CORE = pl.BlockSpec(memory_space=pltpu.VMEM)


def on_device_heads(
    hidden_in, sb_query_w, sb_key_w, sb_value_w, sb_offset,
    delta_query_w, delta_key_w, delta_value_w, decay_w, write_w, write_bias,
    decay_log_scale, decay_shift, head_gain, sb_out_w, delta_out_w,
):
    sp, fs, tp = lax.axis_size("sp"), lax.axis_size("fs"), lax.axis_size("tp")
    rows, half = hidden_in.shape[1:]
    width = half * tp
    length = rows * sp
    heads = decay_log_scale.shape[0]
    cols = sb_query_w.shape[1] // sp
    parts, chunks = 4, 4
    share = rows // tp
    blocks = length // BLOCK
    dma = pltpu.SemaphoreType.DMA
    bf16, f32 = jnp.bfloat16, jnp.float32
    own, incoming = pl.pallas_call(
        layer_kernel,
        name="layer",
        out_shape=(pltpu.VMEM((share, width), bf16),) * 2,
        in_specs=[ANYWHERE] * 16,
        out_specs=(ON_CORE,) * 2,
        scratch_shapes=[
            pltpu.SMEM(sb_offset.shape, f32),
            pltpu.SMEM(decay_log_scale.shape, f32),
            pltpu.SMEM(write_bias.shape, f32),
            pltpu.VMEM((1, head_gain.shape[0]), f32),
            pltpu.VMEM((sp, rows, width), bf16),
            pltpu.VMEM((width, 6 * cols), bf16),
            pltpu.VMEM((2, heads, width), bf16),
            pltpu.VMEM((2 * heads, width), bf16),
            pltpu.VMEM((2 * heads, rows), f32),
            pltpu.VMEM((sp, heads, rows), f32),
            pltpu.VMEM((rows, rows + cols), bf16),
            pltpu.VMEM((3, length, cols), bf16),
            pltpu.VMEM((length, cols), f32),
            pltpu.VMEM((length, cols), f32),
            pltpu.VMEM((cols, cols), f32),
            pltpu.VMEM((blocks, cols + BLOCK, 2 * cols), bf16),
            pltpu.VMEM((blocks, cols + BLOCK, cols), f32),
            pltpu.VMEM((length, cols), bf16),
            pltpu.VMEM((length, cols), bf16),
            pltpu.VMEM((rows, cols * sp), bf16),
            pltpu.VMEM((rows, cols * sp), bf16),
            pltpu.VMEM(sb_out_w.shape, bf16),
            pltpu.VMEM(delta_out_w.shape, bf16),
            pltpu.VMEM((rows, width), f32),
            pltpu.VMEM((chunks, share, width // chunks), bf16),
            dma((2,)), dma((2, sp - 1, parts)), dma((1,)), dma((2 * sp - 1,)),
            dma((1,)), dma((2, 6)), dma((2,)), dma((2,)), dma((2, sp - 1)), dma((11,)),
            dma((2,)), dma((3,)), dma((2,)),
        ],
        compiler_params=pltpu.CompilerParams(
            collective_id=0, has_side_effects=True,
            vmem_limit_bytes=ALL_VMEM - 5 * share * width,
        ),
    )(
        sb_offset, decay_log_scale, write_bias,
        hidden_in.reshape(rows, half), sb_query_w, sb_key_w, sb_value_w,
        delta_query_w, delta_key_w, delta_value_w, decay_w.T, write_w.T,
        decay_shift.reshape(heads, rows), head_gain.reshape(1, -1), sb_out_w, delta_out_w,
    )
    result = (own.astype(f32) + incoming.astype(f32)).astype(bf16)
    return result.reshape(1, share, width)


def on_device(*inputs):
    delta_heads = inputs[11].shape[0]
    square = lax.axis_size("sp") == lax.axis_size("fs") == 4 and lax.axis_size("tp") == 2
    if square and delta_heads == lax.axis_size("sp") and inputs[4].shape[0] % delta_heads == 0:
        return on_device_heads(*inputs)
    return on_device_split(*inputs)


def solution(mesh):
    return jax.shard_map(
        on_device,
        mesh=mesh,
        in_specs=(
            P("fs", "sp", "tp"),
            P("fs", "tp"),
            P("fs", "tp"),
            P("fs", "tp"),
            P("tp"),
            P("fs", "tp"),
            P("fs", "tp"),
            P("fs", "tp"),
            P(None, "tp"),
            P(None, "tp"),
            P("tp"),
            P("tp"),
            P("fs", "tp", "sp"),
            P(),
            P("tp", None),
            P("tp", None),
        ),
        out_specs=P("fs", ("sp", "tp"), None),
        check_vma=False,
    )
```
